512 devices in a mesh: sp: 32 (over z, x), tp: 16 (over y, core).
Axes of the slice: x: 4, y: 8, z: 8, core: 2. Of those that a mesh axis runs over, the one named last changes fastest.
Arguments:
- layer_source_vector: bfloat16 [10240, 2048], P('sp', 'tp'), may hold values from -40 to 40
- attention_lane_source: bfloat16 [10240, 1024], P('sp', 'tp'), may hold values from -6 to 6
- result_valve_logits: bfloat16 [10240, 1024], P('sp', 'tp'), may hold values from -6 to 6
- memory_write_matrix: bfloat16 [10240, 512], P('sp'), may hold values from -6 to 6
- memory_query_matrix: bfloat16 [10240, 512], P('sp'), may hold values from -6 to 6
- increment_logits: bfloat16 [2, 10240, 16], P(None, 'sp', 'tp'), may hold values from -3 to 3
- increment_offset: float32 [2, 16], P(None, 'tp'), may hold values from -16 to -3
- log_fade_speed: float32 [2, 16], P(None, 'tp'), may hold values from 0 to 1.4
- extra_log_fade: float32 [2, 10240, 16], P(None, 'sp', 'tp'), may hold values from -3 to 0
- attention_bypass_factor: float32 [16], P('tp'), may hold values from 0.1 to 1.9
- attention_lane_kernel: bfloat16 [5, 1024], P(None, 'tp'), may hold values from -2.5 to 2.5
- memory_write_kernel: bfloat16 [5, 512], replicated, may hold values from -2.5 to 2.5
- memory_query_kernel: bfloat16 [5, 512], replicated, may hold values from -2.5 to 2.5
- cluster_rescale_factor: float32 [1024], P('tp'), may hold values from 0.1 to 1.9
- blender_result_matrix: bfloat16 [1024, 2048], P(None, 'tp'), may hold values from -0.1875 to 0.1875
- specialist_rescale_factor: float32 [2048], P('tp'), may hold values from 0.1 to 1.9
- chosen_specialists: int32 [10240, 2], P('sp'), may hold values from 0 to 31, all different within a row; in each aligned block of 320 rows (0 to 319, 320 to 639, ...) at most 30 rows name the same one
- specialist_shares: float32 [10240, 2], P('sp'), may hold values from 0.25 to 1.25
- specialist_valve_matrix: bfloat16 [32, 2048, 2048], P('sp', None, 'tp'), may hold values from -0.125 to 0.125
- specialist_raising_matrix: bfloat16 [32, 2048, 2048], P('sp', None, 'tp'), may hold values from -0.125 to 0.125
- specialist_lowering_matrix: bfloat16 [32, 2048, 2048], P('sp', None, 'tp'), may hold values from -0.125 to 0.125
- common_valve_matrix: bfloat16 [2048, 2048], P(None, 'tp'), may hold values from -0.125 to 0.125
- common_raising_matrix: bfloat16 [2048, 2048], P(None, 'tp'), may hold values from -0.125 to 0.125
- common_lowering_matrix: bfloat16 [2048, 2048], P(None, 'tp'), may hold values from -0.125 to 0.125
Outputs:
- result: bfloat16 [10240, 2048], P('sp', 'tp')
The draws below stay inside these ranges and needn't reach their ends.
Inputs may be any that keep to these rules, and one draw needn't show every extreme that they name: `chosen_specialists`: each row names 2 different experts; among the rows of one index of sp no expert is named more than 30 times, a bound that some block reaches there.
All inputs are finite; a program needn't handle non-finite values.
Results may differ from the reference program's by a relative error of at most 0.013.
Values may be sent and summed in bfloat16 or wider, within the bound.
A program may use at most 64 MiB of HBM per device.

```python
import math
import jax
import jax.numpy as jnp
import numpy as np
from jax import lax

D = 2048
HEADS = 16
HEAD_DIM = 64
GROUPS = 4
STATE = 128
CONV = 5
EXP_FF = 2048
SH_FF = 2048
TOP = 2
TOK_DEV = 320
WIDTH = 1024
TOKENS = 10240
EXPERTS = 32
CAP = 30
N_SP = 32


def draw_layer_source_vector(key, part):
    first, second = jax.random.split(key, 2)
    ramp = jnp.exp(math.log(0.5) + math.log(4.0) * jnp.arange(D, dtype=jnp.float32) / (D - 1))
    columns = ramp * jnp.exp(jax.random.uniform(second, (D,), jnp.float32, -0.5, 0.5))
    base = jnp.clip(jax.random.normal(first, (TOKENS, D), jnp.float32), -4.0, 4.0)
    return (base * columns[None, :]).astype(jnp.bfloat16)


def draw_increment_logits(key, part):
    first, second = jax.random.split(key)
    blocks = TOKENS // TOK_DEV
    offset = jax.random.uniform(second, (2, blocks, 1, HEADS), jnp.float32, -0.7, 0.7)
    offset = jnp.broadcast_to(offset, (2, blocks, TOK_DEV, HEADS)).reshape(2, TOKENS, HEADS)
    noise = 0.5 * jnp.clip(jax.random.normal(first, (2, TOKENS, HEADS), jnp.float32), -4.0, 4.0)
    return (noise + offset).astype(jnp.bfloat16)


def draw_increment_offset(key, part):
    first, second, third = jax.random.split(key, 3)
    share = 0.5
    slow = jax.random.uniform(first, (2, HEADS), jnp.float32) < share
    slow_step = jax.random.uniform(second, (2, HEADS), jnp.float32, 0.1, 0.4) / TOKENS
    fast_step = jnp.exp(jax.random.uniform(third, (2, HEADS), jnp.float32, math.log(0.005), math.log(0.02)))
    return jnp.log(jnp.where(slow, slow_step, fast_step)).astype(jnp.float32)


def draw_extra_log_fade(key, part):
    first, second = jax.random.split(key)
    spots = jax.random.randint(first, (2, 4, HEADS), 0, TOKENS)
    strength = jnp.log(jax.random.uniform(second, (2, 4, HEADS), jnp.float32, 0.5, 0.8))
    hits = jnp.arange(TOKENS)[None, None, :, None] == spots[:, :, None, :]
    return jnp.sum(jnp.where(hits, strength[:, :, None, :], 0.0), axis=1).astype(jnp.float32)


def level_of(own_key, extent, shards, low, top_value):
    def one(dim, shards_of):
        steps = jax.random.uniform(jax.random.fold_in(jax.random.fold_in(own_key, 6), dim), (shards_of,), jnp.float32, low / len(shards), top_value / len(shards))
        return jnp.repeat(jnp.exp(steps), extent[dim] // shards_of).reshape((-1,) + (1,) * (len(extent) - dim - 1))

    level = one(*shards[0])
    for cut in shards[1:]:
        level = level * one(*cut)
    return level


def assign_block(rng, own, number, rows, amount, top, limit, lean):
    order = jax.random.permutation(rng, amount)
    packed, common = load_shares(amount, rows * top, limit, lean, True), load_shares(amount, rows * top, limit, lean, False)
    places = jnp.arange(amount)

    def named(lengths, offset_by):
        used = int((lengths > 0).sum())
        fixed = max(1, used // 4)
        passed = fixed + (places - fixed + offset_by * (used - fixed)) % max(1, amount - fixed)
        return jnp.zeros((amount,), jnp.int32).at[order[jnp.where(places < fixed, places, passed)]].set(jnp.asarray(lengths, jnp.int32))

    lengths = jnp.where(number % 4 == 0, named(packed, number // 4), named(common, number - number // 4 - 1))
    mixed = jax.random.permutation(jax.random.fold_in(own, 3), amount)
    source_of, receiver = mixed[0:amount // 2 * 2:2], mixed[1:amount // 2 * 2:2]
    slack = jnp.minimum(lengths[source_of] - 1, limit - lengths[receiver]) // 2
    slack = jnp.where((source_of == order[0]) | (receiver == order[0]) | (lengths[receiver] == 0), 0, jnp.maximum(slack, 0))
    passed = jax.random.randint(jax.random.fold_in(own, 4), (amount // 2,), 0, 1 << 20) % (slack + 1)
    lengths = lengths.at[source_of].add(-passed).at[receiver].add(passed)
    labels = jnp.searchsorted(jnp.cumsum(lengths), jnp.arange(rows * top), side="right").astype(jnp.int32)
    listing = labels.reshape(top, rows).T
    listing = listing[jax.random.permutation(jax.random.fold_in(own, 1), rows)]
    offset_by = jax.random.randint(jax.random.fold_in(own, 2), (rows, 1), 0, top)
    return jnp.take_along_axis(listing, (jnp.arange(top)[None, :] + offset_by) % top, axis=1)


def load_shares(amount, total, reach, skew, full):
    portions = [(1 << 20) // math.isqrt(grade ** skew) + 1 for grade in range(1, amount + 1)]
    largest = reach if full else min(reach, max(-(-total // amount), total * portions[0] // sum(portions)))
    least = 1 if total - largest >= amount - 1 else 0
    holding, rest = [largest] + [least] * (amount - 1), total - largest - least * (amount - 1)
    while rest > 0:
        movable = [i for i in range(1, amount) if holding[i] < largest] or [i for i in range(1, amount) if holding[i] < reach]
        mass, budget = sum([portions[i] for i in movable]), rest
        for i in movable:
            extra = min(reach - holding[i], max(1, budget * portions[i] // mass), rest)
            holding[i] = holding[i] + extra
            rest = rest - extra
    return np.array(holding)


def centred(stream_key, dims, width, reach, cuts=(), kind=jnp.bfloat16):
    entries = width * jax.random.normal(stream_key, dims, jnp.float32)
    if cuts:
        entries = entries * level_of(stream_key, dims, cuts, -0.22, 0.18)
    return jnp.clip(entries, -reach, reach).astype(kind)


def setup_inputs(seed: int = 0) -> dict:
    seeds = jax.random.split(jax.random.key(seed), 25)
    layer_source_vector = draw_layer_source_vector(jax.random.fold_in(seeds[24], 71), 0)
    attention_lane_source = centred(seeds[1], (TOKENS, WIDTH), 1.0, 6.0, ((0, 32), (1, 16)))
    result_valve_logits = centred(seeds[2], (TOKENS, WIDTH), 1.0, 6.0, ((0, 32), (1, 16)))
    memory_write_matrix = centred(seeds[3], (TOKENS, GROUPS * STATE), 1.0, 6.0, ((0, 32),))
    memory_query_matrix = centred(seeds[4], (TOKENS, GROUPS * STATE), 1.0, 6.0, ((0, 32),))
    increment_logits = draw_increment_logits(jax.random.fold_in(seeds[24], 71), 0)
    increment_offset = draw_increment_offset(jax.random.fold_in(seeds[24], 71), 0)
    log_fade_speed = jnp.clip(1.4 * jax.random.uniform(seeds[7], (2, HEADS), jnp.float32) ** level_of(seeds[7], (2, HEADS), ((1, 16),), -0.2, 0.2), 0.0, 1.4)
    extra_log_fade = draw_extra_log_fade(jax.random.fold_in(seeds[24], 71), 0)
    attention_bypass_factor = jnp.clip(1.0 + 0.18 * jax.random.normal(seeds[9], (HEADS,), jnp.float32), 0.1, 1.9)
    attention_lane_kernel = centred(seeds[10], (CONV, WIDTH), CONV ** -0.5, 2.5, ((1, 16),))
    memory_write_kernel = centred(seeds[11], (CONV, GROUPS * STATE), CONV ** -0.5, 2.5)
    memory_query_kernel = centred(seeds[12], (CONV, GROUPS * STATE), CONV ** -0.5, 2.5)
    cluster_rescale_factor = jnp.clip(1.0 + 0.18 * jax.random.normal(seeds[13], (WIDTH,), jnp.float32), 0.1, 1.9)
    blender_result_matrix = centred(seeds[14], (WIDTH, D), WIDTH ** -0.5, 0.1875, ((1, 16),))
    specialist_rescale_factor = jnp.clip(1.0 + 0.18 * jax.random.normal(seeds[15], (D,), jnp.float32), 0.1, 1.9)
    chosen_specialists_keys = jax.random.split(jax.random.fold_in(seeds[16], 1), TOKENS // TOK_DEV)
    chosen_specialists_turns = jax.random.permutation(jax.random.fold_in(seeds[16], 3), TOKENS // TOK_DEV)
    chosen_specialists = jax.vmap(lambda own, number: assign_block(jax.random.fold_in(seeds[16], 2), own, number, TOK_DEV, EXPERTS, TOP, CAP, 1))(chosen_specialists_keys, chosen_specialists_turns).reshape((TOKENS, TOP))
    specialist_shares = jnp.clip(0.25 + 1.0 * jax.random.uniform(seeds[17], (TOKENS, TOP), jnp.float32) ** level_of(seeds[17], (TOKENS, TOP), ((0, 32),), -0.2, 0.2), 0.25, 1.25)
    specialist_valve_matrix = centred(seeds[18], (EXPERTS, D, EXP_FF), D ** -0.5, 0.125, ((0, 32), (2, 16)))
    specialist_raising_matrix = centred(seeds[19], (EXPERTS, D, EXP_FF), D ** -0.5, 0.125, ((0, 32), (2, 16)))
    specialist_lowering_matrix = centred(seeds[20], (EXPERTS, EXP_FF, D), EXP_FF ** -0.5, 0.125, ((0, 32), (2, 16)))
    common_valve_matrix = centred(seeds[21], (D, SH_FF), D ** -0.5, 0.125, ((1, 16),))
    common_raising_matrix = centred(seeds[22], (D, SH_FF), D ** -0.5, 0.125, ((1, 16),))
    common_lowering_matrix = centred(seeds[23], (SH_FF, D), SH_FF ** -0.5, 0.125, ((1, 16),))
    return dict(layer_source_vector=layer_source_vector, attention_lane_source=attention_lane_source, result_valve_logits=result_valve_logits, memory_write_matrix=memory_write_matrix, memory_query_matrix=memory_query_matrix, increment_logits=increment_logits, increment_offset=increment_offset, log_fade_speed=log_fade_speed, extra_log_fade=extra_log_fade, attention_bypass_factor=attention_bypass_factor, attention_lane_kernel=attention_lane_kernel, memory_write_kernel=memory_write_kernel, memory_query_kernel=memory_query_kernel, cluster_rescale_factor=cluster_rescale_factor, blender_result_matrix=blender_result_matrix, specialist_rescale_factor=specialist_rescale_factor, chosen_specialists=chosen_specialists, specialist_shares=specialist_shares, specialist_valve_matrix=specialist_valve_matrix, specialist_raising_matrix=specialist_raising_matrix, specialist_lowering_matrix=specialist_lowering_matrix, common_valve_matrix=common_valve_matrix, common_raising_matrix=common_raising_matrix, common_lowering_matrix=common_lowering_matrix)


def conv_silu(values, taps):
    half = CONV // 2
    length = values.shape[0]
    padded = jnp.pad(values, ((half, half), (0, 0)))
    total = jnp.zeros(values.shape, jnp.float32)
    for offset in range(CONV):
        total = total + padded[offset:offset + length].astype(jnp.float32) * taps[offset].astype(jnp.float32)
    return jax.nn.silu(total).astype(jnp.bfloat16)

def combine_states(earlier, later):
    return (earlier[0] + later[0], jnp.exp(later[0])[:, None, None] * earlier[1] + later[1])

def block_parts(inputs):
    x_block, b_block, c_block, step_block, log_block = inputs
    spread = HEADS // GROUPS
    scores = jnp.einsum('tgn,sgn->gts', c_block.astype(jnp.float32), b_block.astype(jnp.float32), precision=lax.Precision.HIGHEST)
    scores = jnp.repeat(scores, spread, axis=0)
    forward_cum = jnp.cumsum(log_block[0], axis=0)
    backward_cum = jnp.cumsum(log_block[1], axis=0) - log_block[1]
    forward_total = forward_cum[-1]
    backward_total = backward_cum[-1] + log_block[1][-1]
    length = x_block.shape[0]
    position = jnp.arange(length)
    lower = position[:, None] >= position[None, :]
    upper = position[:, None] <= position[None, :]
    forward_gap = forward_cum.T[:, :, None] - forward_cum.T[:, None, :]
    backward_gap = backward_cum.T[:, None, :] - backward_cum.T[:, :, None]
    forward_part = jnp.where(lower, jnp.exp(jnp.where(lower, forward_gap, 0.0)), 0.0) * step_block[0].T[:, None, :]
    backward_part = jnp.where(upper, jnp.exp(jnp.where(upper, backward_gap, 0.0)), 0.0) * step_block[1].T[:, None, :]
    mixing = (scores * (forward_part + backward_part)).astype(jnp.bfloat16)
    inner = jnp.einsum('hts,shp->thp', mixing.astype(jnp.float32), x_block.astype(jnp.float32), precision=lax.Precision.HIGHEST)
    forward_scale = jnp.exp(forward_total[None, :] - forward_cum) * step_block[0]
    backward_scale = jnp.exp(backward_cum) * step_block[1]
    scaled = (jnp.stack([forward_scale, backward_scale])[..., None] * x_block.astype(jnp.float32)[None]).astype(jnp.bfloat16)
    b_heads = jnp.repeat(b_block, spread, axis=1)
    states = jnp.einsum('dshp,shn->dhpn', scaled.astype(jnp.float32), b_heads.astype(jnp.float32), precision=lax.Precision.HIGHEST)
    logs = jnp.stack([forward_total, backward_total])
    return (inner, states, logs)

def run_expert(item):
    rows_in, gate_w, up_w, down_w = item
    hidden = (jax.nn.silu(jnp.dot(rows_in, gate_w, preferred_element_type=jnp.float32)) * jnp.dot(rows_in, up_w, preferred_element_type=jnp.float32)).astype(jnp.bfloat16)
    return jnp.dot(hidden, down_w, preferred_element_type=jnp.float32).astype(jnp.bfloat16)

def reference(layer_source_vector, attention_lane_source, result_valve_logits, memory_write_matrix, memory_query_matrix, increment_logits, increment_offset, log_fade_speed, extra_log_fade, attention_bypass_factor, attention_lane_kernel, memory_write_kernel, memory_query_kernel, cluster_rescale_factor, blender_result_matrix, specialist_rescale_factor, chosen_specialists, specialist_shares, specialist_valve_matrix, specialist_raising_matrix, specialist_lowering_matrix, common_valve_matrix, common_raising_matrix, common_lowering_matrix):
    x_conv = conv_silu(attention_lane_source, attention_lane_kernel)
    b_conv = conv_silu(memory_write_matrix, memory_write_kernel)
    c_conv = conv_silu(memory_query_matrix, memory_query_kernel)
    increment_lengths = jax.nn.softplus(increment_logits.astype(jnp.float32) + increment_offset[:, None, :])
    log_fade_amount = -jnp.exp(log_fade_speed)[:, None, :] * increment_lengths + extra_log_fade
    blocks = N_SP
    x_blocks = x_conv.reshape(blocks, TOK_DEV, HEADS, HEAD_DIM)
    b_blocks = b_conv.reshape(blocks, TOK_DEV, GROUPS, STATE)
    c_blocks = c_conv.reshape(blocks, TOK_DEV, GROUPS, STATE)
    step_blocks = increment_lengths.reshape(2, blocks, TOK_DEV, HEADS).transpose(1, 0, 2, 3)
    log_blocks = log_fade_amount.reshape(2, blocks, TOK_DEV, HEADS).transpose(1, 0, 2, 3)
    inner, states, logs = lax.map(block_parts, (x_blocks, b_blocks, c_blocks, step_blocks, log_blocks))

    def chain_step(carry, item):
        return (combine_states(carry, item), carry)
    zero = (jnp.zeros((HEADS,), jnp.float32), jnp.zeros((HEADS, HEAD_DIM, STATE), jnp.float32))
    _, carried_forward = lax.scan(chain_step, zero, (logs[:, 0], states[:, 0]))
    _, carried_backward = lax.scan(chain_step, zero, (logs[:, 1], states[:, 1]), reverse=True)
    carried = jnp.stack([carried_forward[1], carried_backward[1]], axis=1).astype(jnp.bfloat16)
    c_heads = jnp.repeat(c_blocks, HEADS // GROUPS, axis=2)
    readout = jnp.einsum('kthn,kdhpn->kdthp', c_heads.astype(jnp.float32), carried.astype(jnp.float32), precision=lax.Precision.HIGHEST)
    forward_cum = jnp.cumsum(log_blocks[:, 0], axis=1)
    backward_cum = jnp.cumsum(log_blocks[:, 1], axis=1) - log_blocks[:, 1]
    backward_total = backward_cum[:, -1] + log_blocks[:, 1, -1]
    mixer = inner + jnp.exp(forward_cum)[..., None] * readout[:, 0] + jnp.exp(backward_total[:, None] - backward_cum)[..., None] * readout[:, 1] + attention_bypass_factor[None, None, :, None] * x_blocks.astype(jnp.float32)
    mixer = mixer.reshape(TOKENS, HEADS, HEAD_DIM)
    gated = mixer * jax.nn.silu(result_valve_logits.astype(jnp.float32)).reshape(TOKENS, HEADS, HEAD_DIM)
    grouped = gated.reshape(TOKENS, GROUPS, -1)
    scale = lax.rsqrt(lax.optimization_barrier(jnp.mean(grouped * grouped, axis=-1, keepdims=True)) + 1e-06)
    normed = ((grouped * scale).reshape(TOKENS, WIDTH) * cluster_rescale_factor[None, :]).astype(jnp.bfloat16)
    after_mixer = (layer_source_vector.astype(jnp.float32) + jnp.dot(normed, blender_result_matrix, preferred_element_type=jnp.float32)).astype(jnp.bfloat16)
    resid = after_mixer.astype(jnp.float32)
    features = (resid * lax.rsqrt(lax.optimization_barrier(jnp.mean(resid * resid, axis=1, keepdims=True)) + 1e-06) * specialist_rescale_factor[None, :]).astype(jnp.bfloat16)
    shared_hidden = (jax.nn.silu(jnp.dot(features, common_valve_matrix, preferred_element_type=jnp.float32)) * jnp.dot(features, common_raising_matrix, preferred_element_type=jnp.float32)).astype(jnp.bfloat16)
    shared_out = jnp.dot(shared_hidden, common_lowering_matrix, preferred_element_type=jnp.float32).astype(jnp.bfloat16)
    flat = chosen_specialists.reshape(blocks, TOK_DEV * TOP)
    one_hot = (flat[..., None] == jnp.arange(EXPERTS, dtype=jnp.int32)[None, None, :]).astype(jnp.int32)
    rank = lax.optimization_barrier(jnp.sum((jnp.cumsum(one_hot, axis=1) - one_hot) * one_hot, axis=2))
    place = (jnp.arange(blocks, dtype=jnp.int32)[:, None] * CAP + rank).reshape(-1).astype(jnp.int32)
    expert_flat = flat.reshape(-1).astype(jnp.int32)
    token = (jnp.arange(TOKENS * TOP) // TOP).astype(jnp.int32)
    buffer = jnp.zeros((EXPERTS, blocks * CAP, D), jnp.bfloat16).at[expert_flat, place].set(features[token])
    outputs = lax.map(run_expert, (buffer, specialist_valve_matrix, specialist_raising_matrix, specialist_lowering_matrix))
    picked = outputs[expert_flat, place].astype(jnp.float32).reshape(TOKENS, TOP, D)
    routed = lax.optimization_barrier(jnp.sum(picked * specialist_shares[:, :, None], axis=1))
    return (resid + shared_out.astype(jnp.float32) + routed).astype(jnp.bfloat16)
```

```python
import jax
import jax.numpy as jnp
from jax import lax
from jax.experimental import pallas as pl
from jax.experimental.pallas import tpu as pltpu
from jax.sharding import PartitionSpec as P

D = 2048
HEADS = 16
HEAD_DIM = 64
GROUPS = 4
STATE = 128
CONV = 5

NZ, NX, NY = 8, 4, 8
SP, TP = NZ * NX, NY * 2
T = 320
HALF = T // 2
SLOTS = 32
ROWS = SP * SLOTS
BLOCK = 80
CHUNKS = 2
MESH = pl.DeviceIdType.MESH
F32, BF16 = jnp.float32, jnp.bfloat16


def dot(a, b):
    return jnp.dot(a, b, preferred_element_type=F32)


class Ring:
    def __init__(self, buf, first, rows, sems, index):
        self.buf, self.first, self.rows = buf, first, rows
        self.send, self.recv, self.rsend, self.rrecv = (s.at[index] for s in sems)
        self.sp, tp = lax.axis_index("sp"), lax.axis_index("tp")
        self.y, self.core = tp // 2, tp % 2

    def part(self, chip, core, half=None):
        column = ((chip + 2 * NY) % NY) * 2 + core
        first, rows = self.first, self.rows
        if half is not None:
            rows = rows // 2
            first = first + half * rows
        return self.buf.at[pl.ds(first, rows), pl.ds(pl.multiple_of(column * 128, 128), 128)]

    def hop(self, way, step):
        turn = 1 - 2 * way
        block = self.part(self.y - turn * (step - 1), self.core, way if step == 4 else None)
        return pltpu.make_async_remote_copy(
            src_ref=block,
            dst_ref=block,
            send_sem=self.send.at[4 * way + step - 1],
            recv_sem=self.recv.at[4 * way + step - 1],
            device_id=(self.sp, ((self.y + turn + NY) % NY) * 2 + self.core),
            device_id_type=MESH,
        )

    def landed(self, way, step):
        turn = 1 - 2 * way
        block = self.part(self.y - turn * step, self.core, way if step == 4 else None)
        return pltpu.make_async_remote_copy(
            src_ref=block,
            dst_ref=block,
            send_sem=self.send.at[4 * way + step - 1],
            recv_sem=self.recv.at[4 * way + step - 1],
            device_id=(self.sp, ((self.y + turn + NY) % NY) * 2 + self.core),
            device_id_type=MESH,
        )

    def relay(self, way, step, theirs=False):
        turn = 1 - 2 * way
        core = 1 - self.core if theirs else self.core
        block = self.part(self.y - turn * step, core, way if step == 4 else None)
        slot = 0 if step == 0 else 4 * way + step
        return pltpu.make_async_remote_copy(
            src_ref=block,
            dst_ref=block,
            send_sem=self.rsend.at[slot],
            recv_sem=self.rrecv.at[slot],
            device_id=(self.sp, self.y * 2 + 1 - self.core),
            device_id_type=MESH,
        )

    def start(self):
        self.hop(0, 1).start()
        self.hop(1, 1).start()
        self.relay(0, 0).start()

    def step(self, step):
        for way in (0, 1):
            self.landed(way, step).wait_recv()
            if step < 4:
                self.hop(way, step + 1).start()
            self.relay(way, step).start()

    def finish(self):
        self.relay(0, 0, True).wait_recv()
        for step in range(1, 5):
            for way in (0, 1):
                self.relay(way, step, True).wait_recv()

    def drain(self):
        self.relay(0, 0).wait_send()
        for step in range(1, 5):
            for way in (0, 1):
                self.hop(way, step).wait_send()
                self.relay(way, step).wait_send()


def run(rings):
    for step in range(1, 5):
        for ring in rings:
            ring.step(step)


def kernel(
    st_ref, base_ref, ef_ref, eb_ref, gate_ref, c_ref, ft_ref, src_ref, ch_ref, cht_ref, sh_ref,
    blender_hbm, valve_hbm, raising_hbm, lowering_hbm, cvalve_hbm, craising_hbm, clowering_hbm,
    out_ref,
    rx, tb, rz, ft, wb, wx, wc, wl, wcl, wide, bn, nn, am, ff, sh, xx, hh, dd, oo, ret, pp, qhi, qlo,
    wsem, xs, xr, zs, zr, fs, fr, rsend, rrecv, psend, precv, ds_, dr, os_, or_,
):
    sp, tp = lax.axis_index("sp"), lax.axis_index("tp")
    z, x = sp // NX, sp % NX

    barrier = pltpu.get_barrier_semaphore()

    def greet_tp(k, carry):
        pl.semaphore_signal(barrier, inc=1, device_id=(sp, (tp + k) % TP), device_id_type=MESH)
        return carry

    def greet_sp(k, carry):
        pl.semaphore_signal(barrier, inc=1, device_id=((sp + k) % SP, tp), device_id_type=MESH)
        return carry

    lax.fori_loop(1, TP, greet_tp, 0)
    lax.fori_loop(1, SP, greet_sp, 0)

    loads = [
        pltpu.make_async_copy(blender_hbm, wb, wsem.at[0]),
        pltpu.make_async_copy(valve_hbm.at[0], wx.at[:, pl.ds(0, 128)], wsem.at[1]),
        pltpu.make_async_copy(raising_hbm.at[0], wx.at[:, pl.ds(128, 128)], wsem.at[2]),
        pltpu.make_async_copy(lowering_hbm.at[0], wl, wsem.at[3]),
        pltpu.make_async_copy(cvalve_hbm, wc.at[:, pl.ds(0, 128)], wsem.at[4]),
        pltpu.make_async_copy(craising_hbm, wc.at[:, pl.ds(128, 128)], wsem.at[5]),
        pltpu.make_async_copy(clowering_hbm, wcl, wsem.at[6]),
    ]
    for load in loads:
        load.start()

    rx[x] = st_ref[...]
    ft[tp] = ft_ref[...]
    pl.semaphore_wait(barrier, TP + SP - 2)

    def state_row(k, source):
        return pltpu.make_async_remote_copy(
            src_ref=st_ref,
            dst_ref=rx.at[source],
            send_sem=xs.at[k],
            recv_sem=xr.at[source],
            device_id=(z * NX + (x + k) % NX, tp),
            device_id_type=MESH,
        )

    for k in (2, 1, 3):
        state_row(k, x).start()

    def tile(k, source):
        return pltpu.make_async_remote_copy(
            src_ref=ft_ref,
            dst_ref=ft.at[source],
            send_sem=fs.at[k],
            recv_sem=fr.at[source],
            device_id=(sp, (tp + k) % TP),
            device_id_type=MESH,
        )

    def send_tile(k, carry):
        tile(k, tp).start()
        return carry

    lax.fori_loop(1, TP, send_tile, 0)

    experts = lax.broadcasted_iota(jnp.int32, (T, SP), 1)
    first, second = ch_ref[:, 0:1] == experts, ch_ref[:, 1:2] == experts
    named = jnp.where(first | second, 1.0, 0.0)
    row = lax.broadcasted_iota(jnp.int32, (T, T), 0)
    col = lax.broadcasted_iota(jnp.int32, (T, T), 1)
    lower = jnp.where(col < row, 1.0, 0.0).astype(BF16)
    upper = jnp.where(row < col, 1.0, 0.0).astype(BF16)
    rank = dot(lower, named.astype(BF16))
    rank = jnp.where(named > 0, rank, 99.0).astype(BF16)
    shares = jnp.where(first, sh_ref[:, 0:1], 0.0) + jnp.where(second, sh_ref[:, 1:2], 0.0)
    share_hi = shares.astype(BF16)
    share_lo = (shares - share_hi.astype(F32)).astype(BF16)
    spread = jnp.where(
        lax.broadcasted_iota(jnp.int32, (SP, ROWS), 1) // SLOTS
        == lax.broadcasted_iota(jnp.int32, (SP, ROWS), 0),
        1.0,
        0.0,
    ).astype(BF16)
    place = (lax.broadcasted_iota(jnp.int32, (T, ROWS), 1) % SLOTS).astype(F32)
    here = dot(rank, spread) == place
    qhi[...] = jnp.where(here, dot(share_hi, spread), 0.0).astype(BF16)
    qlo[...] = jnp.where(here, dot(share_lo, spread), 0.0).astype(BF16)
    experts = lax.broadcasted_iota(jnp.int32, (SP, T), 0)
    named = jnp.where((cht_ref[0:1, :] == experts) | (cht_ref[1:2, :] == experts), 1.0, 0.0)
    rank = dot(named.astype(BF16), upper)
    rank = jnp.where(named > 0, rank, 99.0).astype(BF16)
    spread = jnp.where(
        lax.broadcasted_iota(jnp.int32, (ROWS, SP), 0) // SLOTS
        == lax.broadcasted_iota(jnp.int32, (ROWS, SP), 1),
        1.0,
        0.0,
    ).astype(BF16)
    place = (lax.broadcasted_iota(jnp.int32, (ROWS, T), 0) % SLOTS).astype(F32)
    pp[...] = jnp.where(dot(spread, rank) == place, 1.0, 0.0).astype(BF16)

    for k in (1, 2, 3):
        state_row(k, (x + k) % NX).wait_recv()

    def state(block):
        return block[0:64].astype(F32)

    def log_of(block):
        logs = block[64:80].astype(F32)
        return logs[0:1] + logs[1:2] + logs[2:3]

    pad = jnp.zeros((13, 128), BF16)

    def packed(total, log):
        hi = log.astype(BF16)
        rest = log - hi.astype(F32)
        mid = rest.astype(BF16)
        low = (rest - mid.astype(F32)).astype(BF16)
        tail = lax.broadcasted_iota(jnp.int32, (16, 128), 0)
        rows = jnp.where(
            tail == 0,
            hi.astype(F32),
            jnp.where(tail == 1, mid.astype(F32), jnp.where(tail == 2, low.astype(F32), 0.0)),
        )
        return total.astype(BF16), rows.astype(BF16)

    for way in (0, 1):
        total, log = jnp.zeros((64, 128), F32), jnp.zeros((1, 128), F32)
        for i in range(NX) if way == 0 else reversed(range(NX)):
            block = rx[i, way]
            own = log_of(block)
            total = jnp.exp(own) * total + state(block)
            log = log + own
        top, tail = packed(total, log)
        tb[way, 0:64] = top
        tb[way, 64:80] = tail
    rz[z] = tb[0]

    def state_column(k, source):
        return pltpu.make_async_remote_copy(
            src_ref=tb.at[(z + k) // NZ],
            dst_ref=rz.at[source],
            send_sem=zs.at[k],
            recv_sem=zr.at[source],
            device_id=(((z + k) % NZ) * NX + x, tp),
            device_id_type=MESH,
        )

    for k in (4, 3, 5, 2, 6, 1, 7):
        state_column(k, z).start()

    loads[0].wait()
    wide[...] = jnp.zeros(wide.shape, BF16)

    def widen(j, carry):
        block = wb[pl.ds(pl.multiple_of(j * 64, 64), 64), :]
        wide[pl.ds(pl.multiple_of(j * 128, 128), 64), pl.ds(0, 128)] = block
        wide[pl.ds(pl.multiple_of(j * 128 + 64, 64), 64), pl.ds(128, 128)] = block
        return carry

    lax.fori_loop(0, HEADS, widen, 0)

    for k in range(1, NZ):
        state_column(k, (z + k) % NZ).wait_recv()

    carried = []
    for way in (0, 1):
        total = jnp.zeros((64, 128), F32)
        for i in range(NZ) if way == 0 else reversed(range(NZ)):
            block = rz[i]
            passed = (i < z) if way == 0 else (i > z)
            total = jnp.where(passed, jnp.exp(log_of(block)) * total + state(block), total)
        for i in range(NX) if way == 0 else reversed(range(NX)):
            block = rx[i, way]
            passed = (i < x) if way == 0 else (i > x)
            total = jnp.where(passed, jnp.exp(log_of(block)) * total + state(block), total)
        carried.append(total.astype(BF16))

    def read(state_block):
        none = jnp.zeros((64, 128), BF16)
        dims = (((1,), (1,)), ((), ()))
        left = jnp.concatenate([state_block, none], axis=0)
        right = jnp.concatenate([none, state_block], axis=0)
        return lax.dot_general(
            c_ref[0:HALF], left, dims, preferred_element_type=F32
        ) + lax.dot_general(c_ref[HALF:T], right, dims, preferred_element_type=F32)

    mixer = base_ref[...] + ef_ref[...] * read(carried[0]) + eb_ref[...] * read(carried[1])
    mine = pl.ds(pl.multiple_of(tp * 128, 128), 128)
    bn[:, mine] = (mixer * gate_ref[...]).astype(BF16)

    sems = (rsend, rrecv, psend, precv)
    ring = Ring(bn, 0, HALF, sems, 0)
    ring.start()

    def wait_tile(k, carry):
        tile(k, (tp + k) % TP).wait_recv()
        return carry

    lax.fori_loop(1, TP, wait_tile, 0)
    run([ring])
    ring.finish()
    done = [ring]

    left = lax.broadcasted_iota(jnp.int32, (HALF, 128), 1) < 64
    for g in range(GROUPS):
        squares = jnp.zeros((HALF, 128), F32)
        for j in range(4 * g, 4 * g + 4):
            v = bn[:, 128 * j : 128 * j + 128].astype(F32)
            squares = squares + v * v
        top = jnp.sum(jnp.where(left, squares, 0.0), axis=1, keepdims=True)
        bottom = jnp.sum(jnp.where(left, 0.0, squares), axis=1, keepdims=True)
        scale = lax.rsqrt(jnp.where(left, top, bottom) / (4 * HEAD_DIM) + 1e-06)
        for j in range(4 * g, 4 * g + 4):
            v = bn[:, 128 * j : 128 * j + 128].astype(F32)
            nn[:, 128 * j : 128 * j + 128] = (v * scale * ft[j, 1:2]).astype(BF16)
    projected = dot(nn[...], wide[...])
    am[0:HALF, mine] = (src_ref[0:HALF].astype(F32) + projected[:, 0:128]).astype(BF16)
    am[HALF:T, mine] = (src_ref[HALF:T].astype(F32) + projected[:, 128:256]).astype(BF16)

    rings = [Ring(am, i * HALF, HALF, sems, 1 + i) for i in range(2)]
    for ring in rings:
        ring.start()
    run(rings)
    for ring in rings:
        ring.finish()
    done += rings

    squares = jnp.zeros((T, 128), F32)
    for j in range(TP):
        v = am[:, 128 * j : 128 * j + 128].astype(F32)
        squares = squares + v * v
    scale = lax.rsqrt(jnp.sum(squares, axis=1, keepdims=True) / D + 1e-06)
    own = (am[:, mine].astype(F32) * scale * ft[tp, 0:1]).astype(BF16)
    dd[...] = dot(pp[...], own).astype(BF16)

    def rows_of(i):
        return pl.ds(pl.multiple_of(i * SLOTS, SLOTS), SLOTS)

    def deliver(k, source):
        target = (sp + k) % SP
        return pltpu.make_async_remote_copy(
            src_ref=dd.at[rows_of(target)],
            dst_ref=xx.at[rows_of(source), mine],
            send_sem=ds_.at[k],
            recv_sem=dr.at[source],
            device_id=(target, tp),
            device_id_type=MESH,
        )

    def send_rows(k, carry):
        deliver(k, sp).start()
        return carry

    lax.fori_loop(1, SP, send_rows, 0)
    xx[rows_of(sp), mine] = dd[rows_of(sp)]

    for j in range(TP):
        v = am[:, 128 * j : 128 * j + 128].astype(F32)
        ff[:, 128 * j : 128 * j + 128] = (v * scale * ft[j, 0:1]).astype(BF16)
    loads[4].wait()
    loads[5].wait()
    both = dot(ff[...], wc[...])
    sh[:, mine] = (jax.nn.silu(both[:, 0:128]) * both[:, 128:256]).astype(BF16)
    ring = Ring(sh, 0, T, sems, 3)
    ring.start()
    run([ring])

    size = ROWS // CHUNKS
    per = SP // CHUNKS

    def wait_rows(i, carry):
        @pl.when(i != sp)
        def _():
            deliver(1, i).wait_recv()

        return carry

    gathers = []
    for q in range(CHUNKS):
        lax.fori_loop(q * per, (q + 1) * per, wait_rows, 0)
        gathers.append(Ring(xx, q * size, size, sems, 4 + q))
        gathers[-1].start()
    ring.finish()
    done.append(ring)
    loads[6].wait()
    shared = dot(sh[...], wcl[...]).astype(BF16).astype(F32)
    run(gathers)
    done += gathers

    loads[1].wait()
    loads[2].wait()
    hiddens = []
    for q in range(CHUNKS):
        gathers[q].finish()

        def hidden(i, carry):
            at = pl.ds(pl.multiple_of(i * 128, 128), 128)
            both = dot(xx[at, :], wx[...])
            hh[at, mine] = (jax.nn.silu(both[:, 0:128]) * both[:, 128:256]).astype(BF16)
            return carry

        lax.fori_loop(q * size // 128, (q + 1) * size // 128, hidden, 0)
        hiddens.append(Ring(hh, q * size, size, sems, 4 + CHUNKS + q))
        hiddens[-1].start()
    run(hiddens)
    done += hiddens

    def give(i, source):
        return pltpu.make_async_remote_copy(
            src_ref=oo.at[rows_of(i)],
            dst_ref=ret.at[rows_of(source)],
            send_sem=os_.at[i],
            recv_sem=or_.at[source],
            device_id=(i, tp),
            device_id_type=MESH,
        )

    loads[3].wait()
    for q in range(CHUNKS):
        hiddens[q].finish()

        def lowered(i, carry):
            at = pl.ds(pl.multiple_of(i * 128, 128), 128)
            oo[at, :] = dot(hh[at, :], wl[...]).astype(BF16)
            return carry

        lax.fori_loop(q * size // 128, (q + 1) * size // 128, lowered, 0)

        def send_back(k, carry):
            i = q * per + (sp + k) % per

            @pl.when(i != sp)
            def _():
                give(i, sp).start()

            return carry

        lax.fori_loop(0, per, send_back, 0)
    ret[rows_of(sp), :] = oo[rows_of(sp), :]

    def wait_back(k, carry):
        i = (sp + k) % SP
        give(i, i).wait_recv()
        return carry

    lax.fori_loop(1, SP, wait_back, 0)
    routed = dot(qhi[...], ret[...]) + dot(qlo[...], ret[...])
    out_ref[...] = (am[:, mine].astype(F32) + shared + routed).astype(BF16)

    for k in (1, 2, 3):
        state_row(k, x).wait_send()
    for k in range(1, NZ):
        state_column(k, z).wait_send()

    def drain_tp(k, carry):
        tile(k, tp).wait_send()
        return carry

    lax.fori_loop(1, TP, drain_tp, 0)

    def drain_sp(k, carry):
        deliver(k, sp).wait_send()
        give((sp + k) % SP, sp).wait_send()
        return carry

    lax.fori_loop(1, SP, drain_sp, 0)
    for ring in done:
        ring.drain()


def whole(*operands):
    vmem = pl.BlockSpec(memory_space=pltpu.VMEM)
    hbm = pl.BlockSpec(memory_space=pl.ANY)
    rings = 4 + 2 * CHUNKS
    dma = pltpu.SemaphoreType.DMA
    return pl.pallas_call(
        kernel,
        out_shape=jax.ShapeDtypeStruct((T, 128), BF16),
        in_specs=[vmem] * 11 + [hbm] * 7,
        out_specs=vmem,
        scratch_shapes=[
            pltpu.VMEM((NX, 2, BLOCK, 128), BF16),
            pltpu.VMEM((2, BLOCK, 128), BF16),
            pltpu.VMEM((NZ, BLOCK, 128), BF16),
            pltpu.VMEM((TP, 8, 128), F32),
            pltpu.VMEM((1024, 128), BF16),
            pltpu.VMEM((D, 256), BF16),
            pltpu.VMEM((D, 256), BF16),
            pltpu.VMEM((D, 128), BF16),
            pltpu.VMEM((D, 128), BF16),
            pltpu.VMEM((D, 256), BF16),
            pltpu.VMEM((HALF, D), BF16),
            pltpu.VMEM((HALF, D), BF16),
            pltpu.VMEM((T, D), BF16),
            pltpu.VMEM((T, D), BF16),
            pltpu.VMEM((T, D), BF16),
            pltpu.VMEM((ROWS, D), BF16),
            pltpu.VMEM((ROWS, D), BF16),
            pltpu.VMEM((ROWS, 128), BF16),
            pltpu.VMEM((ROWS, 128), BF16),
            pltpu.VMEM((ROWS, 128), BF16),
            pltpu.VMEM((ROWS, T), BF16),
            pltpu.VMEM((T, ROWS), BF16),
            pltpu.VMEM((T, ROWS), BF16),
            dma((7,)),
            dma((NX,)), dma((NX,)),
            dma((NZ,)), dma((NZ,)),
            dma((TP,)), dma((TP,)),
            dma((rings, 8)), dma((rings, 8)), dma((rings, 9)), dma((rings, 9)),
            dma((SP,)), dma((SP,)), dma((SP,)), dma((SP,)),
        ],
        compiler_params=pltpu.CompilerParams(collective_id=0, has_side_effects=True),
        name="mixer_experts",
    )(*operands)


def extended(cells, width):
    count = lax.axis_size("sp")
    ends = count - 1
    head, tail = cells[:width], cells[-width:]
    return jnp.concatenate(
        [
            lax.ppermute(tail, "sp", [(i, (i + 1) % count) for i in range(ends)]),
            cells,
            lax.ppermute(head, "sp", [((i + 1) % count, i) for i in range(ends)]),
        ],
        axis=0,
    )


def halves(rows):
    return jnp.concatenate([rows[:HALF], rows[HALF:]], axis=1)


def shards(
    layer_source_vector,
    attention_lane_source,
    result_valve_logits,
    memory_write_matrix,
    memory_query_matrix,
    increment_logits,
    increment_offset,
    log_fade_speed,
    extra_log_fade,
    attention_bypass_factor,
    attention_lane_kernel,
    memory_write_kernel,
    memory_query_kernel,
    cluster_rescale_factor,
    blender_result_matrix,
    specialist_rescale_factor,
    chosen_specialists,
    specialist_shares,
    specialist_valve_matrix,
    specialist_raising_matrix,
    specialist_lowering_matrix,
    common_valve_matrix,
    common_raising_matrix,
    common_lowering_matrix,
):
    length = attention_lane_source.shape[0]
    channels = attention_lane_source.shape[1]
    group = lax.axis_index("tp") * GROUPS // HEADS
    b_own = lax.dynamic_slice_in_dim(memory_write_matrix, group * STATE, STATE, 1)
    c_own = lax.dynamic_slice_in_dim(memory_query_matrix, group * STATE, STATE, 1)
    joined = jnp.concatenate([attention_lane_source, b_own, c_own], axis=1)
    taps = jnp.concatenate(
        [
            attention_lane_kernel,
            lax.dynamic_slice_in_dim(memory_write_kernel, group * STATE, STATE, 1),
            lax.dynamic_slice_in_dim(memory_query_kernel, group * STATE, STATE, 1),
        ],
        axis=1,
    )
    padded = extended(joined, CONV // 2)
    total = jnp.zeros(joined.shape, F32)
    for offset in range(CONV):
        total = total + padded[offset : offset + length].astype(F32) * taps[offset].astype(F32)
    convolved = jax.nn.silu(total).astype(BF16)
    x_conv = convolved[:, :channels]
    b_conv = convolved[:, channels : channels + STATE]
    c_conv = convolved[:, channels + STATE :]
    steps = jax.nn.softplus(increment_logits[:, :, 0].astype(F32) + increment_offset)
    fades = -jnp.exp(log_fade_speed) * steps + extra_log_fade[:, :, 0]
    forward_cum = jnp.cumsum(fades[0])
    backward_cum = jnp.cumsum(fades[1]) - fades[1]
    forward_total = forward_cum[-1]
    backward_total = backward_cum[-1] + fades[1, -1]
    scores = lax.dot_general(
        c_conv, b_conv, (((1,), (1,)), ((), ())), preferred_element_type=F32
    )
    position = jnp.arange(length)
    lower = position[:, None] >= position[None, :]
    upper = position[:, None] <= position[None, :]
    forward_gap = forward_cum[:, None] - forward_cum[None, :]
    backward_gap = backward_cum[None, :] - backward_cum[:, None]
    mixing = scores * (
        jnp.where(lower, jnp.exp(jnp.where(lower, forward_gap, 0.0)), 0.0) * steps[0][None, :]
        + jnp.where(upper, jnp.exp(jnp.where(upper, backward_gap, 0.0)), 0.0) * steps[1][None, :]
    )
    inner = jnp.dot(mixing.astype(BF16), x_conv, preferred_element_type=F32)
    forward_scale = jnp.exp(forward_total - forward_cum) * steps[0]
    backward_scale = jnp.exp(backward_cum) * steps[1]
    scaled = (
        jnp.stack([forward_scale, backward_scale])[:, :, None] * x_conv.astype(F32)[None]
    ).astype(BF16)
    own_states = jnp.einsum("dsp,sn->dpn", scaled, b_conv, preferred_element_type=F32)
    logs = jnp.stack([forward_total, backward_total])
    hi = lax.reduce_precision(logs, 8, 7)
    mid = lax.reduce_precision(logs - hi, 8, 7)
    low = logs - hi - mid
    tail = jnp.stack([hi, mid, low] + [jnp.zeros_like(hi)] * 13, axis=1)
    states = jnp.concatenate(
        [own_states, jnp.broadcast_to(tail[:, :, None], (2, 16, STATE))], axis=1
    ).astype(BF16)
    base = halves(inner + attention_bypass_factor[0] * x_conv.astype(F32))
    wide = (length, channels)
    from_left = halves(jnp.broadcast_to(jnp.exp(forward_cum)[:, None], wide))
    from_right = halves(jnp.broadcast_to(jnp.exp(backward_total - backward_cum)[:, None], wide))
    gate = halves(jax.nn.silu(result_valve_logits.astype(F32)))
    gains = jnp.concatenate(
        [
            specialist_rescale_factor[None],
            jnp.concatenate([cluster_rescale_factor, cluster_rescale_factor])[None],
            jnp.zeros((6, 128), F32),
        ]
    )
    return whole(
        states, base, from_left, from_right, gate, c_conv, gains, layer_source_vector,
        chosen_specialists, chosen_specialists.T, specialist_shares,
        blender_result_matrix, specialist_valve_matrix, specialist_raising_matrix,
        specialist_lowering_matrix, common_valve_matrix, common_raising_matrix, common_lowering_matrix,
    )


def solution(mesh):
    return jax.shard_map(
        shards,
        mesh=mesh,
        in_specs=(
            P("sp", "tp"),
            P("sp", "tp"),
            P("sp", "tp"),
            P("sp", None),
            P("sp", None),
            P(None, "sp", "tp"),
            P(None, "tp"),
            P(None, "tp"),
            P(None, "sp", "tp"),
            P("tp"),
            P(None, "tp"),
            P(),
            P(),
            P("tp"),
            P(None, "tp"),
            P("tp"),
            P("sp", None),
            P("sp", None),
            P("sp", None, "tp"),
            P("sp", None, "tp"),
            P("sp", None, "tp"),
            P(None, "tp"),
            P(None, "tp"),
            P(None, "tp"),
        ),
        out_specs=P("sp", "tp"),
        check_vma=False,
    )
```

```python
import jax
import jax.numpy as jnp
from jax import lax
from jax.experimental import pallas as pl
from jax.experimental.pallas import tpu as pltpu
from jax.sharding import PartitionSpec as P

D = 2048
HEADS = 16
HEAD_DIM = 64
GROUPS = 4
STATE = 128
CONV = 5

NZ, NX, NY = 8, 4, 8
SP, TP = NZ * NX, NY * 2
T = 320
HALF = T // 2
SLOTS = 32
ROWS = SP * SLOTS
BLOCK = 80
CHUNKS = 2
MESH = pl.DeviceIdType.MESH
F32, BF16 = jnp.float32, jnp.bfloat16


def dot(a, b):
    return jnp.dot(a, b, preferred_element_type=F32)


class Ring:
    def __init__(self, buf, first, rows, sems, index, direct=False):
        self.buf, self.first, self.rows, self.direct = buf, first, rows, direct
        self.send, self.recv, self.rsend, self.rrecv = (s.at[index] for s in sems)
        self.sp, tp = lax.axis_index("sp"), lax.axis_index("tp")
        self.y, self.core = tp // 2, tp % 2

    def part(self, chip, core, half=None):
        column = ((chip + 2 * NY) % NY) * 2 + core
        first, rows = self.first, self.rows
        if half is not None:
            rows = rows // 2
            first = first + half * rows
        return self.buf.at[pl.ds(first, rows), pl.ds(pl.multiple_of(column * 128, 128), 128)]

    def along(self, way, step, chip, far):
        turn = 1 - 2 * way
        block = self.part(chip, self.core, way if step == 4 else None)
        return pltpu.make_async_remote_copy(
            src_ref=block,
            dst_ref=block,
            send_sem=self.send.at[4 * way + step - 1],
            recv_sem=self.recv.at[4 * way + step - 1],
            device_id=(self.sp, ((self.y + turn * far + NY) % NY) * 2 + self.core),
            device_id_type=MESH,
        )

    def hop(self, way, step):
        if self.direct:
            return self.along(way, step, self.y, step)
        return self.along(way, step, self.y - (1 - 2 * way) * (step - 1), 1)

    def landed(self, way, step):
        return self.along(way, step, self.y - (1 - 2 * way) * step, 1)

    def relay(self, way, step, theirs=False):
        turn = 1 - 2 * way
        core = 1 - self.core if theirs else self.core
        block = self.part(self.y - turn * step, core, way if step == 4 else None)
        slot = 0 if step == 0 else 4 * way + step
        return pltpu.make_async_remote_copy(
            src_ref=block,
            dst_ref=block,
            send_sem=self.rsend.at[slot],
            recv_sem=self.rrecv.at[slot],
            device_id=(self.sp, self.y * 2 + 1 - self.core),
            device_id_type=MESH,
        )

    def start(self):
        for step in (4, 3, 2, 1) if self.direct else (1,):
            self.hop(0, step).start()
            self.hop(1, step).start()
        self.relay(0, 0).start()

    def step(self, step):
        for way in (0, 1):
            self.landed(way, step).wait_recv()
            if step < 4 and not self.direct:
                self.hop(way, step + 1).start()
            self.relay(way, step).start()

    def finish(self):
        self.relay(0, 0, True).wait_recv()
        for step in range(1, 5):
            for way in (0, 1):
                self.relay(way, step, True).wait_recv()

    def drain(self):
        self.relay(0, 0).wait_send()
        for step in range(1, 5):
            for way in (0, 1):
                self.hop(way, step).wait_send()
                self.relay(way, step).wait_send()


def run(rings):
    for step in range(1, 5):
        for ring in rings:
            ring.step(step)


def kernel(
    st_ref, base_ref, ef_ref, eb_ref, gate_ref, c_ref, ft_ref, src_ref, ch_ref, cht_ref, sh_ref,
    blender_hbm, valve_hbm, raising_hbm, lowering_hbm, cvalve_hbm, craising_hbm, clowering_hbm,
    out_ref,
    rx, tb, rz, ft, sq, so, wb, wx, wc, wl, wcl, wide, bn, nn, am, ff, sh, xx, hh, dd, oo, ret, pp, qhi, qlo,
    wsem, xs, xr, zs, zr, fs, fr, qs, qr, rsend, rrecv, psend, precv, ds_, dr, os_, or_,
):
    sp, tp = lax.axis_index("sp"), lax.axis_index("tp")
    z, x = sp // NX, sp % NX

    barrier = pltpu.get_barrier_semaphore()

    def greet_tp(k, carry):
        pl.semaphore_signal(barrier, inc=1, device_id=(sp, (tp + k) % TP), device_id_type=MESH)
        return carry

    def greet_sp(k, carry):
        pl.semaphore_signal(barrier, inc=1, device_id=((sp + k) % SP, tp), device_id_type=MESH)
        return carry

    lax.fori_loop(1, TP, greet_tp, 0)
    lax.fori_loop(1, SP, greet_sp, 0)

    loads = [
        pltpu.make_async_copy(blender_hbm, wb, wsem.at[0]),
        pltpu.make_async_copy(valve_hbm.at[0], wx.at[:, pl.ds(0, 128)], wsem.at[1]),
        pltpu.make_async_copy(raising_hbm.at[0], wx.at[:, pl.ds(128, 128)], wsem.at[2]),
        pltpu.make_async_copy(lowering_hbm.at[0], wl, wsem.at[3]),
        pltpu.make_async_copy(cvalve_hbm, wc.at[:, pl.ds(0, 128)], wsem.at[4]),
        pltpu.make_async_copy(craising_hbm, wc.at[:, pl.ds(128, 128)], wsem.at[5]),
        pltpu.make_async_copy(clowering_hbm, wcl, wsem.at[6]),
    ]
    for load in loads:
        load.start()

    rx[x] = st_ref[...]
    ft[tp] = ft_ref[...]
    def state_row(k, source):
        return pltpu.make_async_remote_copy(
            src_ref=st_ref,
            dst_ref=rx.at[source],
            send_sem=xs.at[k],
            recv_sem=xr.at[source],
            device_id=(z * NX + (x + k) % NX, tp),
            device_id_type=MESH,
        )

    def tile(k, source):
        return pltpu.make_async_remote_copy(
            src_ref=ft_ref,
            dst_ref=ft.at[source],
            send_sem=fs.at[k],
            recv_sem=fr.at[source],
            device_id=(sp, (tp + k) % TP),
            device_id_type=MESH,
        )

    def send_tile(k, carry):
        tile(k, tp).start()
        return carry

    experts = lax.broadcasted_iota(jnp.int32, (T, SP), 1)
    first, second = ch_ref[:, 0:1] == experts, ch_ref[:, 1:2] == experts
    named = jnp.where(first | second, 1.0, 0.0)
    row = lax.broadcasted_iota(jnp.int32, (T, T), 0)
    col = lax.broadcasted_iota(jnp.int32, (T, T), 1)
    lower = jnp.where(col < row, 1.0, 0.0).astype(BF16)
    upper = jnp.where(row < col, 1.0, 0.0).astype(BF16)
    rank = dot(lower, named.astype(BF16))
    rank = jnp.where(named > 0, rank, 99.0).astype(BF16)
    shares = jnp.where(first, sh_ref[:, 0:1], 0.0) + jnp.where(second, sh_ref[:, 1:2], 0.0)
    share_hi = shares.astype(BF16)
    share_lo = (shares - share_hi.astype(F32)).astype(BF16)
    spread = jnp.where(
        lax.broadcasted_iota(jnp.int32, (SP, ROWS), 1) // SLOTS
        == lax.broadcasted_iota(jnp.int32, (SP, ROWS), 0),
        1.0,
        0.0,
    ).astype(BF16)
    place = (lax.broadcasted_iota(jnp.int32, (T, ROWS), 1) % SLOTS).astype(F32)
    here = dot(rank, spread) == place
    qhi[...] = jnp.where(here, dot(share_hi, spread), 0.0).astype(BF16)
    qlo[...] = jnp.where(here, dot(share_lo, spread), 0.0).astype(BF16)
    experts = lax.broadcasted_iota(jnp.int32, (SP, T), 0)
    named = jnp.where((cht_ref[0:1, :] == experts) | (cht_ref[1:2, :] == experts), 1.0, 0.0)
    rank = dot(named.astype(BF16), upper)
    rank = jnp.where(named > 0, rank, 99.0).astype(BF16)
    spread = jnp.where(
        lax.broadcasted_iota(jnp.int32, (ROWS, SP), 0) // SLOTS
        == lax.broadcasted_iota(jnp.int32, (ROWS, SP), 1),
        1.0,
        0.0,
    ).astype(BF16)
    place = (lax.broadcasted_iota(jnp.int32, (ROWS, T), 0) % SLOTS).astype(F32)
    pp[...] = jnp.where(dot(spread, rank) == place, 1.0, 0.0).astype(BF16)

    pl.semaphore_wait(barrier, TP + SP - 2)
    for k in (2, 1, 3):
        state_row(k, x).start()
    lax.fori_loop(1, TP, send_tile, 0)

    for k in (1, 2, 3):
        state_row(k, (x + k) % NX).wait_recv()

    def state(block):
        return block[0:64].astype(F32)

    def log_of(block):
        logs = block[64:80].astype(F32)
        return logs[0:1] + logs[1:2] + logs[2:3]

    pad = jnp.zeros((13, 128), BF16)

    def packed(total, log):
        hi = log.astype(BF16)
        rest = log - hi.astype(F32)
        mid = rest.astype(BF16)
        low = (rest - mid.astype(F32)).astype(BF16)
        tail = lax.broadcasted_iota(jnp.int32, (16, 128), 0)
        rows = jnp.where(
            tail == 0,
            hi.astype(F32),
            jnp.where(tail == 1, mid.astype(F32), jnp.where(tail == 2, low.astype(F32), 0.0)),
        )
        return total.astype(BF16), rows.astype(BF16)

    for way in (0, 1):
        total, log = jnp.zeros((64, 128), F32), jnp.zeros((1, 128), F32)
        for i in range(NX) if way == 0 else reversed(range(NX)):
            block = rx[i, way]
            own = log_of(block)
            total = jnp.exp(own) * total + state(block)
            log = log + own
        top, tail = packed(total, log)
        tb[way, 0:64] = top
        tb[way, 64:80] = tail
    rz[z] = tb[0]

    def state_column(k, source):
        return pltpu.make_async_remote_copy(
            src_ref=tb.at[(z + k) // NZ],
            dst_ref=rz.at[source],
            send_sem=zs.at[k],
            recv_sem=zr.at[source],
            device_id=(((z + k) % NZ) * NX + x, tp),
            device_id_type=MESH,
        )

    for k in (4, 3, 5, 2, 6, 1, 7):
        state_column(k, z).start()

    loads[0].wait()
    wide[...] = jnp.zeros(wide.shape, BF16)

    def widen(j, carry):
        block = wb[pl.ds(pl.multiple_of(j * 64, 64), 64), :]
        wide[pl.ds(pl.multiple_of(j * 128, 128), 64), pl.ds(0, 128)] = block
        wide[pl.ds(pl.multiple_of(j * 128 + 64, 64), 64), pl.ds(128, 128)] = block
        return carry

    lax.fori_loop(0, HEADS, widen, 0)

    for k in range(1, NZ):
        state_column(k, (z + k) % NZ).wait_recv()

    carried = []
    for way in (0, 1):
        total = jnp.zeros((64, 128), F32)
        for i in range(NZ) if way == 0 else reversed(range(NZ)):
            block = rz[i]
            passed = (i < z) if way == 0 else (i > z)
            total = jnp.where(passed, jnp.exp(log_of(block)) * total + state(block), total)
        for i in range(NX) if way == 0 else reversed(range(NX)):
            block = rx[i, way]
            passed = (i < x) if way == 0 else (i > x)
            total = jnp.where(passed, jnp.exp(log_of(block)) * total + state(block), total)
        carried.append(total.astype(BF16))

    def read(state_block):
        none = jnp.zeros((64, 128), BF16)
        dims = (((1,), (1,)), ((), ()))
        left = jnp.concatenate([state_block, none], axis=0)
        right = jnp.concatenate([none, state_block], axis=0)
        return lax.dot_general(
            c_ref[0:HALF], left, dims, preferred_element_type=F32
        ) + lax.dot_general(c_ref[HALF:T], right, dims, preferred_element_type=F32)

    mixer = base_ref[...] + ef_ref[...] * read(carried[0]) + eb_ref[...] * read(carried[1])
    mine = pl.ds(pl.multiple_of(tp * 128, 128), 128)
    bn[:, mine] = (mixer * gate_ref[...]).astype(BF16)

    sems = (rsend, rrecv, psend, precv)
    ring = Ring(bn, 0, HALF, sems, 0, direct=True)
    ring.start()

    def wait_tile(k, carry):
        tile(k, (tp + k) % TP).wait_recv()
        return carry

    lax.fori_loop(1, TP, wait_tile, 0)
    run([ring])
    ring.finish()

    left = lax.broadcasted_iota(jnp.int32, (HALF, 128), 1) < 64
    for g in range(GROUPS):
        squares = jnp.zeros((HALF, 128), F32)
        for j in range(4 * g, 4 * g + 4):
            v = bn[:, 128 * j : 128 * j + 128].astype(F32)
            squares = squares + v * v
        top = jnp.sum(jnp.where(left, squares, 0.0), axis=1, keepdims=True)
        bottom = jnp.sum(jnp.where(left, 0.0, squares), axis=1, keepdims=True)
        scale = lax.rsqrt(jnp.where(left, top, bottom) / (4 * HEAD_DIM) + 1e-06)
        for j in range(4 * g, 4 * g + 4):
            v = bn[:, 128 * j : 128 * j + 128].astype(F32)
            nn[:, 128 * j : 128 * j + 128] = (v * scale * ft[j, 1:2]).astype(BF16)
    projected = dot(nn[...], wide[...])
    am[0:HALF] = (src_ref[0:HALF].astype(F32) + projected[:, 0:128]).astype(BF16)
    am[HALF:T] = (src_ref[HALF:T].astype(F32) + projected[:, 128:256]).astype(BF16)

    dims = (((1,), (1,)), ((), ()))
    squares = am[...].astype(F32) * am[...].astype(F32)
    high = squares.astype(BF16)
    rest = (squares - high.astype(F32)).astype(BF16)
    ones = jnp.ones((8, 128), BF16)
    sums = lax.dot_general(ones, high, dims, preferred_element_type=F32) + lax.dot_general(
        ones, rest, dims, preferred_element_type=F32
    )
    line = jnp.concatenate([sums, jnp.zeros((8, 3 * 128 - T), F32)], axis=1)
    level = lax.broadcasted_iota(jnp.int32, (8, 128), 0)
    own = jnp.where(
        level == 0,
        line[:, 0:128],
        jnp.where(level == 1, line[:, 128:256], jnp.where(level == 2, line[:, 256:384], 0.0)),
    )
    sq[tp] = own
    so[...] = own

    def sums_to(k, source):
        return pltpu.make_async_remote_copy(
            src_ref=so,
            dst_ref=sq.at[source],
            send_sem=qs.at[k],
            recv_sem=qr.at[source],
            device_id=(sp, (tp + k) % TP),
            device_id_type=MESH,
        )

    def send_sums(k, carry):
        sums_to((k + 7) % (TP - 1) + 1, tp).start()
        return carry

    lax.fori_loop(0, TP - 1, send_sums, 0)
    ring.drain()

    def wait_sums(k, carry):
        sums_to(k, (tp + k) % TP).wait_recv()
        return carry

    lax.fori_loop(1, TP, wait_sums, 0)
    total = sq[0]
    for j in range(1, TP):
        total = total + sq[j]
    line = jnp.concatenate([total[0:1], total[1:2], total[2:3]], axis=1)
    high = line.astype(BF16).astype(F32)
    middle = (line - high).astype(BF16).astype(F32)
    low = line - high - middle
    level = lax.broadcasted_iota(jnp.int32, (8, 384), 0)
    parts = jnp.where(
        level == 0, high, jnp.where(level == 1, middle, jnp.where(level == 2, low, 0.0))
    ).astype(BF16)
    same = jnp.where(
        lax.broadcasted_iota(jnp.int32, (T, 384), 0) == lax.broadcasted_iota(jnp.int32, (T, 384), 1),
        1.0,
        0.0,
    ).astype(BF16)
    upright = lax.dot_general(same, parts, dims, preferred_element_type=F32)
    scale = lax.rsqrt((upright[:, 0:1] + upright[:, 1:2] + upright[:, 2:3]) / D + 1e-06)
    own = (am[...].astype(F32) * scale * ft_ref[0:1]).astype(BF16)
    ff[:, mine] = own
    dd[...] = dot(pp[...], own).astype(BF16)

    def rows_of(i):
        return pl.ds(pl.multiple_of(i * SLOTS, SLOTS), SLOTS)

    def deliver(k, source):
        target = (sp + k) % SP
        return pltpu.make_async_remote_copy(
            src_ref=dd.at[rows_of(target)],
            dst_ref=xx.at[rows_of(source), mine],
            send_sem=ds_.at[k],
            recv_sem=dr.at[source],
            device_id=(target, tp),
            device_id_type=MESH,
        )

    def send_rows(k, carry):
        deliver(k, sp).start()
        return carry

    lax.fori_loop(1, SP, send_rows, 0)
    xx[rows_of(sp), mine] = dd[rows_of(sp)]

    spread_out = [Ring(ff, i * HALF, HALF, sems, 1 + i) for i in range(2)]
    for ring in spread_out:
        ring.start()

    size = ROWS // CHUNKS
    per = SP // CHUNKS

    def wait_rows(i, carry):
        @pl.when(i != sp)
        def _():
            deliver(1, i).wait_recv()

        return carry

    for step in (1, 2):
        for ring in spread_out:
            ring.step(step)
    gathers = []
    for q in range(CHUNKS):
        lax.fori_loop(q * per, (q + 1) * per, wait_rows, 0)
        gathers.append(Ring(xx, q * size, size, sems, 4 + q))
        gathers[-1].start()
    for step in (3, 4):
        for ring in spread_out:
            ring.step(step)
    for ring in gathers:
        ring.step(1)
    for ring in spread_out:
        ring.finish()
    loads[4].wait()
    loads[5].wait()
    both = dot(ff[...], wc[...])
    sh[:, mine] = (jax.nn.silu(both[:, 0:128]) * both[:, 128:256]).astype(BF16)
    hidden_out = Ring(sh, 0, T, sems, 3)
    hidden_out.start()
    for step in (2, 3, 4):
        for ring in gathers:
            ring.step(step)
        hidden_out.step(step - 1)

    loads[1].wait()
    loads[2].wait()
    hiddens = []
    for q in range(CHUNKS):
        gathers[q].finish()
        at = pl.ds(q * size, size)
        both = dot(xx[at, :], wx[...])
        hh[at, mine] = (jax.nn.silu(both[:, 0:128]) * both[:, 128:256]).astype(BF16)
        hiddens.append(Ring(hh, q * size, size, sems, 4 + CHUNKS + q))
        hiddens[-1].start()
    hidden_out.step(4)
    for k in (1, 2, 3):
        state_row(k, x).wait_send()
    for k in range(1, NZ):
        state_column(k, z).wait_send()

    def drain_tp(k, carry):
        tile(k, tp).wait_send()
        sums_to(k, tp).wait_send()
        return carry

    lax.fori_loop(1, TP, drain_tp, 0)

    def drain_sp(k, carry):
        deliver(k, sp).wait_send()
        return carry

    lax.fori_loop(1, SP, drain_sp, 0)
    for ring in spread_out + gathers:
        ring.drain()
    for ring in hiddens:
        ring.step(1)
    hidden_out.finish()
    loads[6].wait()
    shared = dot(sh[...], wcl[...]).astype(BF16).astype(F32)
    out_ref[...] = shared.astype(BF16)
    hidden_out.drain()
    for step in (2, 3, 4):
        for ring in hiddens:
            ring.step(step)

    def give(i, source):
        return pltpu.make_async_remote_copy(
            src_ref=oo.at[rows_of(i)],
            dst_ref=ret.at[rows_of(source)],
            send_sem=os_.at[i],
            recv_sem=or_.at[source],
            device_id=(i, tp),
            device_id_type=MESH,
        )

    loads[3].wait()
    for q in range(CHUNKS):
        hiddens[q].finish()

        at = pl.ds(q * size, size)
        oo[at, :] = dot(hh[at, :], wl[...]).astype(BF16)

        def send_back(k, carry):
            i = q * per + (sp + k) % per

            @pl.when(i != sp)
            def _():
                give(i, sp).start()

            return carry

        lax.fori_loop(0, per, send_back, 0)
    ret[rows_of(sp), :] = oo[rows_of(sp), :]

    for ring in hiddens:
        ring.drain()

    def wait_back(k, carry):
        i = (sp + k) % SP
        give(i, i).wait_recv()
        give(i, sp).wait_send()
        return carry

    lax.fori_loop(1, SP, wait_back, 0)
    routed = dot(qhi[...], ret[...]) + dot(qlo[...], ret[...])
    out_ref[...] = (am[...].astype(F32) + out_ref[...].astype(F32) + routed).astype(BF16)


def whole(*operands):
    vmem = pl.BlockSpec(memory_space=pltpu.VMEM)
    hbm = pl.BlockSpec(memory_space=pl.ANY)
    rings = 4 + 2 * CHUNKS
    dma = pltpu.SemaphoreType.DMA
    return pl.pallas_call(
        kernel,
        out_shape=jax.ShapeDtypeStruct((T, 128), BF16),
        in_specs=[vmem] * 11 + [hbm] * 7,
        out_specs=vmem,
        scratch_shapes=[
            pltpu.VMEM((NX, 2, BLOCK, 128), BF16),
            pltpu.VMEM((2, BLOCK, 128), BF16),
            pltpu.VMEM((NZ, BLOCK, 128), BF16),
            pltpu.VMEM((TP, 8, 128), F32),
            pltpu.VMEM((TP, 8, 128), F32),
            pltpu.VMEM((8, 128), F32),
            pltpu.VMEM((1024, 128), BF16),
            pltpu.VMEM((D, 256), BF16),
            pltpu.VMEM((D, 256), BF16),
            pltpu.VMEM((D, 128), BF16),
            pltpu.VMEM((D, 128), BF16),
            pltpu.VMEM((D, 256), BF16),
            pltpu.VMEM((HALF, D), BF16),
            pltpu.VMEM((HALF, D), BF16),
            pltpu.VMEM((T, 128), BF16),
            pltpu.VMEM((T, D), BF16),
            pltpu.VMEM((T, D), BF16),
            pltpu.VMEM((ROWS, D), BF16),
            pltpu.VMEM((ROWS, D), BF16),
            pltpu.VMEM((ROWS, 128), BF16),
            pltpu.VMEM((ROWS, 128), BF16),
            pltpu.VMEM((ROWS, 128), BF16),
            pltpu.VMEM((ROWS, T), BF16),
            pltpu.VMEM((T, ROWS), BF16),
            pltpu.VMEM((T, ROWS), BF16),
            dma((7,)),
            dma((NX,)), dma((NX,)),
            dma((NZ,)), dma((NZ,)),
            dma((TP,)), dma((TP,)),
            dma((TP,)), dma((TP,)),
            dma((rings, 8)), dma((rings, 8)), dma((rings, 9)), dma((rings, 9)),
            dma((SP,)), dma((SP,)), dma((SP,)), dma((SP,)),
        ],
        compiler_params=pltpu.CompilerParams(collective_id=0, has_side_effects=True),
        name="mixer_experts",
    )(*operands)


def extended(cells, width):
    count = lax.axis_size("sp")
    ends = count - 1
    head, tail = cells[:width], cells[-width:]
    return jnp.concatenate(
        [
            lax.ppermute(tail, "sp", [(i, (i + 1) % count) for i in range(ends)]),
            cells,
            lax.ppermute(head, "sp", [((i + 1) % count, i) for i in range(ends)]),
        ],
        axis=0,
    )


def halves(rows):
    return jnp.concatenate([rows[:HALF], rows[HALF:]], axis=1)


def shards(
    layer_source_vector,
    attention_lane_source,
    result_valve_logits,
    memory_write_matrix,
    memory_query_matrix,
    increment_logits,
    increment_offset,
    log_fade_speed,
    extra_log_fade,
    attention_bypass_factor,
    attention_lane_kernel,
    memory_write_kernel,
    memory_query_kernel,
    cluster_rescale_factor,
    blender_result_matrix,
    specialist_rescale_factor,
    chosen_specialists,
    specialist_shares,
    specialist_valve_matrix,
    specialist_raising_matrix,
    specialist_lowering_matrix,
    common_valve_matrix,
    common_raising_matrix,
    common_lowering_matrix,
):
    length = attention_lane_source.shape[0]
    channels = attention_lane_source.shape[1]
    group = lax.axis_index("tp") * GROUPS // HEADS
    b_own = lax.dynamic_slice_in_dim(memory_write_matrix, group * STATE, STATE, 1)
    c_own = lax.dynamic_slice_in_dim(memory_query_matrix, group * STATE, STATE, 1)
    joined = jnp.concatenate([attention_lane_source, b_own, c_own], axis=1)
    taps = jnp.concatenate(
        [
            attention_lane_kernel,
            lax.dynamic_slice_in_dim(memory_write_kernel, group * STATE, STATE, 1),
            lax.dynamic_slice_in_dim(memory_query_kernel, group * STATE, STATE, 1),
        ],
        axis=1,
    )
    padded = extended(joined, CONV // 2)
    total = jnp.zeros(joined.shape, F32)
    for offset in range(CONV):
        total = total + padded[offset : offset + length].astype(F32) * taps[offset].astype(F32)
    convolved = jax.nn.silu(total).astype(BF16)
    x_conv = convolved[:, :channels]
    b_conv = convolved[:, channels : channels + STATE]
    c_conv = convolved[:, channels + STATE :]
    steps = jax.nn.softplus(increment_logits[:, :, 0].astype(F32) + increment_offset)
    fades = -jnp.exp(log_fade_speed) * steps + extra_log_fade[:, :, 0]
    forward_cum = jnp.cumsum(fades[0])
    backward_cum = jnp.cumsum(fades[1]) - fades[1]
    forward_total = forward_cum[-1]
    backward_total = backward_cum[-1] + fades[1, -1]
    scores = lax.dot_general(
        c_conv, b_conv, (((1,), (1,)), ((), ())), preferred_element_type=F32
    )
    position = jnp.arange(length)
    lower = position[:, None] >= position[None, :]
    upper = position[:, None] <= position[None, :]
    forward_gap = forward_cum[:, None] - forward_cum[None, :]
    backward_gap = backward_cum[None, :] - backward_cum[:, None]
    mixing = scores * (
        jnp.where(lower, jnp.exp(jnp.where(lower, forward_gap, 0.0)), 0.0) * steps[0][None, :]
        + jnp.where(upper, jnp.exp(jnp.where(upper, backward_gap, 0.0)), 0.0) * steps[1][None, :]
    )
    inner = jnp.dot(mixing.astype(BF16), x_conv, preferred_element_type=F32)
    forward_scale = jnp.exp(forward_total - forward_cum) * steps[0]
    backward_scale = jnp.exp(backward_cum) * steps[1]
    scaled = (
        jnp.stack([forward_scale, backward_scale])[:, :, None] * x_conv.astype(F32)[None]
    ).astype(BF16)
    own_states = jnp.einsum("dsp,sn->dpn", scaled, b_conv, preferred_element_type=F32)
    logs = jnp.stack([forward_total, backward_total])
    hi = lax.reduce_precision(logs, 8, 7)
    mid = lax.reduce_precision(logs - hi, 8, 7)
    low = logs - hi - mid
    tail = jnp.stack([hi, mid, low] + [jnp.zeros_like(hi)] * 13, axis=1)
    states = jnp.concatenate(
        [own_states, jnp.broadcast_to(tail[:, :, None], (2, 16, STATE))], axis=1
    ).astype(BF16)
    base = halves(inner + attention_bypass_factor[0] * x_conv.astype(F32))
    wide = (length, channels)
    from_left = halves(jnp.broadcast_to(jnp.exp(forward_cum)[:, None], wide))
    from_right = halves(jnp.broadcast_to(jnp.exp(backward_total - backward_cum)[:, None], wide))
    gate = halves(jax.nn.silu(result_valve_logits.astype(F32)))
    gains = jnp.concatenate(
        [
            specialist_rescale_factor[None],
            jnp.concatenate([cluster_rescale_factor, cluster_rescale_factor])[None],
            jnp.zeros((6, 128), F32),
        ]
    )
    return whole(
        states, base, from_left, from_right, gate, c_conv, gains, layer_source_vector,
        chosen_specialists, chosen_specialists.T, specialist_shares,
        blender_result_matrix, specialist_valve_matrix, specialist_raising_matrix,
        specialist_lowering_matrix, common_valve_matrix, common_raising_matrix, common_lowering_matrix,
    )


def solution(mesh):
    return jax.shard_map(
        shards,
        mesh=mesh,
        in_specs=(
            P("sp", "tp"),
            P("sp", "tp"),
            P("sp", "tp"),
            P("sp", None),
            P("sp", None),
            P(None, "sp", "tp"),
            P(None, "tp"),
            P(None, "tp"),
            P(None, "sp", "tp"),
            P("tp"),
            P(None, "tp"),
            P(),
            P(),
            P("tp"),
            P(None, "tp"),
            P("tp"),
            P("sp", None),
            P("sp", None),
            P("sp", None, "tp"),
            P("sp", None, "tp"),
            P("sp", None, "tp"),
            P(None, "tp"),
            P(None, "tp"),
            P(None, "tp"),
        ),
        out_specs=P("sp", "tp"),
        check_vma=False,
    )
```

```python
import jax
import jax.numpy as jnp
from jax import lax
from jax.experimental import pallas as pl
from jax.experimental.pallas import tpu as pltpu
from jax.sharding import PartitionSpec as P

D = 2048
HEADS = 16
HEAD_DIM = 64
GROUPS = 4
STATE = 128
CONV = 5

NZ, NX, NY = 8, 4, 8
SP, TP = NZ * NX, NY * 2
T = 320
HALF = T // 2
SLOTS = 32
ROWS = SP * SLOTS
BLOCK = 80
CHUNKS = 2
MESH = pl.DeviceIdType.MESH
F32, BF16 = jnp.float32, jnp.bfloat16


def dot(a, b):
    return jnp.dot(a, b, preferred_element_type=F32)


class Ring:
    def __init__(self, buf, first, rows, sems, index, direct=False):
        self.buf, self.first, self.rows, self.direct = buf, first, rows, direct
        self.out, self.near = sems[0].at[index, 0], sems[0].at[index, 1]
        self.recv = sems[1].at[index]
        self.sp, tp = lax.axis_index("sp"), lax.axis_index("tp")
        self.y, self.core = tp // 2, tp % 2

    def part(self, chip, core, half=None):
        column = ((chip + 2 * NY) % NY) * 2 + core
        first, rows = self.first, self.rows
        if half is not None:
            rows = rows // 2
            first = first + half * rows
        return self.buf.at[pl.ds(first, rows), pl.ds(pl.multiple_of(column * 128, 128), 128)]

    def along(self, way, step, chip, far):
        turn = 1 - 2 * way
        block = self.part(chip, self.core, way if step == 4 else None)
        return pltpu.make_async_remote_copy(
            src_ref=block,
            dst_ref=block,
            send_sem=self.out,
            recv_sem=self.recv.at[4 * way + step - 1],
            device_id=(self.sp, ((self.y + turn * far + NY) % NY) * 2 + self.core),
            device_id_type=MESH,
        )

    def hop(self, way, step):
        if self.direct:
            return self.along(way, step, self.y, step)
        return self.along(way, step, self.y - (1 - 2 * way) * (step - 1), 1)

    def landed(self, way, step):
        return self.along(way, step, self.y - (1 - 2 * way) * step, 1)

    def relay(self, way, step):
        turn = 1 - 2 * way
        return self.over(self.part(self.y - turn * step, self.core, way if step == 4 else None))

    def over(self, block):
        return pltpu.make_async_remote_copy(
            src_ref=block,
            dst_ref=block,
            send_sem=self.out,
            recv_sem=self.near,
            device_id=(self.sp, self.y * 2 + 1 - self.core),
            device_id_type=MESH,
        )

    def several(self, blocks):
        return self.over(self.buf.at[pl.ds(self.first, self.rows), pl.ds(0, 128 * blocks)])

    def start(self):
        for step in (4, 3, 2, 1) if self.direct else (1,):
            self.hop(0, step).start()
            self.hop(1, step).start()
        self.relay(0, 0).start()

    def step(self, step):
        for way in (0, 1):
            self.landed(way, step).wait_recv()
            if step < 4 and not self.direct:
                self.hop(way, step + 1).start()
            self.relay(way, step).start()

    def finish(self):
        self.several(NY).wait_recv()

    def drain(self):
        self.several(2 * NY - 1).wait_send()


def run(rings):
    for step in range(1, 5):
        for ring in rings:
            ring.step(step)


def stacked(rows):
    level = lax.broadcasted_iota(jnp.int32, (8, rows[0].shape[1]), 0)
    total = jnp.zeros(level.shape, F32)
    for k, row in enumerate(rows):
        total = jnp.where(level == k, row, total)
    return total


def three(v):
    high = v.astype(BF16).astype(F32)
    middle = (v - high).astype(BF16).astype(F32)
    return [high, middle, v - high - middle]


def one_hot(shape, test):
    row, col = lax.broadcasted_iota(jnp.int32, shape, 0), lax.broadcasted_iota(jnp.int32, shape, 1)
    return jnp.where(test(row, col), 1.0, 0.0).astype(BF16)


def across(a, b):
    return lax.dot_general(a, b, (((1,), (1,)), ((), ())), preferred_element_type=F32)


def log1p(u):
    series = u * (1 - u * (1 / 2 - u * (1 / 3 - u * (1 / 4 - u * (1 / 5 - u / 6)))))
    return jnp.where(u < 0.03, series, jnp.log(1 + u))


def silu(v):
    return v / (1 + jnp.exp(-v))


def kernel(
    xt_ref, zt_ref, inc_ref, off_ref, spd_ref, fade_ref, byp_ref, xk_ref, bk_ref, ck_ref, gain_ref,
    after_ref, src_ref, cht_ref, sht_ref,
    bm_hbm, cm_hbm, blender_hbm, valve_hbm, raising_hbm, lowering_hbm, cvalve_hbm, craising_hbm, clowering_hbm,
    out_ref,
    xpad, braw, craw, hx, hb, hc, bext, cext, gap, cv, mixed, fto,
    st_ref, rx, tb, rz, ft, sq, so, wb, wx, wc, wl, wcl, wide, bn, nn, am, ff, sh, xx, hh, dd, oo, ret, pp, qhi, qlo,
    wsem, hs, hr, one, dr, rsem, rrecv,
):
    sp, tp = lax.axis_index("sp"), lax.axis_index("tp")
    z, x = sp // NX, sp % NX

    barrier = pltpu.get_barrier_semaphore()

    def greet_tp(k, carry):
        pl.semaphore_signal(barrier, inc=1, device_id=(sp, (tp + k) % TP), device_id_type=MESH)
        return carry

    def greet_sp(k, carry):
        pl.semaphore_signal(barrier, inc=1, device_id=((sp + k) % SP, tp), device_id_type=MESH)
        return carry

    lax.fori_loop(1, TP, greet_tp, 0)
    lax.fori_loop(1, SP, greet_sp, 0)

    at_group = pl.ds(pl.multiple_of((tp // 4) * 128, 128), 128)
    loads = [
        pltpu.make_async_copy(blender_hbm, wb, wsem.at[0]),
        pltpu.make_async_copy(valve_hbm.at[0], wx.at[:, pl.ds(0, 128)], wsem.at[1]),
        pltpu.make_async_copy(raising_hbm.at[0], wx.at[:, pl.ds(128, 128)], wsem.at[2]),
        pltpu.make_async_copy(lowering_hbm.at[0], wl, wsem.at[3]),
        pltpu.make_async_copy(cvalve_hbm, wc.at[:, pl.ds(0, 128)], wsem.at[4]),
        pltpu.make_async_copy(craising_hbm, wc.at[:, pl.ds(128, 128)], wsem.at[5]),
        pltpu.make_async_copy(clowering_hbm, wcl, wsem.at[6]),
    ]
    grouped = [
        pltpu.make_async_copy(bm_hbm.at[:, at_group], braw, wsem.at[7]),
        pltpu.make_async_copy(cm_hbm.at[:, at_group], craw, wsem.at[8]),
    ]
    for load in grouped + loads:
        load.start()

    xpad[...] = jnp.zeros(xpad.shape, BF16)
    xpad[:, 0:T] = xt_ref[...]
    gains = jnp.concatenate([gain_ref[...], gain_ref[...]], axis=1)
    fto[...] = jnp.broadcast_to(gains, (8, 128))
    ft[tp] = fto[...]

    def state_row(k, source):
        return pltpu.make_async_remote_copy(
            src_ref=st_ref,
            dst_ref=rx.at[source],
            send_sem=one.at[0],
            recv_sem=one.at[1],
            device_id=(z * NX + (x + k) % NX, tp),
            device_id_type=MESH,
        )

    def tile(k, source):
        return pltpu.make_async_remote_copy(
            src_ref=fto,
            dst_ref=ft.at[source],
            send_sem=one.at[4],
            recv_sem=one.at[5],
            device_id=(sp, (tp + k) % TP),
            device_id_type=MESH,
        )

    def send_tile(k, carry):
        tile(k, tp).start()
        return carry

    lower = one_hot((T, T), lambda row, col: col < row)
    upper = one_hot((T, T), lambda row, col: row < col)
    same = one_hot((T, T), lambda row, col: row == col)
    experts = lax.broadcasted_iota(jnp.int32, (SP, T), 0)
    first, second = cht_ref[0:1, :] == experts, cht_ref[1:2, :] == experts
    named = jnp.where(first | second, 1.0, 0.0)
    rank = dot(named.astype(BF16), upper)
    rank = jnp.where(named > 0, rank, 99.0).astype(BF16)
    spread = one_hot((ROWS, SP), lambda row, col: row // SLOTS == col)
    place = (lax.broadcasted_iota(jnp.int32, (ROWS, T), 0) % SLOTS).astype(F32)
    pp[...] = jnp.where(dot(spread, rank) == place, 1.0, 0.0).astype(BF16)
    shares = jnp.where(first, sht_ref[0:1, :], 0.0) + jnp.where(second, sht_ref[1:2, :], 0.0)
    share_hi = shares.astype(BF16)
    share_lo = (shares - share_hi.astype(F32)).astype(BF16)
    spread = one_hot((SP, ROWS), lambda row, col: col // SLOTS == row)
    place = (lax.broadcasted_iota(jnp.int32, (T, ROWS), 1) % SLOTS).astype(F32)
    here = dot(across(same, rank).astype(BF16), spread) == place
    qhi[...] = jnp.where(here, dot(across(same, share_hi).astype(BF16), spread), 0.0).astype(BF16)
    qlo[...] = jnp.where(here, dot(across(same, share_lo).astype(BF16), spread), 0.0).astype(BF16)

    steps, fades = [], []
    for d in range(2):
        v = inc_ref[d : d + 1, :].astype(F32) + off_ref[0:1, d : d + 1]
        step = jnp.maximum(v, 0.0) + log1p(jnp.exp(-jnp.abs(v)))
        steps.append(step)
        fades.append(-jnp.exp(spd_ref[0:1, d : d + 1]) * step + fade_ref[d])
    parts = stacked(three(fades[0]) + three(fades[1])).astype(BF16)
    along = dot(parts, upper + same)
    forward_row = along[0:1] + along[1:2] + along[2:3]
    along = dot(parts, upper)
    backward_row = along[3:4] + along[4:5] + along[5:6]
    along = across(lower + same, parts)
    forward_col = along[:, 0:1] + along[:, 1:2] + along[:, 2:3]
    along = across(lower, parts)
    backward_col = along[:, 3:4] + along[:, 4:5] + along[:, 5:6]
    row = lax.broadcasted_iota(jnp.int32, (T, T), 0)
    col = lax.broadcasted_iota(jnp.int32, (T, T), 1)
    gap[...] = (
        jnp.where(row >= col, jnp.exp(forward_col - forward_row), 0.0) * steps[0]
        + jnp.where(row <= col, jnp.exp(backward_row - backward_col), 0.0) * steps[1]
    )
    forward_end = forward_row[:, T - 1 : T]
    backward_end = backward_row[:, T - 1 : T] + fades[1][:, T - 1 : T]
    weigh = [jnp.exp(forward_end - forward_row) * steps[0], jnp.exp(backward_row) * steps[1]]
    seen = [jnp.exp(forward_row), jnp.exp(backward_end - backward_row)]
    cv[...] = stacked(weigh + seen)
    ends = [jnp.broadcast_to(forward_end, (1, 128)), jnp.broadcast_to(backward_end, (1, 128))]

    for load in grouped:
        load.wait()
    pl.semaphore_wait(barrier, TP + SP - 2)

    def halo(side, k):
        there = (sp + 1) % SP if side == 0 else (sp + SP - 1) % SP
        rows = pl.ds(T - 16, 16) if side == 0 else pl.ds(0, 16)
        lanes = pl.ds(256, 128) if side == 0 else pl.ds(0, 128)
        source = (xpad.at[:, lanes], braw.at[rows], craw.at[rows])[k]
        return pltpu.make_async_remote_copy(
            src_ref=source,
            dst_ref=(hx, hb, hc)[k].at[side],
            send_sem=hs.at[3 * side + k],
            recv_sem=hr.at[3 * side + k],
            device_id=(there, tp),
            device_id_type=MESH,
        )

    for k in range(3):
        halo(0, k).start()
        halo(1, k).start()
    lax.fori_loop(1, TP, send_tile, 0)

    taps = across(same[0:64, 0:64], stacked([xk_ref[j : j + 1, :].astype(F32) for j in range(CONV)]).astype(BF16))
    lane = lax.broadcasted_iota(jnp.int32, (64, 128), 1)
    body = xpad[...].astype(F32)
    bext[pl.ds(16, T), :] = braw[...].astype(F32)
    cext[pl.ds(16, T), :] = craw[...].astype(F32)
    for k in range(3):
        halo(0, k).wait_recv()
        halo(1, k).wait_recv()
    before, behind = sp > 0, sp < SP - 1
    last = jnp.where(before, pltpu.roll(hx[0].astype(F32), 64, 1), 0.0)
    coming = jnp.where(behind, pltpu.roll(hx[1].astype(F32), 64, 1), 0.0)
    end = jnp.where(
        lane < 64, body[:, 256:384], jnp.where(lane < 66, coming, jnp.where(lane > 125, last, 0.0))
    )
    cells = jnp.concatenate([body[:, 0:256], end], axis=1)
    total = cells * taps[:, 2:3]
    for j in (0, 1, 3, 4):
        total = total + pltpu.roll(cells, (2 - j) % 384, 1) * taps[:, j : j + 1]
    x_conv = silu(total)[:, 0:T].astype(BF16)
    for ext, halos, kernel_ref in ((bext, hb, bk_ref), (cext, hc, ck_ref)):
        ext[pl.ds(0, 16), :] = jnp.where(before, halos[0].astype(F32), 0.0)
        ext[pl.ds(T + 16, 16), :] = jnp.where(behind, halos[1].astype(F32), 0.0)
        total = jnp.zeros((T, 128), F32)
        for j in range(CONV):
            tap = kernel_ref[j : j + 1, at_group].astype(F32)
            total = total + ext[pl.ds(14 + j, T), :] * tap
        mixed[0 if ext is bext else 1] = silu(total).astype(BF16)
    b_conv, c_conv = mixed[0], mixed[1]

    def packed(total, log):
        tail = jnp.concatenate([stacked(three(log)), jnp.zeros((8, 128), F32)], axis=0)
        return total.astype(BF16), tail.astype(BF16)

    x_wide = x_conv.astype(F32)
    for d in range(2):
        scaled = (cv[d : d + 1, :] * x_wide).astype(BF16)
        top, tail = packed(dot(scaled, b_conv), ends[d])
        st_ref[d, 0:64] = top
        st_ref[d, 64:80] = tail
    rx[x] = st_ref[...]
    for k in (2, 1, 3):
        state_row(k, x).start()
    inner = across(x_conv, (across(c_conv, b_conv) * gap[...]).astype(BF16))
    inner = inner + byp_ref[...] * x_wide
    gate = silu(zt_ref[...].astype(F32))

    def all_rows(k):
        return pltpu.make_async_remote_copy(
            src_ref=rx.at[pl.ds(0, k)],
            dst_ref=rx.at[pl.ds(0, k)],
            send_sem=one.at[0],
            recv_sem=one.at[1],
            device_id=(z * NX + (x + 1) % NX, tp),
            device_id_type=MESH,
        )

    all_rows(NX - 1).wait_recv()

    def state(block):
        return block[0:64].astype(F32)

    def log_of(block):
        logs = block[64:80].astype(F32)
        return logs[0:1] + logs[1:2] + logs[2:3]

    for way in (0, 1):
        total, log = jnp.zeros((64, 128), F32), jnp.zeros((1, 128), F32)
        for i in range(NX) if way == 0 else reversed(range(NX)):
            block = rx[i, way]
            own = log_of(block)
            total = jnp.exp(own) * total + state(block)
            log = log + own
        top, tail = packed(total, log)
        tb[way, 0:64] = top
        tb[way, 64:80] = tail
    rz[z] = tb[0]

    def state_column(k, source):
        return pltpu.make_async_remote_copy(
            src_ref=tb.at[(z + k) // NZ],
            dst_ref=rz.at[source],
            send_sem=one.at[2],
            recv_sem=one.at[3],
            device_id=(((z + k) % NZ) * NX + x, tp),
            device_id_type=MESH,
        )

    for k in (4, 3, 5, 2, 6, 1, 7):
        state_column(k, z).start()

    loads[0].wait()
    wide[...] = jnp.zeros(wide.shape, BF16)

    def widen(j, carry):
        block = wb[pl.ds(pl.multiple_of(j * 64, 64), 64), :]
        wide[pl.ds(pl.multiple_of(j * 128, 128), 64), pl.ds(0, 128)] = block
        wide[pl.ds(pl.multiple_of(j * 128 + 64, 64), 64), pl.ds(128, 128)] = block
        return carry

    lax.fori_loop(0, HEADS, widen, 0)

    def all_columns():
        return pltpu.make_async_remote_copy(
            src_ref=rz.at[pl.ds(0, NZ - 1)],
            dst_ref=rz.at[pl.ds(0, NZ - 1)],
            send_sem=one.at[2],
            recv_sem=one.at[3],
            device_id=(((z + 1) % NZ) * NX + x, tp),
            device_id_type=MESH,
        )

    all_columns().wait_recv()

    carried = []
    for way in (0, 1):
        total = jnp.zeros((64, 128), F32)
        for i in range(NZ) if way == 0 else reversed(range(NZ)):
            block = rz[i]
            passed = (i < z) if way == 0 else (i > z)
            total = jnp.where(passed, jnp.exp(log_of(block)) * total + state(block), total)
        for i in range(NX) if way == 0 else reversed(range(NX)):
            block = rx[i, way]
            passed = (i < x) if way == 0 else (i > x)
            total = jnp.where(passed, jnp.exp(log_of(block)) * total + state(block), total)
        carried.append(total.astype(BF16))

    mixer = inner + cv[2:3, :] * across(carried[0], mixed[1]) + cv[3:4, :] * across(carried[1], mixed[1])
    gated = (mixer * gate).astype(BF16)
    none = jnp.zeros((64, T), BF16)
    upper_half = one_hot((HALF, T), lambda row, col: row == col)
    lower_half = one_hot((HALF, T), lambda row, col: row + HALF == col)
    mine = pl.ds(pl.multiple_of(tp * 128, 128), 128)
    bn[:, mine] = (
        across(upper_half, jnp.concatenate([gated, none], axis=0))
        + across(lower_half, jnp.concatenate([none, gated], axis=0))
    ).astype(BF16)

    sems = (rsem, rrecv)
    ring = Ring(bn, 0, HALF, sems, 0, direct=True)
    ring.start()

    def all_tiles(ref, at):
        return pltpu.make_async_remote_copy(
            src_ref=ref.at[pl.ds(0, TP - 1)],
            dst_ref=ref.at[pl.ds(0, TP - 1)],
            send_sem=one.at[at],
            recv_sem=one.at[at + 1],
            device_id=(sp, (tp + 1) % TP),
            device_id_type=MESH,
        )

    all_tiles(ft, 4).wait_recv()
    run([ring])
    ring.finish()

    left = lax.broadcasted_iota(jnp.int32, (HALF, 128), 1) < 64
    for g in range(GROUPS):
        squares = jnp.zeros((HALF, 128), F32)
        for j in range(4 * g, 4 * g + 4):
            v = bn[:, 128 * j : 128 * j + 128].astype(F32)
            squares = squares + v * v
        top = jnp.sum(jnp.where(left, squares, 0.0), axis=1, keepdims=True)
        bottom = jnp.sum(jnp.where(left, 0.0, squares), axis=1, keepdims=True)
        scale = lax.rsqrt(jnp.where(left, top, bottom) / (4 * HEAD_DIM) + 1e-06)
        for j in range(4 * g, 4 * g + 4):
            v = bn[:, 128 * j : 128 * j + 128].astype(F32)
            nn[:, 128 * j : 128 * j + 128] = (v * scale * ft[j, 0:1]).astype(BF16)
    projected = dot(nn[...], wide[...])
    am[0:HALF] = (src_ref[0:HALF].astype(F32) + projected[:, 0:128]).astype(BF16)
    am[HALF:T] = (src_ref[HALF:T].astype(F32) + projected[:, 128:256]).astype(BF16)

    dims = (((1,), (1,)), ((), ()))
    squares = am[...].astype(F32) * am[...].astype(F32)
    high = squares.astype(BF16)
    rest = (squares - high.astype(F32)).astype(BF16)
    ones = jnp.ones((8, 128), BF16)
    sums = lax.dot_general(ones, high, dims, preferred_element_type=F32) + lax.dot_general(
        ones, rest, dims, preferred_element_type=F32
    )
    line = jnp.concatenate([sums, jnp.zeros((8, 3 * 128 - T), F32)], axis=1)
    level = lax.broadcasted_iota(jnp.int32, (8, 128), 0)
    own = jnp.where(
        level == 0,
        line[:, 0:128],
        jnp.where(level == 1, line[:, 128:256], jnp.where(level == 2, line[:, 256:384], 0.0)),
    )
    sq[tp] = own
    so[...] = own

    def sums_to(k, source):
        return pltpu.make_async_remote_copy(
            src_ref=so,
            dst_ref=sq.at[source],
            send_sem=one.at[6],
            recv_sem=one.at[7],
            device_id=(sp, (tp + k) % TP),
            device_id_type=MESH,
        )

    def send_sums(k, carry):
        sums_to((k + 7) % (TP - 1) + 1, tp).start()
        return carry

    lax.fori_loop(0, TP - 1, send_sums, 0)
    ring.drain()

    all_tiles(sq, 6).wait_recv()
    total = sq[0]
    for j in range(1, TP):
        total = total + sq[j]
    line = jnp.concatenate([total[0:1], total[1:2], total[2:3]], axis=1)
    parts = stacked(three(line)).astype(BF16)
    same = one_hot((T, 384), lambda row, col: row == col)
    upright = lax.dot_general(same, parts, dims, preferred_element_type=F32)
    scale = lax.rsqrt((upright[:, 0:1] + upright[:, 1:2] + upright[:, 2:3]) / D + 1e-06)
    own = (am[...].astype(F32) * scale * after_ref[...]).astype(BF16)
    ff[:, mine] = own
    dd[...] = dot(pp[...], own).astype(BF16)

    def rows_of(i):
        return pl.ds(pl.multiple_of(i * SLOTS, SLOTS), SLOTS)

    def deliver(k, source):
        target = (sp + k) % SP
        return pltpu.make_async_remote_copy(
            src_ref=dd.at[rows_of(target)],
            dst_ref=xx.at[rows_of(source), mine],
            send_sem=one.at[8],
            recv_sem=dr.at[source // (SP // CHUNKS)],
            device_id=(target, tp),
            device_id_type=MESH,
        )

    def send_rows(k, carry):
        deliver(k, sp).start()
        return carry

    lax.fori_loop(1, SP, send_rows, 0)
    xx[rows_of(sp), mine] = dd[rows_of(sp)]

    spread_out = [Ring(ff, i * HALF, HALF, sems, 1 + i) for i in range(2)]
    for ring in spread_out:
        ring.start()

    size = ROWS // CHUNKS
    per = SP // CHUNKS

    def some_rows(ref, first, blocks, sent, received):
        part = ref.at[pl.ds(first, blocks * SLOTS), pl.ds(0, 128)]
        return pltpu.make_async_remote_copy(
            src_ref=part,
            dst_ref=part,
            send_sem=one.at[sent],
            recv_sem=received,
            device_id=((sp + 1) % SP, tp),
            device_id_type=MESH,
        )

    def wait_rows(q):
        @pl.when(sp // per == q)
        def _():
            some_rows(xx, q * size, per - 1, 8, dr.at[q]).wait_recv()

        @pl.when(sp // per != q)
        def _():
            some_rows(xx, q * size, per, 8, dr.at[q]).wait_recv()

    for step in (1, 2):
        for ring in spread_out:
            ring.step(step)
    gathers = []
    for q in range(CHUNKS):
        wait_rows(q)
        gathers.append(Ring(xx, q * size, size, sems, 4 + q))
        gathers[-1].start()
    for step in (3, 4):
        for ring in spread_out:
            ring.step(step)
    for ring in gathers:
        ring.step(1)
    for ring in spread_out:
        ring.finish()
    loads[4].wait()
    loads[5].wait()
    both = dot(ff[...], wc[...])
    sh[:, mine] = (jax.nn.silu(both[:, 0:128]) * both[:, 128:256]).astype(BF16)
    hidden_out = Ring(sh, 0, T, sems, 3)
    hidden_out.start()
    for step in (2, 3, 4):
        for ring in gathers:
            ring.step(step)
        hidden_out.step(step - 1)

    loads[1].wait()
    loads[2].wait()
    hiddens = []
    for q in range(CHUNKS):
        gathers[q].finish()
        at = pl.ds(q * size, size)
        both = dot(xx[at, :], wx[...])
        hh[at, mine] = (jax.nn.silu(both[:, 0:128]) * both[:, 128:256]).astype(BF16)
        hiddens.append(Ring(hh, q * size, size, sems, 4 + CHUNKS + q))
        hiddens[-1].start()
    hidden_out.step(4)
    for side in range(2):
        for k in range(3):
            halo(side, k).wait_send()
    all_rows(NX - 1).wait_send()
    all_columns().wait_send()
    all_tiles(ft, 4).wait_send()
    all_tiles(sq, 6).wait_send()
    some_rows(dd, 0, SP - 1, 8, one.at[9]).wait_send()
    for ring in spread_out + gathers:
        ring.drain()
    for ring in hiddens:
        ring.step(1)
    hidden_out.finish()
    loads[6].wait()
    shared = dot(sh[...], wcl[...]).astype(BF16).astype(F32)
    out_ref[...] = shared.astype(BF16)
    hidden_out.drain()
    for step in (2, 3, 4):
        for ring in hiddens:
            ring.step(step)

    def give(i, source):
        return pltpu.make_async_remote_copy(
            src_ref=oo.at[rows_of(i)],
            dst_ref=ret.at[rows_of(source)],
            send_sem=one.at[10],
            recv_sem=one.at[11],
            device_id=(i, tp),
            device_id_type=MESH,
        )

    loads[3].wait()
    for q in range(CHUNKS):
        hiddens[q].finish()

        at = pl.ds(q * size, size)
        oo[at, :] = dot(hh[at, :], wl[...]).astype(BF16)

        def send_back(k, carry):
            i = q * per + (sp + k) % per

            @pl.when(i != sp)
            def _():
                give(i, sp).start()

            return carry

        lax.fori_loop(0, per, send_back, 0)
    ret[rows_of(sp), :] = oo[rows_of(sp), :]

    for ring in hiddens:
        ring.drain()

    some_rows(ret, 0, SP - 1, 10, one.at[11]).wait_recv()
    some_rows(oo, 0, SP - 1, 10, one.at[11]).wait_send()
    routed = dot(qhi[...], ret[...]) + dot(qlo[...], ret[...])
    out_ref[...] = (am[...].astype(F32) + out_ref[...].astype(F32) + routed).astype(BF16)


def whole(*operands):
    vmem = pl.BlockSpec(memory_space=pltpu.VMEM)
    hbm = pl.BlockSpec(memory_space=pl.ANY)
    rings = 4 + 2 * CHUNKS
    dma = pltpu.SemaphoreType.DMA

    def space(*shape, kind=BF16):
        return pltpu.VMEM(shape, kind)

    return pl.pallas_call(
        kernel,
        out_shape=jax.ShapeDtypeStruct((T, 128), BF16),
        in_specs=[vmem] * 15 + [hbm] * 9,
        out_specs=vmem,
        scratch_shapes=[
            space(64, 384),
            space(T, 128),
            space(T, 128),
            space(2, 64, 128),
            space(2, 16, 128),
            space(2, 16, 128),
            space(T + 32, 128, kind=F32),
            space(T + 32, 128, kind=F32),
            space(T, T, kind=F32),
            space(8, T, kind=F32),
            space(2, T, 128),
            space(8, 128, kind=F32),
            space(2, BLOCK, 128),
            space(NX, 2, BLOCK, 128),
            space(2, BLOCK, 128),
            space(NZ, BLOCK, 128),
            space(TP, 8, 128, kind=F32),
            space(TP, 8, 128, kind=F32),
            space(8, 128, kind=F32),
            space(1024, 128),
            space(D, 256),
            space(D, 256),
            space(D, 128),
            space(D, 128),
            space(D, 256),
            space(HALF, D),
            space(HALF, D),
            space(T, 128),
            space(T, D),
            space(T, D),
            space(ROWS, D),
            space(ROWS, D),
            space(ROWS, 128),
            space(ROWS, 128),
            space(ROWS, 128),
            space(ROWS, T),
            space(T, ROWS),
            space(T, ROWS),
            dma((9,)), dma((6,)), dma((6,)), dma((12,)), dma((CHUNKS,)), dma((rings, 2)), dma((rings, 8)),
        ],
        compiler_params=pltpu.CompilerParams(collective_id=0, has_side_effects=True),
        name="mixer_experts",
    )(*operands)


def shards(
    layer_source_vector,
    attention_lane_source,
    result_valve_logits,
    memory_write_matrix,
    memory_query_matrix,
    increment_logits,
    increment_offset,
    log_fade_speed,
    extra_log_fade,
    attention_bypass_factor,
    attention_lane_kernel,
    memory_write_kernel,
    memory_query_kernel,
    cluster_rescale_factor,
    blender_result_matrix,
    specialist_rescale_factor,
    chosen_specialists,
    specialist_shares,
    specialist_valve_matrix,
    specialist_raising_matrix,
    specialist_lowering_matrix,
    common_valve_matrix,
    common_raising_matrix,
    common_lowering_matrix,
):
    return whole(
        attention_lane_source.T,
        result_valve_logits.T,
        increment_logits.reshape(2, T),
        increment_offset.T,
        log_fade_speed.T,
        extra_log_fade.reshape(2, 1, T),
        attention_bypass_factor.reshape(1, 1),
        attention_lane_kernel,
        memory_write_kernel,
        memory_query_kernel,
        cluster_rescale_factor.reshape(1, 64),
        specialist_rescale_factor.reshape(1, 128),
        layer_source_vector,
        chosen_specialists.T,
        specialist_shares.T,
        memory_write_matrix,
        memory_query_matrix,
        blender_result_matrix,
        specialist_valve_matrix,
        specialist_raising_matrix,
        specialist_lowering_matrix,
        common_valve_matrix,
        common_raising_matrix,
        common_lowering_matrix,
    )


def solution(mesh):
    return jax.shard_map(
        shards,
        mesh=mesh,
        in_specs=(
            P("sp", "tp"),
            P("sp", "tp"),
            P("sp", "tp"),
            P("sp", None),
            P("sp", None),
            P(None, "sp", "tp"),
            P(None, "tp"),
            P(None, "tp"),
            P(None, "sp", "tp"),
            P("tp"),
            P(None, "tp"),
            P(),
            P(),
            P("tp"),
            P(None, "tp"),
            P("tp"),
            P("sp", None),
            P("sp", None),
            P("sp", None, "tp"),
            P("sp", None, "tp"),
            P("sp", None, "tp"),
            P(None, "tp"),
            P(None, "tp"),
            P(None, "tp"),
        ),
        out_specs=P("sp", "tp"),
        check_vma=False,
    )
```

```python
import jax
import jax.numpy as jnp
from jax import lax
from jax.experimental import pallas as pl
from jax.experimental.pallas import tpu as pltpu
from jax.sharding import PartitionSpec as P

D = 2048
HEADS = 16
HEAD_DIM = 64
GROUPS = 4
STATE = 128
CONV = 5

NZ, NX, NY = 8, 4, 8
SP, TP = NZ * NX, NY * 2
T = 320
HALF = T // 2
SLOTS = 32
ROWS = SP * SLOTS
BLOCK = 80
CHUNKS = 2
MESH = pl.DeviceIdType.MESH
F32, BF16 = jnp.float32, jnp.bfloat16


def dot(a, b):
    return jnp.dot(a, b, preferred_element_type=F32)


class Ring:
    def __init__(self, buf, first, rows, sems, index, direct=False, pair=False):
        self.buf, self.first, self.rows, self.direct, self.pair = buf, first, rows, direct, pair
        self.out, self.near = sems[0].at[index, 0], sems[0].at[index, 1]
        self.recv = sems[1].at[index]
        self.sp, tp = lax.axis_index("sp"), lax.axis_index("tp")
        self.y, self.core = tp // 2, tp % 2

    def part(self, chip, core, half=None):
        column, width = ((chip + 2 * NY) % NY) * 2, 128
        if self.pair:
            width = 256
        else:
            column = column + core
        first, rows = self.first, self.rows
        if half is not None:
            rows = rows // 2
            first = first + half * rows
        return self.buf.at[pl.ds(first, rows), pl.ds(pl.multiple_of(column * 128, 128), width)]

    def along(self, way, step, chip, far):
        turn = 1 - 2 * way
        block = self.part(chip, self.core, way if step == 4 else None)
        return pltpu.make_async_remote_copy(
            src_ref=block,
            dst_ref=block,
            send_sem=self.out,
            recv_sem=self.recv.at[4 * way + step - 1],
            device_id=(self.sp, ((self.y + turn * far + NY) % NY) * 2 + self.core),
            device_id_type=MESH,
        )

    def hop(self, way, step):
        if self.direct:
            return self.along(way, step, self.y, step)
        return self.along(way, step, self.y - (1 - 2 * way) * (step - 1), 1)

    def landed(self, way, step):
        return self.along(way, step, self.y - (1 - 2 * way) * step, 1)

    def relay(self, way, step):
        turn = 1 - 2 * way
        return self.over(self.part(self.y - turn * step, self.core, way if step == 4 else None))

    def over(self, block):
        return pltpu.make_async_remote_copy(
            src_ref=block,
            dst_ref=block,
            send_sem=self.out,
            recv_sem=self.near,
            device_id=(self.sp, self.y * 2 + 1 - self.core),
            device_id_type=MESH,
        )

    def several(self, blocks):
        return self.over(self.buf.at[pl.ds(self.first, self.rows), pl.ds(0, 128 * blocks)])

    def start(self):
        for step in (4, 3, 2, 1) if self.direct else (1,):
            self.hop(0, step).start()
            self.hop(1, step).start()
        if not self.pair:
            self.relay(0, 0).start()

    def step(self, step):
        for way in (0, 1):
            self.landed(way, step).wait_recv()
            if step < 4 and not self.direct:
                self.hop(way, step + 1).start()
            if not self.pair:
                self.relay(way, step).start()

    def finish(self):
        self.several(NY).wait_recv()

    def drain(self):
        self.several(2 * NY - (2 if self.pair else 1)).wait_send()


def run(rings):
    for step in range(1, 5):
        for ring in rings:
            ring.step(step)


def stacked(rows):
    level = lax.broadcasted_iota(jnp.int32, (8, rows[0].shape[1]), 0)
    total = jnp.zeros(level.shape, F32)
    for k, row in enumerate(rows):
        total = jnp.where(level == k, row, total)
    return total


def three(v):
    high = v.astype(BF16).astype(F32)
    middle = (v - high).astype(BF16).astype(F32)
    return [high, middle, v - high - middle]


def one_hot(shape, test):
    row, col = lax.broadcasted_iota(jnp.int32, shape, 0), lax.broadcasted_iota(jnp.int32, shape, 1)
    return jnp.where(test(row, col), 1.0, 0.0).astype(BF16)


def across(a, b):
    return lax.dot_general(a, b, (((1,), (1,)), ((), ())), preferred_element_type=F32)


def log1p(u):
    series = u * (1 - u * (1 / 2 - u * (1 / 3 - u * (1 / 4 - u * (1 / 5 - u / 6)))))
    return jnp.where(u < 0.03, series, jnp.log(1 + u))


def silu(v):
    return v / (1 + jnp.exp(-v))


def kernel(
    xt_ref, zt_ref, inc_ref, off_ref, spd_ref, fade_ref, byp_ref, xk_ref, bk_ref, ck_ref, gain_ref,
    after_ref, src_ref, cht_ref, sht_ref,
    bm_hbm, cm_hbm, blender_hbm, valve_hbm, raising_hbm, lowering_hbm, cvalve_hbm, craising_hbm, clowering_hbm,
    out_ref,
    xpad, braw, craw, hx, hb, hc, bext, cext, gap, cv, mixed, fto,
    st_ref, rx, tb, rz, ft, sq, so, wb, wx, wc, wl, wcl, wide, bn, nn, am, ff, sh, xx, hh, dd, ss, sl, oo, ret, pp, qhi, qlo,
    wsem, hs, hr, one, dr, rsem, rrecv,
):
    sp, tp = lax.axis_index("sp"), lax.axis_index("tp")
    z, x = sp // NX, sp % NX
    y, core, side_of = tp // 2, tp % 2, sp // (SP // 2)

    barrier = pltpu.get_barrier_semaphore()

    def greet_tp(k, carry):
        pl.semaphore_signal(barrier, inc=1, device_id=(sp, (tp + k) % TP), device_id_type=MESH)
        return carry

    def greet_sp(k, carry):
        pl.semaphore_signal(barrier, inc=1, device_id=((sp + k) % SP, tp), device_id_type=MESH)
        return carry

    lax.fori_loop(1, TP, greet_tp, 0)
    lax.fori_loop(1, SP, greet_sp, 0)

    def lanes_of(i):
        return pl.ds(pl.multiple_of(i * 128, 128), 128)

    at_group = pl.ds(pl.multiple_of((tp // 4) * 128, 128), 128)
    loads = [
        pltpu.make_async_copy(blender_hbm, wb, wsem.at[0]),
        pltpu.make_async_copy(valve_hbm.at[0], wx.at[:, lanes_of(core)], wsem.at[1]),
        pltpu.make_async_copy(raising_hbm.at[0], wx.at[:, lanes_of(core + 2)], wsem.at[2]),
        pltpu.make_async_copy(lowering_hbm.at[0], wl.at[:, lanes_of(core)], wsem.at[3]),
        pltpu.make_async_copy(cvalve_hbm, wc.at[:, pl.ds(0, 128)], wsem.at[4]),
        pltpu.make_async_copy(craising_hbm, wc.at[:, pl.ds(128, 128)], wsem.at[5]),
        pltpu.make_async_copy(clowering_hbm, wcl, wsem.at[6]),
    ]
    grouped = [
        pltpu.make_async_copy(bm_hbm.at[:, at_group], braw, wsem.at[7]),
        pltpu.make_async_copy(cm_hbm.at[:, at_group], craw, wsem.at[8]),
    ]
    for load in grouped + loads:
        load.start()

    xpad[...] = jnp.zeros(xpad.shape, BF16)
    xpad[:, 0:T] = xt_ref[...]
    gains = jnp.concatenate([gain_ref[...], gain_ref[...]], axis=1)
    fto[...] = jnp.broadcast_to(gains, (8, 128))
    ft[tp] = fto[...]

    def state_row(k, source):
        return pltpu.make_async_remote_copy(
            src_ref=st_ref,
            dst_ref=rx.at[source],
            send_sem=one.at[0],
            recv_sem=one.at[1],
            device_id=(z * NX + (x + k) % NX, tp),
            device_id_type=MESH,
        )

    def tile(k, source):
        return pltpu.make_async_remote_copy(
            src_ref=fto,
            dst_ref=ft.at[source],
            send_sem=one.at[4],
            recv_sem=one.at[5],
            device_id=(sp, (tp + k) % TP),
            device_id_type=MESH,
        )

    def send_tile(k, carry):
        tile(k, tp).start()
        return carry

    lower = one_hot((T, T), lambda row, col: col < row)
    upper = one_hot((T, T), lambda row, col: row < col)
    same = one_hot((T, T), lambda row, col: row == col)
    experts = lax.broadcasted_iota(jnp.int32, (SP, T), 0)
    first, second = cht_ref[0:1, :] == experts, cht_ref[1:2, :] == experts
    named = jnp.where(first | second, 1.0, 0.0)
    rank = dot(named.astype(BF16), upper)
    rank = jnp.where(named > 0, rank, 99.0).astype(BF16)
    spread = one_hot((ROWS, SP), lambda row, col: row // SLOTS == col)
    place = (lax.broadcasted_iota(jnp.int32, (ROWS, T), 0) % SLOTS).astype(F32)
    pp[...] = jnp.where(dot(spread, rank) == place, 1.0, 0.0).astype(BF16)
    shares = jnp.where(first, sht_ref[0:1, :], 0.0) + jnp.where(second, sht_ref[1:2, :], 0.0)
    share_hi = shares.astype(BF16)
    share_lo = (shares - share_hi.astype(F32)).astype(BF16)
    spread = one_hot((SP, ROWS), lambda row, col: col // SLOTS == row)
    place = (lax.broadcasted_iota(jnp.int32, (T, ROWS), 1) % SLOTS).astype(F32)
    here = dot(across(same, rank).astype(BF16), spread) == place
    qhi[...] = jnp.where(here, dot(across(same, share_hi).astype(BF16), spread), 0.0).astype(BF16)
    qlo[...] = jnp.where(here, dot(across(same, share_lo).astype(BF16), spread), 0.0).astype(BF16)

    steps, fades = [], []
    for d in range(2):
        v = inc_ref[d : d + 1, :].astype(F32) + off_ref[0:1, d : d + 1]
        step = jnp.maximum(v, 0.0) + log1p(jnp.exp(-jnp.abs(v)))
        steps.append(step)
        fades.append(-jnp.exp(spd_ref[0:1, d : d + 1]) * step + fade_ref[d])
    parts = stacked(three(fades[0]) + three(fades[1])).astype(BF16)
    along = dot(parts, upper + same)
    forward_row = along[0:1] + along[1:2] + along[2:3]
    along = dot(parts, upper)
    backward_row = along[3:4] + along[4:5] + along[5:6]
    along = across(lower + same, parts)
    forward_col = along[:, 0:1] + along[:, 1:2] + along[:, 2:3]
    along = across(lower, parts)
    backward_col = along[:, 3:4] + along[:, 4:5] + along[:, 5:6]
    row = lax.broadcasted_iota(jnp.int32, (T, T), 0)
    col = lax.broadcasted_iota(jnp.int32, (T, T), 1)
    gap[...] = (
        jnp.where(row >= col, jnp.exp(forward_col - forward_row), 0.0) * steps[0]
        + jnp.where(row <= col, jnp.exp(backward_row - backward_col), 0.0) * steps[1]
    )
    forward_end = forward_row[:, T - 1 : T]
    backward_end = backward_row[:, T - 1 : T] + fades[1][:, T - 1 : T]
    weigh = [jnp.exp(forward_end - forward_row) * steps[0], jnp.exp(backward_row) * steps[1]]
    seen = [jnp.exp(forward_row), jnp.exp(backward_end - backward_row)]
    cv[...] = stacked(weigh + seen)
    ends = [jnp.broadcast_to(forward_end, (1, 128)), jnp.broadcast_to(backward_end, (1, 128))]

    for load in grouped:
        load.wait()
    pl.semaphore_wait(barrier, TP + SP - 2)

    def halo(side, k):
        there = (sp + 1) % SP if side == 0 else (sp + SP - 1) % SP
        rows = pl.ds(T - 16, 16) if side == 0 else pl.ds(0, 16)
        lanes = pl.ds(256, 128) if side == 0 else pl.ds(0, 128)
        source = (xpad.at[:, lanes], braw.at[rows], craw.at[rows])[k]
        return pltpu.make_async_remote_copy(
            src_ref=source,
            dst_ref=(hx, hb, hc)[k].at[side],
            send_sem=hs.at[3 * side + k],
            recv_sem=hr.at[3 * side + k],
            device_id=(there, tp),
            device_id_type=MESH,
        )

    for k in range(3):
        halo(0, k).start()
        halo(1, k).start()
    lax.fori_loop(1, TP, send_tile, 0)

    def to_other(part):
        return pltpu.make_async_remote_copy(
            src_ref=part,
            dst_ref=part,
            send_sem=one.at[12],
            recv_sem=one.at[13],
            device_id=(sp, y * 2 + 1 - core),
            device_id_type=MESH,
        )

    for k in (1, 2, 3):
        loads[k].wait()
    for part in (wx.at[:, lanes_of(core)], wx.at[:, lanes_of(core + 2)], wl.at[:, lanes_of(core)]):
        to_other(part).start()

    taps = across(same[0:64, 0:64], stacked([xk_ref[j : j + 1, :].astype(F32) for j in range(CONV)]).astype(BF16))
    lane = lax.broadcasted_iota(jnp.int32, (64, 128), 1)
    body = xpad[...].astype(F32)
    bext[pl.ds(16, T), :] = braw[...].astype(F32)
    cext[pl.ds(16, T), :] = craw[...].astype(F32)
    for k in range(3):
        halo(0, k).wait_recv()
        halo(1, k).wait_recv()
    before, behind = sp > 0, sp < SP - 1
    last = jnp.where(before, pltpu.roll(hx[0].astype(F32), 64, 1), 0.0)
    coming = jnp.where(behind, pltpu.roll(hx[1].astype(F32), 64, 1), 0.0)
    end = jnp.where(
        lane < 64, body[:, 256:384], jnp.where(lane < 66, coming, jnp.where(lane > 125, last, 0.0))
    )
    cells = jnp.concatenate([body[:, 0:256], end], axis=1)
    total = cells * taps[:, 2:3]
    for j in (0, 1, 3, 4):
        total = total + pltpu.roll(cells, (2 - j) % 384, 1) * taps[:, j : j + 1]
    x_conv = silu(total)[:, 0:T].astype(BF16)
    for ext, halos, kernel_ref in ((bext, hb, bk_ref), (cext, hc, ck_ref)):
        ext[pl.ds(0, 16), :] = jnp.where(before, halos[0].astype(F32), 0.0)
        ext[pl.ds(T + 16, 16), :] = jnp.where(behind, halos[1].astype(F32), 0.0)
        total = jnp.zeros((T, 128), F32)
        for j in range(CONV):
            tap = kernel_ref[j : j + 1, at_group].astype(F32)
            total = total + ext[pl.ds(14 + j, T), :] * tap
        mixed[0 if ext is bext else 1] = silu(total).astype(BF16)
    b_conv, c_conv = mixed[0], mixed[1]

    def packed(total, log):
        tail = jnp.concatenate([stacked(three(log)), jnp.zeros((8, 128), F32)], axis=0)
        return total.astype(BF16), tail.astype(BF16)

    x_wide = x_conv.astype(F32)
    for d in range(2):
        scaled = (cv[d : d + 1, :] * x_wide).astype(BF16)
        top, tail = packed(dot(scaled, b_conv), ends[d])
        st_ref[d, 0:64] = top
        st_ref[d, 64:80] = tail
    rx[x] = st_ref[...]
    for k in (2, 1, 3):
        state_row(k, x).start()
    inner = across(x_conv, (across(c_conv, b_conv) * gap[...]).astype(BF16))
    inner = inner + byp_ref[...] * x_wide
    gate = silu(zt_ref[...].astype(F32))

    def all_rows(k):
        return pltpu.make_async_remote_copy(
            src_ref=rx.at[pl.ds(0, k)],
            dst_ref=rx.at[pl.ds(0, k)],
            send_sem=one.at[0],
            recv_sem=one.at[1],
            device_id=(z * NX + (x + 1) % NX, tp),
            device_id_type=MESH,
        )

    all_rows(NX - 1).wait_recv()

    def state(block):
        return block[0:64].astype(F32)

    def log_of(block):
        logs = block[64:80].astype(F32)
        return logs[0:1] + logs[1:2] + logs[2:3]

    for way in (0, 1):
        total, log = jnp.zeros((64, 128), F32), jnp.zeros((1, 128), F32)
        for i in range(NX) if way == 0 else reversed(range(NX)):
            block = rx[i, way]
            own = log_of(block)
            total = jnp.exp(own) * total + state(block)
            log = log + own
        top, tail = packed(total, log)
        tb[way, 0:64] = top
        tb[way, 64:80] = tail
    rz[z] = tb[0]

    def state_column(k, source):
        return pltpu.make_async_remote_copy(
            src_ref=tb.at[(z + k) // NZ],
            dst_ref=rz.at[source],
            send_sem=one.at[2],
            recv_sem=one.at[3],
            device_id=(((z + k) % NZ) * NX + x, tp),
            device_id_type=MESH,
        )

    for k in (4, 3, 5, 2, 6, 1, 7):
        state_column(k, z).start()

    loads[0].wait()
    wide[...] = jnp.zeros(wide.shape, BF16)

    def widen(j, carry):
        block = wb[pl.ds(pl.multiple_of(j * 64, 64), 64), :]
        wide[pl.ds(pl.multiple_of(j * 128, 128), 64), pl.ds(0, 128)] = block
        wide[pl.ds(pl.multiple_of(j * 128 + 64, 64), 64), pl.ds(128, 128)] = block
        return carry

    lax.fori_loop(0, HEADS, widen, 0)

    def all_columns():
        return pltpu.make_async_remote_copy(
            src_ref=rz.at[pl.ds(0, NZ - 1)],
            dst_ref=rz.at[pl.ds(0, NZ - 1)],
            send_sem=one.at[2],
            recv_sem=one.at[3],
            device_id=(((z + 1) % NZ) * NX + x, tp),
            device_id_type=MESH,
        )

    all_columns().wait_recv()

    carried = []
    for way in (0, 1):
        total = jnp.zeros((64, 128), F32)
        for i in range(NZ) if way == 0 else reversed(range(NZ)):
            block = rz[i]
            passed = (i < z) if way == 0 else (i > z)
            total = jnp.where(passed, jnp.exp(log_of(block)) * total + state(block), total)
        for i in range(NX) if way == 0 else reversed(range(NX)):
            block = rx[i, way]
            passed = (i < x) if way == 0 else (i > x)
            total = jnp.where(passed, jnp.exp(log_of(block)) * total + state(block), total)
        carried.append(total.astype(BF16))

    mixer = inner + cv[2:3, :] * across(carried[0], mixed[1]) + cv[3:4, :] * across(carried[1], mixed[1])
    gated = (mixer * gate).astype(BF16)
    none = jnp.zeros((64, T), BF16)
    upper_half = one_hot((HALF, T), lambda row, col: row == col)
    lower_half = one_hot((HALF, T), lambda row, col: row + HALF == col)
    mine = pl.ds(pl.multiple_of(tp * 128, 128), 128)
    bn[:, mine] = (
        across(upper_half, jnp.concatenate([gated, none], axis=0))
        + across(lower_half, jnp.concatenate([none, gated], axis=0))
    ).astype(BF16)

    sems = (rsem, rrecv)
    ring = Ring(bn, 0, HALF, sems, 0, direct=True)
    ring.start()

    def all_tiles(ref, at):
        return pltpu.make_async_remote_copy(
            src_ref=ref.at[pl.ds(0, TP - 1)],
            dst_ref=ref.at[pl.ds(0, TP - 1)],
            send_sem=one.at[at],
            recv_sem=one.at[at + 1],
            device_id=(sp, (tp + 1) % TP),
            device_id_type=MESH,
        )

    all_tiles(ft, 4).wait_recv()
    run([ring])
    ring.finish()

    left = lax.broadcasted_iota(jnp.int32, (HALF, 128), 1) < 64
    for g in range(GROUPS):
        squares = jnp.zeros((HALF, 128), F32)
        for j in range(4 * g, 4 * g + 4):
            v = bn[:, 128 * j : 128 * j + 128].astype(F32)
            squares = squares + v * v
        top = jnp.sum(jnp.where(left, squares, 0.0), axis=1, keepdims=True)
        bottom = jnp.sum(jnp.where(left, 0.0, squares), axis=1, keepdims=True)
        scale = lax.rsqrt(jnp.where(left, top, bottom) / (4 * HEAD_DIM) + 1e-06)
        for j in range(4 * g, 4 * g + 4):
            v = bn[:, 128 * j : 128 * j + 128].astype(F32)
            nn[:, 128 * j : 128 * j + 128] = (v * scale * ft[j, 0:1]).astype(BF16)
    projected = dot(nn[...], wide[...])
    am[0:HALF] = (src_ref[0:HALF].astype(F32) + projected[:, 0:128]).astype(BF16)
    am[HALF:T] = (src_ref[HALF:T].astype(F32) + projected[:, 128:256]).astype(BF16)

    own = (am[...].astype(F32) * after_ref[...]).astype(BF16)
    ff[:, mine] = own
    dd[...] = dot(pp[...], own).astype(BF16)

    def rows_of(i):
        return pl.ds(pl.multiple_of(i * SLOTS, SLOTS), SLOTS)

    per = SP // 2 // CHUNKS
    size = per * SLOTS
    local = sp % (SP // 2)

    def deliver(k):
        target = (sp + k) % SP
        return pltpu.make_async_remote_copy(
            src_ref=dd.at[rows_of(target)],
            dst_ref=xx.at[rows_of(local), mine],
            send_sem=one.at[8],
            recv_sem=dr.at[local // per],
            device_id=(target, y * 2 + side_of),
            device_id_type=MESH,
        )

    def send_rows(k, carry):
        deliver(k).start()
        return carry

    lax.fori_loop(1, SP, send_rows, 0)

    @pl.when(side_of == core)
    def _():
        xx[rows_of(local), mine] = dd[rows_of(sp)]

    @pl.when(side_of != core)
    def _():
        deliver(0).start()

    spread_out = [Ring(ff, i * HALF, HALF, sems, 1 + i) for i in range(2)]
    for spreading in spread_out:
        spreading.start()

    dims = (((1,), (1,)), ((), ()))
    squares = am[...].astype(F32) * am[...].astype(F32)
    high = squares.astype(BF16)
    rest = (squares - high.astype(F32)).astype(BF16)
    ones = jnp.ones((8, 128), BF16)
    sums = lax.dot_general(ones, high, dims, preferred_element_type=F32) + lax.dot_general(
        ones, rest, dims, preferred_element_type=F32
    )
    line = jnp.concatenate([sums, jnp.zeros((8, 3 * 128 - T), F32)], axis=1)
    level = lax.broadcasted_iota(jnp.int32, (8, 128), 0)
    own = jnp.where(
        level == 0,
        line[:, 0:128],
        jnp.where(level == 1, line[:, 128:256], jnp.where(level == 2, line[:, 256:384], 0.0)),
    )
    sq[tp] = own
    so[...] = own

    def sums_to(k, source):
        return pltpu.make_async_remote_copy(
            src_ref=so,
            dst_ref=sq.at[source],
            send_sem=one.at[6],
            recv_sem=one.at[7],
            device_id=(sp, (tp + k) % TP),
            device_id_type=MESH,
        )

    def send_sums(k, carry):
        sums_to((k + 7) % (TP - 1) + 1, tp).start()
        return carry

    lax.fori_loop(0, TP - 1, send_sums, 0)
    ring.drain()

    def some_rows(ref, first, blocks, sent, received):
        part = ref.at[pl.ds(first, blocks * SLOTS), pl.ds(0, 128)]
        return pltpu.make_async_remote_copy(
            src_ref=part,
            dst_ref=part,
            send_sem=one.at[sent],
            recv_sem=received,
            device_id=((sp + 1) % SP, tp),
            device_id_type=MESH,
        )

    def either(test, less, more):
        @pl.when(test)
        def _():
            less()

        @pl.when(jnp.logical_not(test))
        def _():
            more()

    for step in (1, 2):
        for ring in spread_out:
            ring.step(step)
    gathers = []
    for q in range(CHUNKS):
        either(
            sp // per == core * CHUNKS + q,
            lambda: some_rows(xx, 0, 2 * per - 1, 8, dr.at[q]).wait_recv(),
            lambda: some_rows(xx, 0, 2 * per, 8, dr.at[q]).wait_recv(),
        )
        gathers.append(Ring(xx, q * size, size, sems, 4 + q, pair=True))
        gathers[-1].start()

    all_tiles(sq, 6).wait_recv()
    total = sq[0]
    for j in range(1, TP):
        total = total + sq[j]
    line = jnp.concatenate([total[0:1], total[1:2], total[2:3]], axis=1)
    parts = stacked(three(line)).astype(BF16)
    same = one_hot((T, 384), lambda row, col: row == col)
    upright = across(same, parts)
    scale = lax.rsqrt((upright[:, 0:1] + upright[:, 1:2] + upright[:, 2:3]) / D + 1e-06)
    lane = lax.broadcasted_iota(jnp.int32, (T, 128), 1)
    parts = jnp.zeros((T, 128), F32)
    for k, part in enumerate(three(scale)):
        parts = jnp.where(lane == k, part, parts)
    ss[...] = dot(pp[...], parts.astype(BF16)).astype(BF16)

    def send_scale(k, carry):
        target = (sp + k) % SP
        pltpu.make_async_remote_copy(
            src_ref=ss.at[rows_of(target)],
            dst_ref=sl.at[rows_of(local)],
            send_sem=one.at[14],
            recv_sem=one.at[15],
            device_id=(target, tp),
            device_id_type=MESH,
        ).start()
        return carry

    @pl.when(side_of == core)
    def _():
        lax.fori_loop(1, SP, send_scale, 0)
        sl[rows_of(local), :] = ss[rows_of(sp), :]

    for step in (3, 4):
        for ring in spread_out:
            ring.step(step)
    for ring in gathers:
        ring.step(1)
    for ring in spread_out:
        ring.finish()
    loads[4].wait()
    loads[5].wait()
    both = dot(ff[...], wc[...]) * scale
    sh[:, mine] = (jax.nn.silu(both[:, 0:128]) * both[:, 128:256]).astype(BF16)
    hidden_out = Ring(sh, 0, T, sems, 3)
    hidden_out.start()
    for step in (2, 3, 4):
        for ring in gathers:
            ring.step(step)
        hidden_out.step(step - 1)

    weights = wx.at[:, pl.ds(0, 384)]
    to_other(weights).wait_recv()
    either(
        side_of == core,
        lambda: some_rows(sl, 0, SP // 2 - 1, 14, one.at[15]).wait_recv(),
        lambda: some_rows(sl, 0, SP // 2, 14, one.at[15]).wait_recv(),
    )
    chip = pl.ds(pl.multiple_of(y * 256, 256), 256)
    hiddens = []
    for q in range(CHUNKS):
        at = pl.ds(q * size, size)
        level = sl[at, :].astype(F32)
        level = level[:, 0:1] + level[:, 1:2] + level[:, 2:3]
        both = dot(xx[at, :], wx[...])
        both = both * level
        hh[at, chip] = (jax.nn.silu(both[:, 0:256]) * both[:, 256:512]).astype(BF16)
        hiddens.append(Ring(hh, q * size, size, sems, 4 + CHUNKS + q, pair=True))
        hiddens[-1].start()
    hidden_out.step(4)
    for side in range(2):
        for k in range(3):
            halo(side, k).wait_send()
    all_rows(NX - 1).wait_send()
    all_columns().wait_send()
    all_tiles(ft, 4).wait_send()
    all_tiles(sq, 6).wait_send()
    either(
        side_of == core,
        lambda: some_rows(dd, 0, SP - 1, 8, one.at[9]).wait_send(),
        lambda: some_rows(dd, 0, SP, 8, one.at[9]).wait_send(),
    )

    @pl.when(side_of == core)
    def _():
        some_rows(dd, 0, SP - 1, 14, one.at[9]).wait_send()

    to_other(weights).wait_send()
    for ring in spread_out + gathers:
        ring.drain()
    for ring in hiddens:
        ring.step(1)
    hidden_out.finish()
    loads[6].wait()
    shared = dot(sh[...], wcl[...]).astype(BF16).astype(F32)
    out_ref[...] = shared.astype(BF16)
    hidden_out.drain()
    for step in (2, 3, 4):
        for ring in hiddens:
            ring.step(step)

    def give(i, to_core):
        return pltpu.make_async_remote_copy(
            src_ref=oo.at[rows_of(i), lanes_of(to_core)],
            dst_ref=ret.at[rows_of(sp)],
            send_sem=one.at[10],
            recv_sem=one.at[11],
            device_id=(core * (SP // 2) + i, y * 2 + to_core),
            device_id_type=MESH,
        )

    for q in range(CHUNKS):
        at = pl.ds(q * size, size)
        oo[at, :] = dot(hh[at, :], wl[...]).astype(BF16)

        def send_back(k, carry):
            i = q * per + (sp + k) % per
            here = core * (SP // 2) + i == sp

            @pl.when(jnp.logical_not(here))
            def _():
                give(i, core).start()

            give(i, 1 - core).start()
            return carry

        lax.fori_loop(0, per, send_back, 0)

    @pl.when(side_of == core)
    def _():
        ret[rows_of(sp), :] = oo[rows_of(local), lanes_of(core)]

    for ring in hiddens:
        ring.drain()
    either(
        side_of == core,
        lambda: some_rows(ret, 0, SP - 1, 10, one.at[11]).wait_recv(),
        lambda: some_rows(ret, 0, SP, 10, one.at[11]).wait_recv(),
    )
    either(
        side_of == core,
        lambda: some_rows(ret, 0, SP - 1, 10, one.at[11]).wait_send(),
        lambda: some_rows(ret, 0, SP, 10, one.at[11]).wait_send(),
    )
    routed = dot(qhi[...], ret[...]) + dot(qlo[...], ret[...])
    out_ref[...] = (am[...].astype(F32) + out_ref[...].astype(F32) + routed).astype(BF16)


def whole(*operands):
    vmem = pl.BlockSpec(memory_space=pltpu.VMEM)
    hbm = pl.BlockSpec(memory_space=pl.ANY)
    rings = 4 + 2 * CHUNKS
    dma = pltpu.SemaphoreType.DMA

    def space(*shape, kind=BF16):
        return pltpu.VMEM(shape, kind)

    return pl.pallas_call(
        kernel,
        out_shape=jax.ShapeDtypeStruct((T, 128), BF16),
        in_specs=[vmem] * 15 + [hbm] * 9,
        out_specs=vmem,
        scratch_shapes=[
            space(64, 384),
            space(T, 128),
            space(T, 128),
            space(2, 64, 128),
            space(2, 16, 128),
            space(2, 16, 128),
            space(T + 32, 128, kind=F32),
            space(T + 32, 128, kind=F32),
            space(T, T, kind=F32),
            space(8, T, kind=F32),
            space(2, T, 128),
            space(8, 128, kind=F32),
            space(2, BLOCK, 128),
            space(NX, 2, BLOCK, 128),
            space(2, BLOCK, 128),
            space(NZ, BLOCK, 128),
            space(TP, 8, 128, kind=F32),
            space(TP, 8, 128, kind=F32),
            space(8, 128, kind=F32),
            space(1024, 128),
            space(D, 512),
            space(D, 256),
            space(D, 256),
            space(D, 128),
            space(D, 256),
            space(HALF, D),
            space(HALF, D),
            space(T, 128),
            space(T, D),
            space(T, D),
            space(ROWS // 2, D),
            space(ROWS // 2, D),
            space(ROWS, 128),
            space(ROWS, 128),
            space(ROWS // 2, 128),
            space(ROWS // 2, 256),
            space(ROWS, 128),
            space(ROWS, T),
            space(T, ROWS),
            space(T, ROWS),
            dma((9,)), dma((6,)), dma((6,)), dma((16,)), dma((CHUNKS,)), dma((rings, 2)), dma((rings, 8)),
        ],
        compiler_params=pltpu.CompilerParams(collective_id=0, has_side_effects=True),
        name="mixer_experts",
    )(*operands)


def shards(
    layer_source_vector,
    attention_lane_source,
    result_valve_logits,
    memory_write_matrix,
    memory_query_matrix,
    increment_logits,
    increment_offset,
    log_fade_speed,
    extra_log_fade,
    attention_bypass_factor,
    attention_lane_kernel,
    memory_write_kernel,
    memory_query_kernel,
    cluster_rescale_factor,
    blender_result_matrix,
    specialist_rescale_factor,
    chosen_specialists,
    specialist_shares,
    specialist_valve_matrix,
    specialist_raising_matrix,
    specialist_lowering_matrix,
    common_valve_matrix,
    common_raising_matrix,
    common_lowering_matrix,
):
    return whole(
        attention_lane_source.T,
        result_valve_logits.T,
        increment_logits.reshape(2, T),
        increment_offset.T,
        log_fade_speed.T,
        extra_log_fade.reshape(2, 1, T),
        attention_bypass_factor.reshape(1, 1),
        attention_lane_kernel,
        memory_write_kernel,
        memory_query_kernel,
        cluster_rescale_factor.reshape(1, 64),
        specialist_rescale_factor.reshape(1, 128),
        layer_source_vector,
        chosen_specialists.T,
        specialist_shares.T,
        memory_write_matrix,
        memory_query_matrix,
        blender_result_matrix,
        specialist_valve_matrix,
        specialist_raising_matrix,
        specialist_lowering_matrix,
        common_valve_matrix,
        common_raising_matrix,
        common_lowering_matrix,
    )


def solution(mesh):
    return jax.shard_map(
        shards,
        mesh=mesh,
        in_specs=(
            P("sp", "tp"),
            P("sp", "tp"),
            P("sp", "tp"),
            P("sp", None),
            P("sp", None),
            P(None, "sp", "tp"),
            P(None, "tp"),
            P(None, "tp"),
            P(None, "sp", "tp"),
            P("tp"),
            P(None, "tp"),
            P(),
            P(),
            P("tp"),
            P(None, "tp"),
            P("tp"),
            P("sp", None),
            P("sp", None),
            P("sp", None, "tp"),
            P("sp", None, "tp"),
            P("sp", None, "tp"),
            P(None, "tp"),
            P(None, "tp"),
            P(None, "tp"),
        ),
        out_specs=P("sp", "tp"),
        check_vma=False,
    )
```

```python
import jax
import jax.numpy as jnp
from jax import lax
from jax.experimental import pallas as pl
from jax.experimental.pallas import tpu as pltpu
from jax.sharding import PartitionSpec as P

D = 2048
HEADS = 16
HEAD_DIM = 64
GROUPS = 4
STATE = 128
CONV = 5

NZ, NX, NY = 8, 4, 8
SP, TP = NZ * NX, NY * 2
T = 320
HALF = T // 2
SLOTS = 32
ROWS = SP * SLOTS
CAP = 30
SPLITS = 4
BLOCK = 80
CHUNKS = 2
MESH = pl.DeviceIdType.MESH
F32, BF16 = jnp.float32, jnp.bfloat16


def dot(a, b):
    return jnp.dot(a, b, preferred_element_type=F32)


class Ring:
    def __init__(self, buf, first, rows, sems, index, direct=False, pair=False):
        self.buf, self.first, self.rows, self.direct, self.pair = buf, first, rows, direct, pair
        self.out, self.near = sems[0].at[index, 0], sems[0].at[index, 1]
        self.recv = sems[1].at[index]
        self.sp, tp = lax.axis_index("sp"), lax.axis_index("tp")
        self.y, self.core = tp // 2, tp % 2

    def part(self, chip, core, half=None):
        column, width = ((chip + 2 * NY) % NY) * 2, 128
        if self.pair:
            width = 256
        else:
            column = column + core
        first, rows = self.first, self.rows
        if half is not None:
            cut = (rows // 2 + 15) // 16 * 16
            first, rows = (first, cut) if half == 0 else (first + cut, rows - cut)
        return self.buf.at[pl.ds(first, rows), pl.ds(pl.multiple_of(column * 128, 128), width)]

    def along(self, way, step, chip, far):
        turn = 1 - 2 * way
        block = self.part(chip, self.core, way if step == 4 else None)
        return pltpu.make_async_remote_copy(
            src_ref=block,
            dst_ref=block,
            send_sem=self.out,
            recv_sem=self.recv.at[4 * way + step - 1],
            device_id=(self.sp, ((self.y + turn * far + NY) % NY) * 2 + self.core),
            device_id_type=MESH,
        )

    def hop(self, way, step):
        if self.direct:
            return self.along(way, step, self.y, step)
        return self.along(way, step, self.y - (1 - 2 * way) * (step - 1), 1)

    def landed(self, way, step):
        return self.along(way, step, self.y - (1 - 2 * way) * step, 1)

    def relay(self, way, step):
        turn = 1 - 2 * way
        return self.over(self.part(self.y - turn * step, self.core, way if step == 4 else None))

    def over(self, block):
        return pltpu.make_async_remote_copy(
            src_ref=block,
            dst_ref=block,
            send_sem=self.out,
            recv_sem=self.near,
            device_id=(self.sp, self.y * 2 + 1 - self.core),
            device_id_type=MESH,
        )

    def several(self, blocks):
        return self.over(self.buf.at[pl.ds(self.first, self.rows), pl.ds(0, 128 * blocks)])

    def start(self):
        for step in (4, 3, 2, 1) if self.direct else (1,):
            self.hop(0, step).start()
            self.hop(1, step).start()
        if not self.pair:
            self.relay(0, 0).start()

    def step(self, step):
        for way in (0, 1):
            self.landed(way, step).wait_recv()
            if step < 4 and not self.direct:
                self.hop(way, step + 1).start()
            if not self.pair:
                self.relay(way, step).start()

    def finish(self):
        self.several(NY).wait_recv()

    def drain(self):
        self.several(2 * NY - (2 if self.pair else 1)).wait_send()


def run(rings):
    for step in range(1, 5):
        for ring in rings:
            ring.step(step)


def stacked(rows):
    level = lax.broadcasted_iota(jnp.int32, (8, rows[0].shape[1]), 0)
    total = jnp.zeros(level.shape, F32)
    for k, row in enumerate(rows):
        total = jnp.where(level == k, row, total)
    return total


def three(v):
    high = v.astype(BF16).astype(F32)
    middle = (v - high).astype(BF16).astype(F32)
    return [high, middle, v - high - middle]


def one_hot(shape, test):
    row, col = lax.broadcasted_iota(jnp.int32, shape, 0), lax.broadcasted_iota(jnp.int32, shape, 1)
    return jnp.where(test(row, col), 1.0, 0.0).astype(BF16)


def across(a, b):
    return lax.dot_general(a, b, (((1,), (1,)), ((), ())), preferred_element_type=F32)


def log1p(u):
    series = u * (1 - u * (1 / 2 - u * (1 / 3 - u * (1 / 4 - u * (1 / 5 - u / 6)))))
    return jnp.where(u < 0.03, series, jnp.log(1 + u))


def silu(v):
    return v / (1 + jnp.exp(-v))


def kernel(
    xt_ref, zt_ref, inc_ref, off_ref, spd_ref, fade_ref, byp_ref, xk_ref, bk_ref, ck_ref, gain_ref,
    after_ref, src_ref, cht_ref, sht_ref,
    bm_hbm, cm_hbm, blender_hbm, valve_hbm, raising_hbm, lowering_hbm, cvalve_hbm, craising_hbm, clowering_hbm,
    out_ref,
    xpad, braw, craw, hx, hb, hc, bext, cext, gap, cv, mixed, fto,
    st_ref, rx, tb, rz, ft, sq, so, wb, wx, wc, wl, wcl, wide, bn, nn, am, ff, sh, xl, xx, hh, tot, low, dd, ss, sl, oo, ret, pp, qhi, qlo,
    wsem, hs, hr, one, dr, rsem, rrecv,
):
    sp, tp = lax.axis_index("sp"), lax.axis_index("tp")
    z, x = sp // NX, sp % NX
    y, core, side_of = tp // 2, tp % 2, z % 2

    barrier = pltpu.get_barrier_semaphore()

    def greet_tp(k, carry):
        pl.semaphore_signal(barrier, inc=1, device_id=(sp, (tp + k) % TP), device_id_type=MESH)
        return carry

    def greet_sp(k, carry):
        pl.semaphore_signal(barrier, inc=1, device_id=((sp + k) % SP, tp), device_id_type=MESH)
        return carry

    lax.fori_loop(1, TP, greet_tp, 0)
    lax.fori_loop(1, SP, greet_sp, 0)

    def lanes_of(i):
        return pl.ds(pl.multiple_of(i * 128, 128), 128)

    at_group = pl.ds(pl.multiple_of((tp // 4) * 128, 128), 128)
    loads = [
        pltpu.make_async_copy(blender_hbm, wb, wsem.at[0]),
        pltpu.make_async_copy(valve_hbm.at[0], wx.at[:, lanes_of(core)], wsem.at[1]),
        pltpu.make_async_copy(raising_hbm.at[0], wx.at[:, lanes_of(core + 2)], wsem.at[2]),
        pltpu.make_async_copy(lowering_hbm.at[0], wl.at[:, lanes_of(core)], wsem.at[3]),
        pltpu.make_async_copy(cvalve_hbm, wc.at[:, pl.ds(0, 128)], wsem.at[4]),
        pltpu.make_async_copy(craising_hbm, wc.at[:, pl.ds(128, 128)], wsem.at[5]),
        pltpu.make_async_copy(clowering_hbm, wcl, wsem.at[6]),
    ]
    grouped = [
        pltpu.make_async_copy(bm_hbm.at[:, at_group], braw, wsem.at[7]),
        pltpu.make_async_copy(cm_hbm.at[:, at_group], craw, wsem.at[8]),
    ]
    for load in grouped + loads:
        load.start()

    xpad[...] = jnp.zeros(xpad.shape, BF16)
    xpad[:, 0:T] = xt_ref[...]
    gains = jnp.concatenate([gain_ref[...], gain_ref[...]], axis=1)
    fto[...] = jnp.broadcast_to(gains, (8, 128))
    ft[tp] = fto[...]

    def state_row(k, source):
        return pltpu.make_async_remote_copy(
            src_ref=st_ref,
            dst_ref=rx.at[source],
            send_sem=one.at[0],
            recv_sem=one.at[1],
            device_id=(z * NX + (x + k) % NX, tp),
            device_id_type=MESH,
        )

    def tile(k, source):
        return pltpu.make_async_remote_copy(
            src_ref=fto,
            dst_ref=ft.at[source],
            send_sem=one.at[4],
            recv_sem=one.at[5],
            device_id=(sp, (tp + k) % TP),
            device_id_type=MESH,
        )

    def send_tile(k, carry):
        tile(k, tp).start()
        return carry

    lower = one_hot((T, T), lambda row, col: col < row)
    upper = one_hot((T, T), lambda row, col: row < col)
    same = one_hot((T, T), lambda row, col: row == col)
    experts = lax.broadcasted_iota(jnp.int32, (SP, T), 0)
    first, second = cht_ref[0:1, :] == experts, cht_ref[1:2, :] == experts
    named = jnp.where(first | second, 1.0, 0.0)
    rank = dot(named.astype(BF16), upper)
    rank = jnp.where(named > 0, rank, 99.0).astype(BF16)
    spread = one_hot((ROWS, SP), lambda row, col: row // SLOTS == col)
    place = (lax.broadcasted_iota(jnp.int32, (ROWS, T), 0) % SLOTS).astype(F32)
    pp[...] = jnp.where(dot(spread, rank) == place, 1.0, 0.0).astype(BF16)
    shares = jnp.where(first, sht_ref[0:1, :], 0.0) + jnp.where(second, sht_ref[1:2, :], 0.0)
    share_hi = shares.astype(BF16)
    share_lo = (shares - share_hi.astype(F32)).astype(BF16)
    spread = one_hot((SP, ROWS), lambda row, col: col // SLOTS == row)
    place = (lax.broadcasted_iota(jnp.int32, (T, ROWS), 1) % SLOTS).astype(F32)
    here = dot(across(same, rank).astype(BF16), spread) == place
    qhi[...] = jnp.where(here, dot(across(same, share_hi).astype(BF16), spread), 0.0).astype(BF16)
    qlo[...] = jnp.where(here, dot(across(same, share_lo).astype(BF16), spread), 0.0).astype(BF16)

    steps, fades = [], []
    for d in range(2):
        v = inc_ref[d : d + 1, :].astype(F32) + off_ref[0:1, d : d + 1]
        step = jnp.maximum(v, 0.0) + log1p(jnp.exp(-jnp.abs(v)))
        steps.append(step)
        fades.append(-jnp.exp(spd_ref[0:1, d : d + 1]) * step + fade_ref[d])
    parts = stacked(three(fades[0]) + three(fades[1])).astype(BF16)
    along = dot(parts, upper + same)
    forward_row = along[0:1] + along[1:2] + along[2:3]
    along = dot(parts, upper)
    backward_row = along[3:4] + along[4:5] + along[5:6]
    along = across(lower + same, parts)
    forward_col = along[:, 0:1] + along[:, 1:2] + along[:, 2:3]
    along = across(lower, parts)
    backward_col = along[:, 3:4] + along[:, 4:5] + along[:, 5:6]
    row = lax.broadcasted_iota(jnp.int32, (T, T), 0)
    col = lax.broadcasted_iota(jnp.int32, (T, T), 1)
    gap[...] = (
        jnp.where(row >= col, jnp.exp(forward_col - forward_row), 0.0) * steps[0]
        + jnp.where(row <= col, jnp.exp(backward_row - backward_col), 0.0) * steps[1]
    )
    forward_end = forward_row[:, T - 1 : T]
    backward_end = backward_row[:, T - 1 : T] + fades[1][:, T - 1 : T]
    weigh = [jnp.exp(forward_end - forward_row) * steps[0], jnp.exp(backward_row) * steps[1]]
    seen = [jnp.exp(forward_row), jnp.exp(backward_end - backward_row)]
    cv[...] = stacked(weigh + seen)
    ends = [jnp.broadcast_to(forward_end, (1, 128)), jnp.broadcast_to(backward_end, (1, 128))]

    for load in grouped:
        load.wait()
    pl.semaphore_wait(barrier, TP + SP - 2)

    def halo(side, k):
        there = (sp + 1) % SP if side == 0 else (sp + SP - 1) % SP
        rows = pl.ds(T - 16, 16) if side == 0 else pl.ds(0, 16)
        lanes = pl.ds(256, 128) if side == 0 else pl.ds(0, 128)
        source = (xpad.at[:, lanes], braw.at[rows], craw.at[rows])[k]
        return pltpu.make_async_remote_copy(
            src_ref=source,
            dst_ref=(hx, hb, hc)[k].at[side],
            send_sem=hs.at[3 * side + k],
            recv_sem=hr.at[3 * side + k],
            device_id=(there, tp),
            device_id_type=MESH,
        )

    for k in range(3):
        halo(0, k).start()
        halo(1, k).start()
    lax.fori_loop(1, TP, send_tile, 0)

    def to_other(part):
        return pltpu.make_async_remote_copy(
            src_ref=part,
            dst_ref=part,
            send_sem=one.at[12],
            recv_sem=one.at[13],
            device_id=(sp, y * 2 + 1 - core),
            device_id_type=MESH,
        )

    for k in (1, 2, 3):
        loads[k].wait()
    for part in (wx.at[:, lanes_of(core)], wx.at[:, lanes_of(core + 2)], wl.at[:, lanes_of(core)]):
        to_other(part).start()

    taps = across(same[0:64, 0:64], stacked([xk_ref[j : j + 1, :].astype(F32) for j in range(CONV)]).astype(BF16))
    lane = lax.broadcasted_iota(jnp.int32, (64, 128), 1)
    body = xpad[...].astype(F32)
    bext[pl.ds(16, T), :] = braw[...].astype(F32)
    cext[pl.ds(16, T), :] = craw[...].astype(F32)
    for k in range(3):
        halo(0, k).wait_recv()
        halo(1, k).wait_recv()
    before, behind = sp > 0, sp < SP - 1
    last = jnp.where(before, pltpu.roll(hx[0].astype(F32), 64, 1), 0.0)
    coming = jnp.where(behind, pltpu.roll(hx[1].astype(F32), 64, 1), 0.0)
    end = jnp.where(
        lane < 64, body[:, 256:384], jnp.where(lane < 66, coming, jnp.where(lane > 125, last, 0.0))
    )
    cells = jnp.concatenate([body[:, 0:256], end], axis=1)
    total = cells * taps[:, 2:3]
    for j in (0, 1, 3, 4):
        total = total + pltpu.roll(cells, (2 - j) % 384, 1) * taps[:, j : j + 1]
    x_conv = silu(total)[:, 0:T].astype(BF16)
    for ext, halos, kernel_ref in ((bext, hb, bk_ref), (cext, hc, ck_ref)):
        ext[pl.ds(0, 16), :] = jnp.where(before, halos[0].astype(F32), 0.0)
        ext[pl.ds(T + 16, 16), :] = jnp.where(behind, halos[1].astype(F32), 0.0)
        total = jnp.zeros((T, 128), F32)
        for j in range(CONV):
            tap = kernel_ref[j : j + 1, at_group].astype(F32)
            total = total + ext[pl.ds(14 + j, T), :] * tap
        mixed[0 if ext is bext else 1] = silu(total).astype(BF16)
    b_conv, c_conv = mixed[0], mixed[1]

    def packed(total, log):
        tail = jnp.concatenate([stacked(three(log)), jnp.zeros((8, 128), F32)], axis=0)
        return total.astype(BF16), tail.astype(BF16)

    x_wide = x_conv.astype(F32)
    for d in range(2):
        scaled = (cv[d : d + 1, :] * x_wide).astype(BF16)
        top, tail = packed(dot(scaled, b_conv), ends[d])
        st_ref[d, 0:64] = top
        st_ref[d, 64:80] = tail
    rx[x] = st_ref[...]
    for k in (2, 1, 3):
        state_row(k, x).start()
    inner = across(x_conv, (across(c_conv, b_conv) * gap[...]).astype(BF16))
    inner = inner + byp_ref[...] * x_wide
    gate = silu(zt_ref[...].astype(F32))

    def all_rows(k):
        return pltpu.make_async_remote_copy(
            src_ref=rx.at[pl.ds(0, k)],
            dst_ref=rx.at[pl.ds(0, k)],
            send_sem=one.at[0],
            recv_sem=one.at[1],
            device_id=(z * NX + (x + 1) % NX, tp),
            device_id_type=MESH,
        )

    all_rows(NX - 1).wait_recv()

    def state(block):
        return block[0:64].astype(F32)

    def log_of(block):
        logs = block[64:80].astype(F32)
        return logs[0:1] + logs[1:2] + logs[2:3]

    for way in (0, 1):
        total, log = jnp.zeros((64, 128), F32), jnp.zeros((1, 128), F32)
        for i in range(NX) if way == 0 else reversed(range(NX)):
            block = rx[i, way]
            own = log_of(block)
            total = jnp.exp(own) * total + state(block)
            log = log + own
        top, tail = packed(total, log)
        tb[way, 0:64] = top
        tb[way, 64:80] = tail
    rz[z] = tb[0]

    def state_column(k, source):
        return pltpu.make_async_remote_copy(
            src_ref=tb.at[(z + k) // NZ],
            dst_ref=rz.at[source],
            send_sem=one.at[2],
            recv_sem=one.at[3],
            device_id=(((z + k) % NZ) * NX + x, tp),
            device_id_type=MESH,
        )

    for k in (4, 3, 5, 2, 6, 1, 7):
        state_column(k, z).start()

    loads[0].wait()
    wide[...] = jnp.zeros(wide.shape, BF16)

    def widen(j, carry):
        block = wb[pl.ds(pl.multiple_of(j * 64, 64), 64), :]
        wide[pl.ds(pl.multiple_of(j * 128, 128), 64), pl.ds(0, 128)] = block
        wide[pl.ds(pl.multiple_of(j * 128 + 64, 64), 64), pl.ds(128, 128)] = block
        return carry

    lax.fori_loop(0, HEADS, widen, 0)

    def all_columns():
        return pltpu.make_async_remote_copy(
            src_ref=rz.at[pl.ds(0, NZ - 1)],
            dst_ref=rz.at[pl.ds(0, NZ - 1)],
            send_sem=one.at[2],
            recv_sem=one.at[3],
            device_id=(((z + 1) % NZ) * NX + x, tp),
            device_id_type=MESH,
        )

    all_columns().wait_recv()

    carried = []
    for way in (0, 1):
        total = jnp.zeros((64, 128), F32)
        for i in range(NZ) if way == 0 else reversed(range(NZ)):
            block = rz[i]
            passed = (i < z) if way == 0 else (i > z)
            total = jnp.where(passed, jnp.exp(log_of(block)) * total + state(block), total)
        for i in range(NX) if way == 0 else reversed(range(NX)):
            block = rx[i, way]
            passed = (i < x) if way == 0 else (i > x)
            total = jnp.where(passed, jnp.exp(log_of(block)) * total + state(block), total)
        carried.append(total.astype(BF16))

    mixer = inner + cv[2:3, :] * across(carried[0], mixed[1]) + cv[3:4, :] * across(carried[1], mixed[1])
    gated = (mixer * gate).astype(BF16)
    none = jnp.zeros((64, T), BF16)
    upper_half = one_hot((HALF, T), lambda row, col: row == col)
    lower_half = one_hot((HALF, T), lambda row, col: row + HALF == col)
    mine = pl.ds(pl.multiple_of(tp * 128, 128), 128)
    bn[:, mine] = (
        across(upper_half, jnp.concatenate([gated, none], axis=0))
        + across(lower_half, jnp.concatenate([none, gated], axis=0))
    ).astype(BF16)

    sems = (rsem, rrecv)
    ring = Ring(bn, 0, HALF, sems, 5 + SPLITS, direct=True)
    ring.start()

    def all_tiles(ref, at):
        return pltpu.make_async_remote_copy(
            src_ref=ref.at[pl.ds(0, TP - 1)],
            dst_ref=ref.at[pl.ds(0, TP - 1)],
            send_sem=one.at[at],
            recv_sem=one.at[at + 1],
            device_id=(sp, (tp + 1) % TP),
            device_id_type=MESH,
        )

    all_tiles(ft, 4).wait_recv()
    run([ring])
    ring.finish()

    left = lax.broadcasted_iota(jnp.int32, (HALF, 128), 1) < 64
    for g in range(GROUPS):
        squares = jnp.zeros((HALF, 128), F32)
        for j in range(4 * g, 4 * g + 4):
            v = bn[:, 128 * j : 128 * j + 128].astype(F32)
            squares = squares + v * v
        top = jnp.sum(jnp.where(left, squares, 0.0), axis=1, keepdims=True)
        bottom = jnp.sum(jnp.where(left, 0.0, squares), axis=1, keepdims=True)
        scale = lax.rsqrt(jnp.where(left, top, bottom) / (4 * HEAD_DIM) + 1e-06)
        for j in range(4 * g, 4 * g + 4):
            v = bn[:, 128 * j : 128 * j + 128].astype(F32)
            nn[:, 128 * j : 128 * j + 128] = (v * scale * ft[j, 0:1]).astype(BF16)
    projected = dot(nn[...], wide[...])
    am[0:HALF] = (src_ref[0:HALF].astype(F32) + projected[:, 0:128]).astype(BF16)
    am[HALF:T] = (src_ref[HALF:T].astype(F32) + projected[:, 128:256]).astype(BF16)

    own = (am[...].astype(F32) * after_ref[...]).astype(BF16)
    ff[:, mine] = own
    dd[...] = dot(pp[...], own).astype(BF16)

    def rows_of(i):
        return pl.ds(pl.multiple_of(i * SLOTS, SLOTS), SLOTS)

    per = SP // 2 // CHUNKS
    local = (x % 2) * 8 + (x // 2) * 4 + z // 2

    def deliver(k):
        target = (sp + k) % SP
        return pltpu.make_async_remote_copy(
            src_ref=dd.at[rows_of(target)],
            dst_ref=xl.at[rows_of(local), lanes_of(core)],
            send_sem=one.at[8],
            recv_sem=dr.at[local // per],
            device_id=(target, y * 2 + side_of),
            device_id_type=MESH,
        )

    def outward(m):
        return SP // 2 + (m // 2 + m % 2) * (1 - 2 * (m % 2))

    def send_rows(m, carry):
        deliver(outward(m)).start()
        return carry

    lax.fori_loop(0, SP - 1, send_rows, 0)

    @pl.when(side_of == core)
    def _():
        xl[rows_of(local), lanes_of(core)] = dd[rows_of(sp)]

    @pl.when(side_of != core)
    def _():
        deliver(0).start()

    cells = T // SPLITS
    spread_out = [Ring(ff, i * cells, cells, sems, 4 + i) for i in range(SPLITS)]
    for spreading in spread_out:
        spreading.start()

    dims = (((1,), (1,)), ((), ()))
    squares = am[...].astype(F32) * am[...].astype(F32)
    high = squares.astype(BF16)
    rest = (squares - high.astype(F32)).astype(BF16)
    ones = jnp.ones((8, 128), BF16)
    sums = lax.dot_general(ones, high, dims, preferred_element_type=F32) + lax.dot_general(
        ones, rest, dims, preferred_element_type=F32
    )
    line = jnp.concatenate([sums, jnp.zeros((8, 3 * 128 - T), F32)], axis=1)
    level = lax.broadcasted_iota(jnp.int32, (8, 128), 0)
    own = jnp.where(
        level == 0,
        line[:, 0:128],
        jnp.where(level == 1, line[:, 128:256], jnp.where(level == 2, line[:, 256:384], 0.0)),
    )
    sq[tp] = own
    so[...] = own

    def sums_to(k, source):
        return pltpu.make_async_remote_copy(
            src_ref=so,
            dst_ref=sq.at[source],
            send_sem=one.at[6],
            recv_sem=one.at[7],
            device_id=(sp, (tp + k) % TP),
            device_id_type=MESH,
        )

    def send_sums(k, carry):
        sums_to((k + 7) % (TP - 1) + 1, tp).start()
        return carry

    lax.fori_loop(0, TP - 1, send_sums, 0)
    ring.drain()

    def some_rows(ref, first, blocks, sent, received):
        part = ref.at[pl.ds(first, blocks * SLOTS), pl.ds(0, 128)]
        return pltpu.make_async_remote_copy(
            src_ref=part,
            dst_ref=part,
            send_sem=one.at[sent],
            recv_sem=received,
            device_id=((sp + 1) % SP, tp),
            device_id_type=MESH,
        )

    def either(test, less, more):
        @pl.when(test)
        def _():
            less()

        @pl.when(jnp.logical_not(test))
        def _():
            more()

    for step in (1, 2):
        for ring in spread_out:
            ring.step(step)
    all_tiles(sq, 6).wait_recv()
    total = sq[0]
    for j in range(1, TP):
        total = total + sq[j]
    line = jnp.concatenate([total[0:1], total[1:2], total[2:3]], axis=1)
    parts = stacked(three(line)).astype(BF16)
    same = one_hot((T, 384), lambda row, col: row == col)
    upright = across(same, parts)
    scale = lax.rsqrt((upright[:, 0:1] + upright[:, 1:2] + upright[:, 2:3]) / D + 1e-06)
    lane = lax.broadcasted_iota(jnp.int32, (T, 128), 1)
    parts = jnp.zeros((T, 128), F32)
    for k, part in enumerate(three(scale)):
        parts = jnp.where(lane == k, part, parts)
    ss[...] = dot(pp[...], parts.astype(BF16)).astype(BF16)

    def send_scale(m, carry):
        target = (sp + outward(m)) % SP
        pltpu.make_async_remote_copy(
            src_ref=ss.at[rows_of(target)],
            dst_ref=sl.at[rows_of(local)],
            send_sem=one.at[14],
            recv_sem=one.at[15],
            device_id=(target, tp),
            device_id_type=MESH,
        ).start()
        return carry

    @pl.when(side_of == core)
    def _():
        lax.fori_loop(0, SP - 1, send_scale, 0)
        sl[rows_of(local), :] = ss[rows_of(sp), :]

    for ring in spread_out:
        ring.step(3)
    chip = pl.ds(pl.multiple_of(y * 256, 256), 256)
    packed_rows = per * CAP
    dense = one_hot((packed_rows, per * SLOTS), lambda row, col: row // CAP * SLOTS + row % CAP == col)
    gathers = []
    for q in range(CHUNKS):
        either(
            jnp.logical_and(side_of == core, x % 2 == q),
            lambda: some_rows(xl, 0, 2 * per - 1, 8, dr.at[q]).wait_recv(),
            lambda: some_rows(xl, 0, 2 * per, 8, dr.at[q]).wait_recv(),
        )
        at = pl.ds(q * packed_rows, packed_rows)
        xx[at, chip] = dot(dense, xl[pl.ds(q * per * SLOTS, per * SLOTS), :]).astype(BF16)
        gathers.append(Ring(xx, q * packed_rows, packed_rows, sems, q, pair=True))
        gathers[-1].start()
    for ring in spread_out:
        ring.step(4)
    for ring in spread_out:
        ring.finish()
    loads[4].wait()
    loads[5].wait()
    both = dot(ff[...], wc[...]) * scale
    sh[:, mine] = (jax.nn.silu(both[:, 0:128]) * both[:, 128:256]).astype(BF16)
    hidden_out = Ring(sh, 0, T, sems, 4 + SPLITS)
    hidden_out.start()
    for step in (1, 2, 3):
        for ring in gathers:
            ring.step(step)
        if step > 1:
            hidden_out.step(step - 1)

    def chips(first, count, total, buf, at, weight):
        def add(k, carry):
            part = pl.ds(pl.multiple_of((y + k) % NY * 256, 256), 256)
            total[at, :] += dot(buf[at, part], weight[part, :])
            return carry

        lax.fori_loop(first, first + count, add, 0)

    weights = wx.at[:, pl.ds(0, 384)]
    to_other(weights).wait_recv()
    either(
        side_of == core,
        lambda: some_rows(sl, 0, SP // 2 - 1, 14, one.at[15]).wait_recv(),
        lambda: some_rows(sl, 0, SP // 2, 14, one.at[15]).wait_recv(),
    )
    tot[...] = jnp.zeros(tot.shape, F32)
    levels = []
    for q in range(CHUNKS):
        at = pl.ds(q * packed_rows, packed_rows)
        chips(NY - 3, NY - 1, tot, xx, at, wx)
        level = dot(dense, sl[pl.ds(q * per * SLOTS, per * SLOTS), :])
        levels.append(level[:, 0:1] + level[:, 1:2] + level[:, 2:3])
    hidden_out.step(3)
    hiddens = []
    for q in range(CHUNKS):
        gathers[q].step(4)
        at = pl.ds(q * packed_rows, packed_rows)
        chips(NY // 2, 1, tot, xx, at, wx)
        both = tot[at, :] * levels[q]
        hh[at, chip] = (jax.nn.silu(both[:, 0:256]) * both[:, 256:512]).astype(BF16)
        hiddens.append(Ring(hh, q * packed_rows, packed_rows, sems, 2 + q, pair=True))
        hiddens[-1].start()
    hidden_out.step(4)
    for side in range(2):
        for k in range(3):
            halo(side, k).wait_send()
    all_rows(NX - 1).wait_send()
    all_columns().wait_send()
    all_tiles(ft, 4).wait_send()
    all_tiles(sq, 6).wait_send()
    either(
        side_of == core,
        lambda: some_rows(dd, 0, SP - 1, 8, one.at[9]).wait_send(),
        lambda: some_rows(dd, 0, SP, 8, one.at[9]).wait_send(),
    )

    @pl.when(side_of == core)
    def _():
        some_rows(dd, 0, SP - 1, 14, one.at[9]).wait_send()

    to_other(weights).wait_send()
    for ring in spread_out + gathers:
        ring.drain()
    for ring in hiddens:
        ring.step(1)
    hidden_out.finish()
    loads[6].wait()
    shared = dot(sh[...], wcl[...]).astype(BF16).astype(F32)
    out_ref[...] = shared.astype(BF16)
    hidden_out.drain()
    for step in (2, 3):
        for ring in hiddens:
            ring.step(step)
    low[...] = jnp.zeros(low.shape, F32)
    for q in range(CHUNKS):
        chips(NY - 3, NY - 1, low, hh, pl.ds(q * packed_rows, packed_rows), wl)
    loose = one_hot((per * SLOTS, packed_rows), lambda row, col: col // CAP * SLOTS + col % CAP == row)

    def give(i, to_core):
        return pltpu.make_async_remote_copy(
            src_ref=oo.at[rows_of(i), lanes_of(to_core)],
            dst_ref=ret.at[rows_of(sp)],
            send_sem=one.at[10],
            recv_sem=one.at[11],
            device_id=(((i % 4) * 2 + core) * NX + i // 4 % 2 * 2 + i // 8, y * 2 + to_core),
            device_id_type=MESH,
        )

    for q in range(CHUNKS):
        hiddens[q].step(4)
        at = pl.ds(q * packed_rows, packed_rows)
        chips(NY // 2, 1, low, hh, at, wl)
        oo[pl.ds(q * per * SLOTS, per * SLOTS), :] = dot(loose, low[at, :].astype(BF16)).astype(BF16)

        def send_back(k, carry):
            turn = k // 2
            i = q * per + k % 2 * 4 + (z // 2 + 6 + (turn // 2 + turn % 2) * (1 - 2 * (turn % 2))) % 4
            here = jnp.logical_and(side_of == core, i == local)

            @pl.when(jnp.logical_not(here))
            def _():
                give(i, core).start()

            give(i, 1 - core).start()
            return carry

        lax.fori_loop(0, per, send_back, 0)

    @pl.when(side_of == core)
    def _():
        ret[rows_of(sp), :] = oo[rows_of(local), lanes_of(core)]

    for ring in hiddens:
        ring.drain()
    either(
        side_of == core,
        lambda: some_rows(ret, 0, SP - 1, 10, one.at[11]).wait_recv(),
        lambda: some_rows(ret, 0, SP, 10, one.at[11]).wait_recv(),
    )
    either(
        side_of == core,
        lambda: some_rows(ret, 0, SP - 1, 10, one.at[11]).wait_send(),
        lambda: some_rows(ret, 0, SP, 10, one.at[11]).wait_send(),
    )
    routed = dot(qhi[...], ret[...]) + dot(qlo[...], ret[...])
    out_ref[...] = (am[...].astype(F32) + out_ref[...].astype(F32) + routed).astype(BF16)


def whole(*operands):
    vmem = pl.BlockSpec(memory_space=pltpu.VMEM)
    hbm = pl.BlockSpec(memory_space=pl.ANY)
    rings = 6 + SPLITS
    dma = pltpu.SemaphoreType.DMA

    def space(*shape, kind=BF16):
        return pltpu.VMEM(shape, kind)

    return pl.pallas_call(
        kernel,
        out_shape=jax.ShapeDtypeStruct((T, 128), BF16),
        in_specs=[vmem] * 15 + [hbm] * 9,
        out_specs=vmem,
        scratch_shapes=[
            space(64, 384),
            space(T, 128),
            space(T, 128),
            space(2, 64, 128),
            space(2, 16, 128),
            space(2, 16, 128),
            space(T + 32, 128, kind=F32),
            space(T + 32, 128, kind=F32),
            space(T, T, kind=F32),
            space(8, T, kind=F32),
            space(2, T, 128),
            space(8, 128, kind=F32),
            space(2, BLOCK, 128),
            space(NX, 2, BLOCK, 128),
            space(2, BLOCK, 128),
            space(NZ, BLOCK, 128),
            space(TP, 8, 128, kind=F32),
            space(TP, 8, 128, kind=F32),
            space(8, 128, kind=F32),
            space(1024, 128),
            space(D, 512),
            space(D, 256),
            space(D, 256),
            space(D, 128),
            space(D, 256),
            space(HALF, D),
            space(HALF, D),
            space(T, 128),
            space(T, D),
            space(T, D),
            space(ROWS // 2, 256),
            space(SP // 2 * CAP, D),
            space(SP // 2 * CAP, D),
            space(SP // 2 * CAP, 512, kind=F32),
            space(SP // 2 * CAP, 256, kind=F32),
            space(ROWS, 128),
            space(ROWS, 128),
            space(ROWS // 2, 128),
            space(ROWS // 2, 256),
            space(ROWS, 128),
            space(ROWS, T),
            space(T, ROWS),
            space(T, ROWS),
            dma((9,)), dma((6,)), dma((6,)), dma((16,)), dma((CHUNKS,)), dma((rings, 2)), dma((rings, 8)),
        ],
        compiler_params=pltpu.CompilerParams(collective_id=0, has_side_effects=True),
        name="mixer_experts",
    )(*operands)


def shards(
    layer_source_vector,
    attention_lane_source,
    result_valve_logits,
    memory_write_matrix,
    memory_query_matrix,
    increment_logits,
    increment_offset,
    log_fade_speed,
    extra_log_fade,
    attention_bypass_factor,
    attention_lane_kernel,
    memory_write_kernel,
    memory_query_kernel,
    cluster_rescale_factor,
    blender_result_matrix,
    specialist_rescale_factor,
    chosen_specialists,
    specialist_shares,
    specialist_valve_matrix,
    specialist_raising_matrix,
    specialist_lowering_matrix,
    common_valve_matrix,
    common_raising_matrix,
    common_lowering_matrix,
):
    return whole(
        attention_lane_source.T,
        result_valve_logits.T,
        increment_logits.reshape(2, T),
        increment_offset.T,
        log_fade_speed.T,
        extra_log_fade.reshape(2, 1, T),
        attention_bypass_factor.reshape(1, 1),
        attention_lane_kernel,
        memory_write_kernel,
        memory_query_kernel,
        cluster_rescale_factor.reshape(1, 64),
        specialist_rescale_factor.reshape(1, 128),
        layer_source_vector,
        chosen_specialists.T,
        specialist_shares.T,
        memory_write_matrix,
        memory_query_matrix,
        blender_result_matrix,
        specialist_valve_matrix,
        specialist_raising_matrix,
        specialist_lowering_matrix,
        common_valve_matrix,
        common_raising_matrix,
        common_lowering_matrix,
    )


def solution(mesh):
    return jax.shard_map(
        shards,
        mesh=mesh,
        in_specs=(
            P("sp", "tp"),
            P("sp", "tp"),
            P("sp", "tp"),
            P("sp", None),
            P("sp", None),
            P(None, "sp", "tp"),
            P(None, "tp"),
            P(None, "tp"),
            P(None, "sp", "tp"),
            P("tp"),
            P(None, "tp"),
            P(),
            P(),
            P("tp"),
            P(None, "tp"),
            P("tp"),
            P("sp", None),
            P("sp", None),
            P("sp", None, "tp"),
            P("sp", None, "tp"),
            P("sp", None, "tp"),
            P(None, "tp"),
            P(None, "tp"),
            P(None, "tp"),
        ),
        out_specs=P("sp", "tp"),
        check_vma=False,
    )
```

```python
import jax
import jax.numpy as jnp
from jax import lax
from jax.experimental import pallas as pl
from jax.experimental.pallas import tpu as pltpu
from jax.sharding import PartitionSpec as P

D = 2048
HEADS = 16
HEAD_DIM = 64
GROUPS = 4
STATE = 128
CONV = 5

NZ, NX, NY = 8, 4, 8
SP, TP = NZ * NX, NY * 2
T = 320
HALF = T // 2
SLOTS = 32
ROWS = SP * SLOTS
CAP = 30
SPLITS = 4
BLOCK = 80
CHUNKS = 2
MESH = pl.DeviceIdType.MESH
F32, BF16 = jnp.float32, jnp.bfloat16


def dot(a, b):
    return jnp.dot(a, b, preferred_element_type=F32)


class Ring:
    def __init__(self, buf, first, rows, sems, index, direct=False, pair=False, last=4):
        self.buf, self.first, self.rows = buf, first, rows
        self.direct, self.pair, self.last = direct, pair, last
        self.out, self.near = sems[0].at[index, 0], sems[0].at[index, 1]
        self.recv = sems[1].at[index]
        self.sp, tp = lax.axis_index("sp"), lax.axis_index("tp")
        self.y, self.core = tp // 2, tp % 2

    def part(self, chip, core, half=None):
        column, width = ((chip + 2 * NY) % NY) * 2, 128
        if self.pair:
            width = 256
        else:
            column = column + core
        first, rows = self.first, self.rows
        if half is not None:
            cut = (rows // 2 + 15) // 16 * 16
            first, rows = (first, cut) if half == 0 else (first + cut, rows - cut)
        return self.buf.at[pl.ds(first, rows), pl.ds(pl.multiple_of(column * 128, 128), width)]

    def along(self, way, step, chip, far):
        turn = 1 - 2 * way
        block = self.part(chip, self.core, way if step == 4 else None)
        return pltpu.make_async_remote_copy(
            src_ref=block,
            dst_ref=block,
            send_sem=self.out,
            recv_sem=self.recv.at[4 * way + step - 1],
            device_id=(self.sp, ((self.y + turn * far + NY) % NY) * 2 + self.core),
            device_id_type=MESH,
        )

    def hop(self, way, step):
        if self.direct:
            return self.along(way, step, self.y, step)
        return self.along(way, step, self.y - (1 - 2 * way) * (step - 1), 1)

    def landed(self, way, step):
        return self.along(way, step, self.y - (1 - 2 * way) * step, 1)

    def relay(self, way, step):
        turn = 1 - 2 * way
        return self.over(self.part(self.y - turn * step, self.core, way if step == 4 else None))

    def over(self, block):
        return pltpu.make_async_remote_copy(
            src_ref=block,
            dst_ref=block,
            send_sem=self.out,
            recv_sem=self.near,
            device_id=(self.sp, self.y * 2 + 1 - self.core),
            device_id_type=MESH,
        )

    def several(self, blocks):
        return self.over(self.buf.at[pl.ds(self.first, self.rows), pl.ds(0, 128 * blocks)])

    def start(self):
        for step in (4, 3, 2, 1) if self.direct else (1,):
            self.hop(0, step).start()
            self.hop(1, step).start()
        if not self.pair:
            self.relay(0, 0).start()

    def step(self, step):
        for way in (0, 1):
            self.landed(way, step).wait_recv()
            if step < self.last and not self.direct:
                self.hop(way, step + 1).start()
            if not self.pair:
                self.relay(way, step).start()

    def finish(self):
        self.several(NY).wait_recv()

    def drain(self):
        self.several(2 * NY - (1 if not self.pair else 2 if self.last == 4 else 4)).wait_send()


def run(rings):
    for step in range(1, 5):
        for ring in rings:
            ring.step(step)


def stacked(rows):
    level = lax.broadcasted_iota(jnp.int32, (8, rows[0].shape[1]), 0)
    total = jnp.zeros(level.shape, F32)
    for k, row in enumerate(rows):
        total = jnp.where(level == k, row, total)
    return total


def three(v):
    high = v.astype(BF16).astype(F32)
    middle = (v - high).astype(BF16).astype(F32)
    return [high, middle, v - high - middle]


def one_hot(shape, test):
    row, col = lax.broadcasted_iota(jnp.int32, shape, 0), lax.broadcasted_iota(jnp.int32, shape, 1)
    return jnp.where(test(row, col), 1.0, 0.0).astype(BF16)


def across(a, b):
    return lax.dot_general(a, b, (((1,), (1,)), ((), ())), preferred_element_type=F32)


def log1p(u):
    series = u * (1 - u * (1 / 2 - u * (1 / 3 - u * (1 / 4 - u * (1 / 5 - u / 6)))))
    return jnp.where(u < 0.03, series, jnp.log(1 + u))


def silu(v):
    return v / (1 + jnp.exp(-v))


def kernel(
    xt_ref, zt_ref, inc_ref, off_ref, spd_ref, fade_ref, byp_ref, xk_ref, bk_ref, ck_ref, gain_ref,
    after_ref, src_ref, cht_ref, sht_ref,
    bm_hbm, cm_hbm, blender_hbm, valve_hbm, raising_hbm, lowering_hbm, cvalve_hbm, craising_hbm, clowering_hbm,
    out_ref,
    xpad, braw, craw, hx, hb, hc, bext, cext, gap, cv, mixed, fto,
    st_ref, rx, tb, rz, ft, sq, so, wb, wx, wc, wl, wcl, wide, bn, nn, am, ff, sh, xl, x2, xx, hh, tot, low, dd, d2, ss, sl, oo, ret, pp, qhi, qlo,
    wsem, hs, hr, one, dr, rsem, rrecv,
):
    sp, tp = lax.axis_index("sp"), lax.axis_index("tp")
    z, x = sp // NX, sp % NX
    y, core, side_of = tp // 2, tp % 2, z % 2

    barrier = pltpu.get_barrier_semaphore()

    def greet_tp(k, carry):
        pl.semaphore_signal(barrier, inc=1, device_id=(sp, (tp + k) % TP), device_id_type=MESH)
        return carry

    def greet_sp(k, carry):
        pl.semaphore_signal(barrier, inc=1, device_id=((sp + k) % SP, tp), device_id_type=MESH)
        return carry

    lax.fori_loop(1, TP, greet_tp, 0)
    lax.fori_loop(1, SP, greet_sp, 0)

    def lanes_of(i):
        return pl.ds(pl.multiple_of(i * 128, 128), 128)

    at_group = pl.ds(pl.multiple_of((tp // 4) * 128, 128), 128)
    loads = [
        pltpu.make_async_copy(blender_hbm, wb, wsem.at[0]),
        pltpu.make_async_copy(valve_hbm.at[0], wx.at[:, lanes_of(core)], wsem.at[1]),
        pltpu.make_async_copy(raising_hbm.at[0], wx.at[:, lanes_of(core + 2)], wsem.at[2]),
        pltpu.make_async_copy(lowering_hbm.at[0], wl.at[:, lanes_of(core)], wsem.at[3]),
        pltpu.make_async_copy(cvalve_hbm, wc.at[:, pl.ds(0, 128)], wsem.at[4]),
        pltpu.make_async_copy(craising_hbm, wc.at[:, pl.ds(128, 128)], wsem.at[5]),
        pltpu.make_async_copy(clowering_hbm, wcl, wsem.at[6]),
    ]
    grouped = [
        pltpu.make_async_copy(bm_hbm.at[:, at_group], braw, wsem.at[7]),
        pltpu.make_async_copy(cm_hbm.at[:, at_group], craw, wsem.at[8]),
    ]
    for load in grouped + loads:
        load.start()

    xpad[...] = jnp.zeros(xpad.shape, BF16)
    xpad[:, 0:T] = xt_ref[...]
    gains = jnp.concatenate([gain_ref[...], gain_ref[...]], axis=1)
    fto[...] = jnp.broadcast_to(gains, (8, 128))
    ft[tp] = fto[...]

    def state_row(k, source):
        return pltpu.make_async_remote_copy(
            src_ref=st_ref,
            dst_ref=rx.at[source],
            send_sem=one.at[0],
            recv_sem=one.at[1],
            device_id=(z * NX + (x + k) % NX, tp),
            device_id_type=MESH,
        )

    def tile(k, source):
        return pltpu.make_async_remote_copy(
            src_ref=fto,
            dst_ref=ft.at[source],
            send_sem=one.at[4],
            recv_sem=one.at[5],
            device_id=(sp, (tp + k) % TP),
            device_id_type=MESH,
        )

    def send_tile(k, carry):
        tile(k, tp).start()
        return carry

    lower = one_hot((T, T), lambda row, col: col < row)
    upper = one_hot((T, T), lambda row, col: row < col)
    same = one_hot((T, T), lambda row, col: row == col)
    experts = lax.broadcasted_iota(jnp.int32, (SP, T), 0)
    first, second = cht_ref[0:1, :] == experts, cht_ref[1:2, :] == experts
    named = jnp.where(first | second, 1.0, 0.0)
    rank = dot(named.astype(BF16), upper)
    rank = jnp.where(named > 0, rank, 99.0).astype(BF16)
    spread = one_hot((ROWS, SP), lambda row, col: row // SLOTS == col)
    place = (lax.broadcasted_iota(jnp.int32, (ROWS, T), 0) % SLOTS).astype(F32)
    pp[...] = jnp.where(dot(spread, rank) == place, 1.0, 0.0).astype(BF16)
    shares = jnp.where(first, sht_ref[0:1, :], 0.0) + jnp.where(second, sht_ref[1:2, :], 0.0)
    share_hi = shares.astype(BF16)
    share_lo = (shares - share_hi.astype(F32)).astype(BF16)
    spread = one_hot((SP, ROWS), lambda row, col: col // SLOTS == row)
    place = (lax.broadcasted_iota(jnp.int32, (T, ROWS), 1) % SLOTS).astype(F32)
    here = dot(across(same, rank).astype(BF16), spread) == place
    qhi[...] = jnp.where(here, dot(across(same, share_hi).astype(BF16), spread), 0.0).astype(BF16)
    qlo[...] = jnp.where(here, dot(across(same, share_lo).astype(BF16), spread), 0.0).astype(BF16)

    steps, fades = [], []
    for d in range(2):
        v = inc_ref[d : d + 1, :].astype(F32) + off_ref[0:1, d : d + 1]
        step = jnp.maximum(v, 0.0) + log1p(jnp.exp(-jnp.abs(v)))
        steps.append(step)
        fades.append(-jnp.exp(spd_ref[0:1, d : d + 1]) * step + fade_ref[d])
    parts = stacked(three(fades[0]) + three(fades[1])).astype(BF16)
    along = dot(parts, upper + same)
    forward_row = along[0:1] + along[1:2] + along[2:3]
    along = dot(parts, upper)
    backward_row = along[3:4] + along[4:5] + along[5:6]
    along = across(lower + same, parts)
    forward_col = along[:, 0:1] + along[:, 1:2] + along[:, 2:3]
    along = across(lower, parts)
    backward_col = along[:, 3:4] + along[:, 4:5] + along[:, 5:6]
    row = lax.broadcasted_iota(jnp.int32, (T, T), 0)
    col = lax.broadcasted_iota(jnp.int32, (T, T), 1)
    gap[...] = (
        jnp.where(row >= col, jnp.exp(forward_col - forward_row), 0.0) * steps[0]
        + jnp.where(row <= col, jnp.exp(backward_row - backward_col), 0.0) * steps[1]
    )
    forward_end = forward_row[:, T - 1 : T]
    backward_end = backward_row[:, T - 1 : T] + fades[1][:, T - 1 : T]
    weigh = [jnp.exp(forward_end - forward_row) * steps[0], jnp.exp(backward_row) * steps[1]]
    seen = [jnp.exp(forward_row), jnp.exp(backward_end - backward_row)]
    cv[...] = stacked(weigh + seen)
    ends = [jnp.broadcast_to(forward_end, (1, 128)), jnp.broadcast_to(backward_end, (1, 128))]

    for load in grouped:
        load.wait()
    pl.semaphore_wait(barrier, TP + SP - 2)

    def halo(side, k):
        there = (sp + 1) % SP if side == 0 else (sp + SP - 1) % SP
        rows = pl.ds(T - 16, 16) if side == 0 else pl.ds(0, 16)
        lanes = pl.ds(256, 128) if side == 0 else pl.ds(0, 128)
        source = (xpad.at[:, lanes], braw.at[rows], craw.at[rows])[k]
        return pltpu.make_async_remote_copy(
            src_ref=source,
            dst_ref=(hx, hb, hc)[k].at[side],
            send_sem=hs.at[3 * side + k],
            recv_sem=hr.at[3 * side + k],
            device_id=(there, tp),
            device_id_type=MESH,
        )

    for k in range(3):
        halo(0, k).start()
        halo(1, k).start()
    lax.fori_loop(1, TP, send_tile, 0)

    def to_other(part):
        return pltpu.make_async_remote_copy(
            src_ref=part,
            dst_ref=part,
            send_sem=one.at[12],
            recv_sem=one.at[13],
            device_id=(sp, y * 2 + 1 - core),
            device_id_type=MESH,
        )

    for k in (1, 2, 3):
        loads[k].wait()
    for part in (wx.at[:, lanes_of(core)], wx.at[:, lanes_of(core + 2)], wl.at[:, lanes_of(core)]):
        to_other(part).start()

    taps = across(same[0:64, 0:64], stacked([xk_ref[j : j + 1, :].astype(F32) for j in range(CONV)]).astype(BF16))
    lane = lax.broadcasted_iota(jnp.int32, (64, 128), 1)
    body = xpad[...].astype(F32)
    bext[pl.ds(16, T), :] = braw[...].astype(F32)
    cext[pl.ds(16, T), :] = craw[...].astype(F32)
    for k in range(3):
        halo(0, k).wait_recv()
        halo(1, k).wait_recv()
    before, behind = sp > 0, sp < SP - 1
    last = jnp.where(before, pltpu.roll(hx[0].astype(F32), 64, 1), 0.0)
    coming = jnp.where(behind, pltpu.roll(hx[1].astype(F32), 64, 1), 0.0)
    end = jnp.where(
        lane < 64, body[:, 256:384], jnp.where(lane < 66, coming, jnp.where(lane > 125, last, 0.0))
    )
    cells = jnp.concatenate([body[:, 0:256], end], axis=1)
    total = cells * taps[:, 2:3]
    for j in (0, 1, 3, 4):
        total = total + pltpu.roll(cells, (2 - j) % 384, 1) * taps[:, j : j + 1]
    x_conv = silu(total)[:, 0:T].astype(BF16)
    for ext, halos, kernel_ref in ((bext, hb, bk_ref), (cext, hc, ck_ref)):
        ext[pl.ds(0, 16), :] = jnp.where(before, halos[0].astype(F32), 0.0)
        ext[pl.ds(T + 16, 16), :] = jnp.where(behind, halos[1].astype(F32), 0.0)
        total = jnp.zeros((T, 128), F32)
        for j in range(CONV):
            tap = kernel_ref[j : j + 1, at_group].astype(F32)
            total = total + ext[pl.ds(14 + j, T), :] * tap
        mixed[0 if ext is bext else 1] = silu(total).astype(BF16)
    b_conv, c_conv = mixed[0], mixed[1]

    def packed(total, log):
        tail = jnp.concatenate([stacked(three(log)), jnp.zeros((8, 128), F32)], axis=0)
        return total.astype(BF16), tail.astype(BF16)

    x_wide = x_conv.astype(F32)
    for d in range(2):
        scaled = (cv[d : d + 1, :] * x_wide).astype(BF16)
        top, tail = packed(dot(scaled, b_conv), ends[d])
        st_ref[d, 0:64] = top
        st_ref[d, 64:80] = tail
    rx[x] = st_ref[...]
    for k in (2, 1, 3):
        state_row(k, x).start()
    inner = across(x_conv, (across(c_conv, b_conv) * gap[...]).astype(BF16))
    inner = inner + byp_ref[...] * x_wide
    gate = silu(zt_ref[...].astype(F32))

    def all_rows(k):
        return pltpu.make_async_remote_copy(
            src_ref=rx.at[pl.ds(0, k)],
            dst_ref=rx.at[pl.ds(0, k)],
            send_sem=one.at[0],
            recv_sem=one.at[1],
            device_id=(z * NX + (x + 1) % NX, tp),
            device_id_type=MESH,
        )

    all_rows(NX - 1).wait_recv()

    def state(block):
        return block[0:64].astype(F32)

    def log_of(block):
        logs = block[64:80].astype(F32)
        return logs[0:1] + logs[1:2] + logs[2:3]

    for way in (0, 1):
        total, log = jnp.zeros((64, 128), F32), jnp.zeros((1, 128), F32)
        for i in range(NX) if way == 0 else reversed(range(NX)):
            block = rx[i, way]
            own = log_of(block)
            total = jnp.exp(own) * total + state(block)
            log = log + own
        top, tail = packed(total, log)
        tb[way, 0:64] = top
        tb[way, 64:80] = tail
    rz[z] = tb[0]

    def state_column(k, source):
        return pltpu.make_async_remote_copy(
            src_ref=tb.at[(z + k) // NZ],
            dst_ref=rz.at[source],
            send_sem=one.at[2],
            recv_sem=one.at[3],
            device_id=(((z + k) % NZ) * NX + x, tp),
            device_id_type=MESH,
        )

    for k in (4, 3, 5, 2, 6, 1, 7):
        state_column(k, z).start()

    loads[0].wait()
    wide[...] = jnp.zeros(wide.shape, BF16)

    def widen(j, carry):
        block = wb[pl.ds(pl.multiple_of(j * 64, 64), 64), :]
        wide[pl.ds(pl.multiple_of(j * 128, 128), 64), pl.ds(0, 128)] = block
        wide[pl.ds(pl.multiple_of(j * 128 + 64, 64), 64), pl.ds(128, 128)] = block
        return carry

    lax.fori_loop(0, HEADS, widen, 0)

    def all_columns():
        return pltpu.make_async_remote_copy(
            src_ref=rz.at[pl.ds(0, NZ - 1)],
            dst_ref=rz.at[pl.ds(0, NZ - 1)],
            send_sem=one.at[2],
            recv_sem=one.at[3],
            device_id=(((z + 1) % NZ) * NX + x, tp),
            device_id_type=MESH,
        )

    all_columns().wait_recv()

    carried = []
    for way in (0, 1):
        total = jnp.zeros((64, 128), F32)
        for i in range(NZ) if way == 0 else reversed(range(NZ)):
            block = rz[i]
            passed = (i < z) if way == 0 else (i > z)
            total = jnp.where(passed, jnp.exp(log_of(block)) * total + state(block), total)
        for i in range(NX) if way == 0 else reversed(range(NX)):
            block = rx[i, way]
            passed = (i < x) if way == 0 else (i > x)
            total = jnp.where(passed, jnp.exp(log_of(block)) * total + state(block), total)
        carried.append(total.astype(BF16))

    mixer = inner + cv[2:3, :] * across(carried[0], mixed[1]) + cv[3:4, :] * across(carried[1], mixed[1])
    gated = (mixer * gate).astype(BF16)
    none = jnp.zeros((64, T), BF16)
    upper_half = one_hot((HALF, T), lambda row, col: row == col)
    lower_half = one_hot((HALF, T), lambda row, col: row + HALF == col)
    mine = pl.ds(pl.multiple_of(tp * 128, 128), 128)
    bn[:, mine] = (
        across(upper_half, jnp.concatenate([gated, none], axis=0))
        + across(lower_half, jnp.concatenate([none, gated], axis=0))
    ).astype(BF16)

    sems = (rsem, rrecv)
    ring = Ring(bn, 0, HALF, sems, 6 + SPLITS, direct=True)
    ring.start()

    def all_tiles(ref, at):
        return pltpu.make_async_remote_copy(
            src_ref=ref.at[pl.ds(0, TP - 1)],
            dst_ref=ref.at[pl.ds(0, TP - 1)],
            send_sem=one.at[at],
            recv_sem=one.at[at + 1],
            device_id=(sp, (tp + 1) % TP),
            device_id_type=MESH,
        )

    all_tiles(ft, 4).wait_recv()
    run([ring])
    ring.finish()

    left = lax.broadcasted_iota(jnp.int32, (HALF, 128), 1) < 64
    for g in range(GROUPS):
        squares = jnp.zeros((HALF, 128), F32)
        for j in range(4 * g, 4 * g + 4):
            v = bn[:, 128 * j : 128 * j + 128].astype(F32)
            squares = squares + v * v
        top = jnp.sum(jnp.where(left, squares, 0.0), axis=1, keepdims=True)
        bottom = jnp.sum(jnp.where(left, 0.0, squares), axis=1, keepdims=True)
        scale = lax.rsqrt(jnp.where(left, top, bottom) / (4 * HEAD_DIM) + 1e-06)
        for j in range(4 * g, 4 * g + 4):
            v = bn[:, 128 * j : 128 * j + 128].astype(F32)
            nn[:, 128 * j : 128 * j + 128] = (v * scale * ft[j, 0:1]).astype(BF16)
    projected = dot(nn[...], wide[...])
    am[0:HALF] = (src_ref[0:HALF].astype(F32) + projected[:, 0:128]).astype(BF16)
    am[HALF:T] = (src_ref[HALF:T].astype(F32) + projected[:, 128:256]).astype(BF16)

    own = (am[...].astype(F32) * after_ref[...]).astype(BF16)
    ff[:, mine] = own
    dd[...] = dot(pp[...], own).astype(BF16)

    def rows_of(i):
        return pl.ds(pl.multiple_of(i * SLOTS, SLOTS), SLOTS)

    per = SP // 2 // CHUNKS
    local = (x % 2) * 8 + (x // 2) * 4 + z // 2

    def deliver(k, far=0):
        target = (sp + k) % SP
        return pltpu.make_async_remote_copy(
            src_ref=(d2 if far else dd).at[rows_of(target)],
            dst_ref=(x2 if far else xl).at[rows_of(local), lanes_of(core)],
            send_sem=one.at[9 if far else 8],
            recv_sem=dr.at[local // per + CHUNKS * far],
            device_id=(target, y * 2 + side_of),
            device_id_type=MESH,
        )

    def outward(m):
        return SP // 2 + (m // 2 + m % 2) * (1 - 2 * (m % 2))

    def send_rows(m, carry):
        deliver(outward(m)).start()
        return carry

    lax.fori_loop(0, SP - 1, send_rows, 0)

    @pl.when(side_of == core)
    def _():
        xl[rows_of(local), lanes_of(core)] = dd[rows_of(sp)]

    @pl.when(side_of != core)
    def _():
        deliver(0).start()

    cells = T // SPLITS
    spread_out = [Ring(ff, i * cells, cells, sems, 4 + i) for i in range(SPLITS)]
    for spreading in spread_out:
        spreading.start()

    dims = (((1,), (1,)), ((), ()))
    squares = am[...].astype(F32) * am[...].astype(F32)
    high = squares.astype(BF16)
    rest = (squares - high.astype(F32)).astype(BF16)
    ones = jnp.ones((8, 128), BF16)
    sums = lax.dot_general(ones, high, dims, preferred_element_type=F32) + lax.dot_general(
        ones, rest, dims, preferred_element_type=F32
    )
    line = jnp.concatenate([sums, jnp.zeros((8, 3 * 128 - T), F32)], axis=1)
    level = lax.broadcasted_iota(jnp.int32, (8, 128), 0)
    own = jnp.where(
        level == 0,
        line[:, 0:128],
        jnp.where(level == 1, line[:, 128:256], jnp.where(level == 2, line[:, 256:384], 0.0)),
    )
    sq[tp] = own
    so[...] = own

    def sums_to(k, source):
        return pltpu.make_async_remote_copy(
            src_ref=so,
            dst_ref=sq.at[source],
            send_sem=one.at[6],
            recv_sem=one.at[7],
            device_id=(sp, (tp + k) % TP),
            device_id_type=MESH,
        )

    def send_sums(k, carry):
        sums_to((k + 7) % (TP - 1) + 1, tp).start()
        return carry

    lax.fori_loop(0, TP - 1, send_sums, 0)
    ring.drain()

    def some_rows(ref, first, blocks, sent, received):
        part = ref.at[pl.ds(first, blocks * SLOTS), pl.ds(0, 128)]
        return pltpu.make_async_remote_copy(
            src_ref=part,
            dst_ref=part,
            send_sem=one.at[sent],
            recv_sem=received,
            device_id=((sp + 1) % SP, tp),
            device_id_type=MESH,
        )

    def either(test, less, more):
        @pl.when(test)
        def _():
            less()

        @pl.when(jnp.logical_not(test))
        def _():
            more()

    for step in (1, 2):
        for ring in spread_out:
            ring.step(step)
    chip = pl.ds(pl.multiple_of(y * 256, 256), 256)
    packed_rows = per * CAP
    dense = one_hot((packed_rows, per * SLOTS), lambda row, col: row // CAP * SLOTS + row % CAP == col)
    gathers = []
    for q in range(CHUNKS):
        either(
            jnp.logical_and(side_of == core, x % 2 == q),
            lambda: some_rows(xl, 0, 2 * per - 1, 8, dr.at[q]).wait_recv(),
            lambda: some_rows(xl, 0, 2 * per, 8, dr.at[q]).wait_recv(),
        )
        at = pl.ds(q * packed_rows, packed_rows)
        xx[at, chip] = dot(dense, xl[pl.ds(q * per * SLOTS, per * SLOTS), :]).astype(BF16)
        gathers.append(Ring(xx, q * packed_rows, packed_rows, sems, q, pair=True, last=3))
        gathers[-1].start()
    all_tiles(sq, 6).wait_recv()
    total = sq[0]
    for j in range(1, TP):
        total = total + sq[j]
    line = jnp.concatenate([total[0:1], total[1:2], total[2:3]], axis=1)
    parts = stacked(three(line)).astype(BF16)
    same = one_hot((T, 384), lambda row, col: row == col)
    upright = across(same, parts)
    scale = lax.rsqrt((upright[:, 0:1] + upright[:, 1:2] + upright[:, 2:3]) / D + 1e-06)
    lane = lax.broadcasted_iota(jnp.int32, (T, 128), 1)
    parts = jnp.zeros((T, 128), F32)
    for k, part in enumerate(three(scale)):
        parts = jnp.where(lane == k, part, parts)
    ss[...] = dot(pp[...], parts.astype(BF16)).astype(BF16)

    def send_scale(m, carry):
        target = (sp + outward(m)) % SP
        pltpu.make_async_remote_copy(
            src_ref=ss.at[rows_of(target)],
            dst_ref=sl.at[rows_of(local)],
            send_sem=one.at[14],
            recv_sem=one.at[15],
            device_id=(target, tp),
            device_id_type=MESH,
        ).start()
        return carry

    @pl.when(side_of == core)
    def _():
        lax.fori_loop(0, SP - 1, send_scale, 0)
        sl[rows_of(local), :] = ss[rows_of(sp), :]

    for ring in spread_out:
        ring.step(3)
    for ring in gathers:
        ring.step(1)
    for ring in spread_out:
        ring.step(4)

    opposite = (y + NY // 2) % NY
    d2[...] = dot(pp[...], ff[:, lanes_of(opposite * 2 + core)]).astype(BF16)

    def send_more(m, carry):
        deliver(outward(m), 1).start()
        return carry

    lax.fori_loop(0, SP - 1, send_more, 0)

    @pl.when(side_of == core)
    def _():
        x2[rows_of(local), lanes_of(core)] = d2[rows_of(sp)]

    @pl.when(side_of != core)
    def _():
        deliver(0, 1).start()

    for ring in spread_out:
        ring.finish()
    loads[4].wait()
    loads[5].wait()
    both = dot(ff[...], wc[...]) * scale
    sh[:, mine] = (jax.nn.silu(both[:, 0:128]) * both[:, 128:256]).astype(BF16)
    shared_out = [Ring(sh, i * HALF, HALF, sems, 4 + SPLITS + i) for i in range(2)]
    for ring in shared_out:
        ring.start()
    for ring in gathers:
        ring.step(2)

    def chips(first, count, total, buf, at, weight):
        def add(k, carry):
            part = pl.ds(pl.multiple_of((y + k) % NY * 256, 256), 256)
            total[at, :] += dot(buf[at, part], weight[part, :])
            return carry

        lax.fori_loop(first, first + count, add, 0)

    weights = wx.at[:, pl.ds(0, 384)]
    to_other(weights).wait_recv()
    either(
        side_of == core,
        lambda: some_rows(sl, 0, SP // 2 - 1, 14, one.at[15]).wait_recv(),
        lambda: some_rows(sl, 0, SP // 2, 14, one.at[15]).wait_recv(),
    )
    tot[...] = jnp.zeros(tot.shape, F32)
    levels = []
    for q in range(CHUNKS):
        at = pl.ds(q * packed_rows, packed_rows)
        chips(NY - 2, NY - 3, tot, xx, at, wx)
        either(
            jnp.logical_and(side_of == core, x % 2 == q),
            lambda: some_rows(x2, 0, 2 * per - 1, 9, dr.at[CHUNKS + q]).wait_recv(),
            lambda: some_rows(x2, 0, 2 * per, 9, dr.at[CHUNKS + q]).wait_recv(),
        )
        turned = pl.ds(pl.multiple_of(opposite * 256, 256), 256)
        xx[at, turned] = dot(dense, x2[pl.ds(q * per * SLOTS, per * SLOTS), :]).astype(BF16)
        chips(NY // 2, 1, tot, xx, at, wx)
        level = dot(dense, sl[pl.ds(q * per * SLOTS, per * SLOTS), :])
        levels.append(level[:, 0:1] + level[:, 1:2] + level[:, 2:3])
    hiddens = []
    for q in range(CHUNKS):
        gathers[q].step(3)
        if q == CHUNKS - 1:
            for ring in shared_out:
                ring.step(1)
        at = pl.ds(q * packed_rows, packed_rows)
        chips(3, 1, tot, xx, at, wx)
        chips(NY - 3, 1, tot, xx, at, wx)
        both = tot[at, :] * levels[q]
        hh[at, chip] = (jax.nn.silu(both[:, 0:256]) * both[:, 256:512]).astype(BF16)
        hiddens.append(Ring(hh, q * packed_rows, packed_rows, sems, 2 + q, pair=True))
        hiddens[-1].start()
    for side in range(2):
        for k in range(3):
            halo(side, k).wait_send()
    all_rows(NX - 1).wait_send()
    all_columns().wait_send()
    all_tiles(ft, 4).wait_send()
    all_tiles(sq, 6).wait_send()
    for sent in (8, 9):
        either(
            side_of == core,
            lambda: some_rows(dd, 0, SP - 1, sent, one.at[16]).wait_send(),
            lambda: some_rows(dd, 0, SP, sent, one.at[16]).wait_send(),
        )

    @pl.when(side_of == core)
    def _():
        some_rows(dd, 0, SP - 1, 14, one.at[16]).wait_send()

    to_other(weights).wait_send()
    for ring in spread_out + gathers:
        ring.drain()
    low[...] = jnp.zeros(low.shape, F32)
    for step in (1, 2, 3):
        for ring in hiddens:
            ring.step(step)
        if step == 3:
            for ring in shared_out:
                ring.step(2)
        for q in range(CHUNKS):
            at = pl.ds(q * packed_rows, packed_rows)
            if step == 1:
                chips(NY, 1, low, hh, at, wl)
            chips(step, 1, low, hh, at, wl)
            chips(NY - step, 1, low, hh, at, wl)
    loose = one_hot((per * SLOTS, packed_rows), lambda row, col: col // CAP * SLOTS + col % CAP == row)

    def give(i, to_core):
        return pltpu.make_async_remote_copy(
            src_ref=oo.at[rows_of(i), lanes_of(to_core)],
            dst_ref=ret.at[rows_of(sp)],
            send_sem=one.at[10],
            recv_sem=one.at[11],
            device_id=(((i % 4) * 2 + core) * NX + i // 4 % 2 * 2 + i // 8, y * 2 + to_core),
            device_id_type=MESH,
        )

    for q in range(CHUNKS):
        hiddens[q].step(4)
        at = pl.ds(q * packed_rows, packed_rows)
        chips(NY // 2, 1, low, hh, at, wl)
        oo[pl.ds(q * per * SLOTS, per * SLOTS), :] = dot(loose, low[at, :].astype(BF16)).astype(BF16)

        def send_back(k, carry):
            turn = k // 2
            i = q * per + k % 2 * 4 + (z // 2 + 6 + (turn // 2 + turn % 2) * (1 - 2 * (turn % 2))) % 4
            here = jnp.logical_and(side_of == core, i == local)

            @pl.when(jnp.logical_not(here))
            def _():
                give(i, core).start()

            give(i, 1 - core).start()
            return carry

        lax.fori_loop(0, per, send_back, 0)

    @pl.when(side_of == core)
    def _():
        ret[rows_of(sp), :] = oo[rows_of(local), lanes_of(core)]

    for step in (3, 4):
        for ring in shared_out:
            ring.step(step)
    for ring in shared_out:
        ring.finish()
    loads[6].wait()
    shared = dot(sh[...], wcl[...]).astype(BF16).astype(F32)
    out_ref[...] = shared.astype(BF16)
    for ring in hiddens + shared_out:
        ring.drain()
    either(
        side_of == core,
        lambda: some_rows(ret, 0, SP - 1, 10, one.at[11]).wait_recv(),
        lambda: some_rows(ret, 0, SP, 10, one.at[11]).wait_recv(),
    )
    either(
        side_of == core,
        lambda: some_rows(ret, 0, SP - 1, 10, one.at[11]).wait_send(),
        lambda: some_rows(ret, 0, SP, 10, one.at[11]).wait_send(),
    )
    routed = dot(qhi[...], ret[...]) + dot(qlo[...], ret[...])
    out_ref[...] = (am[...].astype(F32) + out_ref[...].astype(F32) + routed).astype(BF16)


def whole(*operands):
    vmem = pl.BlockSpec(memory_space=pltpu.VMEM)
    hbm = pl.BlockSpec(memory_space=pl.ANY)
    rings = 7 + SPLITS
    dma = pltpu.SemaphoreType.DMA

    def space(*shape, kind=BF16):
        return pltpu.VMEM(shape, kind)

    return pl.pallas_call(
        kernel,
        out_shape=jax.ShapeDtypeStruct((T, 128), BF16),
        in_specs=[vmem] * 15 + [hbm] * 9,
        out_specs=vmem,
        scratch_shapes=[
            space(64, 384),
            space(T, 128),
            space(T, 128),
            space(2, 64, 128),
            space(2, 16, 128),
            space(2, 16, 128),
            space(T + 32, 128, kind=F32),
            space(T + 32, 128, kind=F32),
            space(T, T, kind=F32),
            space(8, T, kind=F32),
            space(2, T, 128),
            space(8, 128, kind=F32),
            space(2, BLOCK, 128),
            space(NX, 2, BLOCK, 128),
            space(2, BLOCK, 128),
            space(NZ, BLOCK, 128),
            space(TP, 8, 128, kind=F32),
            space(TP, 8, 128, kind=F32),
            space(8, 128, kind=F32),
            space(1024, 128),
            space(D, 512),
            space(D, 256),
            space(D, 256),
            space(D, 128),
            space(D, 256),
            space(HALF, D),
            space(HALF, D),
            space(T, 128),
            space(T, D),
            space(T, D),
            space(ROWS // 2, 256),
            space(ROWS // 2, 256),
            space(SP // 2 * CAP, D),
            space(SP // 2 * CAP, D),
            space(SP // 2 * CAP, 512, kind=F32),
            space(SP // 2 * CAP, 256, kind=F32),
            space(ROWS, 128),
            space(ROWS, 128),
            space(ROWS, 128),
            space(ROWS // 2, 128),
            space(ROWS // 2, 256),
            space(ROWS, 128),
            space(ROWS, T),
            space(T, ROWS),
            space(T, ROWS),
            dma((9,)), dma((6,)), dma((6,)), dma((17,)), dma((2 * CHUNKS,)), dma((rings, 2)), dma((rings, 8)),
        ],
        compiler_params=pltpu.CompilerParams(collective_id=0, has_side_effects=True),
        name="mixer_experts",
    )(*operands)


def shards(
    layer_source_vector,
    attention_lane_source,
    result_valve_logits,
    memory_write_matrix,
    memory_query_matrix,
    increment_logits,
    increment_offset,
    log_fade_speed,
    extra_log_fade,
    attention_bypass_factor,
    attention_lane_kernel,
    memory_write_kernel,
    memory_query_kernel,
    cluster_rescale_factor,
    blender_result_matrix,
    specialist_rescale_factor,
    chosen_specialists,
    specialist_shares,
    specialist_valve_matrix,
    specialist_raising_matrix,
    specialist_lowering_matrix,
    common_valve_matrix,
    common_raising_matrix,
    common_lowering_matrix,
):
    return whole(
        attention_lane_source.T,
        result_valve_logits.T,
        increment_logits.reshape(2, T),
        increment_offset.T,
        log_fade_speed.T,
        extra_log_fade.reshape(2, 1, T),
        attention_bypass_factor.reshape(1, 1),
        attention_lane_kernel,
        memory_write_kernel,
        memory_query_kernel,
        cluster_rescale_factor.reshape(1, 64),
        specialist_rescale_factor.reshape(1, 128),
        layer_source_vector,
        chosen_specialists.T,
        specialist_shares.T,
        memory_write_matrix,
        memory_query_matrix,
        blender_result_matrix,
        specialist_valve_matrix,
        specialist_raising_matrix,
        specialist_lowering_matrix,
        common_valve_matrix,
        common_raising_matrix,
        common_lowering_matrix,
    )


def solution(mesh):
    return jax.shard_map(
        shards,
        mesh=mesh,
        in_specs=(
            P("sp", "tp"),
            P("sp", "tp"),
            P("sp", "tp"),
            P("sp", None),
            P("sp", None),
            P(None, "sp", "tp"),
            P(None, "tp"),
            P(None, "tp"),
            P(None, "sp", "tp"),
            P("tp"),
            P(None, "tp"),
            P(),
            P(),
            P("tp"),
            P(None, "tp"),
            P("tp"),
            P("sp", None),
            P("sp", None),
            P("sp", None, "tp"),
            P("sp", None, "tp"),
            P("sp", None, "tp"),
            P(None, "tp"),
            P(None, "tp"),
            P(None, "tp"),
        ),
        out_specs=P("sp", "tp"),
        check_vma=False,
    )
```

```python
import jax
import jax.numpy as jnp
from jax import lax
from jax.experimental import pallas as pl
from jax.experimental.pallas import tpu as pltpu
from jax.sharding import PartitionSpec as P

D = 2048
HEADS = 16
HEAD_DIM = 64
GROUPS = 4
STATE = 128
CONV = 5

NZ, NX, NY = 8, 4, 8
SP, TP = NZ * NX, NY * 2
T = 320
HALF = T // 2
SLOTS = 32
ROWS = SP * SLOTS
CAP = 30
SPLITS = 4
BLOCK = 80
CHUNKS = 2
MESH = pl.DeviceIdType.MESH
F32, BF16 = jnp.float32, jnp.bfloat16


def dot(a, b):
    return jnp.dot(a, b, preferred_element_type=F32)


class Ring:
    def __init__(self, buf, first, rows, sems, index, direct=False, pair=False, last=4):
        self.buf, self.first, self.rows = buf, first, rows
        self.direct, self.pair, self.last = direct, pair, last
        self.out, self.near = sems[0].at[index, 0], sems[0].at[index, 1]
        self.recv = sems[1].at[index]
        self.sp, tp = lax.axis_index("sp"), lax.axis_index("tp")
        self.y, self.core = tp // 2, tp % 2

    def part(self, chip, core, half=None):
        column, width = ((chip + 2 * NY) % NY) * 2, 128
        if self.pair:
            width = 256
        else:
            column = column + core
        first, rows = self.first, self.rows
        if half is not None:
            cut = (rows // 2 + 15) // 16 * 16
            first, rows = (first, cut) if half == 0 else (first + cut, rows - cut)
        return self.buf.at[pl.ds(first, rows), pl.ds(pl.multiple_of(column * 128, 128), width)]

    def along(self, way, step, chip, far):
        turn = 1 - 2 * way
        block = self.part(chip, self.core, way if step == 4 else None)
        return pltpu.make_async_remote_copy(
            src_ref=block,
            dst_ref=block,
            send_sem=self.out,
            recv_sem=self.recv.at[4 * way + step - 1],
            device_id=(self.sp, ((self.y + turn * far + NY) % NY) * 2 + self.core),
            device_id_type=MESH,
        )

    def hop(self, way, step):
        if self.direct:
            return self.along(way, step, self.y, step)
        return self.along(way, step, self.y - (1 - 2 * way) * (step - 1), 1)

    def landed(self, way, step):
        return self.along(way, step, self.y - (1 - 2 * way) * step, 1)

    def relay(self, way, step):
        turn = 1 - 2 * way
        return self.over(self.part(self.y - turn * step, self.core, way if step == 4 else None))

    def over(self, block):
        return pltpu.make_async_remote_copy(
            src_ref=block,
            dst_ref=block,
            send_sem=self.out,
            recv_sem=self.near,
            device_id=(self.sp, self.y * 2 + 1 - self.core),
            device_id_type=MESH,
        )

    def several(self, blocks):
        return self.over(self.buf.at[pl.ds(self.first, self.rows), pl.ds(0, 128 * blocks)])

    def start(self):
        for step in (4, 3, 2, 1) if self.direct else (1,):
            self.hop(0, step).start()
            self.hop(1, step).start()
        if not self.pair:
            self.relay(0, 0).start()

    def step(self, step):
        for way in (0, 1):
            self.landed(way, step).wait_recv()
            if step < self.last and not self.direct:
                self.hop(way, step + 1).start()
            if not self.pair:
                self.relay(way, step).start()

    def finish(self):
        self.several(NY).wait_recv()

    def drain(self):
        self.several(2 * NY - (1 if not self.pair else 2 if self.last == 4 else 4)).wait_send()


def stacked(rows):
    level = lax.broadcasted_iota(jnp.int32, (8, rows[0].shape[1]), 0)
    total = jnp.zeros(level.shape, F32)
    for k, row in enumerate(rows):
        total = jnp.where(level == k, row, total)
    return total


def three(v):
    high = v.astype(BF16).astype(F32)
    middle = (v - high).astype(BF16).astype(F32)
    return [high, middle, v - high - middle]


def one_hot(shape, test):
    row, col = lax.broadcasted_iota(jnp.int32, shape, 0), lax.broadcasted_iota(jnp.int32, shape, 1)
    return jnp.where(test(row, col), 1.0, 0.0).astype(BF16)


def across(a, b):
    return lax.dot_general(a, b, (((1,), (1,)), ((), ())), preferred_element_type=F32)


def log1p(u):
    series = u * (1 - u * (1 / 2 - u * (1 / 3 - u * (1 / 4 - u * (1 / 5 - u / 6)))))
    return jnp.where(u < 0.03, series, jnp.log(1 + u))


def silu(v):
    return v / (1 + jnp.exp(-v))


def kernel(
    xt_ref, zt_ref, inc_ref, off_ref, spd_ref, fade_ref, byp_ref, xk_ref, bk_ref, ck_ref, gain_ref,
    after_ref, src_ref, cht_ref, sht_ref,
    bm_hbm, cm_hbm, blender_hbm, valve_hbm, raising_hbm, lowering_hbm, cvalve_hbm, craising_hbm, clowering_hbm,
    out_ref,
    xpad, braw, craw, hx, hb, hc, bext, cext, gap, cv, mixed, fto,
    st_ref, rx, tb, rz, ft, sq, so, wb, wx, wc, wl, wcl, wide, bn, nn, am, ff, sh, xl, x2, xx, hh, tot, low, dd, d2, ss, sl, outs, theirs, oo, ret, pp, qhi, qlo,
    wsem, hs, hr, one, dr, rsem, rrecv,
):
    sp, tp = lax.axis_index("sp"), lax.axis_index("tp")
    z, x = sp // NX, sp % NX
    y, core, side_of = tp // 2, tp % 2, z % 2

    barrier = pltpu.get_barrier_semaphore()

    def greet_tp(k, carry):
        pl.semaphore_signal(barrier, inc=1, device_id=(sp, (tp + k) % TP), device_id_type=MESH)
        return carry

    def greet_sp(k, carry):
        pl.semaphore_signal(barrier, inc=1, device_id=((sp + k) % SP, tp), device_id_type=MESH)
        return carry

    lax.fori_loop(1, TP, greet_tp, 0)
    lax.fori_loop(1, SP, greet_sp, 0)

    def lanes_of(i):
        return pl.ds(pl.multiple_of(i * 128, 128), 128)

    at_group = pl.ds(pl.multiple_of((tp // 4) * 128, 128), 128)
    loads = [
        pltpu.make_async_copy(blender_hbm, wb, wsem.at[0]),
        pltpu.make_async_copy(valve_hbm.at[0], wx.at[:, lanes_of(core)], wsem.at[1]),
        pltpu.make_async_copy(raising_hbm.at[0], wx.at[:, lanes_of(core + 2)], wsem.at[2]),
        pltpu.make_async_copy(lowering_hbm.at[0], wl.at[:, lanes_of(core)], wsem.at[3]),
        pltpu.make_async_copy(cvalve_hbm, wc.at[:, lanes_of(core)], wsem.at[4]),
        pltpu.make_async_copy(craising_hbm, wc.at[:, lanes_of(core + 2)], wsem.at[5]),
        pltpu.make_async_copy(clowering_hbm, wcl.at[:, lanes_of(core)], wsem.at[6]),
    ]
    grouped = [
        pltpu.make_async_copy(bm_hbm.at[:, at_group], braw, wsem.at[7]),
        pltpu.make_async_copy(cm_hbm.at[:, at_group], craw, wsem.at[8]),
    ]
    for load in grouped + loads:
        load.start()

    xpad[...] = jnp.zeros(xpad.shape, BF16)
    xpad[:, 0:T] = xt_ref[...]
    gains = jnp.concatenate([gain_ref[...], gain_ref[...]], axis=1)
    fto[...] = jnp.broadcast_to(gains, (8, 128))
    ft[tp] = fto[...]

    def state_row(k, source):
        return pltpu.make_async_remote_copy(
            src_ref=st_ref,
            dst_ref=rx.at[source],
            send_sem=one.at[0],
            recv_sem=one.at[1],
            device_id=(z * NX + (x + k) % NX, tp),
            device_id_type=MESH,
        )

    def tile(k, source):
        return pltpu.make_async_remote_copy(
            src_ref=fto,
            dst_ref=ft.at[source],
            send_sem=one.at[4],
            recv_sem=one.at[5],
            device_id=(sp, (tp + k) % TP),
            device_id_type=MESH,
        )

    def send_tile(k, carry):
        tile(k, tp).start()
        return carry

    for load in grouped:
        load.wait()
    pl.semaphore_wait(barrier, TP + SP - 2)

    def halo(side, k):
        there = (sp + 1) % SP if side == 0 else (sp + SP - 1) % SP
        rows = pl.ds(T - 16, 16) if side == 0 else pl.ds(0, 16)
        lanes = pl.ds(256, 128) if side == 0 else pl.ds(0, 128)
        source = (xpad.at[:, lanes], braw.at[rows], craw.at[rows])[k]
        return pltpu.make_async_remote_copy(
            src_ref=source,
            dst_ref=(hx, hb, hc)[k].at[side],
            send_sem=hs.at[3 * side + k],
            recv_sem=hr.at[3 * side + k],
            device_id=(there, tp),
            device_id_type=MESH,
        )

    for k in range(3):
        halo(0, k).start()
        halo(1, k).start()
    lax.fori_loop(1, TP, send_tile, 0)

    lower = one_hot((T, T), lambda row, col: col < row)
    upper = one_hot((T, T), lambda row, col: row < col)
    same = one_hot((T, T), lambda row, col: row == col)
    experts = lax.broadcasted_iota(jnp.int32, (SP, T), 0)
    first, second = cht_ref[0:1, :] == experts, cht_ref[1:2, :] == experts
    named = jnp.where(first | second, 1.0, 0.0)
    rank = dot(named.astype(BF16), upper)
    rank = jnp.where(named > 0, rank, 99.0).astype(BF16)
    spread = one_hot((ROWS, SP), lambda row, col: row // SLOTS == col)
    place = (lax.broadcasted_iota(jnp.int32, (ROWS, T), 0) % SLOTS).astype(F32)
    pp[...] = jnp.where(dot(spread, rank) == place, 1.0, 0.0).astype(BF16)
    shares = jnp.where(first, sht_ref[0:1, :], 0.0) + jnp.where(second, sht_ref[1:2, :], 0.0)
    share_hi = shares.astype(BF16)
    share_lo = (shares - share_hi.astype(F32)).astype(BF16)
    spread = one_hot((SP, ROWS), lambda row, col: col // SLOTS == row)
    place = (lax.broadcasted_iota(jnp.int32, (T, ROWS), 1) % SLOTS).astype(F32)
    here = dot(across(same, rank).astype(BF16), spread) == place
    qhi[...] = jnp.where(here, dot(across(same, share_hi).astype(BF16), spread), 0.0).astype(BF16)
    qlo[...] = jnp.where(here, dot(across(same, share_lo).astype(BF16), spread), 0.0).astype(BF16)

    steps, fades = [], []
    for d in range(2):
        v = inc_ref[d : d + 1, :].astype(F32) + off_ref[0:1, d : d + 1]
        step = jnp.maximum(v, 0.0) + log1p(jnp.exp(-jnp.abs(v)))
        steps.append(step)
        fades.append(-jnp.exp(spd_ref[0:1, d : d + 1]) * step + fade_ref[d])
    parts = stacked(three(fades[0]) + three(fades[1])).astype(BF16)
    along = dot(parts, upper + same)
    forward_row = along[0:1] + along[1:2] + along[2:3]
    along = dot(parts, upper)
    backward_row = along[3:4] + along[4:5] + along[5:6]
    along = across(lower + same, parts)
    forward_col = along[:, 0:1] + along[:, 1:2] + along[:, 2:3]
    along = across(lower, parts)
    backward_col = along[:, 3:4] + along[:, 4:5] + along[:, 5:6]
    row = lax.broadcasted_iota(jnp.int32, (T, T), 0)
    col = lax.broadcasted_iota(jnp.int32, (T, T), 1)
    gap[...] = (
        jnp.where(row >= col, jnp.exp(forward_col - forward_row), 0.0) * steps[0]
        + jnp.where(row <= col, jnp.exp(backward_row - backward_col), 0.0) * steps[1]
    )
    forward_end = forward_row[:, T - 1 : T]
    backward_end = backward_row[:, T - 1 : T] + fades[1][:, T - 1 : T]
    weigh = [jnp.exp(forward_end - forward_row) * steps[0], jnp.exp(backward_row) * steps[1]]
    seen = [jnp.exp(forward_row), jnp.exp(backward_end - backward_row)]
    cv[...] = stacked(weigh + seen)
    ends = [jnp.broadcast_to(forward_end, (1, 128)), jnp.broadcast_to(backward_end, (1, 128))]

    def to_other(part, at):
        return pltpu.make_async_remote_copy(
            src_ref=part,
            dst_ref=part,
            send_sem=one.at[at],
            recv_sem=one.at[at + 1],
            device_id=(sp, y * 2 + 1 - core),
            device_id_type=MESH,
        )

    for k in (1, 2, 3):
        loads[k].wait()
    for part in (wx.at[:, lanes_of(core)], wx.at[:, lanes_of(core + 2)], wl.at[:, lanes_of(core)]):
        to_other(part, 12).start()

    taps = across(same[0:64, 0:64], stacked([xk_ref[j : j + 1, :].astype(F32) for j in range(CONV)]).astype(BF16))
    lane = lax.broadcasted_iota(jnp.int32, (64, 128), 1)
    body = xpad[...].astype(F32)
    bext[pl.ds(16, T), :] = braw[...].astype(F32)
    cext[pl.ds(16, T), :] = craw[...].astype(F32)
    for k in range(3):
        halo(0, k).wait_recv()
        halo(1, k).wait_recv()
    before, behind = sp > 0, sp < SP - 1
    last = jnp.where(before, pltpu.roll(hx[0].astype(F32), 64, 1), 0.0)
    coming = jnp.where(behind, pltpu.roll(hx[1].astype(F32), 64, 1), 0.0)
    end = jnp.where(
        lane < 64, body[:, 256:384], jnp.where(lane < 66, coming, jnp.where(lane > 125, last, 0.0))
    )
    cells = jnp.concatenate([body[:, 0:256], end], axis=1)
    total = cells * taps[:, 2:3]
    for j in (0, 1, 3, 4):
        total = total + pltpu.roll(cells, (2 - j) % 384, 1) * taps[:, j : j + 1]
    x_conv = silu(total)[:, 0:T].astype(BF16)
    for ext, halos, kernel_ref in ((bext, hb, bk_ref), (cext, hc, ck_ref)):
        ext[pl.ds(0, 16), :] = jnp.where(before, halos[0].astype(F32), 0.0)
        ext[pl.ds(T + 16, 16), :] = jnp.where(behind, halos[1].astype(F32), 0.0)
        total = jnp.zeros((T, 128), F32)
        for j in range(CONV):
            tap = kernel_ref[j : j + 1, at_group].astype(F32)
            total = total + ext[pl.ds(14 + j, T), :] * tap
        mixed[0 if ext is bext else 1] = silu(total).astype(BF16)
    b_conv, c_conv = mixed[0], mixed[1]

    def packed(total, log):
        tail = jnp.concatenate([stacked(three(log)), jnp.zeros((8, 128), F32)], axis=0)
        return total.astype(BF16), tail.astype(BF16)

    x_wide = x_conv.astype(F32)
    for d in range(2):
        scaled = (cv[d : d + 1, :] * x_wide).astype(BF16)
        top, tail = packed(dot(scaled, b_conv), ends[d])
        st_ref[d, 0:64] = top
        st_ref[d, 64:80] = tail
    rx[x] = st_ref[...]
    for k in (2, 1, 3):
        state_row(k, x).start()
    inner = across(x_conv, (across(c_conv, b_conv) * gap[...]).astype(BF16))
    inner = inner + byp_ref[...] * x_wide
    gate = silu(zt_ref[...].astype(F32))

    def all_rows(k):
        return pltpu.make_async_remote_copy(
            src_ref=rx.at[pl.ds(0, k)],
            dst_ref=rx.at[pl.ds(0, k)],
            send_sem=one.at[0],
            recv_sem=one.at[1],
            device_id=(z * NX + (x + 1) % NX, tp),
            device_id_type=MESH,
        )

    all_rows(NX - 1).wait_recv()

    def state(block):
        return block[0:64].astype(F32)

    def log_of(block):
        logs = block[64:80].astype(F32)
        return logs[0:1] + logs[1:2] + logs[2:3]

    for way in (0, 1):
        total, log = jnp.zeros((64, 128), F32), jnp.zeros((1, 128), F32)
        for i in range(NX) if way == 0 else reversed(range(NX)):
            block = rx[i, way]
            own = log_of(block)
            total = jnp.exp(own) * total + state(block)
            log = log + own
        top, tail = packed(total, log)
        tb[way, 0:64] = top
        tb[way, 64:80] = tail
    rz[z] = tb[0]

    def state_column(k, source):
        return pltpu.make_async_remote_copy(
            src_ref=tb.at[(z + k) // NZ],
            dst_ref=rz.at[source],
            send_sem=one.at[2],
            recv_sem=one.at[3],
            device_id=(((z + k) % NZ) * NX + x, tp),
            device_id_type=MESH,
        )

    for k in (4, 3, 5, 2, 6, 1, 7):
        state_column(k, z).start()

    for k in (4, 5, 6):
        loads[k].wait()
    for part in (wc.at[:, lanes_of(core)], wc.at[:, lanes_of(core + 2)], wcl.at[:, lanes_of(core)]):
        to_other(part, 18).start()

    loads[0].wait()
    wide[...] = jnp.zeros(wide.shape, BF16)

    def widen(j, carry):
        block = wb[pl.ds(pl.multiple_of(j * 64, 64), 64), :]
        wide[pl.ds(pl.multiple_of(j * 128, 128), 64), pl.ds(0, 128)] = block
        wide[pl.ds(pl.multiple_of(j * 128 + 64, 64), 64), pl.ds(128, 128)] = block
        return carry

    lax.fori_loop(0, HEADS, widen, 0)

    def all_columns():
        return pltpu.make_async_remote_copy(
            src_ref=rz.at[pl.ds(0, NZ - 1)],
            dst_ref=rz.at[pl.ds(0, NZ - 1)],
            send_sem=one.at[2],
            recv_sem=one.at[3],
            device_id=(((z + 1) % NZ) * NX + x, tp),
            device_id_type=MESH,
        )

    all_columns().wait_recv()

    carried = []
    for way in (0, 1):
        total = jnp.zeros((64, 128), F32)
        for i in range(NZ) if way == 0 else reversed(range(NZ)):
            block = rz[i]
            passed = (i < z) if way == 0 else (i > z)
            total = jnp.where(passed, jnp.exp(log_of(block)) * total + state(block), total)
        for i in range(NX) if way == 0 else reversed(range(NX)):
            block = rx[i, way]
            passed = (i < x) if way == 0 else (i > x)
            total = jnp.where(passed, jnp.exp(log_of(block)) * total + state(block), total)
        carried.append(total.astype(BF16))

    mixer = inner + cv[2:3, :] * across(carried[0], mixed[1]) + cv[3:4, :] * across(carried[1], mixed[1])
    gated = (mixer * gate).astype(BF16)
    none = jnp.zeros((64, T), BF16)
    upper_half = one_hot((HALF, T), lambda row, col: row == col)
    lower_half = one_hot((HALF, T), lambda row, col: row + HALF == col)
    mine = pl.ds(pl.multiple_of(tp * 128, 128), 128)
    bn[:, mine] = (
        across(upper_half, jnp.concatenate([gated, none], axis=0))
        + across(lower_half, jnp.concatenate([none, gated], axis=0))
    ).astype(BF16)

    sems = (rsem, rrecv)
    ring = Ring(bn, 0, HALF, sems, 6 + SPLITS, direct=True)
    ring.start()

    def all_tiles(ref, at):
        return pltpu.make_async_remote_copy(
            src_ref=ref.at[pl.ds(0, TP - 1)],
            dst_ref=ref.at[pl.ds(0, TP - 1)],
            send_sem=one.at[at],
            recv_sem=one.at[at + 1],
            device_id=(sp, (tp + 1) % TP),
            device_id_type=MESH,
        )

    all_tiles(ft, 4).wait_recv()
    for step in (4, 3, 2, 1):
        ring.step(step)
    ring.finish()

    left = lax.broadcasted_iota(jnp.int32, (HALF, 128), 1) < 64
    for g in range(GROUPS):
        squares = jnp.zeros((HALF, 128), F32)
        for j in range(4 * g, 4 * g + 4):
            v = bn[:, 128 * j : 128 * j + 128].astype(F32)
            squares = squares + v * v
        top = jnp.sum(jnp.where(left, squares, 0.0), axis=1, keepdims=True)
        bottom = jnp.sum(jnp.where(left, 0.0, squares), axis=1, keepdims=True)
        scale = lax.rsqrt(jnp.where(left, top, bottom) / (4 * HEAD_DIM) + 1e-06)
        for j in range(4 * g, 4 * g + 4):
            v = bn[:, 128 * j : 128 * j + 128].astype(F32)
            nn[:, 128 * j : 128 * j + 128] = (v * scale * ft[j, 0:1]).astype(BF16)
    projected = dot(nn[...], wide[...])
    am[0:HALF] = (src_ref[0:HALF].astype(F32) + projected[:, 0:128]).astype(BF16)
    am[HALF:T] = (src_ref[HALF:T].astype(F32) + projected[:, 128:256]).astype(BF16)

    own = (am[...].astype(F32) * after_ref[...]).astype(BF16)
    ff[:, mine] = own
    dd[...] = dot(pp[...], own).astype(BF16)

    def rows_of(i):
        return pl.ds(pl.multiple_of(i * SLOTS, SLOTS), SLOTS)

    per = SP // 2 // CHUNKS
    local = (x % 2) * 8 + (x // 2) * 4 + z // 2

    def deliver(k, far=0):
        target = (sp + k) % SP
        return pltpu.make_async_remote_copy(
            src_ref=(d2 if far else dd).at[rows_of(target)],
            dst_ref=(x2 if far else xl).at[rows_of(local), lanes_of(core)],
            send_sem=one.at[9 if far else 8],
            recv_sem=dr.at[local // per + CHUNKS * far],
            device_id=(target, y * 2 + side_of),
            device_id_type=MESH,
        )

    def outward(m):
        return SP // 2 + (m // 2 + m % 2) * (1 - 2 * (m % 2))

    def send_rows(m, carry):
        deliver(outward(m)).start()
        return carry

    lax.fori_loop(0, SP - 1, send_rows, 0)

    @pl.when(side_of == core)
    def _():
        xl[rows_of(local), lanes_of(core)] = dd[rows_of(sp)]

    @pl.when(side_of != core)
    def _():
        deliver(0).start()

    cells = T // SPLITS
    spread_out = [Ring(ff, i * cells, cells, sems, 4 + i) for i in range(SPLITS)]
    for spreading in spread_out:
        spreading.start()

    dims = (((1,), (1,)), ((), ()))
    squares = am[...].astype(F32) * am[...].astype(F32)
    high = squares.astype(BF16)
    rest = (squares - high.astype(F32)).astype(BF16)
    ones = jnp.ones((8, 128), BF16)
    sums = lax.dot_general(ones, high, dims, preferred_element_type=F32) + lax.dot_general(
        ones, rest, dims, preferred_element_type=F32
    )
    line = jnp.concatenate([sums, jnp.zeros((8, 3 * 128 - T), F32)], axis=1)
    level = lax.broadcasted_iota(jnp.int32, (8, 128), 0)
    own = jnp.where(
        level == 0,
        line[:, 0:128],
        jnp.where(level == 1, line[:, 128:256], jnp.where(level == 2, line[:, 256:384], 0.0)),
    )
    sq[tp] = own
    so[...] = own

    def sums_to(k, source):
        return pltpu.make_async_remote_copy(
            src_ref=so,
            dst_ref=sq.at[source],
            send_sem=one.at[6],
            recv_sem=one.at[7],
            device_id=(sp, (tp + k) % TP),
            device_id_type=MESH,
        )

    def send_sums(k, carry):
        sums_to((k + 7) % (TP - 1) + 1, tp).start()
        return carry

    lax.fori_loop(0, TP - 1, send_sums, 0)
    ring.drain()

    def some_rows(ref, first, blocks, sent, received):
        part = ref.at[pl.ds(first, blocks * SLOTS), pl.ds(0, 128)]
        return pltpu.make_async_remote_copy(
            src_ref=part,
            dst_ref=part,
            send_sem=one.at[sent],
            recv_sem=received,
            device_id=((sp + 1) % SP, tp),
            device_id_type=MESH,
        )

    def either(test, less, more):
        @pl.when(test)
        def _():
            less()

        @pl.when(jnp.logical_not(test))
        def _():
            more()

    for step in (1, 2, 3):
        for ring in spread_out:
            ring.step(step)
    chip = pl.ds(pl.multiple_of(y * 256, 256), 256)
    packed_rows = per * CAP
    dense = one_hot((packed_rows, per * SLOTS), lambda row, col: row // CAP * SLOTS + row % CAP == col)
    gathers = []
    for q in range(CHUNKS):
        either(
            jnp.logical_and(side_of == core, x % 2 == q),
            lambda: some_rows(xl, 0, 2 * per - 1, 8, dr.at[q]).wait_recv(),
            lambda: some_rows(xl, 0, 2 * per, 8, dr.at[q]).wait_recv(),
        )
        at = pl.ds(q * packed_rows, packed_rows)
        xx[at, chip] = dot(dense, xl[pl.ds(q * per * SLOTS, per * SLOTS), :]).astype(BF16)
        gathers.append(Ring(xx, q * packed_rows, packed_rows, sems, q, pair=True, last=3))
        gathers[-1].start()
    all_tiles(sq, 6).wait_recv()
    total = sq[0]
    for j in range(1, TP):
        total = total + sq[j]
    line = jnp.concatenate([total[0:1], total[1:2], total[2:3]], axis=1)
    parts = stacked(three(line)).astype(BF16)
    same = one_hot((T, 384), lambda row, col: row == col)
    upright = across(same, parts)
    scale = lax.rsqrt((upright[:, 0:1] + upright[:, 1:2] + upright[:, 2:3]) / D + 1e-06)
    lane = lax.broadcasted_iota(jnp.int32, (T, 128), 1)
    parts = jnp.zeros((T, 128), F32)
    for k, part in enumerate(three(scale)):
        parts = jnp.where(lane == k, part, parts)
    ss[...] = dot(pp[...], parts.astype(BF16)).astype(BF16)

    def send_scale(m, carry):
        target = (sp + outward(m)) % SP
        pltpu.make_async_remote_copy(
            src_ref=ss.at[rows_of(target)],
            dst_ref=sl.at[rows_of(local)],
            send_sem=one.at[14],
            recv_sem=one.at[15],
            device_id=(target, tp),
            device_id_type=MESH,
        ).start()
        return carry

    @pl.when(side_of == core)
    def _():
        lax.fori_loop(0, SP - 1, send_scale, 0)
        sl[rows_of(local), :] = ss[rows_of(sp), :]

    for ring in spread_out:
        ring.step(4)

    opposite = (y + NY // 2) % NY
    d2[...] = dot(pp[...], ff[:, lanes_of(opposite * 2 + core)]).astype(BF16)

    def send_more(m, carry):
        deliver(outward(m), 1).start()
        return carry

    lax.fori_loop(0, SP - 1, send_more, 0)

    @pl.when(side_of == core)
    def _():
        x2[rows_of(local), lanes_of(core)] = d2[rows_of(sp)]

    @pl.when(side_of != core)
    def _():
        deliver(0, 1).start()

    for ring in gathers:
        ring.step(1)
    for ring in spread_out:
        ring.finish()
    to_other(wc.at[:, pl.ds(0, 384)], 18).wait_recv()
    rows = pl.ds(pl.multiple_of(core * HALF, 16), HALF)
    both = dot(ff[rows, :], wc[...]) * jnp.where(core == 0, scale[0:HALF], scale[HALF:T])
    sh[rows, chip] = (jax.nn.silu(both[:, 0:256]) * both[:, 256:512]).astype(BF16)
    shared_out = [
        Ring(sh, pl.multiple_of(core * HALF + first, 16), count, sems, 4 + SPLITS + i, pair=True)
        for i, (first, count) in enumerate(((0, 96), (96, 64)))
    ]
    for ring in shared_out:
        ring.start()
    for ring in gathers:
        ring.step(2)

    def chips(first, count, total, buf, at, weight):
        def add(k, carry):
            part = pl.ds(pl.multiple_of((y + k) % NY * 256, 256), 256)
            total[at, :] += dot(buf[at, part], weight[part, :])
            return carry

        lax.fori_loop(first, first + count, add, 0)

    either(
        side_of == core,
        lambda: some_rows(sl, 0, SP // 2 - 1, 14, one.at[15]).wait_recv(),
        lambda: some_rows(sl, 0, SP // 2, 14, one.at[15]).wait_recv(),
    )
    to_other(wx.at[:, pl.ds(0, 384)], 12).wait_recv()
    tot[...] = jnp.zeros(tot.shape, F32)
    levels = []
    for q in range(CHUNKS):
        at = pl.ds(q * packed_rows, packed_rows)
        chips(NY - 2, NY - 3, tot, xx, at, wx)
        either(
            jnp.logical_and(side_of == core, x % 2 == q),
            lambda: some_rows(x2, 0, 2 * per - 1, 9, dr.at[CHUNKS + q]).wait_recv(),
            lambda: some_rows(x2, 0, 2 * per, 9, dr.at[CHUNKS + q]).wait_recv(),
        )
        turned = pl.ds(pl.multiple_of(opposite * 256, 256), 256)
        xx[at, turned] = dot(dense, x2[pl.ds(q * per * SLOTS, per * SLOTS), :]).astype(BF16)
        chips(NY // 2, 1, tot, xx, at, wx)
        level = dot(dense, sl[pl.ds(q * per * SLOTS, per * SLOTS), :])
        levels.append(level[:, 0:1] + level[:, 1:2] + level[:, 2:3])
    hiddens = []
    for q in range(CHUNKS):
        gathers[q].step(3)
        if q == CHUNKS - 1:
            for ring in shared_out:
                ring.step(1)
        at = pl.ds(q * packed_rows, packed_rows)
        chips(3, 1, tot, xx, at, wx)
        chips(NY - 3, 1, tot, xx, at, wx)
        both = tot[at, :] * levels[q]
        hh[at, chip] = (jax.nn.silu(both[:, 0:256]) * both[:, 256:512]).astype(BF16)
        hiddens.append(Ring(hh, q * packed_rows, packed_rows, sems, 2 + q, pair=True))
        hiddens[-1].start()
    for side in range(2):
        for k in range(3):
            halo(side, k).wait_send()
    all_rows(NX - 1).wait_send()
    all_columns().wait_send()
    all_tiles(ft, 4).wait_send()
    all_tiles(sq, 6).wait_send()
    for sent in (8, 9):
        either(
            side_of == core,
            lambda: some_rows(dd, 0, SP - 1, sent, one.at[20]).wait_send(),
            lambda: some_rows(dd, 0, SP, sent, one.at[20]).wait_send(),
        )

    @pl.when(side_of == core)
    def _():
        some_rows(dd, 0, SP - 1, 14, one.at[20]).wait_send()

    to_other(wx.at[:, pl.ds(0, 384)], 12).wait_send()
    to_other(wc.at[:, pl.ds(0, 384)], 18).wait_send()
    for ring in spread_out + gathers:
        ring.drain()
    low[...] = jnp.zeros(low.shape, F32)
    for step in (1, 2, 3):
        for ring in hiddens:
            ring.step(step)
        if step == 3:
            for ring in shared_out:
                ring.step(2)
        for q in range(CHUNKS):
            at = pl.ds(q * packed_rows, packed_rows)
            if step == 1:
                chips(NY, 1, low, hh, at, wl)
            chips(step, 1, low, hh, at, wl)
            chips(NY - step, 1, low, hh, at, wl)
    loose = one_hot((per * SLOTS, packed_rows), lambda row, col: col // CAP * SLOTS + col % CAP == row)

    def give(i, to_core):
        return pltpu.make_async_remote_copy(
            src_ref=oo.at[rows_of(i), lanes_of(to_core)],
            dst_ref=ret.at[rows_of(sp)],
            send_sem=one.at[10],
            recv_sem=one.at[11],
            device_id=(((i % 4) * 2 + core) * NX + i // 4 % 2 * 2 + i // 8, y * 2 + to_core),
            device_id_type=MESH,
        )

    for q in range(CHUNKS):
        hiddens[q].step(4)
        at = pl.ds(q * packed_rows, packed_rows)
        chips(NY // 2, 1, low, hh, at, wl)
        oo[pl.ds(q * per * SLOTS, per * SLOTS), :] = dot(loose, low[at, :].astype(BF16)).astype(BF16)

        def send_back(k, carry):
            turn = k // 2
            i = q * per + k % 2 * 4 + (z // 2 + 6 + (turn // 2 + turn % 2) * (1 - 2 * (turn % 2))) % 4
            here = jnp.logical_and(side_of == core, i == local)

            @pl.when(jnp.logical_not(here))
            def _():
                give(i, core).start()

            give(i, 1 - core).start()
            return carry

        lax.fori_loop(0, per, send_back, 0)

    @pl.when(side_of == core)
    def _():
        ret[rows_of(sp), :] = oo[rows_of(local), lanes_of(core)]

    for step in (3, 4):
        for ring in shared_out:
            ring.step(step)
    lowered = dot(sh[rows, :], wcl[...]).astype(BF16)
    outs[0] = lowered[:, 0:128]
    outs[1] = lowered[:, 128:256]

    def output(source):
        return pltpu.make_async_remote_copy(
            src_ref=outs.at[source],
            dst_ref=theirs,
            send_sem=one.at[16],
            recv_sem=one.at[17],
            device_id=(sp, y * 2 + 1 - core),
            device_id_type=MESH,
        )

    output(1 - core).start()
    for ring in hiddens + shared_out:
        ring.drain()
    either(
        side_of == core,
        lambda: some_rows(ret, 0, SP - 1, 10, one.at[11]).wait_recv(),
        lambda: some_rows(ret, 0, SP, 10, one.at[11]).wait_recv(),
    )
    either(
        side_of == core,
        lambda: some_rows(ret, 0, SP - 1, 10, one.at[11]).wait_send(),
        lambda: some_rows(ret, 0, SP, 10, one.at[11]).wait_send(),
    )
    routed = dot(qhi[...], ret[...]) + dot(qlo[...], ret[...])
    output(1 - core).wait()
    ours, others = outs[core].astype(F32), theirs[...].astype(F32)
    shared = jnp.concatenate(
        [jnp.where(core == 0, ours, others), jnp.where(core == 0, others, ours)], axis=0
    )
    out_ref[...] = (am[...].astype(F32) + shared + routed).astype(BF16)


def whole(*operands):
    vmem = pl.BlockSpec(memory_space=pltpu.VMEM)
    hbm = pl.BlockSpec(memory_space=pl.ANY)
    rings = 7 + SPLITS
    dma = pltpu.SemaphoreType.DMA

    def space(*shape, kind=BF16):
        return pltpu.VMEM(shape, kind)

    return pl.pallas_call(
        kernel,
        out_shape=jax.ShapeDtypeStruct((T, 128), BF16),
        in_specs=[vmem] * 15 + [hbm] * 9,
        out_specs=vmem,
        scratch_shapes=[
            space(64, 384),
            space(T, 128),
            space(T, 128),
            space(2, 64, 128),
            space(2, 16, 128),
            space(2, 16, 128),
            space(T + 32, 128, kind=F32),
            space(T + 32, 128, kind=F32),
            space(T, T, kind=F32),
            space(8, T, kind=F32),
            space(2, T, 128),
            space(8, 128, kind=F32),
            space(2, BLOCK, 128),
            space(NX, 2, BLOCK, 128),
            space(2, BLOCK, 128),
            space(NZ, BLOCK, 128),
            space(TP, 8, 128, kind=F32),
            space(TP, 8, 128, kind=F32),
            space(8, 128, kind=F32),
            space(1024, 128),
            space(D, 512),
            space(D, 512),
            space(D, 256),
            space(D, 256),
            space(D, 256),
            space(HALF, D),
            space(HALF, D),
            space(T, 128),
            space(T, D),
            space(T, D),
            space(ROWS // 2, 256),
            space(ROWS // 2, 256),
            space(SP // 2 * CAP, D),
            space(SP // 2 * CAP, D),
            space(SP // 2 * CAP, 512, kind=F32),
            space(SP // 2 * CAP, 256, kind=F32),
            space(ROWS, 128),
            space(ROWS, 128),
            space(ROWS, 128),
            space(ROWS // 2, 128),
            space(2, HALF, 128),
            space(HALF, 128),
            space(ROWS // 2, 256),
            space(ROWS, 128),
            space(ROWS, T),
            space(T, ROWS),
            space(T, ROWS),
            dma((9,)), dma((6,)), dma((6,)), dma((21,)), dma((2 * CHUNKS,)), dma((rings, 2)), dma((rings, 8)),
        ],
        compiler_params=pltpu.CompilerParams(collective_id=0, has_side_effects=True),
        name="mixer_experts",
    )(*operands)


def shards(
    layer_source_vector,
    attention_lane_source,
    result_valve_logits,
    memory_write_matrix,
    memory_query_matrix,
    increment_logits,
    increment_offset,
    log_fade_speed,
    extra_log_fade,
    attention_bypass_factor,
    attention_lane_kernel,
    memory_write_kernel,
    memory_query_kernel,
    cluster_rescale_factor,
    blender_result_matrix,
    specialist_rescale_factor,
    chosen_specialists,
    specialist_shares,
    specialist_valve_matrix,
    specialist_raising_matrix,
    specialist_lowering_matrix,
    common_valve_matrix,
    common_raising_matrix,
    common_lowering_matrix,
):
    return whole(
        attention_lane_source.T,
        result_valve_logits.T,
        increment_logits.reshape(2, T),
        increment_offset.T,
        log_fade_speed.T,
        extra_log_fade.reshape(2, 1, T),
        attention_bypass_factor.reshape(1, 1),
        attention_lane_kernel,
        memory_write_kernel,
        memory_query_kernel,
        cluster_rescale_factor.reshape(1, 64),
        specialist_rescale_factor.reshape(1, 128),
        layer_source_vector,
        chosen_specialists.T,
        specialist_shares.T,
        memory_write_matrix,
        memory_query_matrix,
        blender_result_matrix,
        specialist_valve_matrix,
        specialist_raising_matrix,
        specialist_lowering_matrix,
        common_valve_matrix,
        common_raising_matrix,
        common_lowering_matrix,
    )


def solution(mesh):
    return jax.shard_map(
        shards,
        mesh=mesh,
        in_specs=(
            P("sp", "tp"),
            P("sp", "tp"),
            P("sp", "tp"),
            P("sp", None),
            P("sp", None),
            P(None, "sp", "tp"),
            P(None, "tp"),
            P(None, "tp"),
            P(None, "sp", "tp"),
            P("tp"),
            P(None, "tp"),
            P(),
            P(),
            P("tp"),
            P(None, "tp"),
            P("tp"),
            P("sp", None),
            P("sp", None),
            P("sp", None, "tp"),
            P("sp", None, "tp"),
            P("sp", None, "tp"),
            P(None, "tp"),
            P(None, "tp"),
            P(None, "tp"),
        ),
        out_specs=P("sp", "tp"),
        check_vma=False,
    )
```

```python
import jax
import jax.numpy as jnp
from jax import lax
from jax.experimental import pallas as pl
from jax.experimental.pallas import tpu as pltpu
from jax.sharding import PartitionSpec as P

D = 2048
HEADS = 16
HEAD_DIM = 64
GROUPS = 4
STATE = 128
CONV = 5

NZ, NX, NY = 8, 4, 8
SP, TP = NZ * NX, NY * 2
T = 320
HALF = T // 2
SLOTS = 32
ROWS = SP * SLOTS
CAP = 30
SPLITS = 4
BLOCK = 80
CHUNKS = 2
PIECE = SLOTS // CHUNKS
MESH = pl.DeviceIdType.MESH
F32, BF16 = jnp.float32, jnp.bfloat16


def dot(a, b):
    return jnp.dot(a, b, preferred_element_type=F32)


class Ring:
    def __init__(self, buf, first, rows, sems, index, direct=False, pair=False, last=4):
        self.buf, self.first, self.rows = buf, first, rows
        self.direct, self.pair, self.last = direct, pair, last
        self.out, self.near = sems[0].at[index, 0], sems[0].at[index, 1]
        self.recv = sems[1].at[index]
        self.sp, tp = lax.axis_index("sp"), lax.axis_index("tp")
        self.y, self.core = tp // 2, tp % 2

    def part(self, chip, core, half=None):
        column, width = ((chip + 2 * NY) % NY) * 2, 128
        if self.pair:
            width = 256
        else:
            column = column + core
        first, rows = self.first, self.rows
        if half is not None:
            cut = (rows // 2 + 15) // 16 * 16
            first, rows = (first, cut) if half == 0 else (first + cut, rows - cut)
        return self.buf.at[pl.ds(first, rows), pl.ds(pl.multiple_of(column * 128, 128), width)]

    def along(self, way, step, chip, far):
        turn = 1 - 2 * way
        block = self.part(chip, self.core, way if step == 4 else None)
        return pltpu.make_async_remote_copy(
            src_ref=block,
            dst_ref=block,
            send_sem=self.out,
            recv_sem=self.recv.at[4 * way + step - 1],
            device_id=(self.sp, ((self.y + turn * far + NY) % NY) * 2 + self.core),
            device_id_type=MESH,
        )

    def hop(self, way, step):
        if self.direct:
            return self.along(way, step, self.y, step)
        return self.along(way, step, self.y - (1 - 2 * way) * (step - 1), 1)

    def landed(self, way, step):
        return self.along(way, step, self.y - (1 - 2 * way) * step, 1)

    def relay(self, way, step):
        turn = 1 - 2 * way
        return self.over(self.part(self.y - turn * step, self.core, way if step == 4 else None))

    def over(self, block):
        return pltpu.make_async_remote_copy(
            src_ref=block,
            dst_ref=block,
            send_sem=self.out,
            recv_sem=self.near,
            device_id=(self.sp, self.y * 2 + 1 - self.core),
            device_id_type=MESH,
        )

    def several(self, blocks):
        return self.over(self.buf.at[pl.ds(self.first, self.rows), pl.ds(0, 128 * blocks)])

    def start(self):
        for step in (4, 3, 2, 1) if self.direct else (1,):
            self.hop(0, step).start()
            self.hop(1, step).start()
        if not self.pair:
            self.relay(0, 0).start()

    def step(self, step):
        for way in (0, 1):
            self.landed(way, step).wait_recv()
            if step < self.last and not self.direct:
                self.hop(way, step + 1).start()
            if not self.pair:
                self.relay(way, step).start()

    def finish(self):
        self.several(NY).wait_recv()

    def drain(self):
        self.several(2 * NY - (1 if not self.pair else 2 if self.last == 4 else 4)).wait_send()


def stacked(rows):
    level = lax.broadcasted_iota(jnp.int32, (8, rows[0].shape[1]), 0)
    total = jnp.zeros(level.shape, F32)
    for k, row in enumerate(rows):
        total = jnp.where(level == k, row, total)
    return total


def three(v):
    high = v.astype(BF16).astype(F32)
    middle = (v - high).astype(BF16).astype(F32)
    return [high, middle, v - high - middle]


def one_hot(shape, test):
    row, col = lax.broadcasted_iota(jnp.int32, shape, 0), lax.broadcasted_iota(jnp.int32, shape, 1)
    return jnp.where(test(row, col), 1.0, 0.0).astype(BF16)


def across(a, b):
    return lax.dot_general(a, b, (((1,), (1,)), ((), ())), preferred_element_type=F32)


def log1p(u):
    series = u * (1 - u * (1 / 2 - u * (1 / 3 - u * (1 / 4 - u * (1 / 5 - u / 6)))))
    return jnp.where(u < 0.03, series, jnp.log(1 + u))


def silu(v):
    return v / (1 + jnp.exp(-v))


def kernel(
    xt_ref, zt_ref, inc_ref, off_ref, spd_ref, fade_ref, byp_ref, xk_ref, bk_ref, ck_ref, gain_ref,
    after_ref, src_ref, cht_ref, sht_ref,
    bm_hbm, cm_hbm, blender_hbm, valve_hbm, raising_hbm, lowering_hbm, cvalve_hbm, craising_hbm, clowering_hbm,
    out_ref,
    xpad, braw, craw, hx, hb, hc, bext, cext, gap, cv, mixed, fto,
    st_ref, rx, tb, rz, ft, sq, so, wb, wx, wc, wl, wcl, wide, bn, nn, am, ff, sh, xl, x2, xx, hh, tot, low, dd, d2, ss, sl, outs, theirs, oo, ret, pp, qhi, qlo,
    wsem, hs, hr, one, dr, rsem, rrecv,
):
    sp, tp = lax.axis_index("sp"), lax.axis_index("tp")
    z, x = sp // NX, sp % NX
    y, core, side_of = tp // 2, tp % 2, z % 2

    barrier = pltpu.get_barrier_semaphore()

    def greet_tp(k, carry):
        pl.semaphore_signal(barrier, inc=1, device_id=(sp, (tp + k) % TP), device_id_type=MESH)
        return carry

    def greet_sp(k, carry):
        pl.semaphore_signal(barrier, inc=1, device_id=((sp + k) % SP, tp), device_id_type=MESH)
        return carry

    lax.fori_loop(1, TP, greet_tp, 0)
    lax.fori_loop(1, SP, greet_sp, 0)

    def lanes_of(i):
        return pl.ds(pl.multiple_of(i * 128, 128), 128)

    at_group = pl.ds(pl.multiple_of((tp // 4) * 128, 128), 128)
    loads = [
        pltpu.make_async_copy(blender_hbm, wb, wsem.at[0]),
        pltpu.make_async_copy(valve_hbm.at[0], wx.at[:, lanes_of(core)], wsem.at[1]),
        pltpu.make_async_copy(raising_hbm.at[0], wx.at[:, lanes_of(core + 2)], wsem.at[2]),
        pltpu.make_async_copy(lowering_hbm.at[0], wl.at[:, lanes_of(core)], wsem.at[3]),
        pltpu.make_async_copy(cvalve_hbm, wc.at[:, lanes_of(core)], wsem.at[4]),
        pltpu.make_async_copy(craising_hbm, wc.at[:, lanes_of(core + 2)], wsem.at[5]),
        pltpu.make_async_copy(clowering_hbm, wcl.at[:, lanes_of(core)], wsem.at[6]),
    ]
    grouped = [
        pltpu.make_async_copy(bm_hbm.at[:, at_group], braw, wsem.at[7]),
        pltpu.make_async_copy(cm_hbm.at[:, at_group], craw, wsem.at[8]),
    ]
    for load in grouped + loads:
        load.start()

    xpad[...] = jnp.zeros(xpad.shape, BF16)
    xpad[:, 0:T] = xt_ref[...]
    gains = jnp.concatenate([gain_ref[...], gain_ref[...]], axis=1)
    fto[...] = jnp.broadcast_to(gains, (8, 128))
    ft[tp] = fto[...]

    def state_row(k, source):
        return pltpu.make_async_remote_copy(
            src_ref=st_ref,
            dst_ref=rx.at[source],
            send_sem=one.at[0],
            recv_sem=one.at[1],
            device_id=(z * NX + (x + k) % NX, tp),
            device_id_type=MESH,
        )

    def tile(k, source):
        return pltpu.make_async_remote_copy(
            src_ref=fto,
            dst_ref=ft.at[source],
            send_sem=one.at[4],
            recv_sem=one.at[5],
            device_id=(sp, (tp + k) % TP),
            device_id_type=MESH,
        )

    def send_tile(k, carry):
        tile(k, tp).start()
        return carry

    for load in grouped:
        load.wait()
    pl.semaphore_wait(barrier, TP + SP - 2)

    def halo(side, k):
        there = (sp + 1) % SP if side == 0 else (sp + SP - 1) % SP
        rows = pl.ds(T - 16, 16) if side == 0 else pl.ds(0, 16)
        lanes = pl.ds(256, 128) if side == 0 else pl.ds(0, 128)
        source = (xpad.at[:, lanes], braw.at[rows], craw.at[rows])[k]
        return pltpu.make_async_remote_copy(
            src_ref=source,
            dst_ref=(hx, hb, hc)[k].at[side],
            send_sem=hs.at[3 * side + k],
            recv_sem=hr.at[3 * side + k],
            device_id=(there, tp),
            device_id_type=MESH,
        )

    for k in range(3):
        halo(0, k).start()
        halo(1, k).start()
    lax.fori_loop(1, TP, send_tile, 0)

    lower = one_hot((T, T), lambda row, col: col < row)
    upper = one_hot((T, T), lambda row, col: row < col)
    same = one_hot((T, T), lambda row, col: row == col)
    experts = lax.broadcasted_iota(jnp.int32, (SP, T), 0)
    first, second = cht_ref[0:1, :] == experts, cht_ref[1:2, :] == experts
    named = jnp.where(first | second, 1.0, 0.0)
    rank = dot(named.astype(BF16), upper)
    rank = jnp.where(named > 0, rank, 99.0).astype(BF16)
    spread = one_hot((ROWS, SP), lambda row, col: row // SLOTS == col)
    place = (lax.broadcasted_iota(jnp.int32, (ROWS, T), 0) % SLOTS).astype(F32)
    pp[...] = jnp.where(dot(spread, rank) == place, 1.0, 0.0).astype(BF16)
    shares = jnp.where(first, sht_ref[0:1, :], 0.0) + jnp.where(second, sht_ref[1:2, :], 0.0)
    share_hi = shares.astype(BF16)
    share_lo = (shares - share_hi.astype(F32)).astype(BF16)
    spread = one_hot((SP, ROWS), lambda row, col: col // SLOTS == row)
    place = (lax.broadcasted_iota(jnp.int32, (T, ROWS), 1) % SLOTS).astype(F32)
    here = dot(across(same, rank).astype(BF16), spread) == place
    qhi[...] = jnp.where(here, dot(across(same, share_hi).astype(BF16), spread), 0.0).astype(BF16)
    qlo[...] = jnp.where(here, dot(across(same, share_lo).astype(BF16), spread), 0.0).astype(BF16)

    steps, fades = [], []
    for d in range(2):
        v = inc_ref[d : d + 1, :].astype(F32) + off_ref[0:1, d : d + 1]
        step = jnp.maximum(v, 0.0) + log1p(jnp.exp(-jnp.abs(v)))
        steps.append(step)
        fades.append(-jnp.exp(spd_ref[0:1, d : d + 1]) * step + fade_ref[d])
    parts = stacked(three(fades[0]) + three(fades[1])).astype(BF16)
    along = dot(parts, upper + same)
    forward_row = along[0:1] + along[1:2] + along[2:3]
    along = dot(parts, upper)
    backward_row = along[3:4] + along[4:5] + along[5:6]
    along = across(lower + same, parts)
    forward_col = along[:, 0:1] + along[:, 1:2] + along[:, 2:3]
    along = across(lower, parts)
    backward_col = along[:, 3:4] + along[:, 4:5] + along[:, 5:6]
    row = lax.broadcasted_iota(jnp.int32, (T, T), 0)
    col = lax.broadcasted_iota(jnp.int32, (T, T), 1)
    gap[...] = (
        jnp.where(row >= col, jnp.exp(forward_col - forward_row), 0.0) * steps[0]
        + jnp.where(row <= col, jnp.exp(backward_row - backward_col), 0.0) * steps[1]
    )
    forward_end = forward_row[:, T - 1 : T]
    backward_end = backward_row[:, T - 1 : T] + fades[1][:, T - 1 : T]
    weigh = [jnp.exp(forward_end - forward_row) * steps[0], jnp.exp(backward_row) * steps[1]]
    seen = [jnp.exp(forward_row), jnp.exp(backward_end - backward_row)]
    cv[...] = stacked(weigh + seen)
    ends = [jnp.broadcast_to(forward_end, (1, 128)), jnp.broadcast_to(backward_end, (1, 128))]

    def to_other(part, at):
        return pltpu.make_async_remote_copy(
            src_ref=part,
            dst_ref=part,
            send_sem=one.at[at],
            recv_sem=one.at[at + 1],
            device_id=(sp, y * 2 + 1 - core),
            device_id_type=MESH,
        )

    for k in (1, 2, 3):
        loads[k].wait()
    for part in (wx.at[:, lanes_of(core)], wx.at[:, lanes_of(core + 2)], wl.at[:, lanes_of(core)]):
        to_other(part, 12).start()

    taps = across(same[0:64, 0:64], stacked([xk_ref[j : j + 1, :].astype(F32) for j in range(CONV)]).astype(BF16))
    lane = lax.broadcasted_iota(jnp.int32, (64, 128), 1)
    body = xpad[...].astype(F32)
    bext[pl.ds(16, T), :] = braw[...].astype(F32)
    cext[pl.ds(16, T), :] = craw[...].astype(F32)
    for k in range(3):
        halo(0, k).wait_recv()
        halo(1, k).wait_recv()
    before, behind = sp > 0, sp < SP - 1
    last = jnp.where(before, pltpu.roll(hx[0].astype(F32), 64, 1), 0.0)
    coming = jnp.where(behind, pltpu.roll(hx[1].astype(F32), 64, 1), 0.0)
    end = jnp.where(
        lane < 64, body[:, 256:384], jnp.where(lane < 66, coming, jnp.where(lane > 125, last, 0.0))
    )
    cells = jnp.concatenate([body[:, 0:256], end], axis=1)
    total = cells * taps[:, 2:3]
    for j in (0, 1, 3, 4):
        total = total + pltpu.roll(cells, (2 - j) % 384, 1) * taps[:, j : j + 1]
    x_conv = silu(total)[:, 0:T].astype(BF16)
    for ext, halos, kernel_ref in ((bext, hb, bk_ref), (cext, hc, ck_ref)):
        ext[pl.ds(0, 16), :] = jnp.where(before, halos[0].astype(F32), 0.0)
        ext[pl.ds(T + 16, 16), :] = jnp.where(behind, halos[1].astype(F32), 0.0)
        total = jnp.zeros((T, 128), F32)
        for j in range(CONV):
            tap = kernel_ref[j : j + 1, at_group].astype(F32)
            total = total + ext[pl.ds(14 + j, T), :] * tap
        mixed[0 if ext is bext else 1] = silu(total).astype(BF16)
    b_conv, c_conv = mixed[0], mixed[1]

    def packed(total, log):
        tail = jnp.concatenate([stacked(three(log)), jnp.zeros((8, 128), F32)], axis=0)
        return total.astype(BF16), tail.astype(BF16)

    x_wide = x_conv.astype(F32)
    for d in range(2):
        scaled = (cv[d : d + 1, :] * x_wide).astype(BF16)
        top, tail = packed(dot(scaled, b_conv), ends[d])
        st_ref[d, 0:64] = top
        st_ref[d, 64:80] = tail
    rx[x] = st_ref[...]
    for k in (2, 1, 3):
        state_row(k, x).start()
    inner = across(x_conv, (across(c_conv, b_conv) * gap[...]).astype(BF16))
    inner = inner + byp_ref[...] * x_wide
    gate = silu(zt_ref[...].astype(F32))

    def all_rows(k):
        return pltpu.make_async_remote_copy(
            src_ref=rx.at[pl.ds(0, k)],
            dst_ref=rx.at[pl.ds(0, k)],
            send_sem=one.at[0],
            recv_sem=one.at[1],
            device_id=(z * NX + (x + 1) % NX, tp),
            device_id_type=MESH,
        )

    all_rows(NX - 1).wait_recv()

    def state(block):
        return block[0:64].astype(F32)

    def log_of(block):
        logs = block[64:80].astype(F32)
        return logs[0:1] + logs[1:2] + logs[2:3]

    for way in (0, 1):
        total, log = jnp.zeros((64, 128), F32), jnp.zeros((1, 128), F32)
        for i in range(NX) if way == 0 else reversed(range(NX)):
            block = rx[i, way]
            own = log_of(block)
            total = jnp.exp(own) * total + state(block)
            log = log + own
        top, tail = packed(total, log)
        tb[way, 0:64] = top
        tb[way, 64:80] = tail
    rz[z] = tb[0]

    def state_column(k, source):
        return pltpu.make_async_remote_copy(
            src_ref=tb.at[(z + k) // NZ],
            dst_ref=rz.at[source],
            send_sem=one.at[2],
            recv_sem=one.at[3],
            device_id=(((z + k) % NZ) * NX + x, tp),
            device_id_type=MESH,
        )

    for k in (4, 3, 5, 2, 6, 1, 7):
        state_column(k, z).start()

    for k in (4, 5, 6):
        loads[k].wait()
    for part in (wc.at[:, lanes_of(core)], wc.at[:, lanes_of(core + 2)], wcl.at[:, lanes_of(core)]):
        to_other(part, 18).start()

    loads[0].wait()
    wide[...] = jnp.zeros(wide.shape, BF16)

    def widen(j, carry):
        block = wb[pl.ds(pl.multiple_of(j * 64, 64), 64), :]
        wide[pl.ds(pl.multiple_of(j * 128, 128), 64), pl.ds(0, 128)] = block
        wide[pl.ds(pl.multiple_of(j * 128 + 64, 64), 64), pl.ds(128, 128)] = block
        return carry

    lax.fori_loop(0, HEADS, widen, 0)

    def all_columns():
        return pltpu.make_async_remote_copy(
            src_ref=rz.at[pl.ds(0, NZ - 1)],
            dst_ref=rz.at[pl.ds(0, NZ - 1)],
            send_sem=one.at[2],
            recv_sem=one.at[3],
            device_id=(((z + 1) % NZ) * NX + x, tp),
            device_id_type=MESH,
        )

    all_columns().wait_recv()

    carried = []
    for way in (0, 1):
        total = jnp.zeros((64, 128), F32)
        for i in range(NZ) if way == 0 else reversed(range(NZ)):
            block = rz[i]
            passed = (i < z) if way == 0 else (i > z)
            total = jnp.where(passed, jnp.exp(log_of(block)) * total + state(block), total)
        for i in range(NX) if way == 0 else reversed(range(NX)):
            block = rx[i, way]
            passed = (i < x) if way == 0 else (i > x)
            total = jnp.where(passed, jnp.exp(log_of(block)) * total + state(block), total)
        carried.append(total.astype(BF16))

    mixer = inner + cv[2:3, :] * across(carried[0], mixed[1]) + cv[3:4, :] * across(carried[1], mixed[1])
    gated = (mixer * gate).astype(BF16)
    none = jnp.zeros((64, T), BF16)
    upper_half = one_hot((HALF, T), lambda row, col: row == col)
    lower_half = one_hot((HALF, T), lambda row, col: row + HALF == col)
    mine = pl.ds(pl.multiple_of(tp * 128, 128), 128)
    bn[:, mine] = (
        across(upper_half, jnp.concatenate([gated, none], axis=0))
        + across(lower_half, jnp.concatenate([none, gated], axis=0))
    ).astype(BF16)

    sems = (rsem, rrecv)
    ring = Ring(bn, 0, HALF, sems, 6 + SPLITS, direct=True)
    ring.start()

    def all_tiles(ref, at):
        return pltpu.make_async_remote_copy(
            src_ref=ref.at[pl.ds(0, TP - 1)],
            dst_ref=ref.at[pl.ds(0, TP - 1)],
            send_sem=one.at[at],
            recv_sem=one.at[at + 1],
            device_id=(sp, (tp + 1) % TP),
            device_id_type=MESH,
        )

    all_tiles(ft, 4).wait_recv()
    for step in (4, 3, 2, 1):
        ring.step(step)
    ring.finish()

    left = lax.broadcasted_iota(jnp.int32, (HALF, 128), 1) < 64
    for g in range(GROUPS):
        squares = jnp.zeros((HALF, 128), F32)
        for j in range(4 * g, 4 * g + 4):
            v = bn[:, 128 * j : 128 * j + 128].astype(F32)
            squares = squares + v * v
        top = jnp.sum(jnp.where(left, squares, 0.0), axis=1, keepdims=True)
        bottom = jnp.sum(jnp.where(left, 0.0, squares), axis=1, keepdims=True)
        scale = lax.rsqrt(jnp.where(left, top, bottom) / (4 * HEAD_DIM) + 1e-06)
        for j in range(4 * g, 4 * g + 4):
            v = bn[:, 128 * j : 128 * j + 128].astype(F32)
            nn[:, 128 * j : 128 * j + 128] = (v * scale * ft[j, 0:1]).astype(BF16)
    projected = dot(nn[...], wide[...])
    am[0:HALF] = (src_ref[0:HALF].astype(F32) + projected[:, 0:128]).astype(BF16)
    am[HALF:T] = (src_ref[HALF:T].astype(F32) + projected[:, 128:256]).astype(BF16)

    own = (am[...].astype(F32) * after_ref[...]).astype(BF16)
    ff[:, mine] = own
    dd[...] = dot(pp[...], own).astype(BF16)

    def rows_of(i):
        return pl.ds(pl.multiple_of(i * SLOTS, SLOTS), SLOTS)

    local = (x % 2) * 8 + (x // 2) * 4 + z // 2
    landing = pl.ds(pl.multiple_of(local * PIECE, PIECE), PIECE)

    def piece_of(i, q):
        return pl.ds(pl.multiple_of(i * SLOTS + q * PIECE, PIECE), PIECE)

    def deliver(k, q):
        target = (sp + k) % SP
        return pltpu.make_async_remote_copy(
            src_ref=dd.at[piece_of(target, q)],
            dst_ref=xl.at[q, landing, lanes_of(core)],
            send_sem=one.at[8],
            recv_sem=dr.at[q],
            device_id=(target, y * 2 + side_of),
            device_id_type=MESH,
        )

    def deliver_more(k):
        target = (sp + k) % SP
        return pltpu.make_async_remote_copy(
            src_ref=d2.at[rows_of(target)],
            dst_ref=x2.at[rows_of(local), lanes_of(core)],
            send_sem=one.at[9],
            recv_sem=dr.at[CHUNKS],
            device_id=(target, y * 2 + side_of),
            device_id_type=MESH,
        )

    def outward(m):
        return SP // 2 + (m // 2 + m % 2) * (1 - 2 * (m % 2))

    for q in range(CHUNKS):

        def send_rows(m, carry):
            deliver(outward(m), q).start()
            return carry

        lax.fori_loop(0, SP - 1, send_rows, 0)

        @pl.when(side_of != core)
        def _():
            deliver(0, q).start()

    @pl.when(side_of == core)
    def _():
        for q in range(CHUNKS):
            xl[q, landing, lanes_of(core)] = dd[piece_of(sp, q)]

    cells = T // SPLITS
    spread_out = [Ring(ff, i * cells, cells, sems, 4 + i) for i in range(SPLITS)]
    for spreading in spread_out:
        spreading.start()

    dims = (((1,), (1,)), ((), ()))
    squares = am[...].astype(F32) * am[...].astype(F32)
    high = squares.astype(BF16)
    rest = (squares - high.astype(F32)).astype(BF16)
    ones = jnp.ones((8, 128), BF16)
    sums = lax.dot_general(ones, high, dims, preferred_element_type=F32) + lax.dot_general(
        ones, rest, dims, preferred_element_type=F32
    )
    line = jnp.concatenate([sums, jnp.zeros((8, 3 * 128 - T), F32)], axis=1)
    level = lax.broadcasted_iota(jnp.int32, (8, 128), 0)
    own = jnp.where(
        level == 0,
        line[:, 0:128],
        jnp.where(level == 1, line[:, 128:256], jnp.where(level == 2, line[:, 256:384], 0.0)),
    )
    sq[tp] = own
    so[...] = own

    def sums_to(k, source):
        return pltpu.make_async_remote_copy(
            src_ref=so,
            dst_ref=sq.at[source],
            send_sem=one.at[6],
            recv_sem=one.at[7],
            device_id=(sp, (tp + k) % TP),
            device_id_type=MESH,
        )

    def send_sums(k, carry):
        sums_to((k + 7) % (TP - 1) + 1, tp).start()
        return carry

    lax.fori_loop(0, TP - 1, send_sums, 0)
    ring.drain()

    def some_rows(ref, first, blocks, sent, received, rows=SLOTS):
        part = ref.at[pl.ds(first, blocks * rows), pl.ds(0, 128)]
        return pltpu.make_async_remote_copy(
            src_ref=part,
            dst_ref=part,
            send_sem=one.at[sent],
            recv_sem=received,
            device_id=((sp + 1) % SP, tp),
            device_id_type=MESH,
        )

    def either(test, less, more):
        @pl.when(test)
        def _():
            less()

        @pl.when(jnp.logical_not(test))
        def _():
            more()

    for step in (1, 2):
        for ring in spread_out:
            ring.step(step)
    chip = pl.ds(pl.multiple_of(y * 256, 256), 256)
    used = [PIECE, CAP - PIECE]
    sources = SP // 2
    spans = [pl.ds(0, sources * used[0]), pl.ds(sources * used[0], sources * used[1])]
    dense = [
        one_hot(
            (sources * used[q], sources * SLOTS),
            lambda row, col: row // used[q] * SLOTS + row % used[q] + q * PIECE == col,
        )
        for q in range(CHUNKS)
    ]
    squeeze = one_hot(
        (sources * used[1], sources * PIECE),
        lambda row, col: row // used[1] * PIECE + row % used[1] == col,
    )
    gathers = []

    def gather(q):
        either(
            side_of == core,
            lambda: some_rows(dd, 0, SP - 1, 8, dr.at[q], PIECE).wait_recv(),
            lambda: some_rows(dd, 0, SP, 8, dr.at[q], PIECE).wait_recv(),
        )
        if used[q] == PIECE:
            xx[spans[q], chip] = xl[q]
        else:
            xx[spans[q], chip] = dot(squeeze, xl[q]).astype(BF16)
        ring = Ring(xx, sources * used[0] * q, sources * used[q], sems, q, pair=True, last=3)
        ring.start()
        gathers.append(ring)

    gather(0)
    all_tiles(sq, 6).wait_recv()
    total = sq[0]
    for j in range(1, TP):
        total = total + sq[j]
    line = jnp.concatenate([total[0:1], total[1:2], total[2:3]], axis=1)
    parts = stacked(three(line)).astype(BF16)
    same = one_hot((T, 384), lambda row, col: row == col)
    upright = across(same, parts)
    scale = lax.rsqrt((upright[:, 0:1] + upright[:, 1:2] + upright[:, 2:3]) / D + 1e-06)
    lane = lax.broadcasted_iota(jnp.int32, (T, 128), 1)
    parts = jnp.zeros((T, 128), F32)
    for k, part in enumerate(three(scale)):
        parts = jnp.where(lane == k, part, parts)
    ss[...] = dot(pp[...], parts.astype(BF16)).astype(BF16)

    def send_scale(m, carry):
        target = (sp + outward(m)) % SP
        pltpu.make_async_remote_copy(
            src_ref=ss.at[rows_of(target)],
            dst_ref=sl.at[rows_of(local)],
            send_sem=one.at[14],
            recv_sem=one.at[15],
            device_id=(target, tp),
            device_id_type=MESH,
        ).start()
        return carry

    @pl.when(side_of == core)
    def _():
        lax.fori_loop(0, SP - 1, send_scale, 0)
        sl[rows_of(local), :] = ss[rows_of(sp), :]

    gather(1)
    for ring in spread_out:
        ring.step(3)
    for ring in gathers:
        ring.step(1)
    for ring in spread_out:
        ring.step(4)

    opposite = (y + NY // 2) % NY
    d2[...] = dot(pp[...], ff[:, lanes_of(opposite * 2 + core)]).astype(BF16)

    def send_more(m, carry):
        deliver_more(outward(m)).start()
        return carry

    lax.fori_loop(0, SP - 1, send_more, 0)

    @pl.when(side_of == core)
    def _():
        x2[rows_of(local), lanes_of(core)] = d2[rows_of(sp)]

    @pl.when(side_of != core)
    def _():
        deliver_more(0).start()

    for ring in spread_out:
        ring.finish()
    to_other(wc.at[:, pl.ds(0, 384)], 18).wait_recv()
    rows = pl.ds(pl.multiple_of(core * HALF, 16), HALF)
    both = dot(ff[rows, :], wc[...]) * jnp.where(core == 0, scale[0:HALF], scale[HALF:T])
    sh[rows, chip] = (jax.nn.silu(both[:, 0:256]) * both[:, 256:512]).astype(BF16)
    shared_out = [
        Ring(sh, pl.multiple_of(core * HALF + first, 16), count, sems, 4 + SPLITS + i, pair=True)
        for i, (first, count) in enumerate(((0, 96), (96, 64)))
    ]
    for ring in shared_out:
        ring.start()
    for ring in gathers:
        ring.step(2)

    def chips(first, count, total, buf, at, weight):
        def add(k, carry):
            part = pl.ds(pl.multiple_of((y + k) % NY * 256, 256), 256)
            total[at, :] += dot(buf[at, part], weight[part, :])
            return carry

        lax.fori_loop(first, first + count, add, 0)

    either(
        side_of == core,
        lambda: some_rows(sl, 0, SP // 2 - 1, 14, one.at[15]).wait_recv(),
        lambda: some_rows(sl, 0, SP // 2, 14, one.at[15]).wait_recv(),
    )
    to_other(wx.at[:, pl.ds(0, 384)], 12).wait_recv()
    tot[...] = jnp.zeros(tot.shape, F32)
    levels = []
    for q in range(CHUNKS):
        chips(NY - 2, NY - 3, tot, xx, spans[q], wx)
    either(
        side_of == core,
        lambda: some_rows(d2, 0, SP - 1, 9, dr.at[CHUNKS]).wait_recv(),
        lambda: some_rows(d2, 0, SP, 9, dr.at[CHUNKS]).wait_recv(),
    )
    turned = pl.ds(pl.multiple_of(opposite * 256, 256), 256)
    for q in range(CHUNKS):
        at = spans[q]
        xx[at, turned] = dot(dense[q], x2[...]).astype(BF16)
        chips(NY // 2, 1, tot, xx, at, wx)
        level = dot(dense[q], sl[...])
        levels.append(level[:, 0:1] + level[:, 1:2] + level[:, 2:3])
    hiddens = []
    for q in range(CHUNKS):
        gathers[q].step(3)
        if q == CHUNKS - 1:
            for ring in shared_out:
                ring.step(1)
        at = spans[q]
        chips(3, 1, tot, xx, at, wx)
        chips(NY - 3, 1, tot, xx, at, wx)
        both = tot[at, :] * levels[q]
        hh[at, chip] = (jax.nn.silu(both[:, 0:256]) * both[:, 256:512]).astype(BF16)
        hiddens.append(Ring(hh, sources * used[0] * q, sources * used[q], sems, 2 + q, pair=True))
        hiddens[-1].start()
    for side in range(2):
        for k in range(3):
            halo(side, k).wait_send()
    all_rows(NX - 1).wait_send()
    all_columns().wait_send()
    all_tiles(ft, 4).wait_send()
    all_tiles(sq, 6).wait_send()
    for sent in (8, 9):
        either(
            side_of == core,
            lambda: some_rows(dd, 0, SP - 1, sent, one.at[20]).wait_send(),
            lambda: some_rows(dd, 0, SP, sent, one.at[20]).wait_send(),
        )

    @pl.when(side_of == core)
    def _():
        some_rows(dd, 0, SP - 1, 14, one.at[20]).wait_send()

    to_other(wx.at[:, pl.ds(0, 384)], 12).wait_send()
    to_other(wc.at[:, pl.ds(0, 384)], 18).wait_send()
    for ring in spread_out + gathers:
        ring.drain()
    low[...] = jnp.zeros(low.shape, F32)
    for step in (1, 2, 3):
        for ring in hiddens:
            ring.step(step)
        if step == 3:
            for ring in shared_out:
                ring.step(2)
        for q in range(CHUNKS):
            at = spans[q]
            if step == 1:
                chips(NY, 1, low, hh, at, wl)
            chips(step, 1, low, hh, at, wl)
            chips(NY - step, 1, low, hh, at, wl)
    loose = [
        one_hot(
            (sources * PIECE, sources * used[q]),
            lambda row, col: col // used[q] * PIECE + col % used[q] == row,
        )
        for q in range(CHUNKS)
    ]

    def give(i, to_core, q):
        return pltpu.make_async_remote_copy(
            src_ref=oo.at[q, pl.ds(pl.multiple_of(i * PIECE, PIECE), PIECE), lanes_of(to_core)],
            dst_ref=ret.at[piece_of(sp, q)],
            send_sem=one.at[10],
            recv_sem=one.at[11],
            device_id=(((i % 4) * 2 + core) * NX + i // 4 % 2 * 2 + i // 8, y * 2 + to_core),
            device_id_type=MESH,
        )

    for q in range(CHUNKS):
        hiddens[q].step(4)
        at = spans[q]
        chips(NY // 2, 1, low, hh, at, wl)
        oo[q] = dot(loose[q], low[at, :].astype(BF16)).astype(BF16)

        def send_back(k, carry):
            turn = k // 4
            i = k % 4 * 4 + (z // 2 + 6 + (turn // 2 + turn % 2) * (1 - 2 * (turn % 2))) % 4
            here = jnp.logical_and(side_of == core, i == local)

            @pl.when(jnp.logical_not(here))
            def _():
                give(i, core, q).start()

            give(i, 1 - core, q).start()
            return carry

        lax.fori_loop(0, sources, send_back, 0)

    @pl.when(side_of == core)
    def _():
        for q in range(CHUNKS):
            ret[piece_of(sp, q), :] = oo[q, landing, lanes_of(core)]

    for step in (3, 4):
        for ring in shared_out:
            ring.step(step)
    lowered = dot(sh[rows, :], wcl[...]).astype(BF16)
    outs[0] = lowered[:, 0:128]
    outs[1] = lowered[:, 128:256]

    def output(source):
        return pltpu.make_async_remote_copy(
            src_ref=outs.at[source],
            dst_ref=theirs,
            send_sem=one.at[16],
            recv_sem=one.at[17],
            device_id=(sp, y * 2 + 1 - core),
            device_id_type=MESH,
        )

    output(1 - core).start()
    for ring in hiddens + shared_out:
        ring.drain()
    either(
        side_of == core,
        lambda: some_rows(ret, 0, SP - 1, 10, one.at[11]).wait_recv(),
        lambda: some_rows(ret, 0, SP, 10, one.at[11]).wait_recv(),
    )
    either(
        side_of == core,
        lambda: some_rows(ret, 0, SP - 1, 10, one.at[11]).wait_send(),
        lambda: some_rows(ret, 0, SP, 10, one.at[11]).wait_send(),
    )
    routed = dot(qhi[...], ret[...]) + dot(qlo[...], ret[...])
    output(1 - core).wait()
    ours, others = outs[core].astype(F32), theirs[...].astype(F32)
    shared = jnp.concatenate(
        [jnp.where(core == 0, ours, others), jnp.where(core == 0, others, ours)], axis=0
    )
    out_ref[...] = (am[...].astype(F32) + shared + routed).astype(BF16)


def whole(*operands):
    vmem = pl.BlockSpec(memory_space=pltpu.VMEM)
    hbm = pl.BlockSpec(memory_space=pl.ANY)
    rings = 7 + SPLITS
    dma = pltpu.SemaphoreType.DMA

    def space(*shape, kind=BF16):
        return pltpu.VMEM(shape, kind)

    return pl.pallas_call(
        kernel,
        out_shape=jax.ShapeDtypeStruct((T, 128), BF16),
        in_specs=[vmem] * 15 + [hbm] * 9,
        out_specs=vmem,
        scratch_shapes=[
            space(64, 384),
            space(T, 128),
            space(T, 128),
            space(2, 64, 128),
            space(2, 16, 128),
            space(2, 16, 128),
            space(T + 32, 128, kind=F32),
            space(T + 32, 128, kind=F32),
            space(T, T, kind=F32),
            space(8, T, kind=F32),
            space(2, T, 128),
            space(8, 128, kind=F32),
            space(2, BLOCK, 128),
            space(NX, 2, BLOCK, 128),
            space(2, BLOCK, 128),
            space(NZ, BLOCK, 128),
            space(TP, 8, 128, kind=F32),
            space(TP, 8, 128, kind=F32),
            space(8, 128, kind=F32),
            space(1024, 128),
            space(D, 512),
            space(D, 512),
            space(D, 256),
            space(D, 256),
            space(D, 256),
            space(HALF, D),
            space(HALF, D),
            space(T, 128),
            space(T, D),
            space(T, D),
            space(2, ROWS // 4, 256),
            space(ROWS // 2, 256),
            space(SP // 2 * CAP, D),
            space(SP // 2 * CAP, D),
            space(SP // 2 * CAP, 512, kind=F32),
            space(SP // 2 * CAP, 256, kind=F32),
            space(ROWS, 128),
            space(ROWS, 128),
            space(ROWS, 128),
            space(ROWS // 2, 128),
            space(2, HALF, 128),
            space(HALF, 128),
            space(2, ROWS // 4, 256),
            space(ROWS, 128),
            space(ROWS, T),
            space(T, ROWS),
            space(T, ROWS),
            dma((9,)), dma((6,)), dma((6,)), dma((21,)), dma((CHUNKS + 1,)), dma((rings, 2)), dma((rings, 8)),
        ],
        compiler_params=pltpu.CompilerParams(collective_id=0, has_side_effects=True),
        name="mixer_experts",
    )(*operands)


def shards(
    layer_source_vector,
    attention_lane_source,
    result_valve_logits,
    memory_write_matrix,
    memory_query_matrix,
    increment_logits,
    increment_offset,
    log_fade_speed,
    extra_log_fade,
    attention_bypass_factor,
    attention_lane_kernel,
    memory_write_kernel,
    memory_query_kernel,
    cluster_rescale_factor,
    blender_result_matrix,
    specialist_rescale_factor,
    chosen_specialists,
    specialist_shares,
    specialist_valve_matrix,
    specialist_raising_matrix,
    specialist_lowering_matrix,
    common_valve_matrix,
    common_raising_matrix,
    common_lowering_matrix,
):
    return whole(
        attention_lane_source.T,
        result_valve_logits.T,
        increment_logits.reshape(2, T),
        increment_offset.T,
        log_fade_speed.T,
        extra_log_fade.reshape(2, 1, T),
        attention_bypass_factor.reshape(1, 1),
        attention_lane_kernel,
        memory_write_kernel,
        memory_query_kernel,
        cluster_rescale_factor.reshape(1, 64),
        specialist_rescale_factor.reshape(1, 128),
        layer_source_vector,
        chosen_specialists.T,
        specialist_shares.T,
        memory_write_matrix,
        memory_query_matrix,
        blender_result_matrix,
        specialist_valve_matrix,
        specialist_raising_matrix,
        specialist_lowering_matrix,
        common_valve_matrix,
        common_raising_matrix,
        common_lowering_matrix,
    )


def solution(mesh):
    return jax.shard_map(
        shards,
        mesh=mesh,
        in_specs=(
            P("sp", "tp"),
            P("sp", "tp"),
            P("sp", "tp"),
            P("sp", None),
            P("sp", None),
            P(None, "sp", "tp"),
            P(None, "tp"),
            P(None, "tp"),
            P(None, "sp", "tp"),
            P("tp"),
            P(None, "tp"),
            P(),
            P(),
            P("tp"),
            P(None, "tp"),
            P("tp"),
            P("sp", None),
            P("sp", None),
            P("sp", None, "tp"),
            P("sp", None, "tp"),
            P("sp", None, "tp"),
            P(None, "tp"),
            P(None, "tp"),
            P(None, "tp"),
        ),
        out_specs=P("sp", "tp"),
        check_vma=False,
    )
```

```python
import jax
import jax.numpy as jnp
from jax import lax
from jax.experimental import pallas as pl
from jax.experimental.pallas import tpu as pltpu
from jax.sharding import PartitionSpec as P

D = 2048
HEADS = 16
HEAD_DIM = 64
GROUPS = 4
STATE = 128
CONV = 5

NZ, NX, NY = 8, 4, 8
SP, TP = NZ * NX, NY * 2
T = 320
HALF = T // 2
SLOTS = 32
ROWS = SP * SLOTS
CAP = 30
SPLITS = 4
BLOCK = 80
CHUNKS = 2
PIECE = SLOTS // CHUNKS
MESH = pl.DeviceIdType.MESH
F32, BF16 = jnp.float32, jnp.bfloat16


def dot(a, b):
    return jnp.dot(a, b, preferred_element_type=F32)


class Ring:
    def __init__(self, buf, first, rows, sems, index, direct=False, pair=False, last=4):
        self.buf, self.first, self.rows = buf, first, rows
        self.direct, self.pair, self.last = direct, pair, last
        self.out, self.near = sems[0].at[index, 0], sems[0].at[index, 1]
        self.recv = sems[1].at[index]
        self.sp, tp = lax.axis_index("sp"), lax.axis_index("tp")
        self.y, self.core = tp // 2, tp % 2

    def part(self, chip, core, half=None):
        column, width = ((chip + 2 * NY) % NY) * 2, 128
        if self.pair:
            width = 256
        else:
            column = column + core
        first, rows = self.first, self.rows
        if half is not None:
            cut = (rows // 2 + 15) // 16 * 16
            first, rows = (first, cut) if half == 0 else (first + cut, rows - cut)
        return self.buf.at[pl.ds(first, rows), pl.ds(pl.multiple_of(column * 128, 128), width)]

    def along(self, way, step, chip, far):
        turn = 1 - 2 * way
        block = self.part(chip, self.core, way if step == 4 else None)
        return pltpu.make_async_remote_copy(
            src_ref=block,
            dst_ref=block,
            send_sem=self.out,
            recv_sem=self.recv.at[4 * way + step - 1],
            device_id=(self.sp, ((self.y + turn * far + NY) % NY) * 2 + self.core),
            device_id_type=MESH,
        )

    def hop(self, way, step):
        if self.direct:
            return self.along(way, step, self.y, step)
        return self.along(way, step, self.y - (1 - 2 * way) * (step - 1), 1)

    def landed(self, way, step):
        return self.along(way, step, self.y - (1 - 2 * way) * step, 1)

    def relay(self, way, step):
        turn = 1 - 2 * way
        return self.over(self.part(self.y - turn * step, self.core, way if step == 4 else None))

    def over(self, block):
        return pltpu.make_async_remote_copy(
            src_ref=block,
            dst_ref=block,
            send_sem=self.out,
            recv_sem=self.near,
            device_id=(self.sp, self.y * 2 + 1 - self.core),
            device_id_type=MESH,
        )

    def several(self, blocks):
        return self.over(self.buf.at[pl.ds(self.first, self.rows), pl.ds(0, 128 * blocks)])

    def start(self):
        for step in (4, 3, 2, 1) if self.direct else (1,):
            self.hop(0, step).start()
            self.hop(1, step).start()
        if not self.pair:
            self.relay(0, 0).start()

    def step(self, step):
        for way in (0, 1):
            self.landed(way, step).wait_recv()
            if step < self.last and not self.direct:
                self.hop(way, step + 1).start()
            if not self.pair:
                self.relay(way, step).start()

    def finish(self):
        self.several(NY).wait_recv()

    def drain(self):
        self.several(2 * NY - (1 if not self.pair else 2 if self.last == 4 else 4)).wait_send()


def stacked(rows):
    level = lax.broadcasted_iota(jnp.int32, (8, rows[0].shape[1]), 0)
    total = jnp.zeros(level.shape, F32)
    for k, row in enumerate(rows):
        total = jnp.where(level == k, row, total)
    return total


def three(v):
    high = v.astype(BF16).astype(F32)
    middle = (v - high).astype(BF16).astype(F32)
    return [high, middle, v - high - middle]


def one_hot(shape, test):
    row, col = lax.broadcasted_iota(jnp.int32, shape, 0), lax.broadcasted_iota(jnp.int32, shape, 1)
    return jnp.where(test(row, col), 1.0, 0.0).astype(BF16)


def across(a, b):
    return lax.dot_general(a, b, (((1,), (1,)), ((), ())), preferred_element_type=F32)


def log1p(u):
    series = u * (1 - u * (1 / 2 - u * (1 / 3 - u * (1 / 4 - u * (1 / 5 - u / 6)))))
    return jnp.where(u < 0.03, series, jnp.log(1 + u))


def silu(v):
    return v / (1 + jnp.exp(-v))


def kernel(
    xt_hbm, zt_hbm, inc_hbm, off_hbm, spd_hbm, fade_hbm, byp_hbm, xk_hbm,
    bk_hbm, ck_hbm, gain_hbm, after_hbm, src_hbm, cht_hbm, sht_hbm,
    bm_hbm, cm_hbm, blender_hbm, valve_hbm, raising_hbm, lowering_hbm, cvalve_hbm, craising_hbm, clowering_hbm,
    out_ref,
    xt_ref, zt_ref, inc_ref, off_ref, spd_ref, fade_ref, byp_ref, xk_ref,
    bk_ref, ck_ref, gain_ref, after_ref, src_ref, cht_ref, sht_ref,
    xpad, braw, craw, hx, hb, hc, bext, cext, gap, cv, mixed, fto,
    st_ref, rx, tb, rz, ft, sq, so, wb, wx, wc, wl, wcl, wide, bn, nn, am, ff, sh, xl, x2, xx, hh, tot, low, dd, d2, ss, sl, outs, theirs, oo, ret, pp, qhi, qlo,
    isem, wsem, hs, hr, one, dr, rsem, rrecv,
):
    sp, tp = lax.axis_index("sp"), lax.axis_index("tp")
    z, x = sp // NX, sp % NX
    y, core, side_of = tp // 2, tp % 2, z % 2

    barrier = pltpu.get_barrier_semaphore()

    def greet_tp(k, carry):
        pl.semaphore_signal(barrier, inc=1, device_id=(sp, (tp + k) % TP), device_id_type=MESH)
        return carry

    def greet_sp(k, carry):
        pl.semaphore_signal(barrier, inc=1, device_id=((sp + k) % SP, tp), device_id_type=MESH)
        return carry

    lax.fori_loop(1, TP, greet_tp, 0)
    lax.fori_loop(1, SP, greet_sp, 0)

    def lanes_of(i):
        return pl.ds(pl.multiple_of(i * 128, 128), 128)

    at_group = pl.ds(pl.multiple_of((tp // 4) * 128, 128), 128)
    loads = [
        pltpu.make_async_copy(blender_hbm, wb, wsem.at[0]),
        pltpu.make_async_copy(valve_hbm.at[0], wx.at[:, lanes_of(core)], wsem.at[1]),
        pltpu.make_async_copy(raising_hbm.at[0], wx.at[:, lanes_of(core + 2)], wsem.at[2]),
        pltpu.make_async_copy(lowering_hbm.at[0], wl.at[:, lanes_of(core)], wsem.at[3]),
        pltpu.make_async_copy(cvalve_hbm, wc.at[:, lanes_of(core)], wsem.at[4]),
        pltpu.make_async_copy(craising_hbm, wc.at[:, lanes_of(core + 2)], wsem.at[5]),
        pltpu.make_async_copy(clowering_hbm, wcl.at[:, lanes_of(core)], wsem.at[6]),
    ]
    grouped = [
        pltpu.make_async_copy(bm_hbm.at[:, at_group], braw, wsem.at[7]),
        pltpu.make_async_copy(cm_hbm.at[:, at_group], craw, wsem.at[8]),
    ]
    small = [
        pltpu.make_async_copy(there, here, isem.at[k])
        for k, (there, here) in enumerate(
            (
                (xt_hbm, xt_ref),
                (zt_hbm, zt_ref),
                (inc_hbm, inc_ref),
                (off_hbm, off_ref),
                (spd_hbm, spd_ref),
                (fade_hbm, fade_ref),
                (byp_hbm, byp_ref),
                (xk_hbm, xk_ref),
                (bk_hbm, bk_ref),
                (ck_hbm, ck_ref),
                (gain_hbm, gain_ref),
                (after_hbm, after_ref),
                (src_hbm, src_ref),
                (cht_hbm, cht_ref),
                (sht_hbm, sht_ref),
            )
        )
    ]
    for load in small + grouped + loads:
        load.start()
    for load in small:
        load.wait()

    xpad[...] = jnp.zeros(xpad.shape, BF16)
    xpad[:, 0:T] = xt_ref[...]
    gains = jnp.concatenate([gain_ref[...], gain_ref[...]], axis=1)
    fto[...] = jnp.broadcast_to(gains, (8, 128))
    ft[tp] = fto[...]

    def state_row(k, source):
        return pltpu.make_async_remote_copy(
            src_ref=st_ref,
            dst_ref=rx.at[source],
            send_sem=one.at[0],
            recv_sem=one.at[1],
            device_id=(z * NX + (x + k) % NX, tp),
            device_id_type=MESH,
        )

    def tile(k, source):
        return pltpu.make_async_remote_copy(
            src_ref=fto,
            dst_ref=ft.at[source],
            send_sem=one.at[4],
            recv_sem=one.at[5],
            device_id=(sp, (tp + k) % TP),
            device_id_type=MESH,
        )

    def send_tile(k, carry):
        tile(k, tp).start()
        return carry

    for load in grouped:
        load.wait()
    pl.semaphore_wait(barrier, TP + SP - 2)

    def halo(side, k):
        there = (sp + 1) % SP if side == 0 else (sp + SP - 1) % SP
        rows = pl.ds(T - 16, 16) if side == 0 else pl.ds(0, 16)
        lanes = pl.ds(256, 128) if side == 0 else pl.ds(0, 128)
        source = (xpad.at[:, lanes], braw.at[rows], craw.at[rows])[k]
        return pltpu.make_async_remote_copy(
            src_ref=source,
            dst_ref=(hx, hb, hc)[k].at[side],
            send_sem=hs.at[3 * side + k],
            recv_sem=hr.at[3 * side + k],
            device_id=(there, tp),
            device_id_type=MESH,
        )

    for k in range(3):
        halo(0, k).start()
        halo(1, k).start()
    lax.fori_loop(1, TP, send_tile, 0)

    lower = one_hot((T, T), lambda row, col: col < row)
    upper = one_hot((T, T), lambda row, col: row < col)
    same = one_hot((T, T), lambda row, col: row == col)
    experts = lax.broadcasted_iota(jnp.int32, (SP, T), 0)
    first, second = cht_ref[0:1, :] == experts, cht_ref[1:2, :] == experts
    named = jnp.where(first | second, 1.0, 0.0)
    rank = dot(named.astype(BF16), upper)
    rank = jnp.where(named > 0, rank, 99.0).astype(BF16)
    spread = one_hot((ROWS, SP), lambda row, col: row // SLOTS == col)
    place = (lax.broadcasted_iota(jnp.int32, (ROWS, T), 0) % SLOTS).astype(F32)
    pp[...] = jnp.where(dot(spread, rank) == place, 1.0, 0.0).astype(BF16)
    shares = jnp.where(first, sht_ref[0:1, :], 0.0) + jnp.where(second, sht_ref[1:2, :], 0.0)
    share_hi = shares.astype(BF16)
    share_lo = (shares - share_hi.astype(F32)).astype(BF16)
    spread = one_hot((SP, ROWS), lambda row, col: col // SLOTS == row)
    place = (lax.broadcasted_iota(jnp.int32, (T, ROWS), 1) % SLOTS).astype(F32)
    here = dot(across(same, rank).astype(BF16), spread) == place
    qhi[...] = jnp.where(here, dot(across(same, share_hi).astype(BF16), spread), 0.0).astype(BF16)
    qlo[...] = jnp.where(here, dot(across(same, share_lo).astype(BF16), spread), 0.0).astype(BF16)

    steps, fades = [], []
    for d in range(2):
        v = inc_ref[d : d + 1, :].astype(F32) + off_ref[0:1, d : d + 1]
        step = jnp.maximum(v, 0.0) + log1p(jnp.exp(-jnp.abs(v)))
        steps.append(step)
        fades.append(-jnp.exp(spd_ref[0:1, d : d + 1]) * step + fade_ref[d])
    parts = stacked(three(fades[0]) + three(fades[1])).astype(BF16)
    along = dot(parts, upper + same)
    forward_row = along[0:1] + along[1:2] + along[2:3]
    along = dot(parts, upper)
    backward_row = along[3:4] + along[4:5] + along[5:6]
    along = across(lower + same, parts)
    forward_col = along[:, 0:1] + along[:, 1:2] + along[:, 2:3]
    along = across(lower, parts)
    backward_col = along[:, 3:4] + along[:, 4:5] + along[:, 5:6]
    row = lax.broadcasted_iota(jnp.int32, (T, T), 0)
    col = lax.broadcasted_iota(jnp.int32, (T, T), 1)
    gap[...] = (
        jnp.where(row >= col, jnp.exp(forward_col - forward_row), 0.0) * steps[0]
        + jnp.where(row <= col, jnp.exp(backward_row - backward_col), 0.0) * steps[1]
    )
    forward_end = forward_row[:, T - 1 : T]
    backward_end = backward_row[:, T - 1 : T] + fades[1][:, T - 1 : T]
    weigh = [jnp.exp(forward_end - forward_row) * steps[0], jnp.exp(backward_row) * steps[1]]
    seen = [jnp.exp(forward_row), jnp.exp(backward_end - backward_row)]
    cv[...] = stacked(weigh + seen)
    ends = [jnp.broadcast_to(forward_end, (1, 128)), jnp.broadcast_to(backward_end, (1, 128))]

    def to_other(part, at):
        return pltpu.make_async_remote_copy(
            src_ref=part,
            dst_ref=part,
            send_sem=one.at[at],
            recv_sem=one.at[at + 1],
            device_id=(sp, y * 2 + 1 - core),
            device_id_type=MESH,
        )

    for k in (1, 2, 3):
        loads[k].wait()
    for part in (wx.at[:, lanes_of(core)], wx.at[:, lanes_of(core + 2)], wl.at[:, lanes_of(core)]):
        to_other(part, 12).start()

    taps = across(same[0:64, 0:64], stacked([xk_ref[j : j + 1, :].astype(F32) for j in range(CONV)]).astype(BF16))
    lane = lax.broadcasted_iota(jnp.int32, (64, 128), 1)
    body = xpad[...].astype(F32)
    bext[pl.ds(16, T), :] = braw[...].astype(F32)
    cext[pl.ds(16, T), :] = craw[...].astype(F32)
    for k in range(3):
        halo(0, k).wait_recv()
        halo(1, k).wait_recv()
    before, behind = sp > 0, sp < SP - 1
    last = jnp.where(before, pltpu.roll(hx[0].astype(F32), 64, 1), 0.0)
    coming = jnp.where(behind, pltpu.roll(hx[1].astype(F32), 64, 1), 0.0)
    end = jnp.where(
        lane < 64, body[:, 256:384], jnp.where(lane < 66, coming, jnp.where(lane > 125, last, 0.0))
    )
    cells = jnp.concatenate([body[:, 0:256], end], axis=1)
    total = cells * taps[:, 2:3]
    for j in (0, 1, 3, 4):
        total = total + pltpu.roll(cells, (2 - j) % 384, 1) * taps[:, j : j + 1]
    x_conv = silu(total)[:, 0:T].astype(BF16)
    for ext, halos, kernel_ref in ((bext, hb, bk_ref), (cext, hc, ck_ref)):
        ext[pl.ds(0, 16), :] = jnp.where(before, halos[0].astype(F32), 0.0)
        ext[pl.ds(T + 16, 16), :] = jnp.where(behind, halos[1].astype(F32), 0.0)
        total = jnp.zeros((T, 128), F32)
        for j in range(CONV):
            tap = kernel_ref[j : j + 1, at_group].astype(F32)
            total = total + ext[pl.ds(14 + j, T), :] * tap
        mixed[0 if ext is bext else 1] = silu(total).astype(BF16)
    b_conv, c_conv = mixed[0], mixed[1]

    def packed(total, log):
        tail = jnp.concatenate([stacked(three(log)), jnp.zeros((8, 128), F32)], axis=0)
        return total.astype(BF16), tail.astype(BF16)

    x_wide = x_conv.astype(F32)
    for d in range(2):
        scaled = (cv[d : d + 1, :] * x_wide).astype(BF16)
        top, tail = packed(dot(scaled, b_conv), ends[d])
        st_ref[d, 0:64] = top
        st_ref[d, 64:80] = tail
    rx[x] = st_ref[...]
    for k in (2, 1, 3):
        state_row(k, x).start()
    inner = across(x_conv, (across(c_conv, b_conv) * gap[...]).astype(BF16))
    inner = inner + byp_ref[0] * x_wide
    gate = silu(zt_ref[...].astype(F32))

    def all_rows(k):
        return pltpu.make_async_remote_copy(
            src_ref=rx.at[pl.ds(0, k)],
            dst_ref=rx.at[pl.ds(0, k)],
            send_sem=one.at[0],
            recv_sem=one.at[1],
            device_id=(z * NX + (x + 1) % NX, tp),
            device_id_type=MESH,
        )

    all_rows(NX - 1).wait_recv()

    def state(block):
        return block[0:64].astype(F32)

    def log_of(block):
        logs = block[64:80].astype(F32)
        return logs[0:1] + logs[1:2] + logs[2:3]

    for way in (0, 1):
        total, log = jnp.zeros((64, 128), F32), jnp.zeros((1, 128), F32)
        for i in range(NX) if way == 0 else reversed(range(NX)):
            block = rx[i, way]
            own = log_of(block)
            total = jnp.exp(own) * total + state(block)
            log = log + own
        top, tail = packed(total, log)
        tb[way, 0:64] = top
        tb[way, 64:80] = tail
    rz[z] = tb[0]

    def state_column(k, source):
        return pltpu.make_async_remote_copy(
            src_ref=tb.at[(z + k) // NZ],
            dst_ref=rz.at[source],
            send_sem=one.at[2],
            recv_sem=one.at[3],
            device_id=(((z + k) % NZ) * NX + x, tp),
            device_id_type=MESH,
        )

    for k in (4, 3, 5, 2, 6, 1, 7):
        state_column(k, z).start()

    for k in (4, 5, 6):
        loads[k].wait()
    for part in (wc.at[:, lanes_of(core)], wc.at[:, lanes_of(core + 2)], wcl.at[:, lanes_of(core)]):
        to_other(part, 18).start()

    loads[0].wait()
    wide[...] = jnp.zeros(wide.shape, BF16)

    def widen(j, carry):
        block = wb[pl.ds(pl.multiple_of(j * 64, 64), 64), :]
        wide[pl.ds(pl.multiple_of(j * 128, 128), 64), pl.ds(0, 128)] = block
        wide[pl.ds(pl.multiple_of(j * 128 + 64, 64), 64), pl.ds(128, 128)] = block
        return carry

    lax.fori_loop(0, HEADS, widen, 0)

    def all_columns():
        return pltpu.make_async_remote_copy(
            src_ref=rz.at[pl.ds(0, NZ - 1)],
            dst_ref=rz.at[pl.ds(0, NZ - 1)],
            send_sem=one.at[2],
            recv_sem=one.at[3],
            device_id=(((z + 1) % NZ) * NX + x, tp),
            device_id_type=MESH,
        )

    all_columns().wait_recv()

    carried = []
    for way in (0, 1):
        total = jnp.zeros((64, 128), F32)
        for i in range(NZ) if way == 0 else reversed(range(NZ)):
            block = rz[i]
            passed = (i < z) if way == 0 else (i > z)
            total = jnp.where(passed, jnp.exp(log_of(block)) * total + state(block), total)
        for i in range(NX) if way == 0 else reversed(range(NX)):
            block = rx[i, way]
            passed = (i < x) if way == 0 else (i > x)
            total = jnp.where(passed, jnp.exp(log_of(block)) * total + state(block), total)
        carried.append(total.astype(BF16))

    mixer = inner + cv[2:3, :] * across(carried[0], mixed[1]) + cv[3:4, :] * across(carried[1], mixed[1])
    gated = (mixer * gate).astype(BF16)
    none = jnp.zeros((64, T), BF16)
    upper_half = one_hot((HALF, T), lambda row, col: row == col)
    lower_half = one_hot((HALF, T), lambda row, col: row + HALF == col)
    mine = pl.ds(pl.multiple_of(tp * 128, 128), 128)
    bn[:, mine] = (
        across(upper_half, jnp.concatenate([gated, none], axis=0))
        + across(lower_half, jnp.concatenate([none, gated], axis=0))
    ).astype(BF16)

    sems = (rsem, rrecv)
    ring = Ring(bn, 0, HALF, sems, 6 + SPLITS, direct=True)
    ring.start()

    def all_tiles(ref, at):
        return pltpu.make_async_remote_copy(
            src_ref=ref.at[pl.ds(0, TP - 1)],
            dst_ref=ref.at[pl.ds(0, TP - 1)],
            send_sem=one.at[at],
            recv_sem=one.at[at + 1],
            device_id=(sp, (tp + 1) % TP),
            device_id_type=MESH,
        )

    all_tiles(ft, 4).wait_recv()
    for step in (4, 3, 2, 1):
        ring.step(step)
    ring.finish()

    left = lax.broadcasted_iota(jnp.int32, (HALF, 128), 1) < 64
    for g in range(GROUPS):
        squares = jnp.zeros((HALF, 128), F32)
        for j in range(4 * g, 4 * g + 4):
            v = bn[:, 128 * j : 128 * j + 128].astype(F32)
            squares = squares + v * v
        top = jnp.sum(jnp.where(left, squares, 0.0), axis=1, keepdims=True)
        bottom = jnp.sum(jnp.where(left, 0.0, squares), axis=1, keepdims=True)
        scale = lax.rsqrt(jnp.where(left, top, bottom) / (4 * HEAD_DIM) + 1e-06)
        for j in range(4 * g, 4 * g + 4):
            v = bn[:, 128 * j : 128 * j + 128].astype(F32)
            nn[:, 128 * j : 128 * j + 128] = (v * scale * ft[j, 0:1]).astype(BF16)
    projected = dot(nn[...], wide[...])
    am[0:HALF] = (src_ref[0:HALF].astype(F32) + projected[:, 0:128]).astype(BF16)
    am[HALF:T] = (src_ref[HALF:T].astype(F32) + projected[:, 128:256]).astype(BF16)

    own = (am[...].astype(F32) * after_ref[...]).astype(BF16)
    ff[:, mine] = own
    cells = T // SPLITS
    spread_out = [Ring(ff, i * cells, cells, sems, 4 + i) for i in range(SPLITS)]
    for spreading in spread_out:
        spreading.start()
    dd[...] = dot(pp[...], own).astype(BF16)

    def rows_of(i):
        return pl.ds(pl.multiple_of(i * SLOTS, SLOTS), SLOTS)

    local = (x % 2) * 8 + (x // 2) * 4 + z // 2
    landing = pl.ds(pl.multiple_of(local * PIECE, PIECE), PIECE)

    def piece_of(i, q):
        return pl.ds(pl.multiple_of(i * SLOTS + q * PIECE, PIECE), PIECE)

    def deliver(k, q):
        target = (sp + k) % SP
        return pltpu.make_async_remote_copy(
            src_ref=dd.at[piece_of(target, q)],
            dst_ref=xl.at[q, landing, lanes_of(core)],
            send_sem=one.at[8],
            recv_sem=dr.at[q],
            device_id=(target, y * 2 + side_of),
            device_id_type=MESH,
        )

    def deliver_more(k):
        target = (sp + k) % SP
        return pltpu.make_async_remote_copy(
            src_ref=d2.at[rows_of(target)],
            dst_ref=x2.at[rows_of(local), lanes_of(core)],
            send_sem=one.at[9],
            recv_sem=dr.at[CHUNKS],
            device_id=(target, y * 2 + side_of),
            device_id_type=MESH,
        )

    def outward(m):
        return SP // 2 + (m // 2 + m % 2) * (1 - 2 * (m % 2))

    for q in range(CHUNKS):

        def send_rows(m, carry):
            deliver(outward(m), q).start()
            return carry

        lax.fori_loop(0, SP - 1, send_rows, 0)

        @pl.when(side_of != core)
        def _():
            deliver(0, q).start()

    @pl.when(side_of == core)
    def _():
        for q in range(CHUNKS):
            xl[q, landing, lanes_of(core)] = dd[piece_of(sp, q)]

    dims = (((1,), (1,)), ((), ()))
    squares = am[...].astype(F32) * am[...].astype(F32)
    high = squares.astype(BF16)
    rest = (squares - high.astype(F32)).astype(BF16)
    ones = jnp.ones((8, 128), BF16)
    sums = lax.dot_general(ones, high, dims, preferred_element_type=F32) + lax.dot_general(
        ones, rest, dims, preferred_element_type=F32
    )
    line = jnp.concatenate([sums, jnp.zeros((8, 3 * 128 - T), F32)], axis=1)
    level = lax.broadcasted_iota(jnp.int32, (8, 128), 0)
    own = jnp.where(
        level == 0,
        line[:, 0:128],
        jnp.where(level == 1, line[:, 128:256], jnp.where(level == 2, line[:, 256:384], 0.0)),
    )
    sq[tp] = own
    so[...] = own

    def sums_to(k, source):
        return pltpu.make_async_remote_copy(
            src_ref=so,
            dst_ref=sq.at[source],
            send_sem=one.at[6],
            recv_sem=one.at[7],
            device_id=(sp, (tp + k) % TP),
            device_id_type=MESH,
        )

    def send_sums(k, carry):
        sums_to((k + 7) % (TP - 1) + 1, tp).start()
        return carry

    lax.fori_loop(0, TP - 1, send_sums, 0)
    ring.drain()

    def some_rows(ref, first, blocks, sent, received, rows=SLOTS):
        part = ref.at[pl.ds(first, blocks * rows), pl.ds(0, 128)]
        return pltpu.make_async_remote_copy(
            src_ref=part,
            dst_ref=part,
            send_sem=one.at[sent],
            recv_sem=received,
            device_id=((sp + 1) % SP, tp),
            device_id_type=MESH,
        )

    def either(test, less, more):
        @pl.when(test)
        def _():
            less()

        @pl.when(jnp.logical_not(test))
        def _():
            more()

    for step in (1, 2):
        for ring in spread_out:
            ring.step(step)
    chip = pl.ds(pl.multiple_of(y * 256, 256), 256)
    used = [PIECE, CAP - PIECE]
    sources = SP // 2
    spans = [pl.ds(0, sources * used[0]), pl.ds(sources * used[0], sources * used[1])]
    dense = [
        one_hot(
            (sources * used[q], sources * SLOTS),
            lambda row, col: row // used[q] * SLOTS + row % used[q] + q * PIECE == col,
        )
        for q in range(CHUNKS)
    ]
    squeeze = one_hot(
        (sources * used[1], sources * PIECE),
        lambda row, col: row // used[1] * PIECE + row % used[1] == col,
    )
    gathers = []

    def gather(q):
        either(
            side_of == core,
            lambda: some_rows(dd, 0, SP - 1, 8, dr.at[q], PIECE).wait_recv(),
            lambda: some_rows(dd, 0, SP, 8, dr.at[q], PIECE).wait_recv(),
        )
        if used[q] == PIECE:
            xx[spans[q], chip] = xl[q]
        else:
            xx[spans[q], chip] = dot(squeeze, xl[q]).astype(BF16)
        ring = Ring(xx, sources * used[0] * q, sources * used[q], sems, q, pair=True, last=3)
        ring.start()
        gathers.append(ring)

    gather(0)
    all_tiles(sq, 6).wait_recv()
    total = sq[0]
    for j in range(1, TP):
        total = total + sq[j]
    line = jnp.concatenate([total[0:1], total[1:2], total[2:3]], axis=1)
    parts = stacked(three(line)).astype(BF16)
    same = one_hot((T, 384), lambda row, col: row == col)
    upright = across(same, parts)
    scale = lax.rsqrt((upright[:, 0:1] + upright[:, 1:2] + upright[:, 2:3]) / D + 1e-06)
    lane = lax.broadcasted_iota(jnp.int32, (T, 128), 1)
    parts = jnp.zeros((T, 128), F32)
    for k, part in enumerate(three(scale)):
        parts = jnp.where(lane == k, part, parts)
    ss[...] = dot(pp[...], parts.astype(BF16)).astype(BF16)

    def send_scale(m, carry):
        target = (sp + outward(m)) % SP
        pltpu.make_async_remote_copy(
            src_ref=ss.at[rows_of(target)],
            dst_ref=sl.at[rows_of(local)],
            send_sem=one.at[14],
            recv_sem=one.at[15],
            device_id=(target, tp),
            device_id_type=MESH,
        ).start()
        return carry

    @pl.when(side_of == core)
    def _():
        lax.fori_loop(0, SP - 1, send_scale, 0)
        sl[rows_of(local), :] = ss[rows_of(sp), :]

    gather(1)
    for ring in spread_out:
        ring.step(3)
    for ring in gathers:
        ring.step(1)
    for ring in spread_out:
        ring.step(4)

    opposite = (y + NY // 2) % NY
    d2[...] = dot(pp[...], ff[:, lanes_of(opposite * 2 + core)]).astype(BF16)

    def send_more(m, carry):
        deliver_more(outward(m)).start()
        return carry

    lax.fori_loop(0, SP - 1, send_more, 0)

    @pl.when(side_of == core)
    def _():
        x2[rows_of(local), lanes_of(core)] = d2[rows_of(sp)]

    @pl.when(side_of != core)
    def _():
        deliver_more(0).start()

    for ring in spread_out:
        ring.finish()
    to_other(wc.at[:, pl.ds(0, 384)], 18).wait_recv()
    rows = pl.ds(pl.multiple_of(core * HALF, 16), HALF)
    both = dot(ff[rows, :], wc[...]) * jnp.where(core == 0, scale[0:HALF], scale[HALF:T])
    sh[rows, chip] = (jax.nn.silu(both[:, 0:256]) * both[:, 256:512]).astype(BF16)
    shared_out = [
        Ring(sh, pl.multiple_of(core * HALF + first, 16), count, sems, 4 + SPLITS + i, pair=True)
        for i, (first, count) in enumerate(((0, 96), (96, 64)))
    ]
    for ring in shared_out:
        ring.start()
    for ring in gathers:
        ring.step(2)

    def chips(first, count, total, buf, at, weight):
        def add(k, carry):
            part = pl.ds(pl.multiple_of((y + k) % NY * 256, 256), 256)
            total[at, :] += dot(buf[at, part], weight[part, :])
            return carry

        lax.fori_loop(first, first + count, add, 0)

    either(
        side_of == core,
        lambda: some_rows(sl, 0, SP // 2 - 1, 14, one.at[15]).wait_recv(),
        lambda: some_rows(sl, 0, SP // 2, 14, one.at[15]).wait_recv(),
    )
    to_other(wx.at[:, pl.ds(0, 384)], 12).wait_recv()
    tot[...] = jnp.zeros(tot.shape, F32)
    levels = []
    for q in range(CHUNKS):
        chips(NY - 2, NY - 3, tot, xx, spans[q], wx)
    either(
        side_of == core,
        lambda: some_rows(d2, 0, SP - 1, 9, dr.at[CHUNKS]).wait_recv(),
        lambda: some_rows(d2, 0, SP, 9, dr.at[CHUNKS]).wait_recv(),
    )
    turned = pl.ds(pl.multiple_of(opposite * 256, 256), 256)
    for q in range(CHUNKS):
        at = spans[q]
        xx[at, turned] = dot(dense[q], x2[...]).astype(BF16)
        chips(NY // 2, 1, tot, xx, at, wx)
        level = dot(dense[q], sl[...])
        levels.append(level[:, 0:1] + level[:, 1:2] + level[:, 2:3])
    hiddens = []
    for q in range(CHUNKS):
        gathers[q].step(3)
        if q == CHUNKS - 1:
            for ring in shared_out:
                ring.step(1)
        at = spans[q]
        chips(3, 1, tot, xx, at, wx)
        chips(NY - 3, 1, tot, xx, at, wx)
        both = tot[at, :] * levels[q]
        hh[at, chip] = (jax.nn.silu(both[:, 0:256]) * both[:, 256:512]).astype(BF16)
        hiddens.append(Ring(hh, sources * used[0] * q, sources * used[q], sems, 2 + q, pair=True))
        hiddens[-1].start()
    for side in range(2):
        for k in range(3):
            halo(side, k).wait_send()
    all_rows(NX - 1).wait_send()
    all_columns().wait_send()
    all_tiles(ft, 4).wait_send()
    all_tiles(sq, 6).wait_send()
    for sent in (8, 9):
        either(
            side_of == core,
            lambda: some_rows(dd, 0, SP - 1, sent, one.at[20]).wait_send(),
            lambda: some_rows(dd, 0, SP, sent, one.at[20]).wait_send(),
        )

    @pl.when(side_of == core)
    def _():
        some_rows(dd, 0, SP - 1, 14, one.at[20]).wait_send()

    to_other(wx.at[:, pl.ds(0, 384)], 12).wait_send()
    to_other(wc.at[:, pl.ds(0, 384)], 18).wait_send()
    for ring in spread_out + gathers:
        ring.drain()
    low[...] = jnp.zeros(low.shape, F32)
    for step in (1, 2, 3):
        for ring in hiddens:
            ring.step(step)
        if step == 3:
            for ring in shared_out:
                ring.step(2)
        for q in range(CHUNKS):
            at = spans[q]
            if step == 1:
                chips(NY, 1, low, hh, at, wl)
            chips(step, 1, low, hh, at, wl)
            chips(NY - step, 1, low, hh, at, wl)
    loose = [
        one_hot(
            (sources * PIECE, sources * used[q]),
            lambda row, col: col // used[q] * PIECE + col % used[q] == row,
        )
        for q in range(CHUNKS)
    ]

    def give(i, to_core, q):
        return pltpu.make_async_remote_copy(
            src_ref=oo.at[q, pl.ds(pl.multiple_of(i * PIECE, PIECE), PIECE), lanes_of(to_core)],
            dst_ref=ret.at[piece_of(sp, q)],
            send_sem=one.at[10],
            recv_sem=one.at[11],
            device_id=(((i % 4) * 2 + core) * NX + i // 4 % 2 * 2 + i // 8, y * 2 + to_core),
            device_id_type=MESH,
        )

    for q in range(CHUNKS):
        hiddens[q].step(4)
        at = spans[q]
        chips(NY // 2, 1, low, hh, at, wl)
        oo[q] = dot(loose[q], low[at, :].astype(BF16)).astype(BF16)

        def send_back(k, carry):
            turn = k // 4
            i = k % 4 * 4 + (z // 2 + 6 + (turn // 2 + turn % 2) * (1 - 2 * (turn % 2))) % 4
            here = jnp.logical_and(side_of == core, i == local)

            @pl.when(jnp.logical_not(here))
            def _():
                give(i, core, q).start()

            give(i, 1 - core, q).start()
            return carry

        lax.fori_loop(0, sources, send_back, 0)

    @pl.when(side_of == core)
    def _():
        for q in range(CHUNKS):
            ret[piece_of(sp, q), :] = oo[q, landing, lanes_of(core)]

    for step in (3, 4):
        for ring in shared_out:
            ring.step(step)
    lowered = dot(sh[rows, :], wcl[...]).astype(BF16)
    outs[0] = lowered[:, 0:128]
    outs[1] = lowered[:, 128:256]

    def output(source):
        return pltpu.make_async_remote_copy(
            src_ref=outs.at[source],
            dst_ref=theirs,
            send_sem=one.at[16],
            recv_sem=one.at[17],
            device_id=(sp, y * 2 + 1 - core),
            device_id_type=MESH,
        )

    output(1 - core).start()
    for ring in hiddens + shared_out:
        ring.drain()
    either(
        side_of == core,
        lambda: some_rows(ret, 0, SP - 1, 10, one.at[11]).wait_recv(),
        lambda: some_rows(ret, 0, SP, 10, one.at[11]).wait_recv(),
    )
    either(
        side_of == core,
        lambda: some_rows(ret, 0, SP - 1, 10, one.at[11]).wait_send(),
        lambda: some_rows(ret, 0, SP, 10, one.at[11]).wait_send(),
    )
    routed = dot(qhi[...], ret[...]) + dot(qlo[...], ret[...])
    output(1 - core).wait()
    ours, others = outs[core].astype(F32), theirs[...].astype(F32)
    shared = jnp.concatenate(
        [jnp.where(core == 0, ours, others), jnp.where(core == 0, others, ours)], axis=0
    )
    out_ref[...] = (am[...].astype(F32) + shared + routed).astype(BF16)


def whole(*operands):
    vmem = pl.BlockSpec(memory_space=pltpu.VMEM)
    hbm = pl.BlockSpec(memory_space=pl.ANY)
    rings = 7 + SPLITS
    dma = pltpu.SemaphoreType.DMA

    def space(*shape, kind=BF16):
        return pltpu.VMEM(shape, kind)

    return pl.pallas_call(
        kernel,
        out_shape=jax.ShapeDtypeStruct((T, 128), BF16),
        in_specs=[hbm] * 24,
        out_specs=vmem,
        scratch_shapes=[
            (pltpu.VMEM if o.ndim > 1 else pltpu.SMEM)(o.shape, o.dtype) for o in operands[:15]
        ]
        + [
            space(64, 384),
            space(T, 128),
            space(T, 128),
            space(2, 64, 128),
            space(2, 16, 128),
            space(2, 16, 128),
            space(T + 32, 128, kind=F32),
            space(T + 32, 128, kind=F32),
            space(T, T, kind=F32),
            space(8, T, kind=F32),
            space(2, T, 128),
            space(8, 128, kind=F32),
            space(2, BLOCK, 128),
            space(NX, 2, BLOCK, 128),
            space(2, BLOCK, 128),
            space(NZ, BLOCK, 128),
            space(TP, 8, 128, kind=F32),
            space(TP, 8, 128, kind=F32),
            space(8, 128, kind=F32),
            space(1024, 128),
            space(D, 512),
            space(D, 512),
            space(D, 256),
            space(D, 256),
            space(D, 256),
            space(HALF, D),
            space(HALF, D),
            space(T, 128),
            space(T, D),
            space(T, D),
            space(2, ROWS // 4, 256),
            space(ROWS // 2, 256),
            space(SP // 2 * CAP, D),
            space(SP // 2 * CAP, D),
            space(SP // 2 * CAP, 512, kind=F32),
            space(SP // 2 * CAP, 256, kind=F32),
            space(ROWS, 128),
            space(ROWS, 128),
            space(ROWS, 128),
            space(ROWS // 2, 128),
            space(2, HALF, 128),
            space(HALF, 128),
            space(2, ROWS // 4, 256),
            space(ROWS, 128),
            space(ROWS, T),
            space(T, ROWS),
            space(T, ROWS),
            dma((15,)), dma((9,)), dma((6,)), dma((6,)), dma((21,)), dma((CHUNKS + 1,)), dma((rings, 2)), dma((rings, 8)),
        ],
        compiler_params=pltpu.CompilerParams(collective_id=0, has_side_effects=True),
        name="mixer_experts",
    )(*operands)


def shards(
    layer_source_vector,
    attention_lane_source,
    result_valve_logits,
    memory_write_matrix,
    memory_query_matrix,
    increment_logits,
    increment_offset,
    log_fade_speed,
    extra_log_fade,
    attention_bypass_factor,
    attention_lane_kernel,
    memory_write_kernel,
    memory_query_kernel,
    cluster_rescale_factor,
    blender_result_matrix,
    specialist_rescale_factor,
    chosen_specialists,
    specialist_shares,
    specialist_valve_matrix,
    specialist_raising_matrix,
    specialist_lowering_matrix,
    common_valve_matrix,
    common_raising_matrix,
    common_lowering_matrix,
):
    return whole(
        attention_lane_source.T,
        result_valve_logits.T,
        increment_logits.reshape(2, T),
        increment_offset.T,
        log_fade_speed.T,
        extra_log_fade.reshape(2, 1, T),
        attention_bypass_factor,
        attention_lane_kernel,
        memory_write_kernel,
        memory_query_kernel,
        cluster_rescale_factor.reshape(1, 64),
        specialist_rescale_factor.reshape(1, 128),
        layer_source_vector,
        chosen_specialists.T,
        specialist_shares.T,
        memory_write_matrix,
        memory_query_matrix,
        blender_result_matrix,
        specialist_valve_matrix,
        specialist_raising_matrix,
        specialist_lowering_matrix,
        common_valve_matrix,
        common_raising_matrix,
        common_lowering_matrix,
    )


def solution(mesh):
    return jax.shard_map(
        shards,
        mesh=mesh,
        in_specs=(
            P("sp", "tp"),
            P("sp", "tp"),
            P("sp", "tp"),
            P("sp", None),
            P("sp", None),
            P(None, "sp", "tp"),
            P(None, "tp"),
            P(None, "tp"),
            P(None, "sp", "tp"),
            P("tp"),
            P(None, "tp"),
            P(),
            P(),
            P("tp"),
            P(None, "tp"),
            P("tp"),
            P("sp", None),
            P("sp", None),
            P("sp", None, "tp"),
            P("sp", None, "tp"),
            P("sp", None, "tp"),
            P(None, "tp"),
            P(None, "tp"),
            P(None, "tp"),
        ),
        out_specs=P("sp", "tp"),
        check_vma=False,
    )
```

```python
import jax
import jax.numpy as jnp
from jax import lax
from jax.experimental import pallas as pl
from jax.experimental.pallas import tpu as pltpu
from jax.sharding import PartitionSpec as P

D = 2048
HEADS = 16
HEAD_DIM = 64
GROUPS = 4
STATE = 128
CONV = 5

NZ, NX, NY = 8, 4, 8
SP, TP = NZ * NX, NY * 2
T = 320
HALF = T // 2
SLOTS = 32
ROWS = SP * SLOTS
CAP = 30
SPLITS = 4
BLOCK = 80
CHUNKS = 2
PIECE = SLOTS // CHUNKS
MESH = pl.DeviceIdType.MESH
F32, BF16 = jnp.float32, jnp.bfloat16


def dot(a, b):
    return jnp.dot(a, b, preferred_element_type=F32)


class Ring:
    def __init__(self, buf, first, rows, sems, index, direct=False, pair=False, last=4):
        self.buf, self.first, self.rows = buf, first, rows
        self.direct, self.pair, self.last = direct, pair, last
        self.out, self.near = sems[0].at[index, 0], sems[0].at[index, 1]
        self.recv = sems[1].at[index]
        self.sp, tp = lax.axis_index("sp"), lax.axis_index("tp")
        self.y, self.core = tp // 2, tp % 2

    def part(self, chip, core, half=None):
        column, width = ((chip + 2 * NY) % NY) * 2, 128
        if self.pair:
            width = 256
        else:
            column = column + core
        first, rows = self.first, self.rows
        if half is not None:
            cut = (rows // 2 + 15) // 16 * 16
            first, rows = (first, cut) if half == 0 else (first + cut, rows - cut)
        return self.buf.at[pl.ds(first, rows), pl.ds(pl.multiple_of(column * 128, 128), width)]

    def along(self, way, step, chip, far):
        turn = 1 - 2 * way
        block = self.part(chip, self.core, way if step == 4 else None)
        return pltpu.make_async_remote_copy(
            src_ref=block,
            dst_ref=block,
            send_sem=self.out,
            recv_sem=self.recv.at[4 * way + step - 1],
            device_id=(self.sp, ((self.y + turn * far + NY) % NY) * 2 + self.core),
            device_id_type=MESH,
        )

    def hop(self, way, step):
        if self.direct:
            return self.along(way, step, self.y, step)
        return self.along(way, step, self.y - (1 - 2 * way) * (step - 1), 1)

    def landed(self, way, step):
        return self.along(way, step, self.y - (1 - 2 * way) * step, 1)

    def relay(self, way, step):
        turn = 1 - 2 * way
        return self.over(self.part(self.y - turn * step, self.core, way if step == 4 else None))

    def over(self, block):
        return pltpu.make_async_remote_copy(
            src_ref=block,
            dst_ref=block,
            send_sem=self.out,
            recv_sem=self.near,
            device_id=(self.sp, self.y * 2 + 1 - self.core),
            device_id_type=MESH,
        )

    def several(self, blocks):
        return self.over(self.buf.at[pl.ds(self.first, self.rows), pl.ds(0, 128 * blocks)])

    def start(self):
        for step in (4, 3, 2, 1) if self.direct else (1,):
            self.hop(0, step).start()
            self.hop(1, step).start()
        if not self.pair:
            self.relay(0, 0).start()

    def step(self, step):
        for way in (0, 1):
            self.landed(way, step).wait_recv()
            if step < self.last and not self.direct:
                self.hop(way, step + 1).start()
            if not self.pair:
                self.relay(way, step).start()

    def finish(self):
        self.several(NY).wait_recv()

    def drain(self):
        self.several(2 * NY - (1 if not self.pair else 2 if self.last == 4 else 4)).wait_send()


def stacked(rows):
    level = lax.broadcasted_iota(jnp.int32, (8, rows[0].shape[1]), 0)
    total = jnp.zeros(level.shape, F32)
    for k, row in enumerate(rows):
        total = jnp.where(level == k, row, total)
    return total


def three(v):
    high = v.astype(BF16).astype(F32)
    middle = (v - high).astype(BF16).astype(F32)
    return [high, middle, v - high - middle]


def one_hot(shape, test):
    row, col = lax.broadcasted_iota(jnp.int32, shape, 0), lax.broadcasted_iota(jnp.int32, shape, 1)
    return jnp.where(test(row, col), 1.0, 0.0).astype(BF16)


def across(a, b):
    return lax.dot_general(a, b, (((1,), (1,)), ((), ())), preferred_element_type=F32)


def log1p(u):
    series = u * (1 - u * (1 / 2 - u * (1 / 3 - u * (1 / 4 - u * (1 / 5 - u / 6)))))
    return jnp.where(u < 0.03, series, jnp.log(1 + u))


def silu(v):
    return v / (1 + jnp.exp(-v))


def kernel(
    xt_hbm, zt_hbm, inc_hbm, off_hbm, spd_hbm, fade_hbm, byp_hbm, xk_hbm,
    bk_hbm, ck_hbm, gain_hbm, after_hbm, src_hbm, cht_hbm, sht_hbm,
    bm_hbm, cm_hbm, blender_hbm, valve_hbm, raising_hbm, lowering_hbm, cvalve_hbm, craising_hbm, clowering_hbm,
    out_ref,
    xt_ref, zt_ref, inc_ref, off_ref, spd_ref, fade_ref, byp_ref, xk_ref,
    bk_ref, ck_ref, gain_ref, after_ref, src_ref, cht_ref, sht_ref,
    xpad, braw, craw, hx, hb, hc, bext, cext, gap, cv, mixed, fto,
    st_ref, rx, tb, rz, ft, sq, so, wb, wx, wc, wl, wcl, wide, bn, nn, am, ff, sh, xl, x2, xx, hh, tot, low, dd, d2, ss, sl, outs, theirs, oo, ret, pp, qhi, qlo,
    isem, wsem, hs, hr, one, dr, rsem, rrecv,
):
    sp, tp = lax.axis_index("sp"), lax.axis_index("tp")
    z, x = sp // NX, sp % NX
    y, core, side_of = tp // 2, tp % 2, z % 2

    barrier = pltpu.get_barrier_semaphore()

    def greet_tp(k, carry):
        pl.semaphore_signal(barrier, inc=1, device_id=(sp, (tp + k) % TP), device_id_type=MESH)
        return carry

    def greet_z(k, carry):
        pl.semaphore_signal(
            barrier, inc=1, device_id=((z + k) % NZ * NX + x, tp), device_id_type=MESH
        )
        return carry

    def greet_x(k, carry):
        pl.semaphore_signal(
            barrier, inc=1, device_id=(z * NX + (x + k) % NX, tp), device_id_type=MESH
        )
        return carry

    def greet_next(k, carry):
        pl.semaphore_signal(
            barrier, inc=1, device_id=((sp + k * (SP - 2) + 1) % SP, tp), device_id_type=MESH
        )
        return carry

    lax.fori_loop(1, TP, greet_tp, 0)
    lax.fori_loop(1, NZ, greet_z, 0)
    lax.fori_loop(1, NX, greet_x, 0)
    lax.fori_loop(0, 2, greet_next, 0)

    def lanes_of(i):
        return pl.ds(pl.multiple_of(i * 128, 128), 128)

    at_group = pl.ds(pl.multiple_of((tp // 4) * 128, 128), 128)
    loads = [
        pltpu.make_async_copy(blender_hbm, wb, wsem.at[0]),
        pltpu.make_async_copy(valve_hbm.at[0], wx.at[:, lanes_of(core)], wsem.at[1]),
        pltpu.make_async_copy(raising_hbm.at[0], wx.at[:, lanes_of(core + 2)], wsem.at[2]),
        pltpu.make_async_copy(lowering_hbm.at[0], wl.at[:, lanes_of(core)], wsem.at[3]),
        pltpu.make_async_copy(cvalve_hbm, wc.at[:, lanes_of(core)], wsem.at[4]),
        pltpu.make_async_copy(craising_hbm, wc.at[:, lanes_of(core + 2)], wsem.at[5]),
        pltpu.make_async_copy(clowering_hbm, wcl.at[:, lanes_of(core)], wsem.at[6]),
    ]
    grouped = [
        pltpu.make_async_copy(bm_hbm.at[:, at_group], braw, wsem.at[7]),
        pltpu.make_async_copy(cm_hbm.at[:, at_group], craw, wsem.at[8]),
    ]
    small = [
        pltpu.make_async_copy(there, here, isem.at[k])
        for k, (there, here) in enumerate(
            (
                (xt_hbm, xt_ref),
                (zt_hbm, zt_ref),
                (inc_hbm, inc_ref),
                (off_hbm, off_ref),
                (spd_hbm, spd_ref),
                (fade_hbm, fade_ref),
                (byp_hbm, byp_ref),
                (xk_hbm, xk_ref),
                (bk_hbm, bk_ref),
                (ck_hbm, ck_ref),
                (gain_hbm, gain_ref),
                (after_hbm, after_ref),
                (src_hbm, src_ref),
                (cht_hbm, cht_ref),
                (sht_hbm, sht_ref),
            )
        )
    ]
    for load in small + grouped + loads:
        load.start()
    for load in small:
        load.wait()

    xpad[...] = jnp.zeros(xpad.shape, BF16)
    xpad[:, 0:T] = xt_ref[...]
    gains = jnp.concatenate([gain_ref[...], gain_ref[...]], axis=1)
    fto[...] = jnp.broadcast_to(gains, (8, 128))
    ft[tp] = fto[...]

    def state_row(k, source):
        return pltpu.make_async_remote_copy(
            src_ref=st_ref,
            dst_ref=rx.at[source],
            send_sem=one.at[0],
            recv_sem=one.at[1],
            device_id=(z * NX + (x + k) % NX, tp),
            device_id_type=MESH,
        )

    def tile(k, source):
        return pltpu.make_async_remote_copy(
            src_ref=fto,
            dst_ref=ft.at[source],
            send_sem=one.at[4],
            recv_sem=one.at[5],
            device_id=(sp, (tp + k) % TP),
            device_id_type=MESH,
        )

    def send_tile(k, carry):
        tile(k, tp).start()
        return carry

    for load in grouped:
        load.wait()
    pl.semaphore_wait(barrier, TP - 1 + NZ - 1 + NX - 1 + 2)

    def halo(side, k):
        there = (sp + 1) % SP if side == 0 else (sp + SP - 1) % SP
        rows = pl.ds(T - 16, 16) if side == 0 else pl.ds(0, 16)
        lanes = pl.ds(256, 128) if side == 0 else pl.ds(0, 128)
        source = (xpad.at[:, lanes], braw.at[rows], craw.at[rows])[k]
        return pltpu.make_async_remote_copy(
            src_ref=source,
            dst_ref=(hx, hb, hc)[k].at[side],
            send_sem=hs.at[3 * side + k],
            recv_sem=hr.at[3 * side + k],
            device_id=(there, tp),
            device_id_type=MESH,
        )

    for k in range(3):
        halo(0, k).start()
        halo(1, k).start()
    lax.fori_loop(1, TP, send_tile, 0)

    lower = one_hot((T, T), lambda row, col: col < row)
    upper = one_hot((T, T), lambda row, col: row < col)
    same = one_hot((T, T), lambda row, col: row == col)
    experts = lax.broadcasted_iota(jnp.int32, (SP, T), 0)
    first, second = cht_ref[0:1, :] == experts, cht_ref[1:2, :] == experts
    named = jnp.where(first | second, 1.0, 0.0)
    rank = dot(named.astype(BF16), upper)
    rank = jnp.where(named > 0, rank, 99.0).astype(BF16)
    spread = one_hot((ROWS, SP), lambda row, col: row // SLOTS == col)
    place = (lax.broadcasted_iota(jnp.int32, (ROWS, T), 0) % SLOTS).astype(F32)
    pp[...] = jnp.where(dot(spread, rank) == place, 1.0, 0.0).astype(BF16)
    shares = jnp.where(first, sht_ref[0:1, :], 0.0) + jnp.where(second, sht_ref[1:2, :], 0.0)
    share_hi = shares.astype(BF16)
    share_lo = (shares - share_hi.astype(F32)).astype(BF16)
    spread = one_hot((SP, ROWS), lambda row, col: col // SLOTS == row)
    place = (lax.broadcasted_iota(jnp.int32, (T, ROWS), 1) % SLOTS).astype(F32)
    here = dot(across(same, rank).astype(BF16), spread) == place
    qhi[...] = jnp.where(here, dot(across(same, share_hi).astype(BF16), spread), 0.0).astype(BF16)
    qlo[...] = jnp.where(here, dot(across(same, share_lo).astype(BF16), spread), 0.0).astype(BF16)

    steps, fades = [], []
    for d in range(2):
        v = inc_ref[d : d + 1, :].astype(F32) + off_ref[0:1, d : d + 1]
        step = jnp.maximum(v, 0.0) + log1p(jnp.exp(-jnp.abs(v)))
        steps.append(step)
        fades.append(-jnp.exp(spd_ref[0:1, d : d + 1]) * step + fade_ref[d])
    parts = stacked(three(fades[0]) + three(fades[1])).astype(BF16)
    along = dot(parts, upper + same)
    forward_row = along[0:1] + along[1:2] + along[2:3]
    along = dot(parts, upper)
    backward_row = along[3:4] + along[4:5] + along[5:6]
    along = across(lower + same, parts)
    forward_col = along[:, 0:1] + along[:, 1:2] + along[:, 2:3]
    along = across(lower, parts)
    backward_col = along[:, 3:4] + along[:, 4:5] + along[:, 5:6]
    row = lax.broadcasted_iota(jnp.int32, (T, T), 0)
    col = lax.broadcasted_iota(jnp.int32, (T, T), 1)
    gap[...] = (
        jnp.where(row >= col, jnp.exp(forward_col - forward_row), 0.0) * steps[0]
        + jnp.where(row <= col, jnp.exp(backward_row - backward_col), 0.0) * steps[1]
    )
    forward_end = forward_row[:, T - 1 : T]
    backward_end = backward_row[:, T - 1 : T] + fades[1][:, T - 1 : T]
    weigh = [jnp.exp(forward_end - forward_row) * steps[0], jnp.exp(backward_row) * steps[1]]
    seen = [jnp.exp(forward_row), jnp.exp(backward_end - backward_row)]
    cv[...] = stacked(weigh + seen)
    ends = [jnp.broadcast_to(forward_end, (1, 128)), jnp.broadcast_to(backward_end, (1, 128))]

    def to_other(part, at):
        return pltpu.make_async_remote_copy(
            src_ref=part,
            dst_ref=part,
            send_sem=one.at[at],
            recv_sem=one.at[at + 1],
            device_id=(sp, y * 2 + 1 - core),
            device_id_type=MESH,
        )


    taps = across(same[0:64, 0:64], stacked([xk_ref[j : j + 1, :].astype(F32) for j in range(CONV)]).astype(BF16))
    lane = lax.broadcasted_iota(jnp.int32, (64, 128), 1)
    body = xpad[...].astype(F32)
    bext[pl.ds(16, T), :] = braw[...].astype(F32)
    cext[pl.ds(16, T), :] = craw[...].astype(F32)
    for k in range(3):
        halo(0, k).wait_recv()
        halo(1, k).wait_recv()
    before, behind = sp > 0, sp < SP - 1
    last = jnp.where(before, pltpu.roll(hx[0].astype(F32), 64, 1), 0.0)
    coming = jnp.where(behind, pltpu.roll(hx[1].astype(F32), 64, 1), 0.0)
    end = jnp.where(
        lane < 64, body[:, 256:384], jnp.where(lane < 66, coming, jnp.where(lane > 125, last, 0.0))
    )
    cells = jnp.concatenate([body[:, 0:256], end], axis=1)
    total = cells * taps[:, 2:3]
    for j in (0, 1, 3, 4):
        total = total + pltpu.roll(cells, (2 - j) % 384, 1) * taps[:, j : j + 1]
    x_conv = silu(total)[:, 0:T].astype(BF16)
    for ext, halos, kernel_ref in ((bext, hb, bk_ref), (cext, hc, ck_ref)):
        ext[pl.ds(0, 16), :] = jnp.where(before, halos[0].astype(F32), 0.0)
        ext[pl.ds(T + 16, 16), :] = jnp.where(behind, halos[1].astype(F32), 0.0)
        total = jnp.zeros((T, 128), F32)
        for j in range(CONV):
            tap = kernel_ref[j : j + 1, at_group].astype(F32)
            total = total + ext[pl.ds(14 + j, T), :] * tap
        mixed[0 if ext is bext else 1] = silu(total).astype(BF16)
    b_conv, c_conv = mixed[0], mixed[1]

    def packed(total, log):
        tail = jnp.concatenate([stacked(three(log)), jnp.zeros((8, 128), F32)], axis=0)
        return total.astype(BF16), tail.astype(BF16)

    x_wide = x_conv.astype(F32)
    for d in range(2):
        scaled = (cv[d : d + 1, :] * x_wide).astype(BF16)
        top, tail = packed(dot(scaled, b_conv), ends[d])
        st_ref[d, 0:64] = top
        st_ref[d, 64:80] = tail
    rx[x] = st_ref[...]
    for k in (2, 1, 3):
        state_row(k, x).start()
    inner = across(x_conv, (across(c_conv, b_conv) * gap[...]).astype(BF16))
    inner = inner + byp_ref[0] * x_wide
    gate = silu(zt_ref[...].astype(F32))

    def all_rows(k):
        return pltpu.make_async_remote_copy(
            src_ref=rx.at[pl.ds(0, k)],
            dst_ref=rx.at[pl.ds(0, k)],
            send_sem=one.at[0],
            recv_sem=one.at[1],
            device_id=(z * NX + (x + 1) % NX, tp),
            device_id_type=MESH,
        )

    all_rows(NX - 1).wait_recv()

    def state(block):
        return block[0:64].astype(F32)

    def log_of(block):
        logs = block[64:80].astype(F32)
        return logs[0:1] + logs[1:2] + logs[2:3]

    for way in (0, 1):
        total, log = jnp.zeros((64, 128), F32), jnp.zeros((1, 128), F32)
        for i in range(NX) if way == 0 else reversed(range(NX)):
            block = rx[i, way]
            own = log_of(block)
            total = jnp.exp(own) * total + state(block)
            log = log + own
        top, tail = packed(total, log)
        tb[way, 0:64] = top
        tb[way, 64:80] = tail
    rz[z] = tb[0]

    def state_column(k, source):
        return pltpu.make_async_remote_copy(
            src_ref=tb.at[(z + k) // NZ],
            dst_ref=rz.at[source],
            send_sem=one.at[2],
            recv_sem=one.at[3],
            device_id=(((z + k) % NZ) * NX + x, tp),
            device_id_type=MESH,
        )

    for k in (4, 3, 5, 2, 6, 1, 7):
        state_column(k, z).start()

    loads[0].wait()
    wide[...] = jnp.zeros(wide.shape, BF16)

    def widen(j, carry):
        block = wb[pl.ds(pl.multiple_of(j * 64, 64), 64), :]
        wide[pl.ds(pl.multiple_of(j * 128, 128), 64), pl.ds(0, 128)] = block
        wide[pl.ds(pl.multiple_of(j * 128 + 64, 64), 64), pl.ds(128, 128)] = block
        return carry

    lax.fori_loop(0, HEADS, widen, 0)

    def all_columns():
        return pltpu.make_async_remote_copy(
            src_ref=rz.at[pl.ds(0, NZ - 1)],
            dst_ref=rz.at[pl.ds(0, NZ - 1)],
            send_sem=one.at[2],
            recv_sem=one.at[3],
            device_id=(((z + 1) % NZ) * NX + x, tp),
            device_id_type=MESH,
        )

    all_columns().wait_recv()

    carried = []
    for way in (0, 1):
        total = jnp.zeros((64, 128), F32)
        for i in range(NZ) if way == 0 else reversed(range(NZ)):
            block = rz[i]
            passed = (i < z) if way == 0 else (i > z)
            total = jnp.where(passed, jnp.exp(log_of(block)) * total + state(block), total)
        for i in range(NX) if way == 0 else reversed(range(NX)):
            block = rx[i, way]
            passed = (i < x) if way == 0 else (i > x)
            total = jnp.where(passed, jnp.exp(log_of(block)) * total + state(block), total)
        carried.append(total.astype(BF16))

    mixer = inner + cv[2:3, :] * across(carried[0], mixed[1]) + cv[3:4, :] * across(carried[1], mixed[1])
    gated = (mixer * gate).astype(BF16)
    none = jnp.zeros((64, T), BF16)
    upper_half = one_hot((HALF, T), lambda row, col: row == col)
    lower_half = one_hot((HALF, T), lambda row, col: row + HALF == col)
    mine = pl.ds(pl.multiple_of(tp * 128, 128), 128)
    bn[:, mine] = (
        across(upper_half, jnp.concatenate([gated, none], axis=0))
        + across(lower_half, jnp.concatenate([none, gated], axis=0))
    ).astype(BF16)

    sems = (rsem, rrecv)
    ring = Ring(bn, 0, HALF, sems, 6 + SPLITS, direct=True)
    ring.start()

    def all_tiles(ref, at):
        return pltpu.make_async_remote_copy(
            src_ref=ref.at[pl.ds(0, TP - 1)],
            dst_ref=ref.at[pl.ds(0, TP - 1)],
            send_sem=one.at[at],
            recv_sem=one.at[at + 1],
            device_id=(sp, (tp + 1) % TP),
            device_id_type=MESH,
        )

    all_tiles(ft, 4).wait_recv()
    for step in (4, 3, 2, 1):
        ring.step(step)
    ring.finish()

    left = lax.broadcasted_iota(jnp.int32, (HALF, 128), 1) < 64
    for g in range(GROUPS):
        squares = jnp.zeros((HALF, 128), F32)
        for j in range(4 * g, 4 * g + 4):
            v = bn[:, 128 * j : 128 * j + 128].astype(F32)
            squares = squares + v * v
        top = jnp.sum(jnp.where(left, squares, 0.0), axis=1, keepdims=True)
        bottom = jnp.sum(jnp.where(left, 0.0, squares), axis=1, keepdims=True)
        scale = lax.rsqrt(jnp.where(left, top, bottom) / (4 * HEAD_DIM) + 1e-06)
        for j in range(4 * g, 4 * g + 4):
            v = bn[:, 128 * j : 128 * j + 128].astype(F32)
            nn[:, 128 * j : 128 * j + 128] = (v * scale * ft[j, 0:1]).astype(BF16)
    projected = dot(nn[...], wide[...])
    am[0:HALF] = (src_ref[0:HALF].astype(F32) + projected[:, 0:128]).astype(BF16)
    am[HALF:T] = (src_ref[HALF:T].astype(F32) + projected[:, 128:256]).astype(BF16)

    own = (am[...].astype(F32) * after_ref[...]).astype(BF16)
    ff[:, mine] = own
    cells = T // SPLITS
    spread_out = [Ring(ff, i * cells, cells, sems, 4 + i) for i in range(SPLITS)]
    for spreading in spread_out:
        spreading.start()
    dd[...] = dot(pp[...], own).astype(BF16)

    def rows_of(i):
        return pl.ds(pl.multiple_of(i * SLOTS, SLOTS), SLOTS)

    local = (x % 2) * 8 + (x // 2) * 4 + z // 2
    landing = pl.ds(pl.multiple_of(local * PIECE, PIECE), PIECE)

    def piece_of(i, q):
        return pl.ds(pl.multiple_of(i * SLOTS + q * PIECE, PIECE), PIECE)

    def deliver(k, q):
        target = (sp + k) % SP
        return pltpu.make_async_remote_copy(
            src_ref=dd.at[piece_of(target, q)],
            dst_ref=xl.at[q, landing, lanes_of(core)],
            send_sem=one.at[8],
            recv_sem=dr.at[q],
            device_id=(target, y * 2 + side_of),
            device_id_type=MESH,
        )

    def deliver_more(k):
        target = (sp + k) % SP
        return pltpu.make_async_remote_copy(
            src_ref=d2.at[rows_of(target)],
            dst_ref=x2.at[rows_of(local), lanes_of(core)],
            send_sem=one.at[9],
            recv_sem=dr.at[CHUNKS],
            device_id=(target, y * 2 + side_of),
            device_id_type=MESH,
        )

    def outward(m):
        return SP // 2 + (m // 2 + m % 2) * (1 - 2 * (m % 2))

    for q in range(CHUNKS):

        def send_rows(m, carry):
            deliver(outward(m), q).start()
            return carry

        lax.fori_loop(0, SP - 1, send_rows, 0)

        @pl.when(side_of != core)
        def _():
            deliver(0, q).start()

    @pl.when(side_of == core)
    def _():
        for q in range(CHUNKS):
            xl[q, landing, lanes_of(core)] = dd[piece_of(sp, q)]

    for k in (4, 5, 6):
        loads[k].wait()
    for part in (wc.at[:, lanes_of(core)], wc.at[:, lanes_of(core + 2)], wcl.at[:, lanes_of(core)]):
        to_other(part, 18).start()

    dims = (((1,), (1,)), ((), ()))
    squares = am[...].astype(F32) * am[...].astype(F32)
    high = squares.astype(BF16)
    rest = (squares - high.astype(F32)).astype(BF16)
    ones = jnp.ones((8, 128), BF16)
    sums = lax.dot_general(ones, high, dims, preferred_element_type=F32) + lax.dot_general(
        ones, rest, dims, preferred_element_type=F32
    )
    line = jnp.concatenate([sums, jnp.zeros((8, 3 * 128 - T), F32)], axis=1)
    level = lax.broadcasted_iota(jnp.int32, (8, 128), 0)
    own = jnp.where(
        level == 0,
        line[:, 0:128],
        jnp.where(level == 1, line[:, 128:256], jnp.where(level == 2, line[:, 256:384], 0.0)),
    )
    sq[tp] = own
    so[...] = own

    def sums_to(k, source):
        return pltpu.make_async_remote_copy(
            src_ref=so,
            dst_ref=sq.at[source],
            send_sem=one.at[6],
            recv_sem=one.at[7],
            device_id=(sp, (tp + k) % TP),
            device_id_type=MESH,
        )

    def send_sums(k, carry):
        sums_to((k + 7) % (TP - 1) + 1, tp).start()
        return carry

    lax.fori_loop(0, TP - 1, send_sums, 0)
    ring.drain()

    def some_rows(ref, first, blocks, sent, received, rows=SLOTS):
        part = ref.at[pl.ds(first, blocks * rows), pl.ds(0, 128)]
        return pltpu.make_async_remote_copy(
            src_ref=part,
            dst_ref=part,
            send_sem=one.at[sent],
            recv_sem=received,
            device_id=((sp + 1) % SP, tp),
            device_id_type=MESH,
        )

    def either(test, less, more):
        @pl.when(test)
        def _():
            less()

        @pl.when(jnp.logical_not(test))
        def _():
            more()

    for step in (1, 2):
        for ring in spread_out:
            ring.step(step)
    chip = pl.ds(pl.multiple_of(y * 256, 256), 256)
    used = [PIECE, CAP - PIECE]
    sources = SP // 2
    spans = [pl.ds(0, sources * used[0]), pl.ds(sources * used[0], sources * used[1])]
    dense = [
        one_hot(
            (sources * used[q], sources * SLOTS),
            lambda row, col: row // used[q] * SLOTS + row % used[q] + q * PIECE == col,
        )
        for q in range(CHUNKS)
    ]
    squeeze = one_hot(
        (sources * used[1], sources * PIECE),
        lambda row, col: row // used[1] * PIECE + row % used[1] == col,
    )
    gathers = []

    def gather(q):
        either(
            side_of == core,
            lambda: some_rows(dd, 0, SP - 1, 8, dr.at[q], PIECE).wait_recv(),
            lambda: some_rows(dd, 0, SP, 8, dr.at[q], PIECE).wait_recv(),
        )
        if used[q] == PIECE:
            xx[spans[q], chip] = xl[q]
        else:
            xx[spans[q], chip] = dot(squeeze, xl[q]).astype(BF16)
        ring = Ring(xx, sources * used[0] * q, sources * used[q], sems, q, pair=True, last=3)
        ring.start()
        gathers.append(ring)

    gather(0)
    all_tiles(sq, 6).wait_recv()
    total = sq[0]
    for j in range(1, TP):
        total = total + sq[j]
    line = jnp.concatenate([total[0:1], total[1:2], total[2:3]], axis=1)
    parts = stacked(three(line)).astype(BF16)
    same = one_hot((T, 384), lambda row, col: row == col)
    upright = across(same, parts)
    scale = lax.rsqrt((upright[:, 0:1] + upright[:, 1:2] + upright[:, 2:3]) / D + 1e-06)
    lane = lax.broadcasted_iota(jnp.int32, (T, 128), 1)
    parts = jnp.zeros((T, 128), F32)
    for k, part in enumerate(three(scale)):
        parts = jnp.where(lane == k, part, parts)
    ss[...] = dot(pp[...], parts.astype(BF16)).astype(BF16)

    def send_scale(m, carry):
        target = (sp + outward(m)) % SP
        pltpu.make_async_remote_copy(
            src_ref=ss.at[rows_of(target)],
            dst_ref=sl.at[rows_of(local)],
            send_sem=one.at[14],
            recv_sem=one.at[15],
            device_id=(target, tp),
            device_id_type=MESH,
        ).start()
        return carry

    @pl.when(side_of == core)
    def _():
        lax.fori_loop(0, SP - 1, send_scale, 0)
        sl[rows_of(local), :] = ss[rows_of(sp), :]

    gather(1)
    for k in (1, 2, 3):
        loads[k].wait()
    for part in (wx.at[:, lanes_of(core)], wx.at[:, lanes_of(core + 2)], wl.at[:, lanes_of(core)]):
        to_other(part, 12).start()
    for ring in spread_out:
        ring.step(3)
    for ring in gathers:
        ring.step(1)
    for ring in spread_out:
        ring.step(4)

    opposite = (y + NY // 2) % NY
    d2[...] = dot(pp[...], ff[:, lanes_of(opposite * 2 + core)]).astype(BF16)

    def send_more(m, carry):
        deliver_more(outward(m)).start()
        return carry

    lax.fori_loop(0, SP - 1, send_more, 0)

    @pl.when(side_of == core)
    def _():
        x2[rows_of(local), lanes_of(core)] = d2[rows_of(sp)]

    @pl.when(side_of != core)
    def _():
        deliver_more(0).start()

    for ring in spread_out:
        ring.finish()
    to_other(wc.at[:, pl.ds(0, 384)], 18).wait_recv()
    rows = pl.ds(pl.multiple_of(core * HALF, 16), HALF)
    both = dot(ff[rows, :], wc[...]) * jnp.where(core == 0, scale[0:HALF], scale[HALF:T])
    sh[rows, chip] = (jax.nn.silu(both[:, 0:256]) * both[:, 256:512]).astype(BF16)
    shared_out = [
        Ring(sh, pl.multiple_of(core * HALF + first, 16), count, sems, 4 + SPLITS + i, pair=True)
        for i, (first, count) in enumerate(((0, 96), (96, 64)))
    ]
    for ring in shared_out:
        ring.start()
    for ring in gathers:
        ring.step(2)

    def chips(first, count, total, buf, at, weight):
        def add(k, carry):
            part = pl.ds(pl.multiple_of((y + k) % NY * 256, 256), 256)
            total[at, :] += dot(buf[at, part], weight[part, :])
            return carry

        lax.fori_loop(first, first + count, add, 0)

    either(
        side_of == core,
        lambda: some_rows(sl, 0, SP // 2 - 1, 14, one.at[15]).wait_recv(),
        lambda: some_rows(sl, 0, SP // 2, 14, one.at[15]).wait_recv(),
    )
    to_other(wx.at[:, pl.ds(0, 384)], 12).wait_recv()
    tot[...] = jnp.zeros(tot.shape, F32)
    levels = []
    for q in range(CHUNKS):
        chips(NY - 2, NY - 3, tot, xx, spans[q], wx)
    either(
        side_of == core,
        lambda: some_rows(d2, 0, SP - 1, 9, dr.at[CHUNKS]).wait_recv(),
        lambda: some_rows(d2, 0, SP, 9, dr.at[CHUNKS]).wait_recv(),
    )
    turned = pl.ds(pl.multiple_of(opposite * 256, 256), 256)
    for q in range(CHUNKS):
        at = spans[q]
        xx[at, turned] = dot(dense[q], x2[...]).astype(BF16)
        chips(NY // 2, 1, tot, xx, at, wx)
        level = dot(dense[q], sl[...])
        levels.append(level[:, 0:1] + level[:, 1:2] + level[:, 2:3])
    hiddens = []
    for q in range(CHUNKS):
        gathers[q].step(3)
        if q == CHUNKS - 1:
            for ring in shared_out:
                ring.step(1)
        at = spans[q]
        chips(3, 1, tot, xx, at, wx)
        chips(NY - 3, 1, tot, xx, at, wx)
        both = tot[at, :] * levels[q]
        hh[at, chip] = (jax.nn.silu(both[:, 0:256]) * both[:, 256:512]).astype(BF16)
        hiddens.append(Ring(hh, sources * used[0] * q, sources * used[q], sems, 2 + q, pair=True))
        hiddens[-1].start()
    for side in range(2):
        for k in range(3):
            halo(side, k).wait_send()
    all_rows(NX - 1).wait_send()
    all_columns().wait_send()
    all_tiles(ft, 4).wait_send()
    all_tiles(sq, 6).wait_send()
    for sent in (8, 9):
        either(
            side_of == core,
            lambda: some_rows(dd, 0, SP - 1, sent, one.at[20]).wait_send(),
            lambda: some_rows(dd, 0, SP, sent, one.at[20]).wait_send(),
        )

    @pl.when(side_of == core)
    def _():
        some_rows(dd, 0, SP - 1, 14, one.at[20]).wait_send()

    to_other(wx.at[:, pl.ds(0, 384)], 12).wait_send()
    to_other(wc.at[:, pl.ds(0, 384)], 18).wait_send()
    for ring in spread_out + gathers:
        ring.drain()
    low[...] = jnp.zeros(low.shape, F32)
    for step in (1, 2, 3):
        for ring in hiddens:
            ring.step(step)
        if step == 3:
            for ring in shared_out:
                ring.step(2)
        for q in range(CHUNKS):
            at = spans[q]
            if step == 1:
                chips(NY, 1, low, hh, at, wl)
            chips(step, 1, low, hh, at, wl)
            chips(NY - step, 1, low, hh, at, wl)
    loose = [
        one_hot(
            (sources * PIECE, sources * used[q]),
            lambda row, col: col // used[q] * PIECE + col % used[q] == row,
        )
        for q in range(CHUNKS)
    ]

    def give(i, to_core, q):
        return pltpu.make_async_remote_copy(
            src_ref=oo.at[q, pl.ds(pl.multiple_of(i * PIECE, PIECE), PIECE), lanes_of(to_core)],
            dst_ref=ret.at[piece_of(sp, q)],
            send_sem=one.at[10],
            recv_sem=one.at[11],
            device_id=(((i % 4) * 2 + core) * NX + i // 4 % 2 * 2 + i // 8, y * 2 + to_core),
            device_id_type=MESH,
        )

    for q in range(CHUNKS):
        hiddens[q].step(4)
        at = spans[q]
        chips(NY // 2, 1, low, hh, at, wl)
        oo[q] = dot(loose[q], low[at, :].astype(BF16)).astype(BF16)

        def send_back(k, carry):
            turn = k // 4
            i = k % 4 * 4 + (z // 2 + 6 + (turn // 2 + turn % 2) * (1 - 2 * (turn % 2))) % 4
            here = jnp.logical_and(side_of == core, i == local)

            @pl.when(jnp.logical_not(here))
            def _():
                give(i, core, q).start()

            give(i, 1 - core, q).start()
            return carry

        lax.fori_loop(0, sources, send_back, 0)

    @pl.when(side_of == core)
    def _():
        for q in range(CHUNKS):
            ret[piece_of(sp, q), :] = oo[q, landing, lanes_of(core)]

    for step in (3, 4):
        for ring in shared_out:
            ring.step(step)
    lowered = dot(sh[rows, :], wcl[...]).astype(BF16)
    outs[0] = lowered[:, 0:128]
    outs[1] = lowered[:, 128:256]

    def output(source):
        return pltpu.make_async_remote_copy(
            src_ref=outs.at[source],
            dst_ref=theirs,
            send_sem=one.at[16],
            recv_sem=one.at[17],
            device_id=(sp, y * 2 + 1 - core),
            device_id_type=MESH,
        )

    output(1 - core).start()
    for ring in hiddens + shared_out:
        ring.drain()
    either(
        side_of == core,
        lambda: some_rows(ret, 0, SP - 1, 10, one.at[11]).wait_recv(),
        lambda: some_rows(ret, 0, SP, 10, one.at[11]).wait_recv(),
    )
    either(
        side_of == core,
        lambda: some_rows(ret, 0, SP - 1, 10, one.at[11]).wait_send(),
        lambda: some_rows(ret, 0, SP, 10, one.at[11]).wait_send(),
    )
    routed = dot(qhi[...], ret[...]) + dot(qlo[...], ret[...])
    output(1 - core).wait()
    ours, others = outs[core].astype(F32), theirs[...].astype(F32)
    shared = jnp.concatenate(
        [jnp.where(core == 0, ours, others), jnp.where(core == 0, others, ours)], axis=0
    )
    out_ref[...] = (am[...].astype(F32) + shared + routed).astype(BF16)


def whole(*operands):
    vmem = pl.BlockSpec(memory_space=pltpu.VMEM)
    hbm = pl.BlockSpec(memory_space=pl.ANY)
    rings = 7 + SPLITS
    dma = pltpu.SemaphoreType.DMA

    def space(*shape, kind=BF16):
        return pltpu.VMEM(shape, kind)

    return pl.pallas_call(
        kernel,
        out_shape=jax.ShapeDtypeStruct((T, 128), BF16),
        in_specs=[hbm] * 24,
        out_specs=vmem,
        scratch_shapes=[
            (pltpu.VMEM if o.ndim > 1 else pltpu.SMEM)(o.shape, o.dtype) for o in operands[:15]
        ]
        + [
            space(64, 384),
            space(T, 128),
            space(T, 128),
            space(2, 64, 128),
            space(2, 16, 128),
            space(2, 16, 128),
            space(T + 32, 128, kind=F32),
            space(T + 32, 128, kind=F32),
            space(T, T, kind=F32),
            space(8, T, kind=F32),
            space(2, T, 128),
            space(8, 128, kind=F32),
            space(2, BLOCK, 128),
            space(NX, 2, BLOCK, 128),
            space(2, BLOCK, 128),
            space(NZ, BLOCK, 128),
            space(TP, 8, 128, kind=F32),
            space(TP, 8, 128, kind=F32),
            space(8, 128, kind=F32),
            space(1024, 128),
            space(D, 512),
            space(D, 512),
            space(D, 256),
            space(D, 256),
            space(D, 256),
            space(HALF, D),
            space(HALF, D),
            space(T, 128),
            space(T, D),
            space(T, D),
            space(2, ROWS // 4, 256),
            space(ROWS // 2, 256),
            space(SP // 2 * CAP, D),
            space(SP // 2 * CAP, D),
            space(SP // 2 * CAP, 512, kind=F32),
            space(SP // 2 * CAP, 256, kind=F32),
            space(ROWS, 128),
            space(ROWS, 128),
            space(ROWS, 128),
            space(ROWS // 2, 128),
            space(2, HALF, 128),
            space(HALF, 128),
            space(2, ROWS // 4, 256),
            space(ROWS, 128),
            space(ROWS, T),
            space(T, ROWS),
            space(T, ROWS),
            dma((15,)), dma((9,)), dma((6,)), dma((6,)), dma((21,)), dma((CHUNKS + 1,)), dma((rings, 2)), dma((rings, 8)),
        ],
        compiler_params=pltpu.CompilerParams(collective_id=0, has_side_effects=True),
        name="mixer_experts",
    )(*operands)


def shards(
    layer_source_vector,
    attention_lane_source,
    result_valve_logits,
    memory_write_matrix,
    memory_query_matrix,
    increment_logits,
    increment_offset,
    log_fade_speed,
    extra_log_fade,
    attention_bypass_factor,
    attention_lane_kernel,
    memory_write_kernel,
    memory_query_kernel,
    cluster_rescale_factor,
    blender_result_matrix,
    specialist_rescale_factor,
    chosen_specialists,
    specialist_shares,
    specialist_valve_matrix,
    specialist_raising_matrix,
    specialist_lowering_matrix,
    common_valve_matrix,
    common_raising_matrix,
    common_lowering_matrix,
):
    return whole(
        attention_lane_source.T,
        result_valve_logits.T,
        increment_logits.reshape(2, T),
        increment_offset.T,
        log_fade_speed.T,
        extra_log_fade.reshape(2, 1, T),
        attention_bypass_factor,
        attention_lane_kernel,
        memory_write_kernel,
        memory_query_kernel,
        cluster_rescale_factor.reshape(1, 64),
        specialist_rescale_factor.reshape(1, 128),
        layer_source_vector,
        chosen_specialists.T,
        specialist_shares.T,
        memory_write_matrix,
        memory_query_matrix,
        blender_result_matrix,
        specialist_valve_matrix,
        specialist_raising_matrix,
        specialist_lowering_matrix,
        common_valve_matrix,
        common_raising_matrix,
        common_lowering_matrix,
    )


def solution(mesh):
    return jax.shard_map(
        shards,
        mesh=mesh,
        in_specs=(
            P("sp", "tp"),
            P("sp", "tp"),
            P("sp", "tp"),
            P("sp", None),
            P("sp", None),
            P(None, "sp", "tp"),
            P(None, "tp"),
            P(None, "tp"),
            P(None, "sp", "tp"),
            P("tp"),
            P(None, "tp"),
            P(),
            P(),
            P("tp"),
            P(None, "tp"),
            P("tp"),
            P("sp", None),
            P("sp", None),
            P("sp", None, "tp"),
            P("sp", None, "tp"),
            P("sp", None, "tp"),
            P(None, "tp"),
            P(None, "tp"),
            P(None, "tp"),
        ),
        out_specs=P("sp", "tp"),
        check_vma=False,
    )
```

```python
import jax
import jax.numpy as jnp
from jax import lax
from jax.experimental import pallas as pl
from jax.experimental.pallas import tpu as pltpu
from jax.sharding import PartitionSpec as P

D = 2048
HEADS = 16
HEAD_DIM = 64
GROUPS = 4
STATE = 128
CONV = 5

NZ, NX, NY = 8, 4, 8
SP, TP = NZ * NX, NY * 2
T = 320
HALF = T // 2
SLOTS = 32
ROWS = SP * SLOTS
CAP = 30
SPLITS = 4
BLOCK = 80
CHUNKS = 2
PIECE = SLOTS // CHUNKS
MESH = pl.DeviceIdType.MESH
F32, BF16 = jnp.float32, jnp.bfloat16


def dot(a, b):
    return jnp.dot(a, b, preferred_element_type=F32)


class Ring:
    def __init__(self, buf, first, rows, sems, index, direct=False, pair=False, last=4):
        self.buf, self.first, self.rows = buf, first, rows
        self.direct, self.pair, self.last = direct, pair, last
        self.out, self.near = sems[0].at[index, 0], sems[0].at[index, 1]
        self.recv = sems[1].at[index]
        self.sp, tp = lax.axis_index("sp"), lax.axis_index("tp")
        self.y, self.core = tp // 2, tp % 2

    def part(self, chip, core, half=None):
        column, width = ((chip + 2 * NY) % NY) * 2, 128
        if self.pair:
            width = 256
        else:
            column = column + core
        first, rows = self.first, self.rows
        if half is not None:
            cut = (rows // 2 + 15) // 16 * 16
            first, rows = (first, cut) if half == 0 else (first + cut, rows - cut)
        return self.buf.at[pl.ds(first, rows), pl.ds(pl.multiple_of(column * 128, 128), width)]

    def along(self, way, step, chip, far):
        turn = 1 - 2 * way
        block = self.part(chip, self.core, way if step == 4 else None)
        return pltpu.make_async_remote_copy(
            src_ref=block,
            dst_ref=block,
            send_sem=self.out,
            recv_sem=self.recv.at[4 * way + step - 1],
            device_id=(self.sp, ((self.y + turn * far + NY) % NY) * 2 + self.core),
            device_id_type=MESH,
        )

    def hop(self, way, step):
        if self.direct:
            return self.along(way, step, self.y, step)
        return self.along(way, step, self.y - (1 - 2 * way) * (step - 1), 1)

    def landed(self, way, step):
        return self.along(way, step, self.y - (1 - 2 * way) * step, 1)

    def relay(self, way, step):
        turn = 1 - 2 * way
        return self.over(self.part(self.y - turn * step, self.core, way if step == 4 else None))

    def over(self, block):
        return pltpu.make_async_remote_copy(
            src_ref=block,
            dst_ref=block,
            send_sem=self.out,
            recv_sem=self.near,
            device_id=(self.sp, self.y * 2 + 1 - self.core),
            device_id_type=MESH,
        )

    def several(self, blocks):
        return self.over(self.buf.at[pl.ds(self.first, self.rows), pl.ds(0, 128 * blocks)])

    def start(self):
        for step in (4, 3, 2, 1) if self.direct else (1,):
            self.hop(0, step).start()
            self.hop(1, step).start()
        if not self.pair:
            self.relay(0, 0).start()

    def step(self, step):
        for way in (0, 1):
            self.landed(way, step).wait_recv()
            if step < self.last and not self.direct:
                self.hop(way, step + 1).start()
            if not self.pair:
                self.relay(way, step).start()

    def finish(self):
        self.several(NY).wait_recv()

    def drain(self):
        self.several(2 * NY - (1 if not self.pair else 2 if self.last == 4 else 4)).wait_send()


def stacked(rows):
    level = lax.broadcasted_iota(jnp.int32, (8, rows[0].shape[1]), 0)
    total = jnp.zeros(level.shape, F32)
    for k, row in enumerate(rows):
        total = jnp.where(level == k, row, total)
    return total


def three(v):
    high = v.astype(BF16).astype(F32)
    middle = (v - high).astype(BF16).astype(F32)
    return [high, middle, v - high - middle]


def one_hot(shape, test):
    row, col = lax.broadcasted_iota(jnp.int32, shape, 0), lax.broadcasted_iota(jnp.int32, shape, 1)
    return jnp.where(test(row, col), 1.0, 0.0).astype(BF16)


def across(a, b):
    return lax.dot_general(a, b, (((1,), (1,)), ((), ())), preferred_element_type=F32)


def log1p(u):
    series = u * (1 - u * (1 / 2 - u * (1 / 3 - u * (1 / 4 - u * (1 / 5 - u / 6)))))
    return jnp.where(u < 0.03, series, jnp.log(1 + u))


def silu(v):
    return v / (1 + jnp.exp(-v))


def kernel(
    xt_hbm, zt_hbm, inc_hbm, off_hbm, spd_hbm, fade_hbm, byp_hbm, xk_hbm,
    bk_hbm, ck_hbm, gain_hbm, after_hbm, src_hbm, cht_hbm, sht_hbm,
    bm_hbm, cm_hbm, blender_hbm, valve_hbm, raising_hbm, lowering_hbm, cvalve_hbm, craising_hbm, clowering_hbm,
    out_ref,
    xt_ref, zt_ref, inc_ref, off_ref, spd_ref, fade_ref, byp_ref, xk_ref,
    bk_ref, ck_ref, gain_ref, after_ref, src_ref, cht_ref, sht_ref,
    xpad, braw, craw, hx, hb, hc, bext, cext, gap, cv, mixed, fto,
    st_ref, rx, tb, rz, ft, sq, so, wb, wx, wc, wl, wcl, wide, bn, nn, am, ff, sh, xl, x2, xx, hh, tot, low, dd, d2, ss, sl, outs, theirs, oo, ret, pp, qhi, qlo,
    isem, wsem, hs, hr, one, dr, rsem, rrecv,
):
    sp, tp = lax.axis_index("sp"), lax.axis_index("tp")
    z, x = sp // NX, sp % NX
    y, core, side_of = tp // 2, tp % 2, z % 2

    barrier = pltpu.get_barrier_semaphore()

    def greet_tp(k, carry):
        pl.semaphore_signal(barrier, inc=1, device_id=(sp, (tp + k) % TP), device_id_type=MESH)
        return carry

    def greet_z(k, carry):
        pl.semaphore_signal(
            barrier, inc=1, device_id=((z + k) % NZ * NX + x, tp), device_id_type=MESH
        )
        return carry

    def greet_x(k, carry):
        pl.semaphore_signal(
            barrier, inc=1, device_id=(z * NX + (x + k) % NX, tp), device_id_type=MESH
        )
        return carry

    def greet_next(k, carry):
        pl.semaphore_signal(
            barrier, inc=1, device_id=((sp + k * (SP - 2) + 1) % SP, tp), device_id_type=MESH
        )
        return carry

    lax.fori_loop(1, TP, greet_tp, 0)
    lax.fori_loop(1, NZ, greet_z, 0)
    lax.fori_loop(1, NX, greet_x, 0)
    lax.fori_loop(0, 2, greet_next, 0)

    def lanes_of(i):
        return pl.ds(pl.multiple_of(i * 128, 128), 128)

    at_group = pl.ds(pl.multiple_of((tp // 4) * 128, 128), 128)
    loads = [
        pltpu.make_async_copy(blender_hbm, wb, wsem.at[0]),
        pltpu.make_async_copy(valve_hbm.at[0], wx.at[:, lanes_of(core)], wsem.at[1]),
        pltpu.make_async_copy(raising_hbm.at[0], wx.at[:, lanes_of(core + 2)], wsem.at[2]),
        pltpu.make_async_copy(lowering_hbm.at[0], wl.at[:, lanes_of(core)], wsem.at[3]),
        pltpu.make_async_copy(cvalve_hbm, wc.at[:, lanes_of(core)], wsem.at[4]),
        pltpu.make_async_copy(craising_hbm, wc.at[:, lanes_of(core + 2)], wsem.at[5]),
        pltpu.make_async_copy(clowering_hbm, wcl.at[:, lanes_of(core)], wsem.at[6]),
    ]
    grouped = [
        pltpu.make_async_copy(bm_hbm.at[:, at_group], braw, wsem.at[7]),
        pltpu.make_async_copy(cm_hbm.at[:, at_group], craw, wsem.at[8]),
    ]
    small = [
        pltpu.make_async_copy(there, here, isem.at[k])
        for k, (there, here) in enumerate(
            (
                (xt_hbm, xt_ref),
                (zt_hbm, zt_ref),
                (inc_hbm, inc_ref),
                (off_hbm, off_ref),
                (spd_hbm, spd_ref),
                (fade_hbm, fade_ref),
                (byp_hbm, byp_ref),
                (xk_hbm, xk_ref),
                (bk_hbm, bk_ref),
                (ck_hbm, ck_ref),
                (gain_hbm, gain_ref),
                (after_hbm, after_ref),
                (src_hbm, src_ref),
                (cht_hbm, cht_ref),
                (sht_hbm, sht_ref),
            )
        )
    ]
    for load in small + grouped + loads:
        load.start()
    for load in small:
        load.wait()

    xpad[...] = jnp.zeros(xpad.shape, BF16)
    xpad[:, 0:T] = xt_ref[...]
    gains = jnp.concatenate([gain_ref[...], gain_ref[...]], axis=1)
    fto[...] = jnp.broadcast_to(gains, (8, 128))
    ft[tp] = fto[...]

    def state_row(k, source):
        return pltpu.make_async_remote_copy(
            src_ref=st_ref,
            dst_ref=rx.at[source],
            send_sem=one.at[0],
            recv_sem=one.at[1],
            device_id=(z * NX + (x + k) % NX, tp),
            device_id_type=MESH,
        )

    def tile(k, source):
        return pltpu.make_async_remote_copy(
            src_ref=fto,
            dst_ref=ft.at[source],
            send_sem=one.at[4],
            recv_sem=one.at[5],
            device_id=(sp, (tp + k) % TP),
            device_id_type=MESH,
        )

    def send_tile(k, carry):
        tile(k, tp).start()
        return carry

    for load in grouped:
        load.wait()
    pl.semaphore_wait(barrier, TP - 1 + NZ - 1 + NX - 1 + 2)

    def halo(side, k):
        there = (sp + 1) % SP if side == 0 else (sp + SP - 1) % SP
        rows = pl.ds(T - 16, 16) if side == 0 else pl.ds(0, 16)
        lanes = pl.ds(256, 128) if side == 0 else pl.ds(0, 128)
        source = (xpad.at[:, lanes], braw.at[rows], craw.at[rows])[k]
        return pltpu.make_async_remote_copy(
            src_ref=source,
            dst_ref=(hx, hb, hc)[k].at[side],
            send_sem=hs.at[3 * side + k],
            recv_sem=hr.at[3 * side + k],
            device_id=(there, tp),
            device_id_type=MESH,
        )

    for k in range(3):
        halo(0, k).start()
        halo(1, k).start()
    lax.fori_loop(1, TP, send_tile, 0)

    lower = one_hot((T, T), lambda row, col: col < row)
    upper = one_hot((T, T), lambda row, col: row < col)
    same = one_hot((T, T), lambda row, col: row == col)
    experts = lax.broadcasted_iota(jnp.int32, (SP, T), 0)
    first, second = cht_ref[0:1, :] == experts, cht_ref[1:2, :] == experts
    named = jnp.where(first | second, 1.0, 0.0)
    rank = dot(named.astype(BF16), upper)
    rank = jnp.where(named > 0, rank, 99.0).astype(BF16)
    spread = one_hot((ROWS, SP), lambda row, col: row // SLOTS == col)
    place = (lax.broadcasted_iota(jnp.int32, (ROWS, T), 0) % SLOTS).astype(F32)
    pp[...] = jnp.where(dot(spread, rank) == place, 1.0, 0.0).astype(BF16)
    shares = jnp.where(first, sht_ref[0:1, :], 0.0) + jnp.where(second, sht_ref[1:2, :], 0.0)
    share_hi = shares.astype(BF16)
    share_lo = (shares - share_hi.astype(F32)).astype(BF16)
    spread = one_hot((SP, ROWS), lambda row, col: col // SLOTS == row)
    place = (lax.broadcasted_iota(jnp.int32, (T, ROWS), 1) % SLOTS).astype(F32)
    here = dot(across(same, rank).astype(BF16), spread) == place
    qhi[...] = jnp.where(here, dot(across(same, share_hi).astype(BF16), spread), 0.0).astype(BF16)
    qlo[...] = jnp.where(here, dot(across(same, share_lo).astype(BF16), spread), 0.0).astype(BF16)

    steps, fades = [], []
    for d in range(2):
        v = inc_ref[d : d + 1, :].astype(F32) + off_ref[0:1, d : d + 1]
        step = jnp.maximum(v, 0.0) + log1p(jnp.exp(-jnp.abs(v)))
        steps.append(step)
        fades.append(-jnp.exp(spd_ref[0:1, d : d + 1]) * step + fade_ref[d])
    parts = stacked(three(fades[0]) + three(fades[1])).astype(BF16)
    along = dot(parts, upper + same)
    forward_row = along[0:1] + along[1:2] + along[2:3]
    along = dot(parts, upper)
    backward_row = along[3:4] + along[4:5] + along[5:6]
    along = across(lower + same, parts)
    forward_col = along[:, 0:1] + along[:, 1:2] + along[:, 2:3]
    along = across(lower, parts)
    backward_col = along[:, 3:4] + along[:, 4:5] + along[:, 5:6]
    row = lax.broadcasted_iota(jnp.int32, (T, T), 0)
    col = lax.broadcasted_iota(jnp.int32, (T, T), 1)
    gap[...] = (
        jnp.where(row >= col, jnp.exp(forward_col - forward_row), 0.0) * steps[0]
        + jnp.where(row <= col, jnp.exp(backward_row - backward_col), 0.0) * steps[1]
    )
    forward_end = forward_row[:, T - 1 : T]
    backward_end = backward_row[:, T - 1 : T] + fades[1][:, T - 1 : T]
    weigh = [jnp.exp(forward_end - forward_row) * steps[0], jnp.exp(backward_row) * steps[1]]
    seen = [jnp.exp(forward_row), jnp.exp(backward_end - backward_row)]
    cv[...] = stacked(weigh + seen)
    ends = [jnp.broadcast_to(forward_end, (1, 128)), jnp.broadcast_to(backward_end, (1, 128))]

    def to_other(part, at):
        return pltpu.make_async_remote_copy(
            src_ref=part,
            dst_ref=part,
            send_sem=one.at[at],
            recv_sem=one.at[at + 1],
            device_id=(sp, y * 2 + 1 - core),
            device_id_type=MESH,
        )


    taps = across(same[0:64, 0:64], stacked([xk_ref[j : j + 1, :].astype(F32) for j in range(CONV)]).astype(BF16))
    lane = lax.broadcasted_iota(jnp.int32, (64, 128), 1)
    body = xpad[...].astype(F32)
    bext[pl.ds(16, T), :] = braw[...].astype(F32)
    cext[pl.ds(16, T), :] = craw[...].astype(F32)
    for k in range(3):
        halo(0, k).wait_recv()
        halo(1, k).wait_recv()
    before, behind = sp > 0, sp < SP - 1
    last = jnp.where(before, pltpu.roll(hx[0].astype(F32), 64, 1), 0.0)
    coming = jnp.where(behind, pltpu.roll(hx[1].astype(F32), 64, 1), 0.0)
    end = jnp.where(
        lane < 64, body[:, 256:384], jnp.where(lane < 66, coming, jnp.where(lane > 125, last, 0.0))
    )
    cells = jnp.concatenate([body[:, 0:256], end], axis=1)
    total = cells * taps[:, 2:3]
    for j in (0, 1, 3, 4):
        total = total + pltpu.roll(cells, (2 - j) % 384, 1) * taps[:, j : j + 1]
    x_conv = silu(total)[:, 0:T].astype(BF16)
    for ext, halos, kernel_ref in ((bext, hb, bk_ref), (cext, hc, ck_ref)):
        ext[pl.ds(0, 16), :] = jnp.where(before, halos[0].astype(F32), 0.0)
        ext[pl.ds(T + 16, 16), :] = jnp.where(behind, halos[1].astype(F32), 0.0)
        total = jnp.zeros((T, 128), F32)
        for j in range(CONV):
            tap = kernel_ref[j : j + 1, at_group].astype(F32)
            total = total + ext[pl.ds(14 + j, T), :] * tap
        mixed[0 if ext is bext else 1] = silu(total).astype(BF16)
    b_conv, c_conv = mixed[0], mixed[1]

    def packed(total, log):
        tail = jnp.concatenate([stacked(three(log)), jnp.zeros((8, 128), F32)], axis=0)
        return total.astype(BF16), tail.astype(BF16)

    x_wide = x_conv.astype(F32)
    for d in range(2):
        scaled = (cv[d : d + 1, :] * x_wide).astype(BF16)
        top, tail = packed(dot(scaled, b_conv), ends[d])
        st_ref[d, 0:64] = top
        st_ref[d, 64:80] = tail
    rx[x] = st_ref[...]
    for k in (2, 1, 3):
        state_row(k, x).start()
    inner = across(x_conv, (across(c_conv, b_conv) * gap[...]).astype(BF16))
    inner = inner + byp_ref[0] * x_wide
    gate = silu(zt_ref[...].astype(F32))

    def all_rows(k):
        return pltpu.make_async_remote_copy(
            src_ref=rx.at[pl.ds(0, k)],
            dst_ref=rx.at[pl.ds(0, k)],
            send_sem=one.at[0],
            recv_sem=one.at[1],
            device_id=(z * NX + (x + 1) % NX, tp),
            device_id_type=MESH,
        )

    all_rows(NX - 1).wait_recv()

    def state(block):
        return block[0:64].astype(F32)

    def log_of(block):
        logs = block[64:80].astype(F32)
        return logs[0:1] + logs[1:2] + logs[2:3]

    for way in (0, 1):
        total, log = jnp.zeros((64, 128), F32), jnp.zeros((1, 128), F32)
        for i in range(NX) if way == 0 else reversed(range(NX)):
            block = rx[i, way]
            own = log_of(block)
            total = jnp.exp(own) * total + state(block)
            log = log + own
        top, tail = packed(total, log)
        tb[way, 0:64] = top
        tb[way, 64:80] = tail
    rz[z] = tb[0]

    def state_column(k, source):
        return pltpu.make_async_remote_copy(
            src_ref=tb.at[(z + k) // NZ],
            dst_ref=rz.at[source],
            send_sem=one.at[2],
            recv_sem=one.at[3],
            device_id=(((z + k) % NZ) * NX + x, tp),
            device_id_type=MESH,
        )

    for k in (4, 3, 5, 2, 6, 1, 7):
        state_column(k, z).start()

    loads[0].wait()
    wide[...] = jnp.zeros(wide.shape, BF16)

    def widen(j, carry):
        block = wb[pl.ds(pl.multiple_of(j * 64, 64), 64), :]
        wide[pl.ds(pl.multiple_of(j * 128, 128), 64), pl.ds(0, 128)] = block
        wide[pl.ds(pl.multiple_of(j * 128 + 64, 64), 64), pl.ds(128, 128)] = block
        return carry

    lax.fori_loop(0, HEADS, widen, 0)

    def all_columns():
        return pltpu.make_async_remote_copy(
            src_ref=rz.at[pl.ds(0, NZ - 1)],
            dst_ref=rz.at[pl.ds(0, NZ - 1)],
            send_sem=one.at[2],
            recv_sem=one.at[3],
            device_id=(((z + 1) % NZ) * NX + x, tp),
            device_id_type=MESH,
        )

    all_columns().wait_recv()

    carried = []
    for way in (0, 1):
        total = jnp.zeros((64, 128), F32)
        for i in range(NZ) if way == 0 else reversed(range(NZ)):
            block = rz[i]
            passed = (i < z) if way == 0 else (i > z)
            total = jnp.where(passed, jnp.exp(log_of(block)) * total + state(block), total)
        for i in range(NX) if way == 0 else reversed(range(NX)):
            block = rx[i, way]
            passed = (i < x) if way == 0 else (i > x)
            total = jnp.where(passed, jnp.exp(log_of(block)) * total + state(block), total)
        carried.append(total.astype(BF16))

    mixer = inner + cv[2:3, :] * across(carried[0], mixed[1]) + cv[3:4, :] * across(carried[1], mixed[1])
    gated = (mixer * gate).astype(BF16)
    none = jnp.zeros((64, T), BF16)
    upper_half = one_hot((HALF, T), lambda row, col: row == col)
    lower_half = one_hot((HALF, T), lambda row, col: row + HALF == col)
    mine = pl.ds(pl.multiple_of(tp * 128, 128), 128)
    bn[:, mine] = (
        across(upper_half, jnp.concatenate([gated, none], axis=0))
        + across(lower_half, jnp.concatenate([none, gated], axis=0))
    ).astype(BF16)

    sems = (rsem, rrecv)
    ring = Ring(bn, 0, HALF, sems, 6 + SPLITS, direct=True)
    ring.start()

    def all_tiles(ref, at):
        return pltpu.make_async_remote_copy(
            src_ref=ref.at[pl.ds(0, TP - 1)],
            dst_ref=ref.at[pl.ds(0, TP - 1)],
            send_sem=one.at[at],
            recv_sem=one.at[at + 1],
            device_id=(sp, (tp + 1) % TP),
            device_id_type=MESH,
        )

    all_tiles(ft, 4).wait_recv()
    for step in (4, 3, 2, 1):
        ring.step(step)
    ring.finish()

    left = lax.broadcasted_iota(jnp.int32, (HALF, 128), 1) < 64
    for g in range(GROUPS):
        squares = jnp.zeros((HALF, 128), F32)
        for j in range(4 * g, 4 * g + 4):
            v = bn[:, 128 * j : 128 * j + 128].astype(F32)
            squares = squares + v * v
        top = jnp.sum(jnp.where(left, squares, 0.0), axis=1, keepdims=True)
        bottom = jnp.sum(jnp.where(left, 0.0, squares), axis=1, keepdims=True)
        scale = lax.rsqrt(jnp.where(left, top, bottom) / (4 * HEAD_DIM) + 1e-06)
        for j in range(4 * g, 4 * g + 4):
            v = bn[:, 128 * j : 128 * j + 128].astype(F32)
            nn[:, 128 * j : 128 * j + 128] = (v * scale * ft[j, 0:1]).astype(BF16)
    projected = dot(nn[...], wide[...])
    am[0:HALF] = (src_ref[0:HALF].astype(F32) + projected[:, 0:128]).astype(BF16)
    am[HALF:T] = (src_ref[HALF:T].astype(F32) + projected[:, 128:256]).astype(BF16)

    own = (am[...].astype(F32) * after_ref[...]).astype(BF16)
    ff[:, mine] = own
    cells = T // SPLITS
    spread_out = [Ring(ff, i * cells, cells, sems, 4 + i) for i in range(SPLITS)]
    for spreading in spread_out:
        spreading.start()
    dd[...] = dot(pp[...], own).astype(BF16)

    def rows_of(i):
        return pl.ds(pl.multiple_of(i * SLOTS, SLOTS), SLOTS)

    local = (x % 2) * 8 + (x // 2) * 4 + z // 2
    landing = pl.ds(pl.multiple_of(local * PIECE, PIECE), PIECE)

    def piece_of(i, q):
        return pl.ds(pl.multiple_of(i * SLOTS + q * PIECE, PIECE), PIECE)

    def deliver(k, q):
        target = (sp + k) % SP
        return pltpu.make_async_remote_copy(
            src_ref=dd.at[piece_of(target, q)],
            dst_ref=xl.at[q, landing, lanes_of(core)],
            send_sem=one.at[8],
            recv_sem=dr.at[q],
            device_id=(target, y * 2 + side_of),
            device_id_type=MESH,
        )

    def deliver_more(k):
        target = (sp + k) % SP
        return pltpu.make_async_remote_copy(
            src_ref=d2.at[rows_of(target)],
            dst_ref=x2.at[rows_of(local), lanes_of(core)],
            send_sem=one.at[9],
            recv_sem=dr.at[CHUNKS],
            device_id=(target, y * 2 + side_of),
            device_id_type=MESH,
        )

    def outward(m):
        return SP // 2 + (m // 2 + m % 2) * (1 - 2 * (m % 2))

    for q in range(CHUNKS):

        def send_rows(m, carry):
            deliver(outward(m), q).start()
            return carry

        lax.fori_loop(0, SP - 1, send_rows, 0)

        @pl.when(side_of != core)
        def _():
            deliver(0, q).start()

    @pl.when(side_of == core)
    def _():
        for q in range(CHUNKS):
            xl[q, landing, lanes_of(core)] = dd[piece_of(sp, q)]

    for k in (4, 5, 6):
        loads[k].wait()
    for part in (wc.at[:, lanes_of(core)], wc.at[:, lanes_of(core + 2)], wcl.at[:, lanes_of(core)]):
        to_other(part, 18).start()

    dims = (((1,), (1,)), ((), ()))
    squares = am[...].astype(F32) * am[...].astype(F32)
    high = squares.astype(BF16)
    rest = (squares - high.astype(F32)).astype(BF16)
    ones = jnp.ones((8, 128), BF16)
    sums = lax.dot_general(ones, high, dims, preferred_element_type=F32) + lax.dot_general(
        ones, rest, dims, preferred_element_type=F32
    )
    line = jnp.concatenate([sums, jnp.zeros((8, 3 * 128 - T), F32)], axis=1)
    level = lax.broadcasted_iota(jnp.int32, (8, 128), 0)
    own = jnp.where(
        level == 0,
        line[:, 0:128],
        jnp.where(level == 1, line[:, 128:256], jnp.where(level == 2, line[:, 256:384], 0.0)),
    )
    sq[tp] = own
    so[...] = own

    def sums_to(k, source):
        return pltpu.make_async_remote_copy(
            src_ref=so,
            dst_ref=sq.at[source],
            send_sem=one.at[6],
            recv_sem=one.at[7],
            device_id=(sp, (tp + k) % TP),
            device_id_type=MESH,
        )

    def send_sums(k, carry):
        sums_to((k + 7) % (TP - 1) + 1, tp).start()
        return carry

    lax.fori_loop(0, TP - 1, send_sums, 0)
    ring.drain()

    def some_rows(ref, first, blocks, sent, received, rows=SLOTS):
        part = ref.at[pl.ds(first, blocks * rows), pl.ds(0, 128)]
        return pltpu.make_async_remote_copy(
            src_ref=part,
            dst_ref=part,
            send_sem=one.at[sent],
            recv_sem=received,
            device_id=((sp + 1) % SP, tp),
            device_id_type=MESH,
        )

    def either(test, less, more):
        @pl.when(test)
        def _():
            less()

        @pl.when(jnp.logical_not(test))
        def _():
            more()

    for step in (1, 2):
        for ring in spread_out:
            ring.step(step)
    chip = pl.ds(pl.multiple_of(y * 256, 256), 256)
    used = [PIECE, CAP - PIECE]
    sources = SP // 2
    spans = [pl.ds(0, sources * used[0]), pl.ds(sources * used[0], sources * used[1])]
    dense = [
        one_hot(
            (sources * used[q], sources * SLOTS),
            lambda row, col: row // used[q] * SLOTS + row % used[q] + q * PIECE == col,
        )
        for q in range(CHUNKS)
    ]
    squeeze = one_hot(
        (sources * used[1], sources * PIECE),
        lambda row, col: row // used[1] * PIECE + row % used[1] == col,
    )
    gathers = []

    def gather(q):
        either(
            side_of == core,
            lambda: some_rows(dd, 0, SP - 1, 8, dr.at[q], PIECE).wait_recv(),
            lambda: some_rows(dd, 0, SP, 8, dr.at[q], PIECE).wait_recv(),
        )
        if used[q] == PIECE:
            xx[spans[q], chip] = xl[q]
        else:
            xx[spans[q], chip] = dot(squeeze, xl[q]).astype(BF16)
        ring = Ring(xx, sources * used[0] * q, sources * used[q], sems, q, pair=True, last=3)
        ring.start()
        gathers.append(ring)

    gather(0)
    all_tiles(sq, 6).wait_recv()
    total = sq[0]
    for j in range(1, TP):
        total = total + sq[j]
    line = jnp.concatenate([total[0:1], total[1:2], total[2:3]], axis=1)
    parts = stacked(three(line)).astype(BF16)
    same = one_hot((T, 384), lambda row, col: row == col)
    upright = across(same, parts)
    scale = lax.rsqrt((upright[:, 0:1] + upright[:, 1:2] + upright[:, 2:3]) / D + 1e-06)
    lane = lax.broadcasted_iota(jnp.int32, (T, 128), 1)
    parts = jnp.zeros((T, 128), F32)
    for k, part in enumerate(three(scale)):
        parts = jnp.where(lane == k, part, parts)
    ss[...] = dot(pp[...], parts.astype(BF16)).astype(BF16)

    def send_scale(m, carry):
        target = (sp + outward(m)) % SP
        pltpu.make_async_remote_copy(
            src_ref=ss.at[rows_of(target)],
            dst_ref=sl.at[rows_of(local)],
            send_sem=one.at[14],
            recv_sem=one.at[15],
            device_id=(target, tp),
            device_id_type=MESH,
        ).start()
        return carry

    @pl.when(side_of == core)
    def _():
        lax.fori_loop(0, SP - 1, send_scale, 0)
        sl[rows_of(local), :] = ss[rows_of(sp), :]

    for ring in spread_out:
        ring.step(3)
    gather(1)
    for k in (1, 2, 3):
        loads[k].wait()
    for part in (wx.at[:, lanes_of(core)], wx.at[:, lanes_of(core + 2)], wl.at[:, lanes_of(core)]):
        to_other(part, 12).start()
    gathers[0].step(1)
    for ring in spread_out:
        ring.step(4)

    opposite = (y + NY // 2) % NY
    d2[...] = dot(pp[...], ff[:, lanes_of(opposite * 2 + core)]).astype(BF16)

    def send_more(m, carry):
        deliver_more(outward(m)).start()
        return carry

    lax.fori_loop(0, SP - 1, send_more, 0)

    @pl.when(side_of == core)
    def _():
        x2[rows_of(local), lanes_of(core)] = d2[rows_of(sp)]

    @pl.when(side_of != core)
    def _():
        deliver_more(0).start()

    gathers[1].step(1)
    for ring in spread_out:
        ring.finish()
    to_other(wc.at[:, pl.ds(0, 384)], 18).wait_recv()
    rows = pl.ds(pl.multiple_of(core * HALF, 16), HALF)
    both = dot(ff[rows, :], wc[...]) * jnp.where(core == 0, scale[0:HALF], scale[HALF:T])
    sh[rows, chip] = (jax.nn.silu(both[:, 0:256]) * both[:, 256:512]).astype(BF16)
    shared_out = [
        Ring(sh, pl.multiple_of(core * HALF + first, 16), count, sems, 4 + SPLITS + i, pair=True)
        for i, (first, count) in enumerate(((0, 96), (96, 64)))
    ]
    for ring in shared_out:
        ring.start()
    for ring in gathers:
        ring.step(2)

    def chips(first, count, total, buf, at, weight):
        def add(k, carry):
            part = pl.ds(pl.multiple_of((y + k) % NY * 256, 256), 256)
            total[at, :] += dot(buf[at, part], weight[part, :])
            return carry

        lax.fori_loop(first, first + count, add, 0)

    either(
        side_of == core,
        lambda: some_rows(sl, 0, SP // 2 - 1, 14, one.at[15]).wait_recv(),
        lambda: some_rows(sl, 0, SP // 2, 14, one.at[15]).wait_recv(),
    )
    to_other(wx.at[:, pl.ds(0, 384)], 12).wait_recv()
    tot[...] = jnp.zeros(tot.shape, F32)
    levels = []
    for q in range(CHUNKS):
        chips(NY - 2, NY - 3, tot, xx, spans[q], wx)
    either(
        side_of == core,
        lambda: some_rows(d2, 0, SP - 1, 9, dr.at[CHUNKS]).wait_recv(),
        lambda: some_rows(d2, 0, SP, 9, dr.at[CHUNKS]).wait_recv(),
    )
    turned = pl.ds(pl.multiple_of(opposite * 256, 256), 256)
    for q in range(CHUNKS):
        at = spans[q]
        xx[at, turned] = dot(dense[q], x2[...]).astype(BF16)
        chips(NY // 2, 1, tot, xx, at, wx)
        level = dot(dense[q], sl[...])
        levels.append(level[:, 0:1] + level[:, 1:2] + level[:, 2:3])
    hiddens = []
    for q in range(CHUNKS):
        gathers[q].step(3)
        if q == CHUNKS - 1:
            for ring in shared_out:
                ring.step(1)
        at = spans[q]
        chips(3, 1, tot, xx, at, wx)
        chips(NY - 3, 1, tot, xx, at, wx)
        both = tot[at, :] * levels[q]
        hh[at, chip] = (jax.nn.silu(both[:, 0:256]) * both[:, 256:512]).astype(BF16)
        hiddens.append(Ring(hh, sources * used[0] * q, sources * used[q], sems, 2 + q, pair=True))
        hiddens[-1].start()
    for side in range(2):
        for k in range(3):
            halo(side, k).wait_send()
    all_rows(NX - 1).wait_send()
    all_columns().wait_send()
    all_tiles(ft, 4).wait_send()
    all_tiles(sq, 6).wait_send()
    for sent in (8, 9):
        either(
            side_of == core,
            lambda: some_rows(dd, 0, SP - 1, sent, one.at[20]).wait_send(),
            lambda: some_rows(dd, 0, SP, sent, one.at[20]).wait_send(),
        )

    @pl.when(side_of == core)
    def _():
        some_rows(dd, 0, SP - 1, 14, one.at[20]).wait_send()

    to_other(wx.at[:, pl.ds(0, 384)], 12).wait_send()
    to_other(wc.at[:, pl.ds(0, 384)], 18).wait_send()
    for ring in spread_out + gathers:
        ring.drain()
    low[...] = jnp.zeros(low.shape, F32)
    for step in (1, 2, 3):
        for ring in hiddens:
            ring.step(step)
        if step == 3:
            for ring in shared_out:
                ring.step(2)
        for q in range(CHUNKS):
            at = spans[q]
            if step == 1:
                chips(NY, 1, low, hh, at, wl)
            chips(step, 1, low, hh, at, wl)
            chips(NY - step, 1, low, hh, at, wl)
    loose = [
        one_hot(
            (sources * PIECE, sources * used[q]),
            lambda row, col: col // used[q] * PIECE + col % used[q] == row,
        )
        for q in range(CHUNKS)
    ]

    def give(i, to_core, q):
        return pltpu.make_async_remote_copy(
            src_ref=oo.at[q, pl.ds(pl.multiple_of(i * PIECE, PIECE), PIECE), lanes_of(to_core)],
            dst_ref=ret.at[piece_of(sp, q)],
            send_sem=one.at[10],
            recv_sem=one.at[11],
            device_id=(((i % 4) * 2 + core) * NX + i // 4 % 2 * 2 + i // 8, y * 2 + to_core),
            device_id_type=MESH,
        )

    for q in range(CHUNKS):
        hiddens[q].step(4)
        at = spans[q]
        chips(NY // 2, 1, low, hh, at, wl)
        oo[q] = dot(loose[q], low[at, :].astype(BF16)).astype(BF16)

        def send_back(k, carry):
            turn = k // 4
            i = k % 4 * 4 + (z // 2 + 6 + (turn // 2 + turn % 2) * (1 - 2 * (turn % 2))) % 4
            here = jnp.logical_and(side_of == core, i == local)

            @pl.when(jnp.logical_not(here))
            def _():
                give(i, core, q).start()

            give(i, 1 - core, q).start()
            return carry

        lax.fori_loop(0, sources, send_back, 0)

    @pl.when(side_of == core)
    def _():
        for q in range(CHUNKS):
            ret[piece_of(sp, q), :] = oo[q, landing, lanes_of(core)]

    for step in (3, 4):
        for ring in shared_out:
            ring.step(step)
    lowered = dot(sh[rows, :], wcl[...]).astype(BF16)
    outs[0] = lowered[:, 0:128]
    outs[1] = lowered[:, 128:256]

    def output(source):
        return pltpu.make_async_remote_copy(
            src_ref=outs.at[source],
            dst_ref=theirs,
            send_sem=one.at[16],
            recv_sem=one.at[17],
            device_id=(sp, y * 2 + 1 - core),
            device_id_type=MESH,
        )

    output(1 - core).start()
    for ring in hiddens + shared_out:
        ring.drain()
    either(
        side_of == core,
        lambda: some_rows(ret, 0, SP - 1, 10, one.at[11]).wait_recv(),
        lambda: some_rows(ret, 0, SP, 10, one.at[11]).wait_recv(),
    )
    either(
        side_of == core,
        lambda: some_rows(ret, 0, SP - 1, 10, one.at[11]).wait_send(),
        lambda: some_rows(ret, 0, SP, 10, one.at[11]).wait_send(),
    )
    routed = dot(qhi[...], ret[...]) + dot(qlo[...], ret[...])
    output(1 - core).wait()
    ours, others = outs[core].astype(F32), theirs[...].astype(F32)
    shared = jnp.concatenate(
        [jnp.where(core == 0, ours, others), jnp.where(core == 0, others, ours)], axis=0
    )
    out_ref[...] = (am[...].astype(F32) + shared + routed).astype(BF16)


def whole(*operands):
    vmem = pl.BlockSpec(memory_space=pltpu.VMEM)
    hbm = pl.BlockSpec(memory_space=pl.ANY)
    rings = 7 + SPLITS
    dma = pltpu.SemaphoreType.DMA

    def space(*shape, kind=BF16):
        return pltpu.VMEM(shape, kind)

    return pl.pallas_call(
        kernel,
        out_shape=jax.ShapeDtypeStruct((T, 128), BF16),
        in_specs=[hbm] * 24,
        out_specs=vmem,
        scratch_shapes=[
            (pltpu.VMEM if o.ndim > 1 else pltpu.SMEM)(o.shape, o.dtype) for o in operands[:15]
        ]
        + [
            space(64, 384),
            space(T, 128),
            space(T, 128),
            space(2, 64, 128),
            space(2, 16, 128),
            space(2, 16, 128),
            space(T + 32, 128, kind=F32),
            space(T + 32, 128, kind=F32),
            space(T, T, kind=F32),
            space(8, T, kind=F32),
            space(2, T, 128),
            space(8, 128, kind=F32),
            space(2, BLOCK, 128),
            space(NX, 2, BLOCK, 128),
            space(2, BLOCK, 128),
            space(NZ, BLOCK, 128),
            space(TP, 8, 128, kind=F32),
            space(TP, 8, 128, kind=F32),
            space(8, 128, kind=F32),
            space(1024, 128),
            space(D, 512),
            space(D, 512),
            space(D, 256),
            space(D, 256),
            space(D, 256),
            space(HALF, D),
            space(HALF, D),
            space(T, 128),
            space(T, D),
            space(T, D),
            space(2, ROWS // 4, 256),
            space(ROWS // 2, 256),
            space(SP // 2 * CAP, D),
            space(SP // 2 * CAP, D),
            space(SP // 2 * CAP, 512, kind=F32),
            space(SP // 2 * CAP, 256, kind=F32),
            space(ROWS, 128),
            space(ROWS, 128),
            space(ROWS, 128),
            space(ROWS // 2, 128),
            space(2, HALF, 128),
            space(HALF, 128),
            space(2, ROWS // 4, 256),
            space(ROWS, 128),
            space(ROWS, T),
            space(T, ROWS),
            space(T, ROWS),
            dma((15,)), dma((9,)), dma((6,)), dma((6,)), dma((21,)), dma((CHUNKS + 1,)), dma((rings, 2)), dma((rings, 8)),
        ],
        compiler_params=pltpu.CompilerParams(collective_id=0, has_side_effects=True),
        name="mixer_experts",
    )(*operands)


def shards(
    layer_source_vector,
    attention_lane_source,
    result_valve_logits,
    memory_write_matrix,
    memory_query_matrix,
    increment_logits,
    increment_offset,
    log_fade_speed,
    extra_log_fade,
    attention_bypass_factor,
    attention_lane_kernel,
    memory_write_kernel,
    memory_query_kernel,
    cluster_rescale_factor,
    blender_result_matrix,
    specialist_rescale_factor,
    chosen_specialists,
    specialist_shares,
    specialist_valve_matrix,
    specialist_raising_matrix,
    specialist_lowering_matrix,
    common_valve_matrix,
    common_raising_matrix,
    common_lowering_matrix,
):
    return whole(
        attention_lane_source.T,
        result_valve_logits.T,
        increment_logits.reshape(2, T),
        increment_offset.T,
        log_fade_speed.T,
        extra_log_fade.reshape(2, 1, T),
        attention_bypass_factor,
        attention_lane_kernel,
        memory_write_kernel,
        memory_query_kernel,
        cluster_rescale_factor.reshape(1, 64),
        specialist_rescale_factor.reshape(1, 128),
        layer_source_vector,
        chosen_specialists.T,
        specialist_shares.T,
        memory_write_matrix,
        memory_query_matrix,
        blender_result_matrix,
        specialist_valve_matrix,
        specialist_raising_matrix,
        specialist_lowering_matrix,
        common_valve_matrix,
        common_raising_matrix,
        common_lowering_matrix,
    )


def solution(mesh):
    return jax.shard_map(
        shards,
        mesh=mesh,
        in_specs=(
            P("sp", "tp"),
            P("sp", "tp"),
            P("sp", "tp"),
            P("sp", None),
            P("sp", None),
            P(None, "sp", "tp"),
            P(None, "tp"),
            P(None, "tp"),
            P(None, "sp", "tp"),
            P("tp"),
            P(None, "tp"),
            P(),
            P(),
            P("tp"),
            P(None, "tp"),
            P("tp"),
            P("sp", None),
            P("sp", None),
            P("sp", None, "tp"),
            P("sp", None, "tp"),
            P("sp", None, "tp"),
            P(None, "tp"),
            P(None, "tp"),
            P(None, "tp"),
        ),
        out_specs=P("sp", "tp"),
        check_vma=False,
    )
```
